32 devices in a mesh: ep: 8 (over z, x), tp: 4 (over y, core).
Axes of the slice: x: 2, y: 2, z: 4, core: 2. Of those that a mesh axis runs over, the one named last changes fastest.
Arguments:
- residual_in: bfloat16 [128, 2048], P('ep'), may hold values from -6 to 6
- lengths: int32 [128], P('ep'), may hold values from 1 to 511, as said below
- kv_cache: bfloat16 [128, 4, 512, 256], P('ep', 'tp'), may hold values from -640 to 640
- norm_gain_attn: float32 [2048], replicated, may hold values from 0.1 to 1.9
- query_weight: bfloat16 [2048, 2048], P(None, 'tp'), may hold values from -0.125 to 0.125
- key_weight: bfloat16 [2048, 512], P(None, 'tp'), may hold values from -0.125 to 0.125
- value_weight: bfloat16 [2048, 512], P(None, 'tp'), may hold values from -0.125 to 0.125
- diff_lambda: float32 [16], P('tp'), may hold values from 0.3 to 0.8
- head_gain: float32 [128], replicated, may hold values from 0.1 to 1.9
- out_weight: bfloat16 [2048, 2048], P(None, 'tp'), may hold values from -0.125 to 0.125
- norm_gain_ffn: float32 [2048], replicated, may hold values from 0.1 to 1.9
- route_ids: int32 [128, 2], P('ep'), may hold values from 0 to 7, as said below
- route_weights: float32 [128, 2], P('ep'), may hold values from 0.1 to 1
- expert_gate: bfloat16 [8, 2048, 512], P('ep', None, 'tp'), may hold values from -0.125 to 0.125
- expert_up: bfloat16 [8, 2048, 512], P('ep', None, 'tp'), may hold values from -0.125 to 0.125
- expert_down: bfloat16 [8, 512, 2048], P('ep', 'tp'), may hold values from -0.25 to 0.25
- dense_gate: bfloat16 [2048, 8192], P(None, 'ep'), may hold values from -0.125 to 0.125
- dense_up: bfloat16 [2048, 8192], P(None, 'ep'), may hold values from -0.125 to 0.125
- dense_down: bfloat16 [8192, 2048], P('ep'), may hold values from -0.0625 to 0.0625
- dense_mix: float32 [2048], replicated, may hold values from -0.125 to 0.125
Outputs:
- layer_out: bfloat16 [128, 2048], P('ep', 'tp')
- new_rows: bfloat16 [128, 4, 256], P('ep', 'tp')
The draws below stay inside these ranges and needn't reach their ends.
Inputs may be any that keep to these rules, and one draw needn't show every extreme that they name: The new token stands at position lengths[b]; some sequence holds 511 positions in every draw. `route_ids`: each row names 2 different experts from one group; the groups are the 4 runs of consecutive expert numbers of equal size. Among the rows of one index of ep no expert is named more than 8 times, and some expert exactly 8 times.
All inputs are finite; a program needn't handle non-finite values.
Results may differ from the reference program's by a relative error of at most 0.008.
The reference program's roundings to bfloat16 on the way count: a program that leaves them out, or rounds other values in their place, can miss the bound.
Values may be sent and summed in bfloat16 or wider, within the bound.
A program may use at most 64 MiB of HBM per device.

```python
import math
import jax
import jax.numpy as jnp
from jax import lax

D = 2048
HEADS = 16
KV_HEADS = 4
QK_DIM = 64
HEAD_DIM = 128
KV_WIDTH = 256
SEQ_DEV = 16
CACHE = 512
TOKENS = 128
EXPERTS = 8
GROUPS = 4
TOPK = 2
EXP_FF = 512
DENSE_FF = 8192
CAP = 8
N_EP = 8
N_TP = 4


def draw_lengths(key, part):
    raw = jax.random.randint(jax.random.fold_in(key, 21), (TOKENS,), 0, CACHE - 1)
    factor = jax.random.randint(jax.random.fold_in(key, 22), (TOKENS // SEQ_DEV, 1), 1, 9)
    spread = jnp.broadcast_to(factor, (TOKENS // SEQ_DEV, SEQ_DEV)).reshape(TOKENS)
    counts = 1 + raw * spread // 8
    longest = jax.random.randint(jax.random.fold_in(key, 23), (), 0, TOKENS)
    return jnp.where(jnp.arange(TOKENS, dtype=jnp.int32) == longest, CACHE - 1, counts).astype(jnp.int32)


def draw_kv_cache(key, part):
    base = jnp.clip(jax.random.normal(key, (TOKENS, KV_HEADS, CACHE, KV_WIDTH), jnp.float32), -6.0, 6.0)
    lane = lax.broadcasted_iota(jnp.int32, (1, 1, 1, KV_WIDTH), 3)
    level = jnp.ones((TOKENS, KV_HEADS, 1, 1), jnp.float32)
    factor = jnp.where(lane < 2 * QK_DIM, 1.75 * level, 1.0)
    return (base * factor).astype(jnp.bfloat16)


def draw_route_ids(key, part):
    blocks = TOKENS // SEQ_DEV
    per_group = EXPERTS // GROUPS
    busy_rows = CAP * per_group // TOPK
    busy = jax.random.randint(jax.random.fold_in(key, 41), (blocks, 1), 0, GROUPS)
    other = (busy + jax.random.randint(jax.random.fold_in(key, 42), (blocks, SEQ_DEV), 1, GROUPS)) % GROUPS
    place = lax.broadcasted_iota(jnp.int32, (blocks, SEQ_DEV), 1)
    ordered = jnp.where(place < busy_rows, busy, other)
    scores = jax.random.randint(jax.random.fold_in(key, 43), (blocks, SEQ_DEV), 0, 1 << 20) * SEQ_DEV + place
    order = jnp.argsort(scores, axis=1)
    group = jnp.take_along_axis(ordered, order, axis=1)
    member = (group[:, :, None] == jnp.arange(GROUPS, dtype=jnp.int32)[None, None, :]).astype(jnp.int32)
    rank = jnp.sum((jnp.cumsum(member, axis=1) - member) * member, axis=2)
    shift = TOPK * jax.random.randint(jax.random.fold_in(key, 44), (blocks, GROUPS), 0, per_group // TOPK)
    offset = jnp.take_along_axis(shift, group, axis=1)
    first = TOPK * rank + offset
    picks = [group * per_group + (first + step) % per_group for step in range(TOPK)]
    return jnp.stack(picks, axis=-1).reshape(TOKENS, TOPK).astype(jnp.int32)


def level_of(key, shape, shards, low, largest):
    def one(position, shards_of):
        steps = jax.random.uniform(jax.random.fold_in(jax.random.fold_in(key, 6), position), (shards_of,), jnp.float32, low / len(shards), largest / len(shards))
        return jnp.repeat(jnp.exp(steps), shape[position] // shards_of).reshape((-1,) + (1,) * (len(shape) - position - 1))

    level = one(*shards[0])
    for cut in shards[1:]:
        level = level * one(*cut)
    return level


def scatter_about(own_key, dims, scale, most, split=(), kind=jnp.bfloat16):
    level = level_of(own_key, dims, split, -0.22, 0.18) if split else 1.0
    array = jax.random.normal(own_key, dims, jnp.float32) * scale * level
    return jnp.minimum(jnp.maximum(array, -most), most).astype(kind)


def setup_inputs(seed: int = 0) -> dict:
    seeds = jax.random.split(jax.random.key(seed), 21)
    return {
        "residual_in": scatter_about(seeds[0], (TOKENS, D), 1.0, 6.0, ((0, 8),)),
        "lengths": draw_lengths(jax.random.fold_in(seeds[20], 71), 0),
        "kv_cache": draw_kv_cache(jax.random.fold_in(seeds[20], 71), 0),
        "norm_gain_attn": jnp.clip(1.0 + 0.18 * jax.random.normal(seeds[3], (D,), jnp.float32), 0.1, 1.9),
        "query_weight": scatter_about(seeds[4], (D, HEADS * 2 * QK_DIM), D ** -0.5, 0.125, ((1, 4),)),
        "key_weight": scatter_about(seeds[5], (D, KV_HEADS * 2 * QK_DIM), D ** -0.5, 0.125, ((1, 4),)),
        "value_weight": scatter_about(seeds[6], (D, KV_HEADS * HEAD_DIM), D ** -0.5, 0.125, ((1, 4),)),
        "diff_lambda": jnp.clip(0.3 + 0.5 * jax.random.uniform(seeds[7], (HEADS,), jnp.float32) ** level_of(seeds[7], (HEADS,), ((0, 4),), -0.2, 0.2), 0.3, 0.8),
        "head_gain": jnp.clip(1.0 + 0.18 * jax.random.normal(seeds[8], (HEAD_DIM,), jnp.float32), 0.1, 1.9),
        "out_weight": scatter_about(seeds[9], (HEADS * HEAD_DIM, D), (HEADS * HEAD_DIM) ** -0.5, 0.125, ((1, 4),)),
        "norm_gain_ffn": jnp.clip(1.0 + 0.18 * jax.random.normal(seeds[10], (D,), jnp.float32), 0.1, 1.9),
        "route_ids": draw_route_ids(jax.random.fold_in(seeds[20], 71), 0),
        "route_weights": jnp.clip(jnp.exp(math.log(1.0) - 2.3025851 * jax.random.uniform(seeds[12], (TOKENS, TOPK), jnp.float32) ** level_of(seeds[12], (TOKENS, TOPK), ((0, 8),), -0.2, 0.2)), 0.1, 1.0),
        "expert_gate": scatter_about(seeds[13], (EXPERTS, D, EXP_FF), D ** -0.5, 0.125, ((0, 8), (2, 4))),
        "expert_up": scatter_about(seeds[14], (EXPERTS, D, EXP_FF), D ** -0.5, 0.125, ((0, 8), (2, 4))),
        "expert_down": scatter_about(seeds[15], (EXPERTS, EXP_FF, D), EXP_FF ** -0.5, 0.25, ((0, 8), (1, 4))),
        "dense_gate": scatter_about(seeds[16], (D, DENSE_FF), D ** -0.5, 0.125, ((1, 8),)),
        "dense_up": scatter_about(seeds[17], (D, DENSE_FF), D ** -0.5, 0.125, ((1, 8),)),
        "dense_down": scatter_about(seeds[18], (DENSE_FF, D), DENSE_FF ** -0.5, 0.0625, ((0, 8),)),
        "dense_mix": scatter_about(seeds[19], (D,), D ** -0.5, 0.125, (), jnp.float32),
    }


EPS = 1e-06

def rms_rows(values, gain):
    mean_sq = lax.optimization_barrier(jnp.mean(values * values, axis=-1, keepdims=True))
    return values * lax.rsqrt(mean_sq + EPS) * gain

def rotate(vectors, positions):
    half = vectors.shape[-1] // 2
    inverse = 10000.0 ** (-jnp.arange(half, dtype=jnp.float32) / half)
    angle = positions[:, None, None, None] * inverse
    cosine = jnp.cos(angle)
    sine = jnp.sin(angle)
    first = vectors[..., :half]
    second = vectors[..., half:]
    return jnp.concatenate([first * cosine - second * sine, first * sine + second * cosine], axis=-1)

def normalize(scores, latest, valid):
    masked = jnp.where(valid, scores, -jnp.inf)
    top = jnp.maximum(lax.optimization_barrier(jnp.max(masked, axis=-1)), latest)
    raised = jnp.where(valid, jnp.exp(jnp.where(valid, scores, 0.0) - top[..., None]), 0.0)
    raised_new = jnp.exp(latest - top)
    total = lax.optimization_barrier(jnp.sum(raised, axis=-1)) + raised_new
    return (raised / total[..., None], raised_new / total)

def attend(query, fresh, cache, lengths, lam):
    count = fresh.shape[0]
    groups = fresh.shape[1]
    share = query.shape[1] // groups
    scale = QK_DIM ** (-0.5)
    grouped = query.astype(jnp.float32).reshape(count, groups, share, 2, QK_DIM)
    latest = fresh.astype(jnp.float32)
    stored = cache.astype(jnp.float32)
    first = jnp.einsum('bgjd,bgkd->bgjk', grouped[:, :, :, 0], stored[..., :QK_DIM]) * scale
    second = jnp.einsum('bgjd,bgkd->bgjk', grouped[:, :, :, 1], stored[..., QK_DIM:2 * QK_DIM]) * scale
    first_new = jnp.einsum('bgjd,bgd->bgj', grouped[:, :, :, 0], latest[..., :QK_DIM]) * scale
    second_new = jnp.einsum('bgjd,bgd->bgj', grouped[:, :, :, 1], latest[..., QK_DIM:2 * QK_DIM]) * scale
    valid = jnp.arange(cache.shape[2], dtype=jnp.int32)[None, None, None, :] < lengths[:, None, None, None]
    prob_one, prob_one_new = normalize(first, first_new, valid)
    prob_two, prob_two_new = normalize(second, second_new, valid)
    weight = lam.reshape(groups, share)[None, :, :, None]
    mapped = (prob_one - weight * prob_two).astype(jnp.bfloat16)
    mapped_new = (prob_one_new - weight[..., 0] * prob_two_new).astype(jnp.bfloat16)
    output = jnp.einsum('bgjk,bgkd->bgjd', mapped.astype(jnp.float32), stored[..., 2 * QK_DIM:])
    output = output + mapped_new.astype(jnp.float32)[..., None] * latest[:, :, None, 2 * QK_DIM:]
    return output.reshape(count, groups * share, HEAD_DIM)

def reference(residual_in, lengths, kv_cache, norm_gain_attn, query_weight, key_weight, value_weight, diff_lambda, head_gain, out_weight, norm_gain_ffn, route_ids, route_weights, expert_gate, expert_up, expert_down, dense_gate, dense_up, dense_down, dense_mix):
    blocks = TOKENS // SEQ_DEV
    resid = residual_in.astype(jnp.float32)
    normed = rms_rows(resid, norm_gain_attn).astype(jnp.bfloat16)
    positions = lengths.astype(jnp.float32)
    query = jnp.dot(normed, query_weight, preferred_element_type=jnp.float32).reshape(TOKENS, HEADS, 2, QK_DIM)
    query = rotate(query, positions).astype(jnp.bfloat16)
    keys = jnp.dot(normed, key_weight, preferred_element_type=jnp.float32).reshape(TOKENS, KV_HEADS, 2, QK_DIM)
    keys = rotate(keys, positions).astype(jnp.bfloat16).reshape(TOKENS, KV_HEADS, 2 * QK_DIM)
    values = jnp.dot(normed, value_weight, preferred_element_type=jnp.float32).reshape(TOKENS, KV_HEADS, HEAD_DIM).astype(jnp.bfloat16)
    fresh = jnp.concatenate([keys, values], axis=-1)

    def per_block(items):
        return attend(items[0], items[1], items[2], items[3], diff_lambda)
    mixed = lax.map(per_block, (query.reshape(blocks, SEQ_DEV, HEADS, 2, QK_DIM), fresh.reshape(blocks, SEQ_DEV, KV_HEADS, KV_WIDTH), kv_cache.reshape(blocks, SEQ_DEV, KV_HEADS, CACHE, KV_WIDTH), lengths.reshape(blocks, SEQ_DEV)))
    mixed = mixed.reshape(TOKENS, HEADS, HEAD_DIM)
    heads_out = rms_rows(mixed, head_gain).astype(jnp.bfloat16).reshape(TOKENS, HEADS * HEAD_DIM)
    stream = (resid + jnp.dot(heads_out, out_weight, preferred_element_type=jnp.float32)).astype(jnp.bfloat16)
    ffn_in = rms_rows(stream.astype(jnp.float32), norm_gain_ffn).astype(jnp.bfloat16)
    flat_ids = route_ids.reshape(blocks, SEQ_DEV * TOPK)
    member = (flat_ids[..., None] == jnp.arange(EXPERTS, dtype=jnp.int32)[None, None, :]).astype(jnp.int32)
    slot = lax.optimization_barrier(jnp.sum((jnp.cumsum(member, axis=1) - member) * member, axis=2))
    block_of = lax.broadcasted_iota(jnp.int32, (blocks, SEQ_DEV * TOPK), 0)
    place = (flat_ids * N_EP + block_of) * CAP + slot
    owner = block_of * SEQ_DEV + lax.broadcasted_iota(jnp.int32, (blocks, SEQ_DEV * TOPK), 1) // TOPK
    table = jnp.zeros((EXPERTS * N_EP * CAP,), jnp.int32).at[place.reshape(-1)].set(owner.reshape(-1))
    quarter = EXP_FF // N_TP

    def expert_rows(items):
        index, w_gate, w_up, w_down = items
        chosen = ffn_in[index]
        gate = jnp.dot(chosen, w_gate, preferred_element_type=jnp.float32)
        upward = jnp.dot(chosen, w_up, preferred_element_type=jnp.float32)
        hidden = (jax.nn.silu(gate) * upward).astype(jnp.bfloat16)
        total = jnp.zeros((chosen.shape[0], D), jnp.float32)
        for part in range(N_TP):
            piece = jnp.dot(hidden[:, part * quarter:(part + 1) * quarter], w_down[part * quarter:(part + 1) * quarter], preferred_element_type=jnp.float32).astype(jnp.bfloat16)
            total = total + lax.optimization_barrier(piece).astype(jnp.float32)
        return total.astype(jnp.bfloat16)
    results = lax.map(expert_rows, (table.reshape(EXPERTS, N_EP * CAP), expert_gate, expert_up, expert_down))
    flat_results = results.reshape(EXPERTS * N_EP * CAP, D)
    picked = flat_results[place.reshape(TOKENS, TOPK)]
    moe = lax.optimization_barrier(jnp.sum(route_weights[..., None] * picked.astype(jnp.float32), axis=1))
    dense_g = jnp.dot(ffn_in, dense_gate, preferred_element_type=jnp.float32)
    dense_u = jnp.dot(ffn_in, dense_up, preferred_element_type=jnp.float32)
    dense_hidden = (jax.nn.silu(dense_g) * dense_u).astype(jnp.bfloat16)
    dense = jnp.dot(dense_hidden, dense_down, preferred_element_type=jnp.float32)
    mix = jax.nn.sigmoid(lax.optimization_barrier(jnp.sum(ffn_in.astype(jnp.float32) * dense_mix, axis=-1)))
    layer_out = (stream.astype(jnp.float32) + moe + mix[:, None] * dense).astype(jnp.bfloat16)
    return (layer_out, fresh)
```

```python
import functools
import math

import jax
import jax.numpy as jnp
from jax import lax
from jax.experimental import pallas as pl
from jax.experimental.pallas import tpu as pltpu
from jax.sharding import PartitionSpec as P

QK_DIM = 64
EPS = 1e-06
MESH = pl.DeviceIdType.MESH
F32 = jnp.float32
BF16 = jnp.bfloat16
LANES = 128
Q_CHUNKS = 4
INNER = 2
CORES = 2


def flip(value, mask):
    bit = 1
    while bit <= mask:
        if mask & bit:
            value = value + bit * (1 - 2 * ((value // bit) % 2))
        bit *= 2
    return value


def each(count, body, order=None):
    if count <= 16:
        for index in order if order is not None else range(count):
            body(index)
    else:

        def step(index, carry):
            body(index)
            return carry

        lax.fori_loop(0, count, step, 0)


def block(start, size):
    return pl.ds(pl.multiple_of(start * size, size), size)


def remote(source, target, send, recv, where):
    return pltpu.make_async_remote_copy(
        src_ref=source,
        dst_ref=target,
        send_sem=send,
        recv_sem=recv,
        device_id=where,
        device_id_type=MESH,
    )


def dot(left, right):
    return jnp.dot(left, right, preferred_element_type=F32)


def column(row):
    count = row.shape[1]
    square = (count, count)
    same = lax.broadcasted_iota(jnp.int32, square, 0) == lax.broadcasted_iota(jnp.int32, square, 1)
    return jnp.sum(jnp.where(same, row, jnp.zeros_like(row)), axis=1, keepdims=True)


def layer_kernel(
    n_ep,
    n_tp,
    split,
    lengths_ref,
    lam_ref,
    resid_ref,
    first_gain_ref,
    head_gain_ref,
    gain_ref,
    mixw_ref,
    ids_ref,
    rw_ref,
    qw_hbm,
    kw_hbm,
    vw_hbm,
    cache_hbm,
    ow_hbm,
    eg_hbm,
    eu_hbm,
    ed_hbm,
    dg_hbm,
    du_hbm,
    dd_hbm,
    out_ref,
    new_ref,
    qw,
    kw,
    vw,
    cache,
    pairs,
    scores,
    mixed,
    heads_ref,
    ow,
    eg,
    eu,
    ed,
    dg,
    du,
    dd,
    heads_all,
    stream,
    ffn,
    mix,
    route,
    eh,
    dh,
    away,
    came,
    summed,
    landed,
    w_sem,
    q_sem,
    cache_sem,
    route_send,
    route_recv,
    heads_send,
    heads_recv,
    first_send,
    second_send,
    relay_send,
    stream_recv,
    pair_send,
    pair_recv,
    back_send,
    back_recv,
):
    e = lax.axis_index("ep")
    t = lax.axis_index("tp")
    half = n_tp // 2
    mate = flip(t, 1)
    core = t % 2
    seqs, width = resid_ref.shape
    quarter = out_ref.shape[1]
    held, _, part = eg.shape
    hid = dg.shape[1]
    rows_all = n_ep * seqs
    evens = [2 * i for i in range(1, half)]

    depth = qw.shape[0] // Q_CHUNKS
    q_loads = [
        pltpu.make_async_copy(
            qw_hbm.at[pl.ds(i * depth, depth), :], qw.at[pl.ds(i * depth, depth), :], q_sem.at[i]
        )
        for i in range(Q_CHUNKS)
    ] + [
        pltpu.make_async_copy(kw_hbm, kw, q_sem.at[Q_CHUNKS]),
        pltpu.make_async_copy(vw_hbm, vw, q_sem.at[Q_CHUNKS + 1]),
    ]
    for load in q_loads:
        load.start()
    cache_loads = [
        pltpu.make_async_copy(cache_hbm.at[s], cache.at[s], cache_sem.at[s]) for s in range(seqs)
    ]
    for load in cache_loads:
        load.start()

    barrier = pltpu.get_barrier_semaphore()

    def greet(index):
        where = (index // half, 2 * (index % half) + core)

        @pl.when(jnp.logical_or(where[0] != e, where[1] != t))
        def _():
            pl.semaphore_signal(barrier, inc=1, device_id=where, device_id_type=MESH)

    each(n_ep * half, greet)
    for i in range(half):
        pl.semaphore_signal(
            barrier, inc=1, device_id=(e, 2 * i + 1 - core), device_id_type=MESH
        )

    if split:
        cols = block(t, hid)
        dense_parts = (dg_hbm.at[:, cols], du_hbm.at[:, cols], dd_hbm.at[cols, :])
    else:
        dense_parts = (dg_hbm, du_hbm, dd_hbm)
    loads = [
        pltpu.make_async_copy(src, dst, w_sem.at[i])
        for i, (src, dst) in enumerate(
            zip((ow_hbm, eg_hbm, eu_hbm) + dense_parts[:2] + (ed_hbm, dense_parts[2]), (ow, eg, eu, dg, du, ed, dd))
        )
    ]

    lane = lax.broadcasted_iota(jnp.int32, (seqs, route.shape[1]), 1)
    table = jnp.zeros((seqs, route.shape[1]), F32)
    for k in range(ids_ref.shape[0]):
        wanted = column(ids_ref[k : k + 1, :])
        table = table + jnp.where(lane == wanted, column(rw_ref[k : k + 1, :]), 0.0)
    own_rows = block(e, seqs)
    route[own_rows, :] = table

    resid = resid_ref[...].astype(F32)
    mean_sq = jnp.mean(resid * resid, axis=-1, keepdims=True)
    normed = (resid * lax.rsqrt(mean_sq + EPS) * first_gain_ref[...]).astype(BF16)
    row = lax.broadcasted_iota(jnp.int32, (seqs, LANES), 0)
    entry = lax.broadcasted_iota(jnp.int32, (seqs, LANES), 1) % QK_DIM
    position = jnp.zeros((seqs, LANES), F32)
    for s in range(seqs):
        position = jnp.where(row == s, lengths_ref[s].astype(F32), position)
    turn = QK_DIM // 2
    power = (entry % turn).astype(F32) * (-1.0 / turn)
    angle = position * jnp.exp(power * math.log(10000.0))
    cosine = jnp.cos(angle)
    sine = jnp.where(entry < turn, -jnp.sin(angle), jnp.sin(angle))

    def rotate(values):
        other = jnp.where(
            entry < turn, pltpu.roll(values, LANES - turn, 1), pltpu.roll(values, turn, 1)
        )
        return (values * cosine + other * sine).astype(BF16).astype(F32)

    query = jnp.zeros((seqs, qw.shape[1]), F32)
    for i in range(Q_CHUNKS):
        q_loads[i].wait()
        query = query + dot(
            normed[:, i * depth : (i + 1) * depth], qw[i * depth : (i + 1) * depth, :]
        )
    for load in q_loads[Q_CHUNKS:]:
        load.wait()
    keys_raw = dot(normed, kw[...])
    values_raw = dot(normed, vw[...])
    for load in loads:
        load.start()

    groups, spots = cache.shape[1], cache.shape[2]
    share = query.shape[1] // LANES // groups
    lower = lax.broadcasted_iota(jnp.int32, (seqs, LANES), 1) < QK_DIM
    fresh = []
    for g in range(groups):
        key = rotate(keys_raw[:, g * LANES : (g + 1) * LANES])
        value = values_raw[:, g * LANES : (g + 1) * LANES].astype(BF16).astype(F32)
        new_ref[:, 2 * g * LANES : (2 * g + 1) * LANES] = key
        new_ref[:, (2 * g + 1) * LANES : (2 * g + 2) * LANES] = value
        fresh.append((key, value))
        for j in range(share):
            at = (g * share + j) * LANES
            head = rotate(query[:, at : at + LANES])
            pairs[g, :, j, :] = jnp.where(lower, head, 0.0)
            pairs[g, :, share + j, :] = jnp.where(lower, 0.0, head)

    pl.semaphore_wait(barrier, n_ep * half - 1 + half)

    def route_copy(d):
        there = (e + d) % n_ep
        return remote(
            route.at[own_rows, :],
            route.at[own_rows, :],
            route_send.at[d - 1],
            route_recv.at[d - 1],
            (there, t),
        )

    def route_wait(d):
        came_from = (e + n_ep - d) % n_ep
        spot = route.at[block(came_from, seqs), :]
        remote(spot, spot, route_send.at[d - 1], route_recv.at[d - 1], (e, t)).wait_recv()

    each(n_ep - 1, lambda i: route_copy(i + 1).start())

    scale = QK_DIM**-0.5
    lines = 2 * share
    for s in range(seqs):
        cache_loads[s].wait()
        for g in range(groups):
            both = pairs[g, s].astype(BF16)
            scores[g, s] = (
                lax.dot_general(
                    both,
                    cache[s, g, :, :LANES],
                    (((1,), (1,)), ((), ())),
                    preferred_element_type=F32,
                )
                * scale
            )
    length = jnp.zeros((seqs, lines, 1), jnp.int32)
    which = lax.broadcasted_iota(jnp.int32, (seqs, lines, 1), 0)
    for s in range(seqs):
        length = jnp.where(which == s, lengths_ref[s], length)
    place = lax.broadcasted_iota(jnp.int32, (seqs, lines, spots), 2)
    valid = place < length
    line = lax.broadcasted_iota(jnp.int32, (lines, 1), 0)
    for g in range(groups):
        key, value = fresh[g]
        latest = jnp.sum(pairs[g] * key[:, None, :], axis=-1, keepdims=True) * scale
        masked = jnp.where(valid, scores[g], -jnp.inf)
        top = jnp.maximum(jnp.max(masked, axis=-1, keepdims=True), latest)
        raised = jnp.exp(masked - top)
        raised_new = jnp.exp(latest - top)
        total = jnp.sum(raised, axis=-1, keepdims=True) + raised_new
        prob = raised / total
        prob_new = jnp.broadcast_to(raised_new / total, (seqs, lines, LANES))
        lam = jnp.zeros((lines, 1), F32)
        for j in range(share):
            lam = jnp.where(line == j, lam_ref[g * share + j], lam)
        scores[g] = prob - lam[None] * pltpu.roll(prob, share, 1)
        new_weight = (prob_new - lam[None] * pltpu.roll(prob_new, share, 1)).astype(BF16).astype(F32)
        fresh_part = new_weight * value[:, None, :]
        for s in range(seqs):
            mixed[g, s] = dot(scores[g, s].astype(BF16), cache[s, g, :, LANES:])
        whole = mixed[g] + fresh_part
        mean_sq = jnp.mean(whole * whole, axis=-1, keepdims=True)
        mixed[g] = whole * lax.rsqrt(mean_sq + EPS) * head_gain_ref[...][None]
        for j in range(share):
            at = (g * share + j) * LANES
            heads_ref[:, at : at + LANES] = mixed[g, :, j, :].astype(BF16)

    def heads_copy(mask):
        return remote(
            heads_ref,
            heads_all.at[mask - 1],
            heads_send.at[mask - 1],
            heads_recv.at[mask - 1],
            (e, flip(t, mask)),
        )

    for mask in range(n_tp - 1, 0, -1):
        heads_copy(mask).start()

    loads[0].wait()
    span = heads_ref.shape[1]
    total = dot(heads_ref[...], ow[block(t, span), :])
    for mask in range(1, n_tp):
        heads_copy(mask).wait_recv()
        total = total + dot(heads_all[mask - 1], ow[block(flip(t, mask), span), :])
    own_cols = block(t, quarter)
    own_stream = (resid_ref[:, own_cols].astype(F32) + total).astype(BF16)
    stream[own_rows, own_cols] = own_stream

    def spot(owner, column):
        return stream.at[block(owner, seqs), block(column, quarter)]

    def owner_of(d):
        return (e + n_ep - d) % n_ep

    def first(d):
        return remote(
            spot(e, t), spot(e, t), first_send.at[d], stream_recv.at[0, d], ((e + d) % n_ep, t)
        )

    def second(d, mask):
        index = mask // 2 if mask != 1 else 0
        where = spot(owner_of(d), t)
        return remote(
            where, where, second_send.at[index, d], stream_recv.at[mask, d], (e, flip(t, mask))
        )

    def relay(d, mask):
        where = spot(owner_of(d), flip(t, mask))
        return remote(
            where, where, relay_send.at[mask // 2 - 1, d], stream_recv.at[mask + 1, d], (e, mate)
        )

    def arrived(d, mask):
        where = spot(owner_of(d), flip(t, mask))
        remote(where, where, first_send.at[d], stream_recv.at[mask, d], (e, t)).wait_recv()

    def spread(d):
        for mask in evens:
            second(d, mask).start()
        second(d, 1).start()

    far_first = sorted(range(1, n_ep), key=lambda d: -min(d, n_ep - d)) if n_ep <= 16 else None
    near_first = [0] + far_first[::-1] if far_first is not None else None
    each(n_ep - 1 if far_first is None else 1, lambda i: first(i + 1).start(), order=None) if far_first is None else [
        first(d).start() for d in far_first
    ]

    def stage_two(d):
        if not (isinstance(d, int) and d == 0):
            arrived(d, 0)
        spread(d)

    def stage_three(d):
        for mask in evens:
            arrived(d, mask)
            relay(d, mask).start()

    def normalise(d):
        arrived(d, 1)
        for mask in evens:
            arrived(d, mask + 1)
        rows = block(owner_of(d), seqs)
        values = stream[rows, :].astype(F32)
        mean_sq = jnp.mean(values * values, axis=-1, keepdims=True)
        scaled = (values * lax.rsqrt(mean_sq + EPS) * gain_ref[...]).astype(BF16)
        ffn[rows, :] = scaled
        inner = jnp.sum(scaled.astype(F32) * mixw_ref[...], axis=-1, keepdims=True)
        mix[rows, :] = jnp.broadcast_to(jax.nn.sigmoid(inner), (seqs, LANES))

    if near_first is not None:
        for i, d in enumerate(near_first):
            stage_two(d)
            if i:
                stage_three(near_first[i - 1])
            if i > 1:
                normalise(near_first[i - 2])
        stage_three(near_first[-1])
        for d in near_first[-2:]:
            normalise(d)
    else:
        stage_two(0)
        each(n_ep - 1, lambda i: stage_two(i + 1))
        each(n_ep, stage_three)
        each(n_ep, normalise)
    each(n_ep - 1, lambda i: route_wait(i + 1))

    many = min(rows_all, 128)
    batches = rows_all // many
    for load in loads[1:5]:
        load.wait()

    def hidden(b):
        rows = block(b, many)
        a = ffn[rows, :]
        for j in range(held):
            eh[j, rows, :] = (jax.nn.silu(dot(a, eg[j])) * dot(a, eu[j])).astype(BF16)
        units = jax.nn.silu(dot(a, dg[...])) * dot(a, du[...])
        if not split:
            own = hid // n_tp
            unit = lax.broadcasted_iota(jnp.int32, units.shape, 1)
            units = jnp.where((unit >= t * own) & (unit < (t + 1) * own), units, 0.0)
        dh[rows, :] = units.astype(BF16)

    each(batches, hidden)
    for load in loads[5:]:
        load.wait()

    def result(b, q):
        rows = block(b, many)
        cols = block(q, quarter)
        total = mix[rows, :1] * dot(dh[rows, :], dd[:, cols])
        lanes = lax.broadcasted_iota(jnp.int32, (many, route.shape[1]), 1)
        for j in range(held):
            weight = jnp.sum(
                jnp.where(lanes == e * held + j, route[rows, :], 0.0), axis=1, keepdims=True
            )
            piece = dot(eh[j, rows, :], ed[j, :, cols]).astype(BF16)
            total = total + weight * piece.astype(F32)
        return total

    def pair(j):
        return remote(away.at[j], came.at[j], pair_send.at[j], pair_recv.at[j], (e, mate))

    for j in range(half):

        def leave(b, j=j):
            away[j, block(b, many), :] = result(b, 2 * j + 1 - core).astype(BF16)

        each(batches, leave)
        pair(j).start()

    me = e * half + t // 2

    def back(j, d):
        there = (e + d) % n_ep
        return remote(
            summed.at[j, block(there, seqs), :],
            landed.at[me],
            back_send.at[j, d],
            back_recv.at[me],
            (there, 2 * j + core),
        )

    def same(j, d):
        return jnp.logical_and(jnp.asarray(d == 0), 2 * j + core == t)

    for j in range(half):

        def keep(b, j=j):
            summed[j, block(b, many), :] = result(b, 2 * j + core).astype(BF16)

        each(batches, keep)
    for j in range(half):
        pair(j).wait_recv()

        def add(b, j=j):
            rows = block(b, many)
            summed[j, rows, :] = (summed[j, rows, :].astype(F32) + came[j, rows, :].astype(F32)).astype(BF16)

        each(batches, add)

        def send(d, j=j):
            @pl.when(jnp.logical_not(same(j, d)))
            def _():
                back(j, d).start()

        each(n_ep, send, order=None if far_first is None else far_first + [0])

    landed[me] = summed[t // 2, own_rows, :]

    def take(index):
        @pl.when(index != me)
        def _():
            where = landed.at[index]
            remote(where, where, back_send.at[0, 0], back_recv.at[index], (e, t)).wait_recv()

    each(n_ep * half, take)
    out_ref[...] = own_stream.astype(F32) + jnp.sum(landed[...].astype(F32), axis=0)

    for mask in range(1, n_tp):
        heads_copy(mask).wait_send()
    each(n_ep - 1, lambda i: route_copy(i + 1).wait_send())
    each(n_ep - 1, lambda i: first(i + 1).wait_send())

    def sent(d):
        second(d, 1).wait_send()
        for mask in evens:
            second(d, mask).wait_send()
            relay(d, mask).wait_send()

    each(n_ep, sent)
    for j in range(half):
        pair(j).wait_send()

        def gone(d, j=j):
            @pl.when(jnp.logical_not(same(j, d)))
            def _():
                back(j, d).wait_send()

        each(n_ep, gone)


def near_kernel(
    n_ep,
    n_tp,
    lengths_hbm,
    lam_hbm,
    resid_hbm,
    first_gain_hbm,
    head_gain_hbm,
    gain_hbm,
    mixw_hbm,
    ids_hbm,
    rw_hbm,
    qw_hbm,
    kw_hbm,
    vw_hbm,
    cache_hbm,
    ow_hbm,
    eg_hbm,
    eu_hbm,
    ed_hbm,
    dg_hbm,
    du_hbm,
    dd_hbm,
    out_ref,
    new_ref,
    lengths_ref,
    lam_ref,
    resid_ref,
    first_gain_ref,
    head_gain_ref,
    gain_ref,
    mixw_ref,
    ids_ref,
    rw_ref,
    qw,
    kw,
    vw,
    cache,
    pairs,
    scores,
    mixed,
    heads_ref,
    ow,
    gu,
    ed,
    dg,
    du,
    dd,
    heads_all,
    mine,
    stream,
    ffn,
    mix,
    route,
    eh,
    dh,
    leaving,
    kept,
    plane_in,
    column_out,
    column_in,
    small_sem,
    q_sem,
    cache_sem,
    w_sem,
    e_sem,
    push_send,
    push_recv,
    route_send,
    route_recv,
    heads_send,
    heads_recv,
    first_send,
    second_send,
    stream_recv,
    plane_send,
    plane_recv,
    column_send,
    column_recv,
):
    e = lax.axis_index("ep")
    t = lax.axis_index("tp")
    planes = n_ep // INNER
    z = e // INNER
    x = e % INNER
    y = t // CORES
    c = t % CORES
    keeper = z % CORES
    odd = (c + z) % CORES
    turns = planes // CORES
    seqs, width = resid_ref.shape
    quarter = out_ref.shape[1]
    part = eg_hbm.shape[2]
    hid = dg.shape[1]
    mate = flip(t, 1)

    small_loads = [
        pltpu.make_async_copy(src, dst, small_sem.at[i])
        for i, (src, dst) in enumerate(
            (
                (resid_hbm, resid_ref),
                (first_gain_hbm, first_gain_ref),
                (lengths_hbm, lengths_ref),
                (ids_hbm, ids_ref),
                (rw_hbm, rw_ref),
                (lam_hbm, lam_ref),
                (head_gain_hbm, head_gain_ref),
                (gain_hbm, gain_ref),
                (mixw_hbm, mixw_ref),
            )
        )
    ]
    for load in small_loads:
        load.start()
    depth = qw.shape[0] // Q_CHUNKS
    q_loads = [
        pltpu.make_async_copy(
            qw_hbm.at[pl.ds(i * depth, depth), :], qw.at[pl.ds(i * depth, depth), :], q_sem.at[i]
        )
        for i in range(Q_CHUNKS)
    ] + [
        pltpu.make_async_copy(kw_hbm, kw, q_sem.at[Q_CHUNKS]),
        pltpu.make_async_copy(vw_hbm, vw, q_sem.at[Q_CHUNKS + 1]),
    ]
    for load in q_loads:
        load.start()
    e_loads = [
        pltpu.make_async_copy(eg_hbm.at[0], gu.at[c, :, :part], e_sem.at[0]),
        pltpu.make_async_copy(eu_hbm.at[0], gu.at[c, :, part:], e_sem.at[1]),
        pltpu.make_async_copy(ed_hbm.at[0], ed.at[block(c, part), :], e_sem.at[2]),
    ]
    for load in e_loads:
        load.start()
    cache_loads = [
        pltpu.make_async_copy(cache_hbm.at[s], cache.at[s], cache_sem.at[s]) for s in range(seqs)
    ]
    for load in cache_loads:
        load.start()

    barrier = pltpu.get_barrier_semaphore()
    for index in range(n_ep * n_tp):
        where = (index // n_tp, index % n_tp)

        @pl.when(jnp.logical_or(where[0] != e, where[1] != t))
        def _():
            pl.semaphore_signal(barrier, inc=1, device_id=where, device_id_type=MESH)

    cols = block(y, hid)
    loads = [
        pltpu.make_async_copy(src, dst, w_sem.at[i])
        for i, (src, dst) in enumerate(
            (
                (ow_hbm, ow),
                (dg_hbm.at[:, cols], dg),
                (du_hbm.at[:, cols], du),
                (dd_hbm.at[cols, :], dd),
            )
        )
    ]

    for load in small_loads[:3]:
        load.wait()
    resid = resid_ref[...].astype(F32)
    mean_sq = jnp.mean(resid * resid, axis=-1, keepdims=True)
    normed = (resid * lax.rsqrt(mean_sq + EPS) * first_gain_ref[...]).astype(BF16)
    row = lax.broadcasted_iota(jnp.int32, (seqs, LANES), 0)
    entry = lax.broadcasted_iota(jnp.int32, (seqs, LANES), 1) % QK_DIM
    position = jnp.zeros((seqs, LANES), F32)
    for s in range(seqs):
        position = jnp.where(row == s, lengths_ref[s].astype(F32), position)
    turn = QK_DIM // 2
    power = (entry % turn).astype(F32) * (-1.0 / turn)
    angle = position * jnp.exp(power * math.log(10000.0))
    cosine = jnp.cos(angle)
    sine = jnp.where(entry < turn, -jnp.sin(angle), jnp.sin(angle))

    def rotate(values):
        other = jnp.where(
            entry < turn, pltpu.roll(values, LANES - turn, 1), pltpu.roll(values, turn, 1)
        )
        return (values * cosine + other * sine).astype(BF16).astype(F32)

    for load in small_loads[3:]:
        load.wait()

    def spot(plane, inner):
        return plane // CORES * INNER + inner

    own_spot = spot(z, x)
    lane = lax.broadcasted_iota(jnp.int32, (seqs, route.shape[2]), 1)
    table = jnp.zeros((seqs, route.shape[2]), F32)
    for k in range(ids_ref.shape[0]):
        wanted = column(ids_ref[k : k + 1, :])
        table = table + jnp.where(lane == wanted, column(rw_ref[k : k + 1, :]), 0.0)

    @pl.when(odd == 0)
    def _():
        route[own_spot] = table

    query = jnp.zeros((seqs, qw.shape[1]), F32)
    for i in range(Q_CHUNKS):
        q_loads[i].wait()
        query = query + dot(
            normed[:, i * depth : (i + 1) * depth], qw[i * depth : (i + 1) * depth, :]
        )
    for load in q_loads[Q_CHUNKS:]:
        load.wait()
    keys_raw = dot(normed, kw[...])
    values_raw = dot(normed, vw[...])
    for load in loads:
        load.start()

    groups, spots = cache.shape[1], cache.shape[2]
    share = query.shape[1] // LANES // groups
    lower = lax.broadcasted_iota(jnp.int32, (seqs, LANES), 1) < QK_DIM
    fresh = []
    for g in range(groups):
        key = rotate(keys_raw[:, g * LANES : (g + 1) * LANES])
        value = values_raw[:, g * LANES : (g + 1) * LANES].astype(BF16).astype(F32)
        new_ref[:, 2 * g * LANES : (2 * g + 1) * LANES] = key.astype(BF16)
        new_ref[:, (2 * g + 1) * LANES : (2 * g + 2) * LANES] = value.astype(BF16)
        fresh.append((key, value))
        for j in range(share):
            at = (g * share + j) * LANES
            head = rotate(query[:, at : at + LANES])
            pairs[g, :, j, :] = jnp.where(lower, head, 0.0)
            pairs[g, :, share + j, :] = jnp.where(lower, 0.0, head)

    pl.semaphore_wait(barrier, n_ep * n_tp - 1)

    def push(index):
        where = (gu.at[c], ed.at[block(c, part), :])[index]
        return remote(where, where, push_send.at[index], push_recv.at[index], (e, mate))

    def pushed(index):
        where = (gu.at[1 - c], ed.at[block(1 - c, part), :])[index]
        remote(where, where, push_send.at[index], push_recv.at[index], (e, mate)).wait_recv()

    for load in e_loads:
        load.wait()
    push(0).start()
    push(1).start()

    def route_copy(mask):
        where = route.at[own_spot]
        return remote(
            where, where, route_send.at[mask - 1], route_recv.at[own_spot], (flip(e, mask), t)
        )

    @pl.when(odd == 0)
    def _():
        for mask in range(1, n_ep):
            route_copy(mask).start()

    scale = QK_DIM**-0.5
    lines = 2 * share
    for s in range(seqs):
        cache_loads[s].wait()
        for g in range(groups):
            both = pairs[g, s].astype(BF16)
            scores[g, s] = (
                lax.dot_general(
                    both,
                    cache[s, g, :, :LANES],
                    (((1,), (1,)), ((), ())),
                    preferred_element_type=F32,
                )
                * scale
            )
    length = jnp.zeros((seqs, lines, 1), jnp.int32)
    which = lax.broadcasted_iota(jnp.int32, (seqs, lines, 1), 0)
    for s in range(seqs):
        length = jnp.where(which == s, lengths_ref[s], length)
    place = lax.broadcasted_iota(jnp.int32, (seqs, lines, spots), 2)
    valid = place < length
    line = lax.broadcasted_iota(jnp.int32, (lines, 1), 0)
    for g in range(groups):
        key, value = fresh[g]
        latest = jnp.sum(pairs[g] * key[:, None, :], axis=-1, keepdims=True) * scale
        masked = jnp.where(valid, scores[g], -jnp.inf)
        top = jnp.maximum(jnp.max(masked, axis=-1, keepdims=True), latest)
        raised = jnp.exp(masked - top)
        raised_new = jnp.exp(latest - top)
        total = jnp.sum(raised, axis=-1, keepdims=True) + raised_new
        prob = raised / total
        prob_new = jnp.broadcast_to(raised_new / total, (seqs, lines, LANES))
        lam = jnp.zeros((lines, 1), F32)
        for j in range(share):
            lam = jnp.where(line == j, lam_ref[g * share + j], lam)
        scores[g] = prob - lam[None] * pltpu.roll(prob, share, 1)
        new_weight = (prob_new - lam[None] * pltpu.roll(prob_new, share, 1)).astype(BF16).astype(F32)
        fresh_part = new_weight * value[:, None, :]
        for s in range(seqs):
            mixed[g, s] = dot(scores[g, s].astype(BF16), cache[s, g, :, LANES:])
        whole = mixed[g] + fresh_part
        mean_sq = jnp.mean(whole * whole, axis=-1, keepdims=True)
        mixed[g] = whole * lax.rsqrt(mean_sq + EPS) * head_gain_ref[...][None]
        for j in range(share):
            at = (g * share + j) * LANES
            heads_ref[:, at : at + LANES] = mixed[g, :, j, :].astype(BF16)

    def heads_copy(mask):
        return remote(
            heads_ref,
            heads_all.at[mask - 1],
            heads_send.at[mask - 1],
            heads_recv.at[mask - 1],
            (e, flip(t, mask)),
        )

    for mask in range(n_tp - 1, 0, -1):
        heads_copy(mask).start()

    loads[0].wait()
    span = heads_ref.shape[1]
    total = dot(heads_ref[...], ow[block(t, span), :])
    for mask in range(1, n_tp):
        heads_copy(mask).wait_recv()
        total = total + dot(heads_all[mask - 1], ow[block(flip(t, mask), span), :])
    own_cols = block(t, quarter)
    own_stream = (resid_ref[:, own_cols].astype(F32) + total).astype(BF16)
    mine[...] = own_stream

    around = ((1, 1), (1, 0), (0, 1))

    def at_spot(where, owner):
        return stream.at[block(where, seqs), block(owner, quarter)]

    def to_plane(step):
        dx, dy = around[step]
        there = (z * INNER + flip(x, dx), flip(y, dy) * CORES + keeper)
        return remote(
            mine, at_spot(own_spot, t), first_send.at[step], stream_recv.at[own_spot, t], there
        )

    def to_column(d):
        there = (flip(z, d) * INNER + x, y * CORES + keeper)
        return remote(
            mine,
            at_spot(own_spot, t),
            first_send.at[len(around) + d],
            stream_recv.at[own_spot, t],
            there,
        )

    def to_mate():
        return remote(
            mine,
            at_spot(own_spot, t),
            first_send.at[len(around)],
            stream_recv.at[own_spot, t],
            (e, mate),
        )

    for d in range(planes - 1, 0, -1):
        to_column(d).start()
    for step in range(len(around)):
        to_plane(step).start()

    @pl.when(odd == 1)
    def _():
        to_mate().start()

    @pl.when(odd == 0)
    def _():
        stream[block(own_spot, seqs), own_cols] = own_stream

    near = z + odd * (1 - 2 * (z % 2))

    def plane_of(i):
        return flip(near, 2 * i)

    def arrived(where, owner):
        spot_ref = at_spot(where, owner)
        remote(
            spot_ref, spot_ref, first_send.at[0], stream_recv.at[where, owner], (e, t)
        ).wait_recv()

    def forward(i, core, step):
        dx, dy = around[step]
        owner = y * CORES + core
        where = spot(plane_of(i), x)
        spot_ref = at_spot(where, owner)
        return remote(
            spot_ref,
            spot_ref,
            second_send.at[i, core, step],
            stream_recv.at[where, owner],
            (z * INNER + flip(x, dx), flip(y, dy) * CORES + c),
        )

    def relay(i):
        for core in range(CORES):
            arrived(spot(plane_of(i), x), y * CORES + core)
            for step in range(len(around)):
                forward(i, core, step).start()

    def gather(i):
        if i == 0:

            @pl.when(odd == 1)
            def _():
                relay(0)

            @pl.when(odd == 0)
            def _():
                arrived(own_spot, mate)
        else:
            relay(i)

    def normalise(i):
        for inner in (0, 1):
            where = spot(plane_of(i), flip(x, inner))
            for core in range(CORES):
                arrived(where, flip(y, 1) * CORES + core)
            if inner:
                for core in range(CORES):
                    arrived(where, y * CORES + core)
            rows = block(where, seqs)
            values = stream[rows, :].astype(F32)
            mean_sq = jnp.mean(values * values, axis=-1, keepdims=True)
            scaled = (values * lax.rsqrt(mean_sq + EPS) * gain_ref[...]).astype(BF16)
            ffn[rows, :] = scaled
            inside = jnp.sum(scaled.astype(F32) * mixw_ref[...], axis=-1, keepdims=True)
            mix[rows, :] = jnp.broadcast_to(jax.nn.sigmoid(inside), (seqs, LANES))

    for i in range(turns):
        gather(i)
    for i in range(turns):
        normalise(i)

    for i in range(turns):
        for inner in range(INNER):
            where = spot(plane_of(i), inner)

            def route_wait(where=where):
                spot_ref = route.at[where]
                remote(
                    spot_ref, spot_ref, route_send.at[0], route_recv.at[where], (e, t)
                ).wait_recv()

            if i == 0:

                @pl.when(jnp.logical_or(odd == 1, inner != x))
                def _():
                    route_wait()
            else:
                route_wait()

    rows_all = ffn.shape[0]
    pushed(0)
    pushed(1)
    for load in loads[1:3]:
        load.wait()
    a = ffn[...]
    for core in range(CORES):
        both = dot(a, gu[core])
        eh[:, core * part : (core + 1) * part] = (
            jax.nn.silu(both[:, :part]) * both[:, part:]
        ).astype(BF16)
    dh[...] = (jax.nn.silu(dot(a, dg[...])) * dot(a, du[...])).astype(BF16)
    loads[3].wait()

    lanes = lax.broadcasted_iota(jnp.int32, (rows_all, route.shape[2]), 1)
    weight = jnp.sum(
        jnp.where(lanes == e, route[...].reshape(rows_all, route.shape[2]), 0.0),
        axis=1,
        keepdims=True,
    )

    def leave(i, dy, core, step):
        dx = around[step][0]
        where = spot(plane_of(i), flip(x, dx))
        return remote(
            leaving.at[dy, core, block(where, seqs), :],
            plane_in.at[i, core, step],
            plane_send.at[i, core, step],
            plane_recv.at[i, core, step],
            (z * INNER + flip(x, dx), flip(y, dy) * CORES + c),
        )

    order = range(turns - 1, -1, -1)
    for dy in (1, 0):
        for core in range(CORES):
            cols = block(flip(y, dy) * CORES + core, quarter)
            total = mix[:, :1] * dot(dh[...], dd[:, cols]) + weight * dot(eh[...], ed[:, cols])
            leaving[dy, core] = total.astype(BF16)
            if not dy:
                kept[core] = total
            for i in order:
                for step in range(len(around)):
                    if around[step][1] == dy:
                        leave(i, dy, core, step).start()

    def own_plane(i):
        return jnp.logical_and(odd == 0, i == 0)

    def climb(i, core):
        return remote(
            column_out.at[i, core],
            column_in.at[odd + 2 * i],
            column_send.at[i, core],
            column_recv.at[odd + 2 * i],
            (plane_of(i) * INNER + x, y * CORES + core),
        )

    def stays(i, core):
        return jnp.logical_and(own_plane(i), c == core)

    for i in order:
        for core in range(CORES):
            gathered = kept[core, block(spot(plane_of(i), x), seqs), :]
            for step in range(len(around)):
                leave(i, around[step][1], core, step).wait_recv()
                gathered = gathered + plane_in[i, core, step].astype(F32)
            column_out[i, core] = gathered.astype(BF16)

            @pl.when(jnp.logical_not(stays(i, core)))
            def _(i=i, core=core):
                climb(i, core).start()

    def took(d):
        where = column_in.at[d]
        remote(where, where, column_send.at[0, 0], column_recv.at[d], (e, t)).wait_recv()

    @pl.when(odd == 0)
    def _():
        column_in[0] = column_out[0, c]

    @pl.when(odd == 1)
    def _():
        took(0)

    for d in range(1, planes):
        took(d)
    out_ref[...] = (
        own_stream.astype(F32) + jnp.sum(column_in[...].astype(F32), axis=0)
    ).astype(BF16)

    push(0).wait_send()
    push(1).wait_send()
    for mask in range(1, n_tp):
        heads_copy(mask).wait_send()

    @pl.when(odd == 0)
    def _():
        for mask in range(1, n_ep):
            route_copy(mask).wait_send()

    for d in range(1, planes):
        to_column(d).wait_send()
    for step in range(len(around)):
        to_plane(step).wait_send()

    @pl.when(odd == 1)
    def _():
        to_mate().wait_send()

    for i in range(turns):
        for core in range(CORES):
            for step in range(len(around)):

                def forwarded(i=i, core=core, step=step):
                    forward(i, core, step).wait_send()

                if i == 0:
                    pl.when(odd == 1)(forwarded)
                else:
                    forwarded()
                leave(i, around[step][1], core, step).wait_send()

            @pl.when(jnp.logical_not(stays(i, core)))
            def _(i=i, core=core):
                climb(i, core).wait_send()


def near_call(n_ep, n_tp, arrays):
    (
        residual_in,
        lengths,
        kv_cache,
        norm_gain_attn,
        query_weight,
        key_weight,
        value_weight,
        diff_lambda,
        head_gain,
        out_weight,
        norm_gain_ffn,
        route_ids,
        route_weights,
        expert_gate,
        expert_up,
        expert_down,
        dense_gate,
        dense_up,
        dense_down,
        dense_mix,
    ) = arrays
    seqs, width = residual_in.shape
    held = lambda value: pltpu.with_memory_space_constraint(value, pltpu.HBM)
    groups, spots = kv_cache.shape[1:3]
    share = diff_lambda.shape[0] // groups
    inner = query_weight.shape[1]
    quarter = out_weight.shape[1]
    part = expert_gate.shape[2]
    hid = dense_gate.shape[1] // (n_tp // CORES)
    turns = n_ep // INNER // CORES
    blocks = turns * INNER
    rows = blocks * seqs
    lanes = -(-n_ep // LANES) * LANES
    topk = route_ids.shape[1]
    vmem = pl.BlockSpec(memory_space=pltpu.VMEM)
    hbm = pl.BlockSpec(memory_space=pltpu.HBM)
    dma = pltpu.SemaphoreType.DMA
    layer_out, fresh = pl.pallas_call(
        functools.partial(near_kernel, n_ep, n_tp),
        out_shape=(
            jax.ShapeDtypeStruct((seqs, quarter), BF16),
            jax.ShapeDtypeStruct((seqs, groups * kv_cache.shape[3]), BF16),
        ),
        in_specs=[hbm] * 20,
        out_specs=(vmem, vmem),
        scratch_shapes=[
            pltpu.SMEM(lengths.shape, jnp.int32),
            pltpu.SMEM(diff_lambda.shape, F32),
            pltpu.VMEM(residual_in.shape, BF16),
            pltpu.VMEM((1, width), F32),
            pltpu.VMEM((1, head_gain.shape[0]), F32),
            pltpu.VMEM((1, width), F32),
            pltpu.VMEM((1, width), F32),
            pltpu.VMEM((topk, seqs), jnp.int32),
            pltpu.VMEM((topk, seqs), F32),
            pltpu.VMEM(query_weight.shape, BF16),
            pltpu.VMEM(key_weight.shape, BF16),
            pltpu.VMEM(value_weight.shape, BF16),
            pltpu.VMEM(kv_cache.shape, BF16),
            pltpu.VMEM((groups, seqs, 2 * share, LANES), F32),
            pltpu.VMEM((groups, seqs, 2 * share, spots), F32),
            pltpu.VMEM((groups, seqs, 2 * share, LANES), F32),
            pltpu.VMEM((seqs, inner), BF16),
            pltpu.VMEM(out_weight.shape, BF16),
            pltpu.VMEM((CORES, width, 2 * part), BF16),
            pltpu.VMEM((CORES * part, width), BF16),
            pltpu.VMEM((width, hid), BF16),
            pltpu.VMEM((width, hid), BF16),
            pltpu.VMEM((hid, width), BF16),
            pltpu.VMEM((n_tp - 1, seqs, inner), BF16),
            pltpu.VMEM((seqs, quarter), BF16),
            pltpu.VMEM((rows, width), BF16),
            pltpu.VMEM((rows, width), BF16),
            pltpu.VMEM((rows, LANES), F32),
            pltpu.VMEM((blocks, seqs, lanes), F32),
            pltpu.VMEM((rows, CORES * part), BF16),
            pltpu.VMEM((rows, hid), BF16),
            pltpu.VMEM((2, CORES, rows, quarter), BF16),
            pltpu.VMEM((CORES, rows, quarter), F32),
            pltpu.VMEM((turns, CORES, 3, seqs, quarter), BF16),
            pltpu.VMEM((turns, CORES, seqs, quarter), BF16),
            pltpu.VMEM((n_ep // INNER, seqs, quarter), BF16),
            dma((9,)),
            dma((Q_CHUNKS + 2,)),
            dma((seqs,)),
            dma((4,)),
            dma((3,)),
            dma((2,)),
            dma((2,)),
            dma((n_ep - 1,)),
            dma((blocks,)),
            dma((n_tp - 1,)),
            dma((n_tp - 1,)),
            dma((3 + n_ep // INNER,)),
            dma((turns, CORES, 3)),
            dma((blocks, n_tp)),
            dma((turns, CORES, 3)),
            dma((turns, CORES, 3)),
            dma((turns, CORES)),
            dma((n_ep // INNER,)),
        ],
        compiler_params=pltpu.CompilerParams(
            collective_id=0, has_side_effects=True, vmem_limit_bytes=36 * 1024 * 1024
        ),
    )(
        held(lengths),
        held(diff_lambda),
        held(residual_in),
        held(norm_gain_attn[None, :]),
        held(head_gain[None, :]),
        held(norm_gain_ffn[None, :]),
        held(dense_mix[None, :]),
        held(route_ids.T),
        held(route_weights.T),
        held(query_weight),
        held(key_weight),
        held(value_weight),
        held(kv_cache),
        held(out_weight),
        held(expert_gate),
        held(expert_up),
        held(expert_down),
        held(dense_gate),
        held(dense_up),
        held(dense_down),
    )
    return layer_out, fresh.reshape(seqs, groups, kv_cache.shape[3])


def on_device(
    residual_in,
    lengths,
    kv_cache,
    norm_gain_attn,
    query_weight,
    key_weight,
    value_weight,
    diff_lambda,
    head_gain,
    out_weight,
    norm_gain_ffn,
    route_ids,
    route_weights,
    expert_gate,
    expert_up,
    expert_down,
    dense_gate,
    dense_up,
    dense_down,
    dense_mix,
):
    n_ep = lax.axis_size("ep")
    n_tp = lax.axis_size("tp")
    half = n_tp // 2
    if (
        n_tp == 2 * CORES
        and n_ep in (4, 8, 16)
        and expert_gate.shape[0] == 1
        and dense_gate.shape[1] // half % LANES == 0
        and expert_gate.shape[2] % LANES == 0
    ):
        return near_call(
            n_ep,
            n_tp,
            (
                residual_in,
                lengths,
                kv_cache,
                norm_gain_attn,
                query_weight,
                key_weight,
                value_weight,
                diff_lambda,
                head_gain,
                out_weight,
                norm_gain_ffn,
                route_ids,
                route_weights,
                expert_gate,
                expert_up,
                expert_down,
                dense_gate,
                dense_up,
                dense_down,
                dense_mix,
            ),
        )
    seqs, width = residual_in.shape
    groups, spots = kv_cache.shape[1:3]
    share = diff_lambda.shape[0] // groups
    inner = query_weight.shape[1]
    quarter = out_weight.shape[1]
    held, _, part = expert_gate.shape
    rows = n_ep * seqs
    own = dense_gate.shape[1] // n_tp
    split = own % LANES == 0
    hid = own if split else dense_gate.shape[1]
    lanes = -(-n_ep * held // LANES) * LANES
    vmem = pl.BlockSpec(memory_space=pltpu.VMEM)
    smem = pl.BlockSpec(memory_space=pltpu.SMEM)
    hbm = pl.BlockSpec(memory_space=pl.ANY)
    dma = pltpu.SemaphoreType.DMA
    layer_out, fresh = pl.pallas_call(
        functools.partial(layer_kernel, n_ep, n_tp, split),
        out_shape=(
            jax.ShapeDtypeStruct((seqs, quarter), F32),
            jax.ShapeDtypeStruct((seqs, groups * kv_cache.shape[3]), F32),
        ),
        in_specs=[smem] * 2 + [vmem] * 7 + [hbm] * 11,
        out_specs=(vmem, vmem),
        scratch_shapes=[
            pltpu.VMEM(query_weight.shape, BF16),
            pltpu.VMEM(key_weight.shape, BF16),
            pltpu.VMEM(value_weight.shape, BF16),
            pltpu.VMEM(kv_cache.shape, BF16),
            pltpu.VMEM((groups, seqs, 2 * share, LANES), F32),
            pltpu.VMEM((groups, seqs, 2 * share, spots), F32),
            pltpu.VMEM((groups, seqs, 2 * share, LANES), F32),
            pltpu.VMEM((seqs, inner), BF16),
            pltpu.VMEM(out_weight.shape, BF16),
            pltpu.VMEM(expert_gate.shape, BF16),
            pltpu.VMEM(expert_up.shape, BF16),
            pltpu.VMEM(expert_down.shape, BF16),
            pltpu.VMEM((width, hid), BF16),
            pltpu.VMEM((width, hid), BF16),
            pltpu.VMEM((hid, width), BF16),
            pltpu.VMEM((n_tp - 1, seqs, inner), BF16),
            pltpu.VMEM((rows, width), BF16),
            pltpu.VMEM((rows, width), BF16),
            pltpu.VMEM((rows, LANES), F32),
            pltpu.VMEM((rows, lanes), F32),
            pltpu.VMEM((held, rows, part), BF16),
            pltpu.VMEM((rows, hid), BF16),
            pltpu.VMEM((half, rows, quarter), BF16),
            pltpu.VMEM((half, rows, quarter), BF16),
            pltpu.VMEM((half, rows, quarter), BF16),
            pltpu.VMEM((n_ep * half, seqs, quarter), BF16),
            dma((7,)),
            dma((Q_CHUNKS + 2,)),
            dma((seqs,)),
            dma((n_ep - 1,)),
            dma((n_ep - 1,)),
            dma((n_tp - 1,)),
            dma((n_tp - 1,)),
            dma((n_ep,)),
            dma((half, n_ep)),
            dma((max(half - 1, 1), n_ep)),
            dma((n_tp, n_ep)),
            dma((half,)),
            dma((half,)),
            dma((half, n_ep)),
            dma((n_ep * half,)),
        ],
        compiler_params=pltpu.CompilerParams(
            collective_id=0, has_side_effects=True, vmem_limit_bytes=60 * 1024 * 1024
        ),
    )(
        lengths,
        diff_lambda,
        residual_in,
        norm_gain_attn[None, :],
        head_gain[None, :],
        norm_gain_ffn[None, :],
        dense_mix[None, :],
        route_ids.T,
        route_weights.T,
        query_weight,
        key_weight,
        value_weight,
        kv_cache,
        out_weight,
        expert_gate,
        expert_up,
        expert_down,
        dense_gate,
        dense_up,
        dense_down,
    )
    new_rows = fresh.astype(BF16).reshape(seqs, groups, kv_cache.shape[3])
    return (layer_out.astype(BF16), new_rows)


def solution(mesh):
    placed = (
        P("ep", None),
        P("ep"),
        P("ep", "tp", None, None),
        P(),
        P(None, "tp"),
        P(None, "tp"),
        P(None, "tp"),
        P("tp"),
        P(),
        P(None, "tp"),
        P(),
        P("ep", None),
        P("ep", None),
        P("ep", None, "tp"),
        P("ep", None, "tp"),
        P("ep", "tp", None),
        P(None, "ep"),
        P(None, "ep"),
        P("ep", None),
        P(),
    )
    return jax.shard_map(
        on_device,
        mesh=mesh,
        in_specs=placed,
        out_specs=(P("ep", "tp"), P("ep", "tp", None)),
        check_vma=False,
    )
```

```python
import functools
import math

import jax
import jax.numpy as jnp
from jax import lax
from jax.experimental import pallas as pl
from jax.experimental.pallas import tpu as pltpu
from jax.sharding import PartitionSpec as P

QK_DIM = 64
EPS = 1e-06
MESH = pl.DeviceIdType.MESH
F32 = jnp.float32
BF16 = jnp.bfloat16
LANES = 128
Q_CHUNKS = 4
INNER = 2
CORES = 2
CACHE_CHUNKS = 4


def flip(value, mask):
    bit = 1
    while bit <= mask:
        if mask & bit:
            value = value + bit * (1 - 2 * ((value // bit) % 2))
        bit *= 2
    return value


def each(count, body, order=None):
    if count <= 16:
        for index in order if order is not None else range(count):
            body(index)
    else:

        def step(index, carry):
            body(index)
            return carry

        lax.fori_loop(0, count, step, 0)


def block(start, size):
    return pl.ds(pl.multiple_of(start * size, size), size)


def remote(source, target, send, recv, where):
    return pltpu.make_async_remote_copy(
        src_ref=source,
        dst_ref=target,
        send_sem=send,
        recv_sem=recv,
        device_id=where,
        device_id_type=MESH,
    )


def dot(left, right):
    return jnp.dot(left, right, preferred_element_type=F32)


def column(row):
    count = row.shape[1]
    square = (count, count)
    same = lax.broadcasted_iota(jnp.int32, square, 0) == lax.broadcasted_iota(jnp.int32, square, 1)
    return jnp.sum(jnp.where(same, row, jnp.zeros_like(row)), axis=1, keepdims=True)


def layer_kernel(
    n_ep,
    n_tp,
    split,
    lengths_ref,
    lam_ref,
    resid_ref,
    first_gain_ref,
    head_gain_ref,
    gain_ref,
    mixw_ref,
    ids_ref,
    rw_ref,
    qw_hbm,
    kw_hbm,
    vw_hbm,
    cache_hbm,
    ow_hbm,
    eg_hbm,
    eu_hbm,
    ed_hbm,
    dg_hbm,
    du_hbm,
    dd_hbm,
    out_ref,
    new_ref,
    qw,
    kw,
    vw,
    cache,
    pairs,
    scores,
    mixed,
    heads_ref,
    ow,
    eg,
    eu,
    ed,
    dg,
    du,
    dd,
    heads_all,
    stream,
    ffn,
    mix,
    route,
    eh,
    dh,
    away,
    came,
    summed,
    landed,
    w_sem,
    q_sem,
    cache_sem,
    route_send,
    route_recv,
    heads_send,
    heads_recv,
    first_send,
    second_send,
    relay_send,
    stream_recv,
    pair_send,
    pair_recv,
    back_send,
    back_recv,
):
    e = lax.axis_index("ep")
    t = lax.axis_index("tp")
    half = n_tp // 2
    mate = flip(t, 1)
    core = t % 2
    seqs, width = resid_ref.shape
    quarter = out_ref.shape[1]
    held, _, part = eg.shape
    hid = dg.shape[1]
    rows_all = n_ep * seqs
    evens = [2 * i for i in range(1, half)]

    depth = qw.shape[0] // Q_CHUNKS
    q_loads = [
        pltpu.make_async_copy(
            qw_hbm.at[pl.ds(i * depth, depth), :], qw.at[pl.ds(i * depth, depth), :], q_sem.at[i]
        )
        for i in range(Q_CHUNKS)
    ] + [
        pltpu.make_async_copy(kw_hbm, kw, q_sem.at[Q_CHUNKS]),
        pltpu.make_async_copy(vw_hbm, vw, q_sem.at[Q_CHUNKS + 1]),
    ]
    for load in q_loads:
        load.start()
    cache_loads = [
        pltpu.make_async_copy(cache_hbm.at[s], cache.at[s], cache_sem.at[s]) for s in range(seqs)
    ]
    for load in cache_loads:
        load.start()

    barrier = pltpu.get_barrier_semaphore()

    def greet(index):
        where = (index // half, 2 * (index % half) + core)

        @pl.when(jnp.logical_or(where[0] != e, where[1] != t))
        def _():
            pl.semaphore_signal(barrier, inc=1, device_id=where, device_id_type=MESH)

    each(n_ep * half, greet)
    for i in range(half):
        pl.semaphore_signal(
            barrier, inc=1, device_id=(e, 2 * i + 1 - core), device_id_type=MESH
        )

    if split:
        cols = block(t, hid)
        dense_parts = (dg_hbm.at[:, cols], du_hbm.at[:, cols], dd_hbm.at[cols, :])
    else:
        dense_parts = (dg_hbm, du_hbm, dd_hbm)
    loads = [
        pltpu.make_async_copy(src, dst, w_sem.at[i])
        for i, (src, dst) in enumerate(
            zip((ow_hbm, eg_hbm, eu_hbm) + dense_parts[:2] + (ed_hbm, dense_parts[2]), (ow, eg, eu, dg, du, ed, dd))
        )
    ]

    lane = lax.broadcasted_iota(jnp.int32, (seqs, route.shape[1]), 1)
    table = jnp.zeros((seqs, route.shape[1]), F32)
    for k in range(ids_ref.shape[0]):
        wanted = column(ids_ref[k : k + 1, :])
        table = table + jnp.where(lane == wanted, column(rw_ref[k : k + 1, :]), 0.0)
    own_rows = block(e, seqs)
    route[own_rows, :] = table

    resid = resid_ref[...].astype(F32)
    mean_sq = jnp.mean(resid * resid, axis=-1, keepdims=True)
    normed = (resid * lax.rsqrt(mean_sq + EPS) * first_gain_ref[...]).astype(BF16)
    row = lax.broadcasted_iota(jnp.int32, (seqs, LANES), 0)
    entry = lax.broadcasted_iota(jnp.int32, (seqs, LANES), 1) % QK_DIM
    position = jnp.zeros((seqs, LANES), F32)
    for s in range(seqs):
        position = jnp.where(row == s, lengths_ref[s].astype(F32), position)
    turn = QK_DIM // 2
    power = (entry % turn).astype(F32) * (-1.0 / turn)
    angle = position * jnp.exp(power * math.log(10000.0))
    cosine = jnp.cos(angle)
    sine = jnp.where(entry < turn, -jnp.sin(angle), jnp.sin(angle))

    def rotate(values):
        other = jnp.where(
            entry < turn, pltpu.roll(values, LANES - turn, 1), pltpu.roll(values, turn, 1)
        )
        return (values * cosine + other * sine).astype(BF16).astype(F32)

    query = jnp.zeros((seqs, qw.shape[1]), F32)
    for i in range(Q_CHUNKS):
        q_loads[i].wait()
        query = query + dot(
            normed[:, i * depth : (i + 1) * depth], qw[i * depth : (i + 1) * depth, :]
        )
    for load in q_loads[Q_CHUNKS:]:
        load.wait()
    keys_raw = dot(normed, kw[...])
    values_raw = dot(normed, vw[...])
    for load in loads:
        load.start()

    groups, spots = cache.shape[1], cache.shape[2]
    share = query.shape[1] // LANES // groups
    lower = lax.broadcasted_iota(jnp.int32, (seqs, LANES), 1) < QK_DIM
    fresh = []
    for g in range(groups):
        key = rotate(keys_raw[:, g * LANES : (g + 1) * LANES])
        value = values_raw[:, g * LANES : (g + 1) * LANES].astype(BF16).astype(F32)
        new_ref[:, 2 * g * LANES : (2 * g + 1) * LANES] = key
        new_ref[:, (2 * g + 1) * LANES : (2 * g + 2) * LANES] = value
        fresh.append((key, value))
        for j in range(share):
            at = (g * share + j) * LANES
            head = rotate(query[:, at : at + LANES])
            pairs[g, :, j, :] = jnp.where(lower, head, 0.0)
            pairs[g, :, share + j, :] = jnp.where(lower, 0.0, head)

    pl.semaphore_wait(barrier, n_ep * half - 1 + half)

    def route_copy(d):
        there = (e + d) % n_ep
        return remote(
            route.at[own_rows, :],
            route.at[own_rows, :],
            route_send.at[d - 1],
            route_recv.at[d - 1],
            (there, t),
        )

    def route_wait(d):
        came_from = (e + n_ep - d) % n_ep
        spot = route.at[block(came_from, seqs), :]
        remote(spot, spot, route_send.at[d - 1], route_recv.at[d - 1], (e, t)).wait_recv()

    each(n_ep - 1, lambda i: route_copy(i + 1).start())

    scale = QK_DIM**-0.5
    lines = 2 * share
    for s in range(seqs):
        cache_loads[s].wait()
        for g in range(groups):
            both = pairs[g, s].astype(BF16)
            scores[g, s] = (
                lax.dot_general(
                    both,
                    cache[s, g, :, :LANES],
                    (((1,), (1,)), ((), ())),
                    preferred_element_type=F32,
                )
                * scale
            )
    length = jnp.zeros((seqs, lines, 1), jnp.int32)
    which = lax.broadcasted_iota(jnp.int32, (seqs, lines, 1), 0)
    for s in range(seqs):
        length = jnp.where(which == s, lengths_ref[s], length)
    place = lax.broadcasted_iota(jnp.int32, (seqs, lines, spots), 2)
    valid = place < length
    line = lax.broadcasted_iota(jnp.int32, (lines, 1), 0)
    for g in range(groups):
        key, value = fresh[g]
        latest = jnp.sum(pairs[g] * key[:, None, :], axis=-1, keepdims=True) * scale
        masked = jnp.where(valid, scores[g], -jnp.inf)
        top = jnp.maximum(jnp.max(masked, axis=-1, keepdims=True), latest)
        raised = jnp.exp(masked - top)
        raised_new = jnp.exp(latest - top)
        total = jnp.sum(raised, axis=-1, keepdims=True) + raised_new
        prob = raised / total
        prob_new = jnp.broadcast_to(raised_new / total, (seqs, lines, LANES))
        lam = jnp.zeros((lines, 1), F32)
        for j in range(share):
            lam = jnp.where(line == j, lam_ref[g * share + j], lam)
        scores[g] = prob - lam[None] * pltpu.roll(prob, share, 1)
        new_weight = (prob_new - lam[None] * pltpu.roll(prob_new, share, 1)).astype(BF16).astype(F32)
        fresh_part = new_weight * value[:, None, :]
        for s in range(seqs):
            mixed[g, s] = dot(scores[g, s].astype(BF16), cache[s, g, :, LANES:])
        whole = mixed[g] + fresh_part
        mean_sq = jnp.mean(whole * whole, axis=-1, keepdims=True)
        mixed[g] = whole * lax.rsqrt(mean_sq + EPS) * head_gain_ref[...][None]
        for j in range(share):
            at = (g * share + j) * LANES
            heads_ref[:, at : at + LANES] = mixed[g, :, j, :].astype(BF16)

    def heads_copy(mask):
        return remote(
            heads_ref,
            heads_all.at[mask - 1],
            heads_send.at[mask - 1],
            heads_recv.at[mask - 1],
            (e, flip(t, mask)),
        )

    for mask in range(n_tp - 1, 0, -1):
        heads_copy(mask).start()

    loads[0].wait()
    span = heads_ref.shape[1]
    total = dot(heads_ref[...], ow[block(t, span), :])
    for mask in range(1, n_tp):
        heads_copy(mask).wait_recv()
        total = total + dot(heads_all[mask - 1], ow[block(flip(t, mask), span), :])
    own_cols = block(t, quarter)
    own_stream = (resid_ref[:, own_cols].astype(F32) + total).astype(BF16)
    stream[own_rows, own_cols] = own_stream

    def spot(owner, column):
        return stream.at[block(owner, seqs), block(column, quarter)]

    def owner_of(d):
        return (e + n_ep - d) % n_ep

    def first(d):
        return remote(
            spot(e, t), spot(e, t), first_send.at[d], stream_recv.at[0, d], ((e + d) % n_ep, t)
        )

    def second(d, mask):
        index = mask // 2 if mask != 1 else 0
        where = spot(owner_of(d), t)
        return remote(
            where, where, second_send.at[index, d], stream_recv.at[mask, d], (e, flip(t, mask))
        )

    def relay(d, mask):
        where = spot(owner_of(d), flip(t, mask))
        return remote(
            where, where, relay_send.at[mask // 2 - 1, d], stream_recv.at[mask + 1, d], (e, mate)
        )

    def arrived(d, mask):
        where = spot(owner_of(d), flip(t, mask))
        remote(where, where, first_send.at[d], stream_recv.at[mask, d], (e, t)).wait_recv()

    def spread(d):
        for mask in evens:
            second(d, mask).start()
        second(d, 1).start()

    far_first = sorted(range(1, n_ep), key=lambda d: -min(d, n_ep - d)) if n_ep <= 16 else None
    near_first = [0] + far_first[::-1] if far_first is not None else None
    each(n_ep - 1 if far_first is None else 1, lambda i: first(i + 1).start(), order=None) if far_first is None else [
        first(d).start() for d in far_first
    ]

    def stage_two(d):
        if not (isinstance(d, int) and d == 0):
            arrived(d, 0)
        spread(d)

    def stage_three(d):
        for mask in evens:
            arrived(d, mask)
            relay(d, mask).start()

    def normalise(d):
        arrived(d, 1)
        for mask in evens:
            arrived(d, mask + 1)
        rows = block(owner_of(d), seqs)
        values = stream[rows, :].astype(F32)
        mean_sq = jnp.mean(values * values, axis=-1, keepdims=True)
        scaled = (values * lax.rsqrt(mean_sq + EPS) * gain_ref[...]).astype(BF16)
        ffn[rows, :] = scaled
        inner = jnp.sum(scaled.astype(F32) * mixw_ref[...], axis=-1, keepdims=True)
        mix[rows, :] = jnp.broadcast_to(jax.nn.sigmoid(inner), (seqs, LANES))

    if near_first is not None:
        for i, d in enumerate(near_first):
            stage_two(d)
            if i:
                stage_three(near_first[i - 1])
            if i > 1:
                normalise(near_first[i - 2])
        stage_three(near_first[-1])
        for d in near_first[-2:]:
            normalise(d)
    else:
        stage_two(0)
        each(n_ep - 1, lambda i: stage_two(i + 1))
        each(n_ep, stage_three)
        each(n_ep, normalise)
    each(n_ep - 1, lambda i: route_wait(i + 1))

    many = min(rows_all, 128)
    batches = rows_all // many
    for load in loads[1:5]:
        load.wait()

    def hidden(b):
        rows = block(b, many)
        a = ffn[rows, :]
        for j in range(held):
            eh[j, rows, :] = (jax.nn.silu(dot(a, eg[j])) * dot(a, eu[j])).astype(BF16)
        units = jax.nn.silu(dot(a, dg[...])) * dot(a, du[...])
        if not split:
            own = hid // n_tp
            unit = lax.broadcasted_iota(jnp.int32, units.shape, 1)
            units = jnp.where((unit >= t * own) & (unit < (t + 1) * own), units, 0.0)
        dh[rows, :] = units.astype(BF16)

    each(batches, hidden)
    for load in loads[5:]:
        load.wait()

    def result(b, q):
        rows = block(b, many)
        cols = block(q, quarter)
        total = mix[rows, :1] * dot(dh[rows, :], dd[:, cols])
        lanes = lax.broadcasted_iota(jnp.int32, (many, route.shape[1]), 1)
        for j in range(held):
            weight = jnp.sum(
                jnp.where(lanes == e * held + j, route[rows, :], 0.0), axis=1, keepdims=True
            )
            piece = dot(eh[j, rows, :], ed[j, :, cols]).astype(BF16)
            total = total + weight * piece.astype(F32)
        return total

    def pair(j):
        return remote(away.at[j], came.at[j], pair_send.at[j], pair_recv.at[j], (e, mate))

    for j in range(half):

        def leave(b, j=j):
            away[j, block(b, many), :] = result(b, 2 * j + 1 - core).astype(BF16)

        each(batches, leave)
        pair(j).start()

    me = e * half + t // 2

    def back(j, d):
        there = (e + d) % n_ep
        return remote(
            summed.at[j, block(there, seqs), :],
            landed.at[me],
            back_send.at[j, d],
            back_recv.at[me],
            (there, 2 * j + core),
        )

    def same(j, d):
        return jnp.logical_and(jnp.asarray(d == 0), 2 * j + core == t)

    for j in range(half):

        def keep(b, j=j):
            summed[j, block(b, many), :] = result(b, 2 * j + core).astype(BF16)

        each(batches, keep)
    for j in range(half):
        pair(j).wait_recv()

        def add(b, j=j):
            rows = block(b, many)
            summed[j, rows, :] = (summed[j, rows, :].astype(F32) + came[j, rows, :].astype(F32)).astype(BF16)

        each(batches, add)

        def send(d, j=j):
            @pl.when(jnp.logical_not(same(j, d)))
            def _():
                back(j, d).start()

        each(n_ep, send, order=None if far_first is None else far_first + [0])

    landed[me] = summed[t // 2, own_rows, :]

    def take(index):
        @pl.when(index != me)
        def _():
            where = landed.at[index]
            remote(where, where, back_send.at[0, 0], back_recv.at[index], (e, t)).wait_recv()

    each(n_ep * half, take)
    out_ref[...] = own_stream.astype(F32) + jnp.sum(landed[...].astype(F32), axis=0)

    for mask in range(1, n_tp):
        heads_copy(mask).wait_send()
    each(n_ep - 1, lambda i: route_copy(i + 1).wait_send())
    each(n_ep - 1, lambda i: first(i + 1).wait_send())

    def sent(d):
        second(d, 1).wait_send()
        for mask in evens:
            second(d, mask).wait_send()
            relay(d, mask).wait_send()

    each(n_ep, sent)
    for j in range(half):
        pair(j).wait_send()

        def gone(d, j=j):
            @pl.when(jnp.logical_not(same(j, d)))
            def _():
                back(j, d).wait_send()

        each(n_ep, gone)


def near_kernel(
    n_ep,
    n_tp,
    lengths_hbm,
    lam_hbm,
    resid_hbm,
    first_gain_hbm,
    head_gain_hbm,
    gain_hbm,
    mixw_hbm,
    ids_hbm,
    rw_hbm,
    qw_hbm,
    kw_hbm,
    vw_hbm,
    cache_hbm,
    ow_hbm,
    eg_hbm,
    eu_hbm,
    ed_hbm,
    dg_hbm,
    du_hbm,
    dd_hbm,
    out_ref,
    new_ref,
    lengths_ref,
    lam_ref,
    resid_ref,
    first_gain_ref,
    head_gain_ref,
    gain_ref,
    mixw_ref,
    ids_ref,
    rw_ref,
    qkv,
    cache,
    pairs,
    asked,
    scores,
    mixed,
    heads_ref,
    ow,
    gu,
    ed,
    dg,
    du,
    dd,
    heads_all,
    mine,
    stream,
    ffn,
    mix,
    route,
    eh,
    dh,
    leaving,
    kept,
    plane_in,
    column_out,
    column_in,
    local_sem,
    push_send,
    push_recv,
    route_send,
    route_recv,
    heads_send,
    heads_recv,
    chunk_send,
    climb_recv,
    group_recv,
    plane_recv,
    column_recv,
):
    e = lax.axis_index("ep")
    t = lax.axis_index("tp")
    planes = n_ep // INNER
    z = e // INNER
    x = e % INNER
    y = t // CORES
    c = t % CORES
    keeper = z % CORES
    odd = (c + z) % CORES
    turns = planes // CORES
    seqs, width = resid_ref.shape
    quarter = out_ref.shape[1]
    part = eg_hbm.shape[2]
    hid = dg.shape[1]
    mate = flip(t, 1)

    def gather_loads(sem, *routes):
        return [pltpu.make_async_copy(src, dst, local_sem.at[sem]) for src, dst in routes]

    first_loads = gather_loads(
        0, (resid_hbm, resid_ref), (first_gain_hbm, first_gain_ref), (lengths_hbm, lengths_ref)
    )
    for load in first_loads:
        load.start()
    depth = qkv.shape[0] // Q_CHUNKS
    inner = qw_hbm.shape[1]
    side = kw_hbm.shape[1]
    for i in range(Q_CHUNKS):
        deep = pl.ds(i * depth, depth)
        for load in gather_loads(
            1 + i,
            (qw_hbm.at[deep, :], qkv.at[deep, :inner]),
            (kw_hbm.at[deep, :], qkv.at[deep, inner : inner + side]),
            (vw_hbm.at[deep, :], qkv.at[deep, inner + side :]),
        ):
            load.start()

    barrier = pltpu.get_barrier_semaphore()
    for index in range(n_ep * n_tp):
        where = (index // n_tp, index % n_tp)

        @pl.when(jnp.logical_or(where[0] != e, where[1] != t))
        def _():
            pl.semaphore_signal(barrier, inc=1, device_id=where, device_id_type=MESH)

    for load in first_loads:
        load.wait()
    bunch = seqs // CACHE_CHUNKS
    cache_loads = [
        gather_loads(
            1 + Q_CHUNKS + i,
            (cache_hbm.at[pl.ds(i * bunch, bunch)], cache.at[pl.ds(i * bunch, bunch)]),
        )[0]
        for i in range(CACHE_CHUNKS)
    ]
    for load in cache_loads:
        load.start()
    late = 1 + Q_CHUNKS + CACHE_CHUNKS
    late_loads = gather_loads(
        late,
        (ids_hbm, ids_ref),
        (rw_hbm, rw_ref),
        (lam_hbm, lam_ref),
        (head_gain_hbm, head_gain_ref),
        (gain_hbm, gain_ref),
        (mixw_hbm, mixw_ref),
    )
    for load in late_loads:
        load.start()
    cols = block(y, hid)
    e_loads = gather_loads(
        late + 1, (eg_hbm.at[0], gu.at[c, :, :part]), (eu_hbm.at[0], gu.at[c, :, part:])
    ) + gather_loads(late + 2, (ed_hbm.at[0], ed.at[block(c, part), :]))
    loads = [
        gather_loads(1 + i, route)[0]
        for i, route in enumerate(
            (
                (ow_hbm, ow),
                (dg_hbm.at[:, cols], dg),
                (du_hbm.at[:, cols], du),
                (dd_hbm.at[cols, :], dd),
            )
        )
    ]
    resid = resid_ref[...].astype(F32)
    mean_sq = jnp.mean(resid * resid, axis=-1, keepdims=True)
    normed = (resid * lax.rsqrt(mean_sq + EPS) * first_gain_ref[...]).astype(BF16)
    row = lax.broadcasted_iota(jnp.int32, (seqs, LANES), 0)
    entry = lax.broadcasted_iota(jnp.int32, (seqs, LANES), 1) % QK_DIM
    position = jnp.zeros((seqs, LANES), F32)
    for s in range(seqs):
        position = jnp.where(row == s, lengths_ref[s].astype(F32), position)
    turn = QK_DIM // 2
    power = (entry % turn).astype(F32) * (-1.0 / turn)
    angle = position * jnp.exp(power * math.log(10000.0))
    cosine = jnp.cos(angle)
    sine = jnp.where(entry < turn, -jnp.sin(angle), jnp.sin(angle))

    def rotate(values):
        other = jnp.where(
            entry < turn, pltpu.roll(values, LANES - turn, 1), pltpu.roll(values, turn, 1)
        )
        return (values * cosine + other * sine).astype(BF16).astype(F32)

    def spot(plane, inner):
        return plane // CORES * INNER + inner

    own_spot = spot(z, x)
    projected = jnp.zeros((seqs, qkv.shape[1]), F32)
    for i in range(Q_CHUNKS):
        deep = pl.ds(i * depth, depth)
        pltpu.make_async_copy(qkv.at[deep, :], qkv.at[deep, :], local_sem.at[1 + i]).wait()
        projected = projected + dot(normed[:, i * depth : (i + 1) * depth], qkv[deep, :])
    query = projected[:, :inner]
    keys_raw = projected[:, inner : inner + side]
    values_raw = projected[:, inner + side :]
    for load in e_loads + loads:
        load.start()

    groups, spots = cache.shape[1], cache.shape[2]
    share = query.shape[1] // LANES // groups
    scale = QK_DIM**-0.5
    lines = 2 * share
    lower = lax.broadcasted_iota(jnp.int32, (seqs, LANES), 1) < QK_DIM
    fresh = []
    for g in range(groups):
        key = rotate(keys_raw[:, g * LANES : (g + 1) * LANES])
        value = values_raw[:, g * LANES : (g + 1) * LANES].astype(BF16).astype(F32)
        new_ref[:, 2 * g * LANES : (2 * g + 1) * LANES] = key.astype(BF16)
        new_ref[:, (2 * g + 1) * LANES : (2 * g + 2) * LANES] = value.astype(BF16)
        fresh.append((key, value))
        for j in range(share):
            at = (g * share + j) * LANES
            head = rotate(query[:, at : at + LANES])
            pairs[g, :, j, :] = jnp.where(lower, head, 0.0)
            pairs[g, :, share + j, :] = jnp.where(lower, 0.0, head)
        spread = (pairs[g] * scale).reshape(seqs * lines, LANES).astype(BF16)
        turn_of = lax.broadcasted_iota(jnp.int32, spread.shape, 0) // lines % 2
        asked[g, :, :LANES] = jnp.where(turn_of == 0, spread, jnp.zeros_like(spread))
        asked[g, :, LANES:] = jnp.where(turn_of == 0, jnp.zeros_like(spread), spread)

    pl.semaphore_wait(barrier, n_ep * n_tp - 1)

    def push(index):
        where = (gu.at[c], ed.at[block(c, part), :])[index]
        return remote(where, where, push_send.at[0], push_recv.at[index], (e, mate))

    def pushed(index):
        where = (gu.at[1 - c], ed.at[block(1 - c, part), :])[index]
        remote(where, where, push_send.at[0], push_recv.at[index], (e, mate)).wait_recv()

    def beside(s, g, lanes):
        return jnp.concatenate([cache[s, g, :, lanes], cache[s + 1, g, :, lanes]], axis=1)

    for s in range(0, seqs, 2):
        if s % bunch == 0:
            cache_loads[s // bunch].wait()
        for g in range(groups):
            scores[g, s : s + 2] = lax.dot_general(
                asked[g, s * lines : (s + 2) * lines, :],
                beside(s, g, slice(0, LANES)),
                (((1,), (1,)), ((), ())),
                preferred_element_type=F32,
            ).reshape(2, lines, spots)
    for load in late_loads:
        load.wait()
    length = jnp.zeros((seqs, lines, 1), jnp.int32)
    which = lax.broadcasted_iota(jnp.int32, (seqs, lines, 1), 0)
    for s in range(seqs):
        length = jnp.where(which == s, lengths_ref[s], length)
    place = lax.broadcasted_iota(jnp.int32, (seqs, lines, spots), 2)
    valid = place < length
    line = lax.broadcasted_iota(jnp.int32, (lines, 1), 0)
    for g in range(groups):
        key, value = fresh[g]
        latest = jnp.sum(pairs[g] * key[:, None, :], axis=-1, keepdims=True) * scale
        masked = jnp.where(valid, scores[g], -jnp.inf)
        top = jnp.maximum(jnp.max(masked, axis=-1, keepdims=True), latest)
        raised = jnp.exp(masked - top)
        raised_new = jnp.exp(latest - top)
        total = jnp.sum(raised, axis=-1, keepdims=True) + raised_new
        lam = jnp.full((lines, 1), 1.0, F32)
        for j in range(share):
            lam = jnp.where(line == share + j, lam_ref[g * share + j], lam)
        part_of = lam[None] / total
        prob = raised * part_of
        prob_new = jnp.broadcast_to(raised_new * part_of, (seqs, lines, LANES))
        weights = (prob - pltpu.roll(prob, share, 1)).astype(BF16)
        new_weight = (prob_new - pltpu.roll(prob_new, share, 1)).astype(BF16).astype(F32)
        fresh_part = new_weight * value[:, None, :]
        for s in range(0, seqs, 2):
            both = dot(
                weights[s : s + 2].reshape(2 * lines, spots), beside(s, g, slice(LANES, None))
            )
            mixed[g, s] = both[:lines, :LANES]
            mixed[g, s + 1] = both[lines:, LANES:]
        whole = mixed[g] + fresh_part
        mean_sq = jnp.mean(whole * whole, axis=-1, keepdims=True)
        mixed[g] = whole * lax.rsqrt(mean_sq + EPS) * head_gain_ref[...][None]
        for j in range(share):
            at = (g * share + j) * LANES
            heads_ref[:, at : at + LANES] = mixed[g, :, j, :].astype(BF16)

    def heads_copy(mask):
        return remote(
            heads_ref,
            heads_all.at[mask - 1],
            heads_send.at[0],
            heads_recv.at[mask // CORES],
            (e, flip(t, mask)),
        )

    for mask in range(n_tp - 1, 0, -1):
        heads_copy(mask).start()

    for load in e_loads:
        load.wait()
    push(0).start()
    push(1).start()

    lane = lax.broadcasted_iota(jnp.int32, (seqs, route.shape[2]), 1)
    table = jnp.zeros((seqs, route.shape[2]), F32)
    for k in range(ids_ref.shape[0]):
        wanted = column(ids_ref[k : k + 1, :])
        table = table + jnp.where(lane == wanted, column(rw_ref[k : k + 1, :]), 0.0)

    @pl.when(odd == 0)
    def _():
        route[own_spot] = table

    def route_copy(mask):
        where = route.at[own_spot]
        return remote(
            where, where, route_send.at[0], route_recv.at[0], (flip(e, mask), t)
        )

    @pl.when(odd == 0)
    def _():
        for mask in range(1, n_ep):
            route_copy(mask).start()


    loads[0].wait()
    span = heads_ref.shape[1]
    total = dot(heads_ref[...], ow[block(t, span), :])
    for far in range(n_tp // CORES):
        batch = heads_all.at[pl.ds(0, 1) if far == 0 else pl.ds(far * CORES - 1, CORES)]
        remote(batch, batch, heads_send.at[0], heads_recv.at[far], (e, t)).wait_recv()
        for mask in range(max(far * CORES, 1), (far + 1) * CORES):
            total = total + dot(heads_all[mask - 1], ow[block(flip(t, mask), span), :])
    own_cols = block(t, quarter)
    own_stream = (resid_ref[:, own_cols].astype(F32) + total).astype(BF16)
    mine[...] = own_stream

    around = ((1, 1), (1, 0), (0, 1))

    def at_spot(where, owner):
        return stream.at[block(where, seqs), block(owner, quarter)]

    def to_plane(step):
        dx, dy = around[step]
        there = (z * INNER + flip(x, dx), flip(y, dy) * CORES + keeper)
        return remote(
            mine, at_spot(own_spot, t), chunk_send.at[0], group_recv.at[0, dx], there
        )

    def to_column(d):
        there = (flip(z, d) * INNER + x, y * CORES + keeper)
        return remote(
            mine, at_spot(own_spot, t), chunk_send.at[0], climb_recv.at[d // CORES, c], there
        )

    def to_mate():
        return remote(
            mine, at_spot(own_spot, t), chunk_send.at[0], climb_recv.at[0, c], (e, mate)
        )

    for d in range(planes - 1, 0, -1):
        to_column(d).start()
    for step in range(len(around)):
        to_plane(step).start()

    @pl.when(odd == 1)
    def _():
        to_mate().start()

    @pl.when(odd == 0)
    def _():
        stream[block(own_spot, seqs), own_cols] = own_stream

    near = z + odd * (1 - 2 * (z % 2))

    def plane_of(i):
        return flip(near, 2 * i)

    def arrived(i, core):
        where = at_spot(spot(plane_of(i), x), y * CORES + core)
        remote(where, where, chunk_send.at[0], climb_recv.at[i, core], (e, t)).wait_recv()

    def forward(i, core, step):
        dx, dy = around[step]
        where = at_spot(spot(plane_of(i), x), y * CORES + core)
        return remote(
            where,
            where,
            chunk_send.at[0],
            group_recv.at[i, dx],
            (z * INNER + flip(x, dx), flip(y, dy) * CORES + c),
        )

    def relay(i):
        for core in range(CORES):
            arrived(i, core)
            for step in range(len(around)):
                forward(i, core, step).start()

    def gather(i):
        if i == 0:

            @pl.when(odd == 1)
            def _():
                relay(0)

            @pl.when(odd == 0)
            def _():
                arrived(0, 1 - c)
        else:
            relay(i)

    def normalise(i):
        for inner in range(INNER):
            rows = block(spot(plane_of(i), flip(x, inner)), seqs)
            came = stream.at[rows, :] if inner else stream.at[rows, block(flip(y, 1), CORES * quarter)]
            remote(came, came, chunk_send.at[0], group_recv.at[i, inner], (e, t)).wait_recv()
            values = stream[rows, :].astype(F32)
            mean_sq = jnp.mean(values * values, axis=-1, keepdims=True)
            scaled = (values * lax.rsqrt(mean_sq + EPS) * gain_ref[...]).astype(BF16)
            ffn[rows, :] = scaled
            inside = jnp.sum(scaled.astype(F32) * mixw_ref[...], axis=-1, keepdims=True)
            mix[rows, :] = jnp.broadcast_to(jax.nn.sigmoid(inside), (seqs, LANES))

    for i in range(turns):
        gather(i)
    for i in range(turns):
        normalise(i)

    def route_wait(count):
        where = route.at[pl.ds(0, count)]
        remote(where, where, route_send.at[0], route_recv.at[0], (e, t)).wait_recv()

    @pl.when(odd == 0)
    def _():
        route_wait(route.shape[0] - 1)

    @pl.when(odd == 1)
    def _():
        route_wait(route.shape[0])

    rows_all = ffn.shape[0]
    pushed(0)
    pushed(1)
    for load in loads[1:3]:
        load.wait()
    a = ffn[...]
    for core in range(CORES):
        both = dot(a, gu[core])
        eh[:, core * part : (core + 1) * part] = (
            jax.nn.silu(both[:, :part]) * both[:, part:]
        ).astype(BF16)
    dh[...] = (jax.nn.silu(dot(a, dg[...])) * dot(a, du[...])).astype(BF16)
    loads[3].wait()

    lanes = lax.broadcasted_iota(jnp.int32, (rows_all, route.shape[2]), 1)
    weight = jnp.sum(
        jnp.where(lanes == e, route[...].reshape(rows_all, route.shape[2]), 0.0),
        axis=1,
        keepdims=True,
    )

    def leave(i, core, step):
        dx, dy = around[step]
        where = spot(plane_of(i), flip(x, dx))
        return remote(
            leaving.at[dy, block(where, seqs), pl.ds(core * quarter, quarter)],
            plane_in.at[i, core, step],
            chunk_send.at[0],
            plane_recv.at[i, core],
            (z * INNER + flip(x, dx), flip(y, dy) * CORES + c),
        )

    order = range(turns - 1, -1, -1)
    for dy in (1, 0):
        cols = block(flip(y, dy), CORES * quarter)
        total = mix[:, :1] * dot(dh[...], dd[:, cols]) + weight * dot(eh[...], ed[:, cols])
        leaving[dy] = total.astype(BF16)
        if not dy:
            kept[...] = total
        for i in order:
            for core in range(CORES):
                for step in range(len(around)):
                    if around[step][1] == dy:
                        leave(i, core, step).start()

    def own_plane(i):
        return jnp.logical_and(odd == 0, i == 0)

    def climb(i, core):
        return remote(
            column_out.at[i, core],
            column_in.at[odd + 2 * i],
            chunk_send.at[0],
            column_recv.at[0],
            (plane_of(i) * INNER + x, y * CORES + core),
        )

    def stays(i, core):
        return jnp.logical_and(own_plane(i), c == core)

    for i in order:
        for core in range(CORES):
            gathered = kept[block(spot(plane_of(i), x), seqs), core * quarter : (core + 1) * quarter]
            came = plane_in.at[i, core]
            remote(came, came, chunk_send.at[0], plane_recv.at[i, core], (e, t)).wait_recv()
            for step in range(len(around)):
                gathered = gathered + plane_in[i, core, step].astype(F32)
            column_out[i, core] = gathered.astype(BF16)

            @pl.when(jnp.logical_not(stays(i, core)))
            def _(i=i, core=core):
                climb(i, core).start()

    def took(start):
        where = column_in.at[pl.ds(start, planes - start)]
        remote(where, where, chunk_send.at[0], column_recv.at[0], (e, t)).wait_recv()

    @pl.when(odd == 0)
    def _():
        column_in[0] = column_out[0, c]
        took(1)

    @pl.when(odd == 1)
    def _():
        took(0)

    out_ref[...] = (
        own_stream.astype(F32) + jnp.sum(column_in[...].astype(F32), axis=0)
    ).astype(BF16)

    push(0).wait_send()
    push(1).wait_send()
    remote(heads_all, heads_all, heads_send.at[0], heads_recv.at[0], (e, t)).wait_send()

    def drained(count):
        where = ow.at[pl.ds(0, count * seqs), :]
        remote(where, where, chunk_send.at[0], column_recv.at[0], (e, t)).wait_send()

    hops = len(around)
    always = planes - 1 + hops + 2 * turns * CORES * hops + turns * CORES

    @pl.when(odd == 0)
    def _():
        for mask in range(1, n_ep):
            route_copy(mask).wait_send()
        drained(always - CORES * hops - 1)

    @pl.when(odd == 1)
    def _():
        drained(always + 1)


def near_call(n_ep, n_tp, arrays):
    (
        residual_in,
        lengths,
        kv_cache,
        norm_gain_attn,
        query_weight,
        key_weight,
        value_weight,
        diff_lambda,
        head_gain,
        out_weight,
        norm_gain_ffn,
        route_ids,
        route_weights,
        expert_gate,
        expert_up,
        expert_down,
        dense_gate,
        dense_up,
        dense_down,
        dense_mix,
    ) = arrays
    seqs, width = residual_in.shape
    held = lambda value: pltpu.with_memory_space_constraint(value, pltpu.HBM)
    groups, spots = kv_cache.shape[1:3]
    share = diff_lambda.shape[0] // groups
    inner = query_weight.shape[1]
    quarter = out_weight.shape[1]
    part = expert_gate.shape[2]
    hid = dense_gate.shape[1] // (n_tp // CORES)
    turns = n_ep // INNER // CORES
    blocks = turns * INNER
    rows = blocks * seqs
    lanes = -(-n_ep // LANES) * LANES
    topk = route_ids.shape[1]
    vmem = pl.BlockSpec(memory_space=pltpu.VMEM)
    hbm = pl.BlockSpec(memory_space=pltpu.HBM)
    dma = pltpu.SemaphoreType.DMA
    layer_out, fresh = pl.pallas_call(
        functools.partial(near_kernel, n_ep, n_tp),
        out_shape=(
            jax.ShapeDtypeStruct((seqs, quarter), BF16),
            jax.ShapeDtypeStruct((seqs, groups * kv_cache.shape[3]), BF16),
        ),
        in_specs=[hbm] * 20,
        out_specs=(vmem, vmem),
        scratch_shapes=[
            pltpu.SMEM(lengths.shape, jnp.int32),
            pltpu.SMEM(diff_lambda.shape, F32),
            pltpu.VMEM(residual_in.shape, BF16),
            pltpu.VMEM((1, width), F32),
            pltpu.VMEM((1, head_gain.shape[0]), F32),
            pltpu.VMEM((1, width), F32),
            pltpu.VMEM((1, width), F32),
            pltpu.VMEM((topk, seqs), jnp.int32),
            pltpu.VMEM((topk, seqs), F32),
            pltpu.VMEM((width, inner + key_weight.shape[1] + value_weight.shape[1]), BF16),
            pltpu.VMEM(kv_cache.shape, BF16),
            pltpu.VMEM((groups, seqs, 2 * share, LANES), F32),
            pltpu.VMEM((groups, seqs * 2 * share, 2 * LANES), BF16),
            pltpu.VMEM((groups, seqs, 2 * share, spots), F32),
            pltpu.VMEM((groups, seqs, 2 * share, LANES), F32),
            pltpu.VMEM((seqs, inner), BF16),
            pltpu.VMEM(out_weight.shape, BF16),
            pltpu.VMEM((CORES, width, 2 * part), BF16),
            pltpu.VMEM((CORES * part, width), BF16),
            pltpu.VMEM((width, hid), BF16),
            pltpu.VMEM((width, hid), BF16),
            pltpu.VMEM((hid, width), BF16),
            pltpu.VMEM((n_tp - 1, seqs, inner), BF16),
            pltpu.VMEM((seqs, quarter), BF16),
            pltpu.VMEM((rows, width), BF16),
            pltpu.VMEM((rows, width), BF16),
            pltpu.VMEM((rows, LANES), F32),
            pltpu.VMEM((blocks, seqs, lanes), F32),
            pltpu.VMEM((rows, CORES * part), BF16),
            pltpu.VMEM((rows, hid), BF16),
            pltpu.VMEM((2, rows, CORES * quarter), BF16),
            pltpu.VMEM((rows, CORES * quarter), F32),
            pltpu.VMEM((turns, CORES, 3, seqs, quarter), BF16),
            pltpu.VMEM((turns, CORES, seqs, quarter), BF16),
            pltpu.VMEM((n_ep // INNER, seqs, quarter), BF16),
            dma((Q_CHUNKS + CACHE_CHUNKS + 4,)),
            dma((1,)),
            dma((2,)),
            dma((1,)),
            dma((1,)),
            dma((1,)),
            dma((n_tp // CORES,)),
            dma((1,)),
            dma((turns, CORES)),
            dma((turns, INNER)),
            dma((turns, CORES)),
            dma((1,)),
        ],
        compiler_params=pltpu.CompilerParams(
            collective_id=0, has_side_effects=True, vmem_limit_bytes=36 * 1024 * 1024
        ),
    )(
        held(lengths),
        held(diff_lambda),
        held(residual_in),
        held(norm_gain_attn[None, :]),
        held(head_gain[None, :]),
        held(norm_gain_ffn[None, :]),
        held(dense_mix[None, :]),
        held(route_ids.T),
        held(route_weights.T),
        held(query_weight),
        held(key_weight),
        held(value_weight),
        held(kv_cache),
        held(out_weight),
        held(expert_gate),
        held(expert_up),
        held(expert_down),
        held(dense_gate),
        held(dense_up),
        held(dense_down),
    )
    return layer_out, fresh.reshape(seqs, groups, kv_cache.shape[3])


def on_device(
    residual_in,
    lengths,
    kv_cache,
    norm_gain_attn,
    query_weight,
    key_weight,
    value_weight,
    diff_lambda,
    head_gain,
    out_weight,
    norm_gain_ffn,
    route_ids,
    route_weights,
    expert_gate,
    expert_up,
    expert_down,
    dense_gate,
    dense_up,
    dense_down,
    dense_mix,
):
    n_ep = lax.axis_size("ep")
    n_tp = lax.axis_size("tp")
    half = n_tp // 2
    if (
        n_tp == 2 * CORES
        and n_ep in (4, 8, 16)
        and expert_gate.shape[0] == 1
        and dense_gate.shape[1] // half % LANES == 0
        and expert_gate.shape[2] % LANES == 0
    ):
        return near_call(
            n_ep,
            n_tp,
            (
                residual_in,
                lengths,
                kv_cache,
                norm_gain_attn,
                query_weight,
                key_weight,
                value_weight,
                diff_lambda,
                head_gain,
                out_weight,
                norm_gain_ffn,
                route_ids,
                route_weights,
                expert_gate,
                expert_up,
                expert_down,
                dense_gate,
                dense_up,
                dense_down,
                dense_mix,
            ),
        )
    seqs, width = residual_in.shape
    groups, spots = kv_cache.shape[1:3]
    share = diff_lambda.shape[0] // groups
    inner = query_weight.shape[1]
    quarter = out_weight.shape[1]
    held, _, part = expert_gate.shape
    rows = n_ep * seqs
    own = dense_gate.shape[1] // n_tp
    split = own % LANES == 0
    hid = own if split else dense_gate.shape[1]
    lanes = -(-n_ep * held // LANES) * LANES
    vmem = pl.BlockSpec(memory_space=pltpu.VMEM)
    smem = pl.BlockSpec(memory_space=pltpu.SMEM)
    hbm = pl.BlockSpec(memory_space=pl.ANY)
    dma = pltpu.SemaphoreType.DMA
    layer_out, fresh = pl.pallas_call(
        functools.partial(layer_kernel, n_ep, n_tp, split),
        out_shape=(
            jax.ShapeDtypeStruct((seqs, quarter), F32),
            jax.ShapeDtypeStruct((seqs, groups * kv_cache.shape[3]), F32),
        ),
        in_specs=[smem] * 2 + [vmem] * 7 + [hbm] * 11,
        out_specs=(vmem, vmem),
        scratch_shapes=[
            pltpu.VMEM(query_weight.shape, BF16),
            pltpu.VMEM(key_weight.shape, BF16),
            pltpu.VMEM(value_weight.shape, BF16),
            pltpu.VMEM(kv_cache.shape, BF16),
            pltpu.VMEM((groups, seqs, 2 * share, LANES), F32),
            pltpu.VMEM((groups, seqs, 2 * share, spots), F32),
            pltpu.VMEM((groups, seqs, 2 * share, LANES), F32),
            pltpu.VMEM((seqs, inner), BF16),
            pltpu.VMEM(out_weight.shape, BF16),
            pltpu.VMEM(expert_gate.shape, BF16),
            pltpu.VMEM(expert_up.shape, BF16),
            pltpu.VMEM(expert_down.shape, BF16),
            pltpu.VMEM((width, hid), BF16),
            pltpu.VMEM((width, hid), BF16),
            pltpu.VMEM((hid, width), BF16),
            pltpu.VMEM((n_tp - 1, seqs, inner), BF16),
            pltpu.VMEM((rows, width), BF16),
            pltpu.VMEM((rows, width), BF16),
            pltpu.VMEM((rows, LANES), F32),
            pltpu.VMEM((rows, lanes), F32),
            pltpu.VMEM((held, rows, part), BF16),
            pltpu.VMEM((rows, hid), BF16),
            pltpu.VMEM((half, rows, quarter), BF16),
            pltpu.VMEM((half, rows, quarter), BF16),
            pltpu.VMEM((half, rows, quarter), BF16),
            pltpu.VMEM((n_ep * half, seqs, quarter), BF16),
            dma((7,)),
            dma((Q_CHUNKS + 2,)),
            dma((seqs,)),
            dma((n_ep - 1,)),
            dma((n_ep - 1,)),
            dma((n_tp - 1,)),
            dma((n_tp - 1,)),
            dma((n_ep,)),
            dma((half, n_ep)),
            dma((max(half - 1, 1), n_ep)),
            dma((n_tp, n_ep)),
            dma((half,)),
            dma((half,)),
            dma((half, n_ep)),
            dma((n_ep * half,)),
        ],
        compiler_params=pltpu.CompilerParams(
            collective_id=0, has_side_effects=True, vmem_limit_bytes=60 * 1024 * 1024
        ),
    )(
        lengths,
        diff_lambda,
        residual_in,
        norm_gain_attn[None, :],
        head_gain[None, :],
        norm_gain_ffn[None, :],
        dense_mix[None, :],
        route_ids.T,
        route_weights.T,
        query_weight,
        key_weight,
        value_weight,
        kv_cache,
        out_weight,
        expert_gate,
        expert_up,
        expert_down,
        dense_gate,
        dense_up,
        dense_down,
    )
    new_rows = fresh.astype(BF16).reshape(seqs, groups, kv_cache.shape[3])
    return (layer_out.astype(BF16), new_rows)


def solution(mesh):
    placed = (
        P("ep", None),
        P("ep"),
        P("ep", "tp", None, None),
        P(),
        P(None, "tp"),
        P(None, "tp"),
        P(None, "tp"),
        P("tp"),
        P(),
        P(None, "tp"),
        P(),
        P("ep", None),
        P("ep", None),
        P("ep", None, "tp"),
        P("ep", None, "tp"),
        P("ep", "tp", None),
        P(None, "ep"),
        P(None, "ep"),
        P("ep", None),
        P(),
    )
    return jax.shard_map(
        on_device,
        mesh=mesh,
        in_specs=placed,
        out_specs=(P("ep", "tp"), P("ep", "tp", None)),
        check_vma=False,
    )
```

```python
import functools
import math

import jax
import jax.numpy as jnp
from jax import lax
from jax.experimental import pallas as pl
from jax.experimental.pallas import tpu as pltpu
from jax.sharding import PartitionSpec as P

QK_DIM = 64
EPS = 1e-06
MESH = pl.DeviceIdType.MESH
F32 = jnp.float32
BF16 = jnp.bfloat16
LANES = 128
Q_CHUNKS = 4
INNER = 2
CORES = 2
RELAY = 1
CACHE_CHUNKS = 4


def flip(value, mask):
    bit = 1
    while bit <= mask:
        if mask & bit:
            value = value + bit * (1 - 2 * ((value // bit) % 2))
        bit *= 2
    return value


def each(count, body, order=None):
    if count <= 16:
        for index in order if order is not None else range(count):
            body(index)
    else:

        def step(index, carry):
            body(index)
            return carry

        lax.fori_loop(0, count, step, 0)


def block(start, size):
    return pl.ds(pl.multiple_of(start * size, size), size)


def remote(source, target, send, recv, where):
    return pltpu.make_async_remote_copy(
        src_ref=source,
        dst_ref=target,
        send_sem=send,
        recv_sem=recv,
        device_id=where,
        device_id_type=MESH,
    )


def dot(left, right):
    return jnp.dot(left, right, preferred_element_type=F32)


def column(row):
    count = row.shape[1]
    square = (count, count)
    same = lax.broadcasted_iota(jnp.int32, square, 0) == lax.broadcasted_iota(jnp.int32, square, 1)
    return jnp.sum(jnp.where(same, row, jnp.zeros_like(row)), axis=1, keepdims=True)


def layer_kernel(
    n_ep,
    n_tp,
    split,
    lengths_ref,
    lam_ref,
    resid_ref,
    first_gain_ref,
    head_gain_ref,
    gain_ref,
    mixw_ref,
    ids_ref,
    rw_ref,
    qw_hbm,
    kw_hbm,
    vw_hbm,
    cache_hbm,
    ow_hbm,
    eg_hbm,
    eu_hbm,
    ed_hbm,
    dg_hbm,
    du_hbm,
    dd_hbm,
    out_ref,
    new_ref,
    qw,
    kw,
    vw,
    cache,
    pairs,
    scores,
    mixed,
    heads_ref,
    ow,
    eg,
    eu,
    ed,
    dg,
    du,
    dd,
    heads_all,
    stream,
    ffn,
    mix,
    route,
    eh,
    dh,
    away,
    came,
    summed,
    landed,
    w_sem,
    q_sem,
    cache_sem,
    route_send,
    route_recv,
    heads_send,
    heads_recv,
    first_send,
    second_send,
    relay_send,
    stream_recv,
    pair_send,
    pair_recv,
    back_send,
    back_recv,
):
    e = lax.axis_index("ep")
    t = lax.axis_index("tp")
    half = n_tp // 2
    mate = flip(t, 1)
    core = t % 2
    seqs, width = resid_ref.shape
    quarter = out_ref.shape[1]
    held, _, part = eg.shape
    hid = dg.shape[1]
    rows_all = n_ep * seqs
    evens = [2 * i for i in range(1, half)]

    depth = qw.shape[0] // Q_CHUNKS
    q_loads = [
        pltpu.make_async_copy(
            qw_hbm.at[pl.ds(i * depth, depth), :], qw.at[pl.ds(i * depth, depth), :], q_sem.at[i]
        )
        for i in range(Q_CHUNKS)
    ] + [
        pltpu.make_async_copy(kw_hbm, kw, q_sem.at[Q_CHUNKS]),
        pltpu.make_async_copy(vw_hbm, vw, q_sem.at[Q_CHUNKS + 1]),
    ]
    for load in q_loads:
        load.start()
    cache_loads = [
        pltpu.make_async_copy(cache_hbm.at[s], cache.at[s], cache_sem.at[s]) for s in range(seqs)
    ]
    for load in cache_loads:
        load.start()

    barrier = pltpu.get_barrier_semaphore()

    def greet(index):
        where = (index // half, 2 * (index % half) + core)

        @pl.when(jnp.logical_or(where[0] != e, where[1] != t))
        def _():
            pl.semaphore_signal(barrier, inc=1, device_id=where, device_id_type=MESH)

    each(n_ep * half, greet)
    for i in range(half):
        pl.semaphore_signal(
            barrier, inc=1, device_id=(e, 2 * i + 1 - core), device_id_type=MESH
        )

    if split:
        cols = block(t, hid)
        dense_parts = (dg_hbm.at[:, cols], du_hbm.at[:, cols], dd_hbm.at[cols, :])
    else:
        dense_parts = (dg_hbm, du_hbm, dd_hbm)
    loads = [
        pltpu.make_async_copy(src, dst, w_sem.at[i])
        for i, (src, dst) in enumerate(
            zip((ow_hbm, eg_hbm, eu_hbm) + dense_parts[:2] + (ed_hbm, dense_parts[2]), (ow, eg, eu, dg, du, ed, dd))
        )
    ]

    lane = lax.broadcasted_iota(jnp.int32, (seqs, route.shape[1]), 1)
    table = jnp.zeros((seqs, route.shape[1]), F32)
    for k in range(ids_ref.shape[0]):
        wanted = column(ids_ref[k : k + 1, :])
        table = table + jnp.where(lane == wanted, column(rw_ref[k : k + 1, :]), 0.0)
    own_rows = block(e, seqs)
    route[own_rows, :] = table

    resid = resid_ref[...].astype(F32)
    mean_sq = jnp.mean(resid * resid, axis=-1, keepdims=True)
    normed = (resid * lax.rsqrt(mean_sq + EPS) * first_gain_ref[...]).astype(BF16)
    row = lax.broadcasted_iota(jnp.int32, (seqs, LANES), 0)
    entry = lax.broadcasted_iota(jnp.int32, (seqs, LANES), 1) % QK_DIM
    position = jnp.zeros((seqs, LANES), F32)
    for s in range(seqs):
        position = jnp.where(row == s, lengths_ref[s].astype(F32), position)
    turn = QK_DIM // 2
    power = (entry % turn).astype(F32) * (-1.0 / turn)
    angle = position * jnp.exp(power * math.log(10000.0))
    cosine = jnp.cos(angle)
    sine = jnp.where(entry < turn, -jnp.sin(angle), jnp.sin(angle))

    def rotate(values):
        other = jnp.where(
            entry < turn, pltpu.roll(values, LANES - turn, 1), pltpu.roll(values, turn, 1)
        )
        return (values * cosine + other * sine).astype(BF16).astype(F32)

    query = jnp.zeros((seqs, qw.shape[1]), F32)
    for i in range(Q_CHUNKS):
        q_loads[i].wait()
        query = query + dot(
            normed[:, i * depth : (i + 1) * depth], qw[i * depth : (i + 1) * depth, :]
        )
    for load in q_loads[Q_CHUNKS:]:
        load.wait()
    keys_raw = dot(normed, kw[...])
    values_raw = dot(normed, vw[...])
    for load in loads:
        load.start()

    groups, spots = cache.shape[1], cache.shape[2]
    share = query.shape[1] // LANES // groups
    lower = lax.broadcasted_iota(jnp.int32, (seqs, LANES), 1) < QK_DIM
    fresh = []
    for g in range(groups):
        key = rotate(keys_raw[:, g * LANES : (g + 1) * LANES])
        value = values_raw[:, g * LANES : (g + 1) * LANES].astype(BF16).astype(F32)
        new_ref[:, 2 * g * LANES : (2 * g + 1) * LANES] = key
        new_ref[:, (2 * g + 1) * LANES : (2 * g + 2) * LANES] = value
        fresh.append((key, value))
        for j in range(share):
            at = (g * share + j) * LANES
            head = rotate(query[:, at : at + LANES])
            pairs[g, :, j, :] = jnp.where(lower, head, 0.0)
            pairs[g, :, share + j, :] = jnp.where(lower, 0.0, head)

    pl.semaphore_wait(barrier, n_ep * half - 1 + half)

    def route_copy(d):
        there = (e + d) % n_ep
        return remote(
            route.at[own_rows, :],
            route.at[own_rows, :],
            route_send.at[d - 1],
            route_recv.at[d - 1],
            (there, t),
        )

    def route_wait(d):
        came_from = (e + n_ep - d) % n_ep
        spot = route.at[block(came_from, seqs), :]
        remote(spot, spot, route_send.at[d - 1], route_recv.at[d - 1], (e, t)).wait_recv()

    each(n_ep - 1, lambda i: route_copy(i + 1).start())

    scale = QK_DIM**-0.5
    lines = 2 * share
    for s in range(seqs):
        cache_loads[s].wait()
        for g in range(groups):
            both = pairs[g, s].astype(BF16)
            scores[g, s] = (
                lax.dot_general(
                    both,
                    cache[s, g, :, :LANES],
                    (((1,), (1,)), ((), ())),
                    preferred_element_type=F32,
                )
                * scale
            )
    length = jnp.zeros((seqs, lines, 1), jnp.int32)
    which = lax.broadcasted_iota(jnp.int32, (seqs, lines, 1), 0)
    for s in range(seqs):
        length = jnp.where(which == s, lengths_ref[s], length)
    place = lax.broadcasted_iota(jnp.int32, (seqs, lines, spots), 2)
    valid = place < length
    line = lax.broadcasted_iota(jnp.int32, (lines, 1), 0)
    for g in range(groups):
        key, value = fresh[g]
        latest = jnp.sum(pairs[g] * key[:, None, :], axis=-1, keepdims=True) * scale
        masked = jnp.where(valid, scores[g], -jnp.inf)
        top = jnp.maximum(jnp.max(masked, axis=-1, keepdims=True), latest)
        raised = jnp.exp(masked - top)
        raised_new = jnp.exp(latest - top)
        total = jnp.sum(raised, axis=-1, keepdims=True) + raised_new
        prob = raised / total
        prob_new = jnp.broadcast_to(raised_new / total, (seqs, lines, LANES))
        lam = jnp.zeros((lines, 1), F32)
        for j in range(share):
            lam = jnp.where(line == j, lam_ref[g * share + j], lam)
        scores[g] = prob - lam[None] * pltpu.roll(prob, share, 1)
        new_weight = (prob_new - lam[None] * pltpu.roll(prob_new, share, 1)).astype(BF16).astype(F32)
        fresh_part = new_weight * value[:, None, :]
        for s in range(seqs):
            mixed[g, s] = dot(scores[g, s].astype(BF16), cache[s, g, :, LANES:])
        whole = mixed[g] + fresh_part
        mean_sq = jnp.mean(whole * whole, axis=-1, keepdims=True)
        mixed[g] = whole * lax.rsqrt(mean_sq + EPS) * head_gain_ref[...][None]
        for j in range(share):
            at = (g * share + j) * LANES
            heads_ref[:, at : at + LANES] = mixed[g, :, j, :].astype(BF16)

    def heads_copy(mask):
        return remote(
            heads_ref,
            heads_all.at[mask - 1],
            heads_send.at[mask - 1],
            heads_recv.at[mask - 1],
            (e, flip(t, mask)),
        )

    for mask in range(n_tp - 1, 0, -1):
        heads_copy(mask).start()

    loads[0].wait()
    span = heads_ref.shape[1]
    total = dot(heads_ref[...], ow[block(t, span), :])
    for mask in range(1, n_tp):
        heads_copy(mask).wait_recv()
        total = total + dot(heads_all[mask - 1], ow[block(flip(t, mask), span), :])
    own_cols = block(t, quarter)
    own_stream = (resid_ref[:, own_cols].astype(F32) + total).astype(BF16)
    stream[own_rows, own_cols] = own_stream

    def spot(owner, column):
        return stream.at[block(owner, seqs), block(column, quarter)]

    def owner_of(d):
        return (e + n_ep - d) % n_ep

    def first(d):
        return remote(
            spot(e, t), spot(e, t), first_send.at[d], stream_recv.at[0, d], ((e + d) % n_ep, t)
        )

    def second(d, mask):
        index = mask // 2 if mask != 1 else 0
        where = spot(owner_of(d), t)
        return remote(
            where, where, second_send.at[index, d], stream_recv.at[mask, d], (e, flip(t, mask))
        )

    def relay(d, mask):
        where = spot(owner_of(d), flip(t, mask))
        return remote(
            where, where, relay_send.at[mask // 2 - 1, d], stream_recv.at[mask + 1, d], (e, mate)
        )

    def arrived(d, mask):
        where = spot(owner_of(d), flip(t, mask))
        remote(where, where, first_send.at[d], stream_recv.at[mask, d], (e, t)).wait_recv()

    def spread(d):
        for mask in evens:
            second(d, mask).start()
        second(d, 1).start()

    far_first = sorted(range(1, n_ep), key=lambda d: -min(d, n_ep - d)) if n_ep <= 16 else None
    near_first = [0] + far_first[::-1] if far_first is not None else None
    each(n_ep - 1 if far_first is None else 1, lambda i: first(i + 1).start(), order=None) if far_first is None else [
        first(d).start() for d in far_first
    ]

    def stage_two(d):
        if not (isinstance(d, int) and d == 0):
            arrived(d, 0)
        spread(d)

    def stage_three(d):
        for mask in evens:
            arrived(d, mask)
            relay(d, mask).start()

    def normalise(d):
        arrived(d, 1)
        for mask in evens:
            arrived(d, mask + 1)
        rows = block(owner_of(d), seqs)
        values = stream[rows, :].astype(F32)
        mean_sq = jnp.mean(values * values, axis=-1, keepdims=True)
        scaled = (values * lax.rsqrt(mean_sq + EPS) * gain_ref[...]).astype(BF16)
        ffn[rows, :] = scaled
        inner = jnp.sum(scaled.astype(F32) * mixw_ref[...], axis=-1, keepdims=True)
        mix[rows, :] = jnp.broadcast_to(jax.nn.sigmoid(inner), (seqs, LANES))

    if near_first is not None:
        for i, d in enumerate(near_first):
            stage_two(d)
            if i:
                stage_three(near_first[i - 1])
            if i > 1:
                normalise(near_first[i - 2])
        stage_three(near_first[-1])
        for d in near_first[-2:]:
            normalise(d)
    else:
        stage_two(0)
        each(n_ep - 1, lambda i: stage_two(i + 1))
        each(n_ep, stage_three)
        each(n_ep, normalise)
    each(n_ep - 1, lambda i: route_wait(i + 1))

    many = min(rows_all, 128)
    batches = rows_all // many
    for load in loads[1:5]:
        load.wait()

    def hidden(b):
        rows = block(b, many)
        a = ffn[rows, :]
        for j in range(held):
            eh[j, rows, :] = (jax.nn.silu(dot(a, eg[j])) * dot(a, eu[j])).astype(BF16)
        units = jax.nn.silu(dot(a, dg[...])) * dot(a, du[...])
        if not split:
            own = hid // n_tp
            unit = lax.broadcasted_iota(jnp.int32, units.shape, 1)
            units = jnp.where((unit >= t * own) & (unit < (t + 1) * own), units, 0.0)
        dh[rows, :] = units.astype(BF16)

    each(batches, hidden)
    for load in loads[5:]:
        load.wait()

    def result(b, q):
        rows = block(b, many)
        cols = block(q, quarter)
        total = mix[rows, :1] * dot(dh[rows, :], dd[:, cols])
        lanes = lax.broadcasted_iota(jnp.int32, (many, route.shape[1]), 1)
        for j in range(held):
            weight = jnp.sum(
                jnp.where(lanes == e * held + j, route[rows, :], 0.0), axis=1, keepdims=True
            )
            piece = dot(eh[j, rows, :], ed[j, :, cols]).astype(BF16)
            total = total + weight * piece.astype(F32)
        return total

    def pair(j):
        return remote(away.at[j], came.at[j], pair_send.at[j], pair_recv.at[j], (e, mate))

    for j in range(half):

        def leave(b, j=j):
            away[j, block(b, many), :] = result(b, 2 * j + 1 - core).astype(BF16)

        each(batches, leave)
        pair(j).start()

    me = e * half + t // 2

    def back(j, d):
        there = (e + d) % n_ep
        return remote(
            summed.at[j, block(there, seqs), :],
            landed.at[me],
            back_send.at[j, d],
            back_recv.at[me],
            (there, 2 * j + core),
        )

    def same(j, d):
        return jnp.logical_and(jnp.asarray(d == 0), 2 * j + core == t)

    for j in range(half):

        def keep(b, j=j):
            summed[j, block(b, many), :] = result(b, 2 * j + core).astype(BF16)

        each(batches, keep)
    for j in range(half):
        pair(j).wait_recv()

        def add(b, j=j):
            rows = block(b, many)
            summed[j, rows, :] = (summed[j, rows, :].astype(F32) + came[j, rows, :].astype(F32)).astype(BF16)

        each(batches, add)

        def send(d, j=j):
            @pl.when(jnp.logical_not(same(j, d)))
            def _():
                back(j, d).start()

        each(n_ep, send, order=None if far_first is None else far_first + [0])

    landed[me] = summed[t // 2, own_rows, :]

    def take(index):
        @pl.when(index != me)
        def _():
            where = landed.at[index]
            remote(where, where, back_send.at[0, 0], back_recv.at[index], (e, t)).wait_recv()

    each(n_ep * half, take)
    out_ref[...] = own_stream.astype(F32) + jnp.sum(landed[...].astype(F32), axis=0)

    for mask in range(1, n_tp):
        heads_copy(mask).wait_send()
    each(n_ep - 1, lambda i: route_copy(i + 1).wait_send())
    each(n_ep - 1, lambda i: first(i + 1).wait_send())

    def sent(d):
        second(d, 1).wait_send()
        for mask in evens:
            second(d, mask).wait_send()
            relay(d, mask).wait_send()

    each(n_ep, sent)
    for j in range(half):
        pair(j).wait_send()

        def gone(d, j=j):
            @pl.when(jnp.logical_not(same(j, d)))
            def _():
                back(j, d).wait_send()

        each(n_ep, gone)


def near_kernel(
    n_ep,
    n_tp,
    lengths_hbm,
    lam_hbm,
    resid_hbm,
    first_gain_hbm,
    head_gain_hbm,
    gain_hbm,
    mixw_hbm,
    ids_hbm,
    rw_hbm,
    qw_hbm,
    kw_hbm,
    vw_hbm,
    cache_hbm,
    ow_hbm,
    eg_hbm,
    eu_hbm,
    ed_hbm,
    dg_hbm,
    du_hbm,
    dd_hbm,
    out_ref,
    new_ref,
    lengths_ref,
    lam_ref,
    resid_ref,
    first_gain_ref,
    head_gain_ref,
    gain_ref,
    mixw_ref,
    ids_ref,
    rw_ref,
    qkv,
    cache,
    pairs,
    asked,
    scores,
    mixed,
    heads_ref,
    ow,
    gu,
    ed,
    dg,
    du,
    dd,
    heads_all,
    mine,
    stream,
    ffn,
    route,
    eh,
    dh,
    leaving,
    kept,
    plane_in,
    column_out,
    column_in,
    local_sem,
    push_send,
    push_recv,
    route_send,
    route_recv,
    heads_send,
    heads_recv,
    chunk_send,
    climb_recv,
    group_recv,
    plane_recv,
    column_recv,
):
    e = lax.axis_index("ep")
    t = lax.axis_index("tp")
    planes = n_ep // INNER
    z = e // INNER
    x = e % INNER
    y = t // CORES
    c = t % CORES
    keeper = z % CORES
    odd = (c + z) % CORES
    turns = planes // CORES
    seqs, width = resid_ref.shape
    quarter = out_ref.shape[1]
    part = eg_hbm.shape[2]
    hid = dg.shape[1]
    mate = flip(t, 1)

    def gather_loads(sem, *routes):
        return [pltpu.make_async_copy(src, dst, local_sem.at[sem]) for src, dst in routes]

    first_loads = gather_loads(
        0, (resid_hbm, resid_ref), (first_gain_hbm, first_gain_ref), (lengths_hbm, lengths_ref)
    )
    for load in first_loads:
        load.start()
    depth = qkv.shape[0] // Q_CHUNKS
    inner = qw_hbm.shape[1]
    side = kw_hbm.shape[1]
    for i in range(Q_CHUNKS):
        deep = pl.ds(i * depth, depth)
        for load in gather_loads(
            1 + i,
            (qw_hbm.at[deep, :], qkv.at[deep, :inner]),
            (kw_hbm.at[deep, :], qkv.at[deep, inner : inner + side]),
            (vw_hbm.at[deep, :], qkv.at[deep, inner + side :]),
        ):
            load.start()

    barrier = pltpu.get_barrier_semaphore()
    for index in range(n_ep * n_tp):
        where = (index // n_tp, index % n_tp)

        @pl.when(jnp.logical_or(where[0] != e, where[1] != t))
        def _():
            pl.semaphore_signal(barrier, inc=1, device_id=where, device_id_type=MESH)

    for load in first_loads:
        load.wait()
    bunch = seqs // CACHE_CHUNKS
    cache_loads = [
        gather_loads(
            1 + Q_CHUNKS + i,
            (cache_hbm.at[pl.ds(i * bunch, bunch)], cache.at[pl.ds(i * bunch, bunch)]),
        )[0]
        for i in range(CACHE_CHUNKS)
    ]
    for load in cache_loads:
        load.start()
    late = 1 + Q_CHUNKS + CACHE_CHUNKS
    late_loads = gather_loads(
        late,
        (ids_hbm, ids_ref),
        (rw_hbm, rw_ref),
        (lam_hbm, lam_ref),
        (head_gain_hbm, head_gain_ref),
        (gain_hbm, gain_ref),
        (mixw_hbm, mixw_ref),
    )
    for load in late_loads:
        load.start()
    cols = block(y, hid)
    e_loads = gather_loads(
        late + 1, (eg_hbm.at[0], gu.at[c, :, :part]), (eu_hbm.at[0], gu.at[c, :, part:])
    ) + gather_loads(late + 2, (ed_hbm.at[0], ed.at[block(c, part), :]))
    loads = [
        gather_loads(1 + i, route)[0]
        for i, route in enumerate(
            (
                (ow_hbm, ow),
                (dg_hbm.at[:, cols], dg),
                (du_hbm.at[:, cols], du),
                (dd_hbm.at[cols, :], dd),
            )
        )
    ]
    resid = resid_ref[...].astype(F32)
    mean_sq = jnp.mean(resid * resid, axis=-1, keepdims=True)
    normed = (resid * lax.rsqrt(mean_sq + EPS) * first_gain_ref[...]).astype(BF16)
    row = lax.broadcasted_iota(jnp.int32, (seqs, LANES), 0)
    entry = lax.broadcasted_iota(jnp.int32, (seqs, LANES), 1) % QK_DIM
    position = jnp.zeros((seqs, LANES), F32)
    for s in range(seqs):
        position = jnp.where(row == s, lengths_ref[s].astype(F32), position)
    turn = QK_DIM // 2
    power = (entry % turn).astype(F32) * (-1.0 / turn)
    angle = position * jnp.exp(power * math.log(10000.0))
    cosine = jnp.cos(angle)
    sine = jnp.where(entry < turn, -jnp.sin(angle), jnp.sin(angle))

    def rotate(values):
        other = jnp.where(
            entry < turn, pltpu.roll(values, LANES - turn, 1), pltpu.roll(values, turn, 1)
        )
        return (values * cosine + other * sine).astype(BF16).astype(F32)

    def spot(plane, inner):
        return plane // CORES * INNER + inner

    own_spot = spot(z, x)
    projected = jnp.zeros((seqs, qkv.shape[1]), F32)
    for i in range(Q_CHUNKS):
        deep = pl.ds(i * depth, depth)
        pltpu.make_async_copy(qkv.at[deep, :], qkv.at[deep, :], local_sem.at[1 + i]).wait()
        projected = projected + dot(normed[:, i * depth : (i + 1) * depth], qkv[deep, :])
    query = projected[:, :inner]
    keys_raw = projected[:, inner : inner + side]
    values_raw = projected[:, inner + side :]
    for load in e_loads + loads:
        load.start()

    groups, spots = cache.shape[1], cache.shape[2]
    share = query.shape[1] // LANES // groups
    scale = QK_DIM**-0.5
    lines = 2 * share
    lower = lax.broadcasted_iota(jnp.int32, (seqs, LANES), 1) < QK_DIM
    fresh = []
    for g in range(groups):
        key = rotate(keys_raw[:, g * LANES : (g + 1) * LANES])
        value = values_raw[:, g * LANES : (g + 1) * LANES].astype(BF16).astype(F32)
        new_ref[:, 2 * g * LANES : (2 * g + 1) * LANES] = key.astype(BF16)
        new_ref[:, (2 * g + 1) * LANES : (2 * g + 2) * LANES] = value.astype(BF16)
        fresh.append((key, value))
        for j in range(share):
            at = (g * share + j) * LANES
            head = rotate(query[:, at : at + LANES])
            pairs[g, :, j, :] = jnp.where(lower, head, 0.0)
            pairs[g, :, share + j, :] = jnp.where(lower, 0.0, head)
        spread = (pairs[g] * scale).reshape(seqs * lines, LANES).astype(BF16)
        turn_of = lax.broadcasted_iota(jnp.int32, spread.shape, 0) // lines % 2
        asked[g, :, :LANES] = jnp.where(turn_of == 0, spread, jnp.zeros_like(spread))
        asked[g, :, LANES:] = jnp.where(turn_of == 0, jnp.zeros_like(spread), spread)

    def push(index):
        where = (gu.at[c], ed.at[block(c, part), :])[index]
        return remote(where, where, push_send.at[0], push_recv.at[index], (e, mate))

    def pushed(index):
        where = (gu.at[1 - c], ed.at[block(1 - c, part), :])[index]
        remote(where, where, push_send.at[0], push_recv.at[index], (e, mate)).wait_recv()

    def beside(s, g, lanes):
        return jnp.concatenate([cache[s, g, :, lanes], cache[s + 1, g, :, lanes]], axis=1)

    for s in range(0, seqs, 2):
        if s % bunch == 0:
            cache_loads[s // bunch].wait()
        for g in range(groups):
            scores[g, s : s + 2] = lax.dot_general(
                asked[g, s * lines : (s + 2) * lines, :],
                beside(s, g, slice(0, LANES)),
                (((1,), (1,)), ((), ())),
                preferred_element_type=F32,
            ).reshape(2, lines, spots)
    for load in late_loads:
        load.wait()
    length = jnp.zeros((seqs, lines, 1), jnp.int32)
    which = lax.broadcasted_iota(jnp.int32, (seqs, lines, 1), 0)
    for s in range(seqs):
        length = jnp.where(which == s, lengths_ref[s], length)
    place = lax.broadcasted_iota(jnp.int32, (seqs, lines, spots), 2)
    valid = place < length
    line = lax.broadcasted_iota(jnp.int32, (lines, 1), 0)
    for g in range(groups):
        key, value = fresh[g]
        latest = jnp.sum(pairs[g] * key[:, None, :], axis=-1, keepdims=True) * scale
        masked = jnp.where(valid, scores[g], -jnp.inf)
        top = jnp.maximum(jnp.max(masked, axis=-1, keepdims=True), latest)
        raised = jnp.exp(masked - top)
        raised_new = jnp.exp(latest - top)
        total = jnp.sum(raised, axis=-1, keepdims=True) + raised_new
        lam = jnp.full((lines, 1), 1.0, F32)
        for j in range(share):
            lam = jnp.where(line == share + j, lam_ref[g * share + j], lam)
        part_of = lam[None] / total
        prob = raised * part_of
        prob_new = jnp.broadcast_to(raised_new * part_of, (seqs, lines, LANES))
        weights = (prob - pltpu.roll(prob, share, 1)).astype(BF16)
        new_weight = (prob_new - pltpu.roll(prob_new, share, 1)).astype(BF16).astype(F32)
        fresh_part = new_weight * value[:, None, :]
        for s in range(0, seqs, 2):
            both = dot(
                weights[s : s + 2].reshape(2 * lines, spots), beside(s, g, slice(LANES, None))
            )
            mixed[g, s] = both[:lines, :LANES]
            mixed[g, s + 1] = both[lines:, LANES:]
        whole = mixed[g] + fresh_part
        mean_sq = jnp.mean(whole * whole, axis=-1, keepdims=True)
        mixed[g] = whole * lax.rsqrt(mean_sq + EPS) * head_gain_ref[...][None]
        for j in range(share):
            at = (g * share + j) * LANES
            heads_ref[:, at : at + LANES] = mixed[g, :, j, :].astype(BF16)

    def heads_copy(mask):
        return remote(
            heads_ref,
            heads_all.at[mask - 1],
            heads_send.at[0],
            heads_recv.at[mask // CORES],
            (e, flip(t, mask)),
        )

    pl.semaphore_wait(barrier, n_ep * n_tp - 1)
    for mask in range(n_tp - 1, 0, -1):
        heads_copy(mask).start()

    for load in e_loads:
        load.wait()
    push(0).start()
    push(1).start()

    lane = lax.broadcasted_iota(jnp.int32, (seqs, route.shape[2]), 1)
    table = jnp.zeros((seqs, route.shape[2]), F32)
    for k in range(ids_ref.shape[0]):
        wanted = column(ids_ref[k : k + 1, :])
        table = table + jnp.where(lane == wanted, column(rw_ref[k : k + 1, :]), 0.0)

    @pl.when(odd == 0)
    def _():
        route[own_spot] = table

    def route_copy(mask):
        where = route.at[own_spot]
        return remote(
            where, where, route_send.at[0], route_recv.at[0], (flip(e, mask), t)
        )

    @pl.when(odd == 0)
    def _():
        for mask in range(1, n_ep):
            route_copy(mask).start()


    loads[0].wait()
    span = heads_ref.shape[1]
    total = dot(heads_ref[...], ow[block(t, span), :])
    for far in range(n_tp // CORES):
        batch = heads_all.at[pl.ds(0, 1) if far == 0 else pl.ds(far * CORES - 1, CORES)]
        remote(batch, batch, heads_send.at[0], heads_recv.at[far], (e, t)).wait_recv()
        for mask in range(max(far * CORES, 1), (far + 1) * CORES):
            total = total + dot(heads_all[mask - 1], ow[block(flip(t, mask), span), :])
    own_cols = block(t, quarter)
    own_stream = (resid_ref[:, own_cols].astype(F32) + total).astype(BF16)
    mine[...] = own_stream

    around = ((1, 1), (1, 0), (0, 1))
    last = turns - 1
    edge = jnp.logical_or(z == 0, z == planes - 1)
    far = jnp.logical_and(edge, odd == 1)

    def chunk(group, owner):
        return stream.at[block(group, seqs), block(owner, quarter)]

    def to_plane(step):
        dx, dy = around[step]
        there = (z * INNER + flip(x, dx), flip(y, dy) * CORES + keeper)
        return remote(
            mine, chunk(e, t), chunk_send.at[0], group_recv.at[z // CORES, dx], there
        )

    def to_column(d):
        core = jnp.where(z == planes - 1, keeper, RELAY) if d == planes - 1 else RELAY
        there = (flip(z, d) * INNER + x, y * CORES + core)
        return remote(mine, chunk(e, t), chunk_send.at[0], climb_recv.at[z, c], there)

    def to_mate():
        return remote(mine, chunk(e, t), chunk_send.at[0], climb_recv.at[z, c], (e, mate))

    def to_far(step):
        dx, dy = around[step]
        there = (flip(z, planes - 1) * INNER + flip(x, dx), flip(y, dy) * CORES + keeper)
        return remote(
            mine, chunk(e, t), chunk_send.at[0], group_recv.at[z // CORES, dx], there
        )

    for d in range(planes - 2, 0, -1):
        to_column(d).start()

    @pl.when(z == planes - 1)
    def _():
        for step in range(len(around)):
            to_far(step).start()

    to_column(planes - 1).start()
    for step in range(len(around)):
        to_plane(step).start()

    @pl.when(odd == 1)
    def _():
        to_mate().start()

    @pl.when(odd == 0)
    def _():
        stream[block(e, seqs), own_cols] = own_stream

    near = z + odd * (1 - 2 * (z % 2))

    def plane_of(i):
        return flip(near, 2 * i)

    def arrived(plane, core):
        where = chunk(plane * INNER + x, y * CORES + core)
        remote(where, where, chunk_send.at[0], climb_recv.at[plane, core], (e, t)).wait_recv()

    def forward(plane, core, step):
        dx, dy = around[step]
        where = chunk(plane * INNER + x, y * CORES + core)
        return remote(
            where,
            where,
            chunk_send.at[0],
            group_recv.at[plane // CORES, dx],
            (z * INNER + flip(x, dx), flip(y, dy) * CORES + plane % CORES),
        )

    def hand_over(plane, core):
        where = chunk(plane * INNER + x, y * CORES + core)
        return remote(where, where, chunk_send.at[0], climb_recv.at[plane, core], (e, mate))

    @pl.when(c == RELAY)
    def _():
        for plane in range(planes):
            passes = plane != z
            if plane == planes - 1:
                passes = jnp.logical_and(passes, z != 0)

            @pl.when(passes)
            def _(plane=plane):
                for core in range(CORES):
                    arrived(plane, core)
                    for step in range(len(around)):
                        forward(plane, core, step).start()
                    if plane % CORES != RELAY:
                        hand_over(plane, core).start()

    def normalise(i):
        plane = CORES * i + c

        @pl.when(plane == z)
        def _():
            arrived(plane, 1 - c)

        leapt = jnp.logical_and(plane == planes - 1, z == 0)

        @pl.when(jnp.logical_and(plane != z, jnp.logical_or(c != RELAY, leapt)))
        def _():
            for core in range(CORES):
                arrived(plane, core)

        for inner in range(INNER):
            group = plane * INNER + flip(x, inner)
            came = stream.at[
                block(group, seqs),
                pl.ds(0, width) if inner else block(flip(y, 1), CORES * quarter),
            ]
            remote(
                came, came, chunk_send.at[0], group_recv.at[plane // CORES, inner], (e, t)
            ).wait_recv()
            values = stream[block(group, seqs), :].astype(F32)
            mean_sq = jnp.mean(values * values, axis=-1, keepdims=True)
            scaled = (values * lax.rsqrt(mean_sq + EPS) * gain_ref[...]).astype(BF16)
            ffn[block(spot(plane, flip(x, inner)), seqs), :] = scaled

    for i in range(turns):
        normalise(i)

    def route_wait(count):
        where = route.at[pl.ds(0, count)]
        remote(where, where, route_send.at[0], route_recv.at[0], (e, t)).wait_recv()

    @pl.when(odd == 0)
    def _():
        route_wait(route.shape[0] - 1)

    @pl.when(odd == 1)
    def _():
        route_wait(route.shape[0])

    rows_all = ffn.shape[0]
    pushed(0)
    pushed(1)
    for load in loads[1:]:
        load.wait()
    a = ffn[...]
    dh[...] = (jax.nn.silu(dot(a, dg[...])) * dot(a, du[...])).astype(BF16)
    for core in range(CORES):
        both = dot(a, gu[core])
        eh[:, core * part : (core + 1) * part] = (
            jax.nn.silu(both[:, :part]) * both[:, part:]
        ).astype(BF16)
    blend = jax.nn.sigmoid(jnp.sum(a.astype(F32) * mixw_ref[...], axis=-1, keepdims=True))
    lanes = lax.broadcasted_iota(jnp.int32, (rows_all, route.shape[2]), 1)
    weight = jnp.sum(
        jnp.where(lanes == e, route[...].reshape(rows_all, route.shape[2]), 0.0),
        axis=1,
        keepdims=True,
    )
    half = CORES * quarter
    for dy in (1, 0):
        cols = block(flip(y, dy), half)
        total = blend * dot(dh[...], dd[:, cols]) + weight * dot(eh[...], ed[:, cols])
        leaving[dy] = total.astype(BF16)
        if not dy:
            kept[...] = total

    def leave(i, core, step):
        dx, dy = around[step]
        where = spot(plane_of(i), flip(x, dx))
        return remote(
            leaving.at[dy, block(where, seqs), pl.ds(core * quarter, quarter)],
            plane_in.at[i, core, step],
            chunk_send.at[0],
            plane_recv.at[i, core],
            (z * INNER + flip(x, dx), flip(y, dy) * CORES + c),
        )

    def leap(core, step):
        dx, dy = around[step] if step < len(around) else (0, 0)
        where = spot(plane_of(last), flip(x, dx))
        return remote(
            leaving.at[dy, block(where, seqs), pl.ds(core * quarter, quarter)],
            column_in.at[planes - 1 + (step + 1) % (len(around) + 1)],
            chunk_send.at[0],
            column_recv.at[0],
            (plane_of(last) * INNER + flip(x, dx), flip(y, dy) * CORES + core),
        )

    order = range(turns - 1, -1, -1)
    for dy in (1, 0):
        steps = [step for step in range(len(around)) if around[step][1] == dy]

        @pl.when(far)
        def _():
            for step in steps + [len(around)] * (1 - dy):
                for core in range(CORES):
                    leap(core, step).start()

        for i in order:

            def depart(i=i):
                for core in range(CORES):
                    for step in steps:
                        leave(i, core, step).start()

            if i == last:
                pl.when(jnp.logical_not(far))(depart)
            else:
                depart()

    def own_plane(i):
        return jnp.logical_and(odd == 0, i == 0)

    def climb(i, core):
        return remote(
            column_out.at[i, core],
            column_in.at[odd + 2 * i],
            chunk_send.at[0],
            column_recv.at[0],
            (plane_of(i) * INNER + x, y * CORES + core),
        )

    def stays(i, core):
        return jnp.logical_and(own_plane(i), c == core)

    def rise(i):
        for core in range(CORES):
            gathered = kept[block(spot(plane_of(i), x), seqs), core * quarter : (core + 1) * quarter]
            came = plane_in.at[i, core]
            remote(came, came, chunk_send.at[0], plane_recv.at[i, core], (e, t)).wait_recv()
            for step in range(len(around)):
                gathered = gathered + plane_in[i, core, step].astype(F32)
            column_out[i, core] = gathered.astype(BF16)

            @pl.when(jnp.logical_not(stays(i, core)))
            def _(i=i, core=core):
                climb(i, core).start()

    for i in order:
        if i == last:

            @pl.when(jnp.logical_not(far))
            def _(i=i):
                rise(i)
        else:
            rise(i)

    def took(start, stop):
        where = column_in.at[pl.ds(start, stop - start)]
        remote(where, where, chunk_send.at[0], column_recv.at[0], (e, t)).wait_recv()

    @pl.when(odd == 0)
    def _():
        column_in[0] = column_out[0, c]

    def finish(stop):
        for parity in range(2):

            @pl.when(odd == parity)
            def _(parity=parity):
                took(1 - parity, stop)

        out_ref[...] = (
            own_stream.astype(F32) + jnp.sum(column_in[:stop].astype(F32), axis=0)
        ).astype(BF16)

    @pl.when(edge)
    def _():
        finish(planes + len(around))

    @pl.when(jnp.logical_not(edge))
    def _():
        finish(planes)

    push(0).wait_send()
    push(1).wait_send()
    remote(heads_all, heads_all, heads_send.at[0], heads_recv.at[0], (e, t)).wait_send()

    def drained(count):
        where = ow.at[pl.ds(0, count * seqs), :]
        remote(where, where, chunk_send.at[0], column_recv.at[0], (e, t)).wait_send()

    hops = len(around)
    @pl.when(odd == 0)
    def _():
        for mask in range(1, n_ep):
            route_copy(mask).wait_send()

    for level in range(planes):
        for core in range(CORES):
            count = planes - 1 + hops + turns * CORES * (hops + 1)
            count += hops if level == planes - 1 else 0
            count += 1 if (level + core) % CORES else -1
            for plane in range(planes) if core == RELAY else ():
                if plane != level and plane - level != planes - 1:
                    count += CORES * (hops + (plane % CORES != RELAY))

            @pl.when(jnp.logical_and(z == level, c == core))
            def _(count=count):
                drained(count)


def near_call(n_ep, n_tp, arrays):
    (
        residual_in,
        lengths,
        kv_cache,
        norm_gain_attn,
        query_weight,
        key_weight,
        value_weight,
        diff_lambda,
        head_gain,
        out_weight,
        norm_gain_ffn,
        route_ids,
        route_weights,
        expert_gate,
        expert_up,
        expert_down,
        dense_gate,
        dense_up,
        dense_down,
        dense_mix,
    ) = arrays
    seqs, width = residual_in.shape
    held = lambda value: pltpu.with_memory_space_constraint(value, pltpu.HBM)
    groups, spots = kv_cache.shape[1:3]
    share = diff_lambda.shape[0] // groups
    inner = query_weight.shape[1]
    quarter = out_weight.shape[1]
    part = expert_gate.shape[2]
    hid = dense_gate.shape[1] // (n_tp // CORES)
    turns = n_ep // INNER // CORES
    blocks = turns * INNER
    rows = blocks * seqs
    lanes = -(-n_ep // LANES) * LANES
    topk = route_ids.shape[1]
    vmem = pl.BlockSpec(memory_space=pltpu.VMEM)
    hbm = pl.BlockSpec(memory_space=pltpu.HBM)
    dma = pltpu.SemaphoreType.DMA
    layer_out, fresh = pl.pallas_call(
        functools.partial(near_kernel, n_ep, n_tp),
        out_shape=(
            jax.ShapeDtypeStruct((seqs, quarter), BF16),
            jax.ShapeDtypeStruct((seqs, groups * kv_cache.shape[3]), BF16),
        ),
        in_specs=[hbm] * 20,
        out_specs=(vmem, vmem),
        scratch_shapes=[
            pltpu.SMEM(lengths.shape, jnp.int32),
            pltpu.SMEM(diff_lambda.shape, F32),
            pltpu.VMEM(residual_in.shape, BF16),
            pltpu.VMEM((1, width), F32),
            pltpu.VMEM((1, head_gain.shape[0]), F32),
            pltpu.VMEM((1, width), F32),
            pltpu.VMEM((1, width), F32),
            pltpu.VMEM((topk, seqs), jnp.int32),
            pltpu.VMEM((topk, seqs), F32),
            pltpu.VMEM((width, inner + key_weight.shape[1] + value_weight.shape[1]), BF16),
            pltpu.VMEM(kv_cache.shape, BF16),
            pltpu.VMEM((groups, seqs, 2 * share, LANES), F32),
            pltpu.VMEM((groups, seqs * 2 * share, 2 * LANES), BF16),
            pltpu.VMEM((groups, seqs, 2 * share, spots), F32),
            pltpu.VMEM((groups, seqs, 2 * share, LANES), F32),
            pltpu.VMEM((seqs, inner), BF16),
            pltpu.VMEM(out_weight.shape, BF16),
            pltpu.VMEM((CORES, width, 2 * part), BF16),
            pltpu.VMEM((CORES * part, width), BF16),
            pltpu.VMEM((width, hid), BF16),
            pltpu.VMEM((width, hid), BF16),
            pltpu.VMEM((hid, width), BF16),
            pltpu.VMEM((n_tp - 1, seqs, inner), BF16),
            pltpu.VMEM((seqs, quarter), BF16),
            pltpu.VMEM((n_ep * seqs, width), BF16),
            pltpu.VMEM((rows, width), BF16),
            pltpu.VMEM((blocks, seqs, lanes), F32),
            pltpu.VMEM((rows, CORES * part), BF16),
            pltpu.VMEM((rows, hid), BF16),
            pltpu.VMEM((2, rows, CORES * quarter), BF16),
            pltpu.VMEM((rows, CORES * quarter), F32),
            pltpu.VMEM((turns, CORES, 3, seqs, quarter), BF16),
            pltpu.VMEM((turns, CORES, seqs, quarter), BF16),
            pltpu.VMEM((n_ep // INNER + 3, seqs, quarter), BF16),
            dma((Q_CHUNKS + CACHE_CHUNKS + 4,)),
            dma((1,)),
            dma((2,)),
            dma((1,)),
            dma((1,)),
            dma((1,)),
            dma((n_tp // CORES,)),
            dma((1,)),
            dma((n_ep // INNER, CORES)),
            dma((turns, INNER)),
            dma((turns, CORES)),
            dma((1,)),
        ],
        compiler_params=pltpu.CompilerParams(
            collective_id=0, has_side_effects=True, vmem_limit_bytes=36 * 1024 * 1024
        ),
    )(
        held(lengths),
        held(diff_lambda),
        held(residual_in),
        held(norm_gain_attn[None, :]),
        held(head_gain[None, :]),
        held(norm_gain_ffn[None, :]),
        held(dense_mix[None, :]),
        held(route_ids.T),
        held(route_weights.T),
        held(query_weight),
        held(key_weight),
        held(value_weight),
        held(kv_cache),
        held(out_weight),
        held(expert_gate),
        held(expert_up),
        held(expert_down),
        held(dense_gate),
        held(dense_up),
        held(dense_down),
    )
    return layer_out, fresh.reshape(seqs, groups, kv_cache.shape[3])


def on_device(
    residual_in,
    lengths,
    kv_cache,
    norm_gain_attn,
    query_weight,
    key_weight,
    value_weight,
    diff_lambda,
    head_gain,
    out_weight,
    norm_gain_ffn,
    route_ids,
    route_weights,
    expert_gate,
    expert_up,
    expert_down,
    dense_gate,
    dense_up,
    dense_down,
    dense_mix,
):
    n_ep = lax.axis_size("ep")
    n_tp = lax.axis_size("tp")
    half = n_tp // 2
    if (
        n_tp == 2 * CORES
        and n_ep in (4, 8, 16)
        and expert_gate.shape[0] == 1
        and dense_gate.shape[1] // half % LANES == 0
        and expert_gate.shape[2] % LANES == 0
    ):
        return near_call(
            n_ep,
            n_tp,
            (
                residual_in,
                lengths,
                kv_cache,
                norm_gain_attn,
                query_weight,
                key_weight,
                value_weight,
                diff_lambda,
                head_gain,
                out_weight,
                norm_gain_ffn,
                route_ids,
                route_weights,
                expert_gate,
                expert_up,
                expert_down,
                dense_gate,
                dense_up,
                dense_down,
                dense_mix,
            ),
        )
    seqs, width = residual_in.shape
    groups, spots = kv_cache.shape[1:3]
    share = diff_lambda.shape[0] // groups
    inner = query_weight.shape[1]
    quarter = out_weight.shape[1]
    held, _, part = expert_gate.shape
    rows = n_ep * seqs
    own = dense_gate.shape[1] // n_tp
    split = own % LANES == 0
    hid = own if split else dense_gate.shape[1]
    lanes = -(-n_ep * held // LANES) * LANES
    vmem = pl.BlockSpec(memory_space=pltpu.VMEM)
    smem = pl.BlockSpec(memory_space=pltpu.SMEM)
    hbm = pl.BlockSpec(memory_space=pl.ANY)
    dma = pltpu.SemaphoreType.DMA
    layer_out, fresh = pl.pallas_call(
        functools.partial(layer_kernel, n_ep, n_tp, split),
        out_shape=(
            jax.ShapeDtypeStruct((seqs, quarter), F32),
            jax.ShapeDtypeStruct((seqs, groups * kv_cache.shape[3]), F32),
        ),
        in_specs=[smem] * 2 + [vmem] * 7 + [hbm] * 11,
        out_specs=(vmem, vmem),
        scratch_shapes=[
            pltpu.VMEM(query_weight.shape, BF16),
            pltpu.VMEM(key_weight.shape, BF16),
            pltpu.VMEM(value_weight.shape, BF16),
            pltpu.VMEM(kv_cache.shape, BF16),
            pltpu.VMEM((groups, seqs, 2 * share, LANES), F32),
            pltpu.VMEM((groups, seqs, 2 * share, spots), F32),
            pltpu.VMEM((groups, seqs, 2 * share, LANES), F32),
            pltpu.VMEM((seqs, inner), BF16),
            pltpu.VMEM(out_weight.shape, BF16),
            pltpu.VMEM(expert_gate.shape, BF16),
            pltpu.VMEM(expert_up.shape, BF16),
            pltpu.VMEM(expert_down.shape, BF16),
            pltpu.VMEM((width, hid), BF16),
            pltpu.VMEM((width, hid), BF16),
            pltpu.VMEM((hid, width), BF16),
            pltpu.VMEM((n_tp - 1, seqs, inner), BF16),
            pltpu.VMEM((rows, width), BF16),
            pltpu.VMEM((rows, width), BF16),
            pltpu.VMEM((rows, LANES), F32),
            pltpu.VMEM((rows, lanes), F32),
            pltpu.VMEM((held, rows, part), BF16),
            pltpu.VMEM((rows, hid), BF16),
            pltpu.VMEM((half, rows, quarter), BF16),
            pltpu.VMEM((half, rows, quarter), BF16),
            pltpu.VMEM((half, rows, quarter), BF16),
            pltpu.VMEM((n_ep * half, seqs, quarter), BF16),
            dma((7,)),
            dma((Q_CHUNKS + 2,)),
            dma((seqs,)),
            dma((n_ep - 1,)),
            dma((n_ep - 1,)),
            dma((n_tp - 1,)),
            dma((n_tp - 1,)),
            dma((n_ep,)),
            dma((half, n_ep)),
            dma((max(half - 1, 1), n_ep)),
            dma((n_tp, n_ep)),
            dma((half,)),
            dma((half,)),
            dma((half, n_ep)),
            dma((n_ep * half,)),
        ],
        compiler_params=pltpu.CompilerParams(
            collective_id=0, has_side_effects=True, vmem_limit_bytes=60 * 1024 * 1024
        ),
    )(
        lengths,
        diff_lambda,
        residual_in,
        norm_gain_attn[None, :],
        head_gain[None, :],
        norm_gain_ffn[None, :],
        dense_mix[None, :],
        route_ids.T,
        route_weights.T,
        query_weight,
        key_weight,
        value_weight,
        kv_cache,
        out_weight,
        expert_gate,
        expert_up,
        expert_down,
        dense_gate,
        dense_up,
        dense_down,
    )
    new_rows = fresh.astype(BF16).reshape(seqs, groups, kv_cache.shape[3])
    return (layer_out.astype(BF16), new_rows)


def solution(mesh):
    placed = (
        P("ep", None),
        P("ep"),
        P("ep", "tp", None, None),
        P(),
        P(None, "tp"),
        P(None, "tp"),
        P(None, "tp"),
        P("tp"),
        P(),
        P(None, "tp"),
        P(),
        P("ep", None),
        P("ep", None),
        P("ep", None, "tp"),
        P("ep", None, "tp"),
        P("ep", "tp", None),
        P(None, "ep"),
        P(None, "ep"),
        P("ep", None),
        P(),
    )
    return jax.shard_map(
        on_device,
        mesh=mesh,
        in_specs=placed,
        out_specs=(P("ep", "tp"), P("ep", "tp", None)),
        check_vma=False,
    )
```

```python
import functools
import math

import jax
import jax.numpy as jnp
from jax import lax
from jax.experimental import pallas as pl
from jax.experimental.pallas import tpu as pltpu
from jax.sharding import PartitionSpec as P

QK_DIM = 64
EPS = 1e-06
MESH = pl.DeviceIdType.MESH
F32 = jnp.float32
BF16 = jnp.bfloat16
LANES = 128
Q_CHUNKS = 4
INNER = 2
CORES = 2
RELAY = 1
CACHE_CHUNKS = 4


def flip(value, mask):
    bit = 1
    while bit <= mask:
        if mask & bit:
            value = value + bit * (1 - 2 * ((value // bit) % 2))
        bit *= 2
    return value


def each(count, body, order=None):
    if count <= 16:
        for index in order if order is not None else range(count):
            body(index)
    else:

        def step(index, carry):
            body(index)
            return carry

        lax.fori_loop(0, count, step, 0)


def block(start, size):
    return pl.ds(pl.multiple_of(start * size, size), size)


def remote(source, target, send, recv, where):
    return pltpu.make_async_remote_copy(
        src_ref=source,
        dst_ref=target,
        send_sem=send,
        recv_sem=recv,
        device_id=where,
        device_id_type=MESH,
    )


def dot(left, right):
    return jnp.dot(left, right, preferred_element_type=F32)


def column(row):
    count = row.shape[1]
    square = (count, count)
    same = lax.broadcasted_iota(jnp.int32, square, 0) == lax.broadcasted_iota(jnp.int32, square, 1)
    return jnp.sum(jnp.where(same, row, jnp.zeros_like(row)), axis=1, keepdims=True)


def layer_kernel(
    n_ep,
    n_tp,
    split,
    lengths_ref,
    lam_ref,
    resid_ref,
    first_gain_ref,
    head_gain_ref,
    gain_ref,
    mixw_ref,
    ids_ref,
    rw_ref,
    qw_hbm,
    kw_hbm,
    vw_hbm,
    cache_hbm,
    ow_hbm,
    eg_hbm,
    eu_hbm,
    ed_hbm,
    dg_hbm,
    du_hbm,
    dd_hbm,
    out_ref,
    new_ref,
    qw,
    kw,
    vw,
    cache,
    pairs,
    scores,
    mixed,
    heads_ref,
    ow,
    eg,
    eu,
    ed,
    dg,
    du,
    dd,
    heads_all,
    stream,
    ffn,
    mix,
    route,
    eh,
    dh,
    away,
    came,
    summed,
    landed,
    w_sem,
    q_sem,
    cache_sem,
    route_send,
    route_recv,
    heads_send,
    heads_recv,
    first_send,
    second_send,
    relay_send,
    stream_recv,
    pair_send,
    pair_recv,
    back_send,
    back_recv,
):
    e = lax.axis_index("ep")
    t = lax.axis_index("tp")
    half = n_tp // 2
    mate = flip(t, 1)
    core = t % 2
    seqs, width = resid_ref.shape
    quarter = out_ref.shape[1]
    held, _, part = eg.shape
    hid = dg.shape[1]
    rows_all = n_ep * seqs
    evens = [2 * i for i in range(1, half)]

    depth = qw.shape[0] // Q_CHUNKS
    q_loads = [
        pltpu.make_async_copy(
            qw_hbm.at[pl.ds(i * depth, depth), :], qw.at[pl.ds(i * depth, depth), :], q_sem.at[i]
        )
        for i in range(Q_CHUNKS)
    ] + [
        pltpu.make_async_copy(kw_hbm, kw, q_sem.at[Q_CHUNKS]),
        pltpu.make_async_copy(vw_hbm, vw, q_sem.at[Q_CHUNKS + 1]),
    ]
    for load in q_loads:
        load.start()
    cache_loads = [
        pltpu.make_async_copy(cache_hbm.at[s], cache.at[s], cache_sem.at[s]) for s in range(seqs)
    ]
    for load in cache_loads:
        load.start()

    barrier = pltpu.get_barrier_semaphore()

    def greet(index):
        where = (index // half, 2 * (index % half) + core)

        @pl.when(jnp.logical_or(where[0] != e, where[1] != t))
        def _():
            pl.semaphore_signal(barrier, inc=1, device_id=where, device_id_type=MESH)

    each(n_ep * half, greet)
    for i in range(half):
        pl.semaphore_signal(
            barrier, inc=1, device_id=(e, 2 * i + 1 - core), device_id_type=MESH
        )

    if split:
        cols = block(t, hid)
        dense_parts = (dg_hbm.at[:, cols], du_hbm.at[:, cols], dd_hbm.at[cols, :])
    else:
        dense_parts = (dg_hbm, du_hbm, dd_hbm)
    loads = [
        pltpu.make_async_copy(src, dst, w_sem.at[i])
        for i, (src, dst) in enumerate(
            zip((ow_hbm, eg_hbm, eu_hbm) + dense_parts[:2] + (ed_hbm, dense_parts[2]), (ow, eg, eu, dg, du, ed, dd))
        )
    ]

    lane = lax.broadcasted_iota(jnp.int32, (seqs, route.shape[1]), 1)
    table = jnp.zeros((seqs, route.shape[1]), F32)
    for k in range(ids_ref.shape[0]):
        wanted = column(ids_ref[k : k + 1, :])
        table = table + jnp.where(lane == wanted, column(rw_ref[k : k + 1, :]), 0.0)
    own_rows = block(e, seqs)
    route[own_rows, :] = table

    resid = resid_ref[...].astype(F32)
    mean_sq = jnp.mean(resid * resid, axis=-1, keepdims=True)
    normed = (resid * lax.rsqrt(mean_sq + EPS) * first_gain_ref[...]).astype(BF16)
    row = lax.broadcasted_iota(jnp.int32, (seqs, LANES), 0)
    entry = lax.broadcasted_iota(jnp.int32, (seqs, LANES), 1) % QK_DIM
    position = jnp.zeros((seqs, LANES), F32)
    for s in range(seqs):
        position = jnp.where(row == s, lengths_ref[s].astype(F32), position)
    turn = QK_DIM // 2
    power = (entry % turn).astype(F32) * (-1.0 / turn)
    angle = position * jnp.exp(power * math.log(10000.0))
    cosine = jnp.cos(angle)
    sine = jnp.where(entry < turn, -jnp.sin(angle), jnp.sin(angle))

    def rotate(values):
        other = jnp.where(
            entry < turn, pltpu.roll(values, LANES - turn, 1), pltpu.roll(values, turn, 1)
        )
        return (values * cosine + other * sine).astype(BF16).astype(F32)

    query = jnp.zeros((seqs, qw.shape[1]), F32)
    for i in range(Q_CHUNKS):
        q_loads[i].wait()
        query = query + dot(
            normed[:, i * depth : (i + 1) * depth], qw[i * depth : (i + 1) * depth, :]
        )
    for load in q_loads[Q_CHUNKS:]:
        load.wait()
    keys_raw = dot(normed, kw[...])
    values_raw = dot(normed, vw[...])
    for load in loads:
        load.start()

    groups, spots = cache.shape[1], cache.shape[2]
    share = query.shape[1] // LANES // groups
    lower = lax.broadcasted_iota(jnp.int32, (seqs, LANES), 1) < QK_DIM
    fresh = []
    for g in range(groups):
        key = rotate(keys_raw[:, g * LANES : (g + 1) * LANES])
        value = values_raw[:, g * LANES : (g + 1) * LANES].astype(BF16).astype(F32)
        new_ref[:, 2 * g * LANES : (2 * g + 1) * LANES] = key
        new_ref[:, (2 * g + 1) * LANES : (2 * g + 2) * LANES] = value
        fresh.append((key, value))
        for j in range(share):
            at = (g * share + j) * LANES
            head = rotate(query[:, at : at + LANES])
            pairs[g, :, j, :] = jnp.where(lower, head, 0.0)
            pairs[g, :, share + j, :] = jnp.where(lower, 0.0, head)

    pl.semaphore_wait(barrier, n_ep * half - 1 + half)

    def route_copy(d):
        there = (e + d) % n_ep
        return remote(
            route.at[own_rows, :],
            route.at[own_rows, :],
            route_send.at[d - 1],
            route_recv.at[d - 1],
            (there, t),
        )

    def route_wait(d):
        came_from = (e + n_ep - d) % n_ep
        spot = route.at[block(came_from, seqs), :]
        remote(spot, spot, route_send.at[d - 1], route_recv.at[d - 1], (e, t)).wait_recv()

    each(n_ep - 1, lambda i: route_copy(i + 1).start())

    scale = QK_DIM**-0.5
    lines = 2 * share
    for s in range(seqs):
        cache_loads[s].wait()
        for g in range(groups):
            both = pairs[g, s].astype(BF16)
            scores[g, s] = (
                lax.dot_general(
                    both,
                    cache[s, g, :, :LANES],
                    (((1,), (1,)), ((), ())),
                    preferred_element_type=F32,
                )
                * scale
            )
    length = jnp.zeros((seqs, lines, 1), jnp.int32)
    which = lax.broadcasted_iota(jnp.int32, (seqs, lines, 1), 0)
    for s in range(seqs):
        length = jnp.where(which == s, lengths_ref[s], length)
    place = lax.broadcasted_iota(jnp.int32, (seqs, lines, spots), 2)
    valid = place < length
    line = lax.broadcasted_iota(jnp.int32, (lines, 1), 0)
    for g in range(groups):
        key, value = fresh[g]
        latest = jnp.sum(pairs[g] * key[:, None, :], axis=-1, keepdims=True) * scale
        masked = jnp.where(valid, scores[g], -jnp.inf)
        top = jnp.maximum(jnp.max(masked, axis=-1, keepdims=True), latest)
        raised = jnp.exp(masked - top)
        raised_new = jnp.exp(latest - top)
        total = jnp.sum(raised, axis=-1, keepdims=True) + raised_new
        prob = raised / total
        prob_new = jnp.broadcast_to(raised_new / total, (seqs, lines, LANES))
        lam = jnp.zeros((lines, 1), F32)
        for j in range(share):
            lam = jnp.where(line == j, lam_ref[g * share + j], lam)
        scores[g] = prob - lam[None] * pltpu.roll(prob, share, 1)
        new_weight = (prob_new - lam[None] * pltpu.roll(prob_new, share, 1)).astype(BF16).astype(F32)
        fresh_part = new_weight * value[:, None, :]
        for s in range(seqs):
            mixed[g, s] = dot(scores[g, s].astype(BF16), cache[s, g, :, LANES:])
        whole = mixed[g] + fresh_part
        mean_sq = jnp.mean(whole * whole, axis=-1, keepdims=True)
        mixed[g] = whole * lax.rsqrt(mean_sq + EPS) * head_gain_ref[...][None]
        for j in range(share):
            at = (g * share + j) * LANES
            heads_ref[:, at : at + LANES] = mixed[g, :, j, :].astype(BF16)

    def heads_copy(mask):
        return remote(
            heads_ref,
            heads_all.at[mask - 1],
            heads_send.at[mask - 1],
            heads_recv.at[mask - 1],
            (e, flip(t, mask)),
        )

    for mask in range(n_tp - 1, 0, -1):
        heads_copy(mask).start()

    loads[0].wait()
    span = heads_ref.shape[1]
    total = dot(heads_ref[...], ow[block(t, span), :])
    for mask in range(1, n_tp):
        heads_copy(mask).wait_recv()
        total = total + dot(heads_all[mask - 1], ow[block(flip(t, mask), span), :])
    own_cols = block(t, quarter)
    own_stream = (resid_ref[:, own_cols].astype(F32) + total).astype(BF16)
    stream[own_rows, own_cols] = own_stream

    def spot(owner, column):
        return stream.at[block(owner, seqs), block(column, quarter)]

    def owner_of(d):
        return (e + n_ep - d) % n_ep

    def first(d):
        return remote(
            spot(e, t), spot(e, t), first_send.at[d], stream_recv.at[0, d], ((e + d) % n_ep, t)
        )

    def second(d, mask):
        index = mask // 2 if mask != 1 else 0
        where = spot(owner_of(d), t)
        return remote(
            where, where, second_send.at[index, d], stream_recv.at[mask, d], (e, flip(t, mask))
        )

    def relay(d, mask):
        where = spot(owner_of(d), flip(t, mask))
        return remote(
            where, where, relay_send.at[mask // 2 - 1, d], stream_recv.at[mask + 1, d], (e, mate)
        )

    def arrived(d, mask):
        where = spot(owner_of(d), flip(t, mask))
        remote(where, where, first_send.at[d], stream_recv.at[mask, d], (e, t)).wait_recv()

    def spread(d):
        for mask in evens:
            second(d, mask).start()
        second(d, 1).start()

    far_first = sorted(range(1, n_ep), key=lambda d: -min(d, n_ep - d)) if n_ep <= 16 else None
    near_first = [0] + far_first[::-1] if far_first is not None else None
    each(n_ep - 1 if far_first is None else 1, lambda i: first(i + 1).start(), order=None) if far_first is None else [
        first(d).start() for d in far_first
    ]

    def stage_two(d):
        if not (isinstance(d, int) and d == 0):
            arrived(d, 0)
        spread(d)

    def stage_three(d):
        for mask in evens:
            arrived(d, mask)
            relay(d, mask).start()

    def normalise(d):
        arrived(d, 1)
        for mask in evens:
            arrived(d, mask + 1)
        rows = block(owner_of(d), seqs)
        values = stream[rows, :].astype(F32)
        mean_sq = jnp.mean(values * values, axis=-1, keepdims=True)
        scaled = (values * lax.rsqrt(mean_sq + EPS) * gain_ref[...]).astype(BF16)
        ffn[rows, :] = scaled
        inner = jnp.sum(scaled.astype(F32) * mixw_ref[...], axis=-1, keepdims=True)
        mix[rows, :] = jnp.broadcast_to(jax.nn.sigmoid(inner), (seqs, LANES))

    if near_first is not None:
        for i, d in enumerate(near_first):
            stage_two(d)
            if i:
                stage_three(near_first[i - 1])
            if i > 1:
                normalise(near_first[i - 2])
        stage_three(near_first[-1])
        for d in near_first[-2:]:
            normalise(d)
    else:
        stage_two(0)
        each(n_ep - 1, lambda i: stage_two(i + 1))
        each(n_ep, stage_three)
        each(n_ep, normalise)
    each(n_ep - 1, lambda i: route_wait(i + 1))

    many = min(rows_all, 128)
    batches = rows_all // many
    for load in loads[1:5]:
        load.wait()

    def hidden(b):
        rows = block(b, many)
        a = ffn[rows, :]
        for j in range(held):
            eh[j, rows, :] = (jax.nn.silu(dot(a, eg[j])) * dot(a, eu[j])).astype(BF16)
        units = jax.nn.silu(dot(a, dg[...])) * dot(a, du[...])
        if not split:
            own = hid // n_tp
            unit = lax.broadcasted_iota(jnp.int32, units.shape, 1)
            units = jnp.where((unit >= t * own) & (unit < (t + 1) * own), units, 0.0)
        dh[rows, :] = units.astype(BF16)

    each(batches, hidden)
    for load in loads[5:]:
        load.wait()

    def result(b, q):
        rows = block(b, many)
        cols = block(q, quarter)
        total = mix[rows, :1] * dot(dh[rows, :], dd[:, cols])
        lanes = lax.broadcasted_iota(jnp.int32, (many, route.shape[1]), 1)
        for j in range(held):
            weight = jnp.sum(
                jnp.where(lanes == e * held + j, route[rows, :], 0.0), axis=1, keepdims=True
            )
            piece = dot(eh[j, rows, :], ed[j, :, cols]).astype(BF16)
            total = total + weight * piece.astype(F32)
        return total

    def pair(j):
        return remote(away.at[j], came.at[j], pair_send.at[j], pair_recv.at[j], (e, mate))

    for j in range(half):

        def leave(b, j=j):
            away[j, block(b, many), :] = result(b, 2 * j + 1 - core).astype(BF16)

        each(batches, leave)
        pair(j).start()

    me = e * half + t // 2

    def back(j, d):
        there = (e + d) % n_ep
        return remote(
            summed.at[j, block(there, seqs), :],
            landed.at[me],
            back_send.at[j, d],
            back_recv.at[me],
            (there, 2 * j + core),
        )

    def same(j, d):
        return jnp.logical_and(jnp.asarray(d == 0), 2 * j + core == t)

    for j in range(half):

        def keep(b, j=j):
            summed[j, block(b, many), :] = result(b, 2 * j + core).astype(BF16)

        each(batches, keep)
    for j in range(half):
        pair(j).wait_recv()

        def add(b, j=j):
            rows = block(b, many)
            summed[j, rows, :] = (summed[j, rows, :].astype(F32) + came[j, rows, :].astype(F32)).astype(BF16)

        each(batches, add)

        def send(d, j=j):
            @pl.when(jnp.logical_not(same(j, d)))
            def _():
                back(j, d).start()

        each(n_ep, send, order=None if far_first is None else far_first + [0])

    landed[me] = summed[t // 2, own_rows, :]

    def take(index):
        @pl.when(index != me)
        def _():
            where = landed.at[index]
            remote(where, where, back_send.at[0, 0], back_recv.at[index], (e, t)).wait_recv()

    each(n_ep * half, take)
    out_ref[...] = own_stream.astype(F32) + jnp.sum(landed[...].astype(F32), axis=0)

    for mask in range(1, n_tp):
        heads_copy(mask).wait_send()
    each(n_ep - 1, lambda i: route_copy(i + 1).wait_send())
    each(n_ep - 1, lambda i: first(i + 1).wait_send())

    def sent(d):
        second(d, 1).wait_send()
        for mask in evens:
            second(d, mask).wait_send()
            relay(d, mask).wait_send()

    each(n_ep, sent)
    for j in range(half):
        pair(j).wait_send()

        def gone(d, j=j):
            @pl.when(jnp.logical_not(same(j, d)))
            def _():
                back(j, d).wait_send()

        each(n_ep, gone)


def near_kernel(
    n_ep,
    n_tp,
    lengths_hbm,
    lam_hbm,
    resid_hbm,
    first_gain_hbm,
    head_gain_hbm,
    gain_hbm,
    mixw_hbm,
    ids_hbm,
    rw_hbm,
    qw_hbm,
    kw_hbm,
    vw_hbm,
    cache_hbm,
    ow_hbm,
    eg_hbm,
    eu_hbm,
    ed_hbm,
    dg_hbm,
    du_hbm,
    dd_hbm,
    out_ref,
    new_ref,
    lengths_ref,
    lam_ref,
    resid_ref,
    first_gain_ref,
    head_gain_ref,
    gain_ref,
    mixw_ref,
    ids_ref,
    rw_ref,
    qkv,
    cache,
    pairs,
    asked,
    scores,
    mixed,
    heads_ref,
    ow,
    gu,
    ed,
    dg,
    du,
    dd,
    heads_all,
    mine,
    stream,
    ffn,
    route,
    eh,
    dh,
    leaving,
    kept,
    plane_in,
    column_out,
    column_in,
    local_sem,
    push_send,
    push_recv,
    route_send,
    route_recv,
    heads_send,
    heads_recv,
    chunk_send,
    climb_recv,
    group_recv,
    plane_recv,
    column_recv,
):
    e = lax.axis_index("ep")
    t = lax.axis_index("tp")
    planes = n_ep // INNER
    z = e // INNER
    x = e % INNER
    y = t // CORES
    c = t % CORES
    keeper = z % CORES
    odd = (c + z) % CORES
    turns = planes // CORES
    seqs, width = resid_ref.shape
    quarter = out_ref.shape[1]
    part = eg_hbm.shape[2]
    hid = dg.shape[1]
    mate = flip(t, 1)

    def gather_loads(sem, *routes):
        return [pltpu.make_async_copy(src, dst, local_sem.at[sem]) for src, dst in routes]

    first_loads = gather_loads(
        0, (resid_hbm, resid_ref), (first_gain_hbm, first_gain_ref), (lengths_hbm, lengths_ref)
    )
    for load in first_loads:
        load.start()
    depth = qkv.shape[0] // Q_CHUNKS
    inner = qw_hbm.shape[1]
    side = kw_hbm.shape[1]
    for i in range(Q_CHUNKS):
        deep = pl.ds(i * depth, depth)
        for load in gather_loads(
            1 + i,
            (qw_hbm.at[deep, :], qkv.at[deep, :inner]),
            (kw_hbm.at[deep, :], qkv.at[deep, inner : inner + side]),
            (vw_hbm.at[deep, :], qkv.at[deep, inner + side :]),
        ):
            load.start()

    barrier = pltpu.get_barrier_semaphore()
    for index in range(n_ep * n_tp):
        where = (index // n_tp, index % n_tp)

        @pl.when(jnp.logical_or(where[0] != e, where[1] != t))
        def _():
            pl.semaphore_signal(barrier, inc=1, device_id=where, device_id_type=MESH)

    for load in first_loads:
        load.wait()
    bunch = seqs // CACHE_CHUNKS
    cache_loads = [
        gather_loads(
            1 + Q_CHUNKS + i,
            (cache_hbm.at[pl.ds(i * bunch, bunch)], cache.at[pl.ds(i * bunch, bunch)]),
        )[0]
        for i in range(CACHE_CHUNKS)
    ]
    for load in cache_loads:
        load.start()
    late = 1 + Q_CHUNKS + CACHE_CHUNKS
    late_loads = gather_loads(
        late,
        (ids_hbm, ids_ref),
        (rw_hbm, rw_ref),
        (lam_hbm, lam_ref),
        (head_gain_hbm, head_gain_ref),
        (gain_hbm, gain_ref),
        (mixw_hbm, mixw_ref),
    )
    for load in late_loads:
        load.start()
    cols = block(y, hid)
    e_loads = gather_loads(
        late + 1, (eg_hbm.at[0], gu.at[c, :, :part]), (eu_hbm.at[0], gu.at[c, :, part:])
    ) + gather_loads(late + 2, (ed_hbm.at[0], ed.at[block(c, part), :]))
    loads = [
        gather_loads(1 + i, route)[0]
        for i, route in enumerate(
            (
                (ow_hbm, ow),
                (dg_hbm.at[:, cols], dg),
                (du_hbm.at[:, cols], du),
                (dd_hbm.at[cols, :], dd),
            )
        )
    ]
    resid = resid_ref[...].astype(F32)
    mean_sq = jnp.mean(resid * resid, axis=-1, keepdims=True)
    normed = (resid * lax.rsqrt(mean_sq + EPS) * first_gain_ref[...]).astype(BF16)
    row = lax.broadcasted_iota(jnp.int32, (seqs, LANES), 0)
    entry = lax.broadcasted_iota(jnp.int32, (seqs, LANES), 1) % QK_DIM
    position = jnp.zeros((seqs, LANES), F32)
    for s in range(seqs):
        position = jnp.where(row == s, lengths_ref[s].astype(F32), position)
    turn = QK_DIM // 2
    power = (entry % turn).astype(F32) * (-1.0 / turn)
    angle = position * jnp.exp(power * math.log(10000.0))
    cosine = jnp.cos(angle)
    sine = jnp.where(entry < turn, -jnp.sin(angle), jnp.sin(angle))

    def rotate(values):
        other = jnp.where(
            entry < turn, pltpu.roll(values, LANES - turn, 1), pltpu.roll(values, turn, 1)
        )
        return (values * cosine + other * sine).astype(BF16).astype(F32)

    def spot(plane, inner):
        return plane // CORES * INNER + inner

    own_spot = spot(z, x)
    projected = jnp.zeros((seqs, qkv.shape[1]), F32)
    for i in range(Q_CHUNKS):
        deep = pl.ds(i * depth, depth)
        pltpu.make_async_copy(qkv.at[deep, :], qkv.at[deep, :], local_sem.at[1 + i]).wait()
        projected = projected + dot(normed[:, i * depth : (i + 1) * depth], qkv[deep, :])
    query = projected[:, :inner]
    keys_raw = projected[:, inner : inner + side]
    values_raw = projected[:, inner + side :]
    for load in e_loads + loads:
        load.start()

    groups, spots = cache.shape[1], cache.shape[2]
    share = query.shape[1] // LANES // groups
    scale = QK_DIM**-0.5
    lines = 2 * share
    lower = lax.broadcasted_iota(jnp.int32, (seqs, LANES), 1) < QK_DIM
    fresh = []
    for g in range(groups):
        key = rotate(keys_raw[:, g * LANES : (g + 1) * LANES])
        value = values_raw[:, g * LANES : (g + 1) * LANES].astype(BF16).astype(F32)
        new_ref[:, 2 * g * LANES : (2 * g + 1) * LANES] = key.astype(BF16)
        new_ref[:, (2 * g + 1) * LANES : (2 * g + 2) * LANES] = value.astype(BF16)
        fresh.append((key, value))
        for j in range(share):
            at = (g * share + j) * LANES
            head = rotate(query[:, at : at + LANES])
            pairs[g, :, j, :] = jnp.where(lower, head, 0.0)
            pairs[g, :, share + j, :] = jnp.where(lower, 0.0, head)
        spread = (pairs[g] * scale).reshape(seqs * lines, LANES).astype(BF16)
        turn_of = lax.broadcasted_iota(jnp.int32, spread.shape, 0) // lines % 2
        asked[g, :, :LANES] = jnp.where(turn_of == 0, spread, jnp.zeros_like(spread))
        asked[g, :, LANES:] = jnp.where(turn_of == 0, jnp.zeros_like(spread), spread)

    def push(index):
        where = (gu.at[c], ed.at[block(c, part), :])[index]
        return remote(where, where, push_send.at[0], push_recv.at[index], (e, mate))

    def pushed(index):
        where = (gu.at[1 - c], ed.at[block(1 - c, part), :])[index]
        remote(where, where, push_send.at[0], push_recv.at[index], (e, mate)).wait_recv()

    def beside(s, g, lanes):
        return jnp.concatenate([cache[s, g, :, lanes], cache[s + 1, g, :, lanes]], axis=1)

    place = lax.broadcasted_iota(jnp.int32, (bunch, lines, spots), 2)
    line = lax.broadcasted_iota(jnp.int32, (lines, 1), 0)

    def score(start):
        for s in range(start, start + bunch, 2):
            for g in range(groups):
                scores[g, s : s + 2] = lax.dot_general(
                    asked[g, s * lines : (s + 2) * lines, :],
                    beside(s, g, slice(0, LANES)),
                    (((1,), (1,)), ((), ())),
                    preferred_element_type=F32,
                ).reshape(2, lines, spots)

    def attend(start):
        stop = start + bunch
        length = jnp.zeros((bunch, lines, 1), jnp.int32)
        which = lax.broadcasted_iota(jnp.int32, (bunch, lines, 1), 0)
        for s in range(bunch):
            length = jnp.where(which == s, lengths_ref[start + s], length)
        valid = place < length
        for g in range(groups):
            key, value = (half[start:stop] for half in fresh[g])
            latest = jnp.sum(pairs[g, start:stop] * key[:, None, :], axis=-1, keepdims=True) * scale
            masked = jnp.where(valid, scores[g, start:stop], -jnp.inf)
            top = jnp.maximum(jnp.max(masked, axis=-1, keepdims=True), latest)
            raised = jnp.exp(masked - top)
            raised_new = jnp.exp(latest - top)
            total = jnp.sum(raised, axis=-1, keepdims=True) + raised_new
            lam = jnp.full((lines, 1), 1.0, F32)
            for j in range(share):
                lam = jnp.where(line == share + j, lam_ref[g * share + j], lam)
            part_of = lam[None] / total
            prob = raised * part_of
            prob_new = jnp.broadcast_to(raised_new * part_of, (bunch, lines, LANES))
            weights = (prob - pltpu.roll(prob, share, 1)).astype(BF16)
            new_weight = (
                (prob_new - pltpu.roll(prob_new, share, 1)).astype(BF16).astype(F32)
            )
            fresh_part = new_weight * value[:, None, :]
            for s in range(0, bunch, 2):
                both = dot(
                    weights[s : s + 2].reshape(2 * lines, spots),
                    beside(start + s, g, slice(LANES, None)),
                )
                mixed[g, start + s] = both[:lines, :LANES]
                mixed[g, start + s + 1] = both[lines:, LANES:]
            whole = mixed[g, start:stop] + fresh_part
            mean_sq = jnp.mean(whole * whole, axis=-1, keepdims=True)
            mixed[g, start:stop] = whole * lax.rsqrt(mean_sq + EPS) * head_gain_ref[...][None]

    for i in range(CACHE_CHUNKS):
        if i == CACHE_CHUNKS - 1:
            for load in late_loads:
                load.wait()
        cache_loads[i].wait()
        score(i * bunch)
        if i == CACHE_CHUNKS - 1:
            for k in range(CACHE_CHUNKS):
                attend(k * bunch)
    for g in range(groups):
        for j in range(share):
            at = (g * share + j) * LANES
            heads_ref[:, at : at + LANES] = mixed[g, :, j, :].astype(BF16)

    def heads_copy(mask):
        return remote(
            heads_ref,
            heads_all.at[mask - 1],
            heads_send.at[0],
            heads_recv.at[mask // CORES],
            (e, flip(t, mask)),
        )

    pl.semaphore_wait(barrier, n_ep * n_tp - 1)
    for mask in range(n_tp - 1, 0, -1):
        heads_copy(mask).start()

    for load in e_loads:
        load.wait()
    push(0).start()
    push(1).start()

    lane = lax.broadcasted_iota(jnp.int32, (seqs, route.shape[2]), 1)
    table = jnp.zeros((seqs, route.shape[2]), F32)
    for k in range(ids_ref.shape[0]):
        wanted = column(ids_ref[k : k + 1, :])
        table = table + jnp.where(lane == wanted, column(rw_ref[k : k + 1, :]), 0.0)

    @pl.when(odd == 0)
    def _():
        route[own_spot] = table

    def route_copy(mask):
        where = route.at[own_spot]
        return remote(
            where, where, route_send.at[0], route_recv.at[0], (flip(e, mask), t)
        )

    @pl.when(odd == 0)
    def _():
        for mask in range(1, n_ep):
            route_copy(mask).start()


    loads[0].wait()
    span = heads_ref.shape[1]
    total = dot(heads_ref[...], ow[block(t, span), :])
    for far in range(n_tp // CORES):
        batch = heads_all.at[pl.ds(0, 1) if far == 0 else pl.ds(far * CORES - 1, CORES)]
        remote(batch, batch, heads_send.at[0], heads_recv.at[far], (e, t)).wait_recv()
        for mask in range(max(far * CORES, 1), (far + 1) * CORES):
            total = total + dot(heads_all[mask - 1], ow[block(flip(t, mask), span), :])
    own_cols = block(t, quarter)
    own_stream = (resid_ref[:, own_cols].astype(F32) + total).astype(BF16)
    mine[...] = own_stream

    around = ((1, 1), (1, 0), (0, 1))
    last = turns - 1
    edge = jnp.logical_or(z == 0, z == planes - 1)
    far = jnp.logical_and(edge, odd == 1)

    def chunk(group, owner):
        return stream.at[block(group, seqs), block(owner, quarter)]

    def to_plane(step):
        dx, dy = around[step]
        there = (z * INNER + flip(x, dx), flip(y, dy) * CORES + keeper)
        return remote(
            mine, chunk(e, t), chunk_send.at[0], group_recv.at[z // CORES, dx], there
        )

    def to_column(d):
        core = jnp.where(z == planes - 1, keeper, RELAY) if d == planes - 1 else RELAY
        there = (flip(z, d) * INNER + x, y * CORES + core)
        return remote(mine, chunk(e, t), chunk_send.at[0], climb_recv.at[z, c], there)

    def to_mate():
        return remote(mine, chunk(e, t), chunk_send.at[0], climb_recv.at[z, c], (e, mate))

    def to_far(step):
        dx, dy = around[step]
        there = (flip(z, planes - 1) * INNER + flip(x, dx), flip(y, dy) * CORES + keeper)
        return remote(
            mine, chunk(e, t), chunk_send.at[0], group_recv.at[z // CORES, dx], there
        )

    for d in range(planes - 2, 0, -1):
        to_column(d).start()

    @pl.when(z == planes - 1)
    def _():
        for step in range(len(around)):
            to_far(step).start()

    to_column(planes - 1).start()
    for step in range(len(around)):
        to_plane(step).start()

    @pl.when(odd == 1)
    def _():
        to_mate().start()

    @pl.when(odd == 0)
    def _():
        stream[block(e, seqs), own_cols] = own_stream

    near = z + odd * (1 - 2 * (z % 2))

    def plane_of(i):
        return flip(near, 2 * i)

    def arrived(plane, core):
        where = chunk(plane * INNER + x, y * CORES + core)
        remote(where, where, chunk_send.at[0], climb_recv.at[plane, core], (e, t)).wait_recv()

    def forward(plane, core, step):
        dx, dy = around[step]
        where = chunk(plane * INNER + x, y * CORES + core)
        return remote(
            where,
            where,
            chunk_send.at[0],
            group_recv.at[plane // CORES, dx],
            (z * INNER + flip(x, dx), flip(y, dy) * CORES + plane % CORES),
        )

    def hand_over(plane, core):
        where = chunk(plane * INNER + x, y * CORES + core)
        return remote(where, where, chunk_send.at[0], climb_recv.at[plane, core], (e, mate))

    @pl.when(c == RELAY)
    def _():
        for plane in range(planes):
            passes = plane != z
            if plane == planes - 1:
                passes = jnp.logical_and(passes, z != 0)

            @pl.when(passes)
            def _(plane=plane):
                for core in range(CORES):
                    arrived(plane, core)
                    for step in range(len(around)):
                        forward(plane, core, step).start()
                    if plane % CORES != RELAY:
                        hand_over(plane, core).start()

    def normalise(i):
        plane = CORES * i + c

        @pl.when(plane == z)
        def _():
            arrived(plane, 1 - c)

        leapt = jnp.logical_and(plane == planes - 1, z == 0)

        @pl.when(jnp.logical_and(plane != z, jnp.logical_or(c != RELAY, leapt)))
        def _():
            for core in range(CORES):
                arrived(plane, core)

        for inner in range(INNER):
            group = plane * INNER + flip(x, inner)
            came = stream.at[
                block(group, seqs),
                pl.ds(0, width) if inner else block(flip(y, 1), CORES * quarter),
            ]
            remote(
                came, came, chunk_send.at[0], group_recv.at[plane // CORES, inner], (e, t)
            ).wait_recv()
            values = stream[block(group, seqs), :].astype(F32)
            mean_sq = jnp.mean(values * values, axis=-1, keepdims=True)
            scaled = (values * lax.rsqrt(mean_sq + EPS) * gain_ref[...]).astype(BF16)
            ffn[block(spot(plane, flip(x, inner)), seqs), :] = scaled

    for i in range(turns):
        normalise(i)

    def route_wait(count):
        where = route.at[pl.ds(0, count)]
        remote(where, where, route_send.at[0], route_recv.at[0], (e, t)).wait_recv()

    @pl.when(odd == 0)
    def _():
        route_wait(route.shape[0] - 1)

    @pl.when(odd == 1)
    def _():
        route_wait(route.shape[0])

    rows_all = ffn.shape[0]
    pushed(0)
    pushed(1)
    for load in loads[1:]:
        load.wait()
    a = ffn[...]
    for core in range(CORES):
        both = dot(a, gu[core])
        eh[:, core * part : (core + 1) * part] = (
            jax.nn.silu(both[:, :part]) * both[:, part:]
        ).astype(BF16)
    for at in range(0, hid, 2 * LANES):
        piece = slice(at, at + 2 * LANES)
        dh[:, piece] = (jax.nn.silu(dot(a, dg[:, piece])) * dot(a, du[:, piece])).astype(BF16)
    blend = jax.nn.sigmoid(jnp.sum(a.astype(F32) * mixw_ref[...], axis=-1, keepdims=True))
    lanes = lax.broadcasted_iota(jnp.int32, (rows_all, route.shape[2]), 1)
    weight = jnp.sum(
        jnp.where(lanes == e, route[...].reshape(rows_all, route.shape[2]), 0.0),
        axis=1,
        keepdims=True,
    )
    half = CORES * quarter
    def project(dy):
        cols = block(flip(y, dy), half)
        sparse = weight * dot(eh[...], ed[:, cols])
        return sparse + blend * dot(dh[...], dd[:, cols])

    leaving[1] = project(1).astype(BF16)

    def leave(i, core, step):
        dx, dy = around[step]
        where = spot(plane_of(i), flip(x, dx))
        return remote(
            leaving.at[dy, block(where, seqs), pl.ds(core * quarter, quarter)],
            plane_in.at[i, core, step],
            chunk_send.at[0],
            plane_recv.at[i, core],
            (z * INNER + flip(x, dx), flip(y, dy) * CORES + c),
        )

    def leap(core, step):
        dx, dy = around[step] if step < len(around) else (0, 0)
        where = spot(plane_of(last), flip(x, dx))
        return remote(
            leaving.at[dy, block(where, seqs), pl.ds(core * quarter, quarter)],
            column_in.at[planes - 1 + (step + 1) % (len(around) + 1)],
            chunk_send.at[0],
            column_recv.at[0],
            (plane_of(last) * INNER + flip(x, dx), flip(y, dy) * CORES + core),
        )

    order = range(turns - 1, -1, -1)
    for dy in (1, 0):
        if not dy:
            total = project(0)
            leaving[0] = total.astype(BF16)
            kept[...] = total
        steps = [step for step in range(len(around)) if around[step][1] == dy]

        @pl.when(far)
        def _():
            for step in steps + [len(around)] * (1 - dy):
                for core in range(CORES):
                    leap(core, step).start()

        for i in order:

            def depart(i=i):
                for core in range(CORES):
                    for step in steps:
                        leave(i, core, step).start()

            if i == last:
                pl.when(jnp.logical_not(far))(depart)
            else:
                depart()

    def own_plane(i):
        return jnp.logical_and(odd == 0, i == 0)

    def climb(i, core):
        return remote(
            column_out.at[i, core],
            column_in.at[odd + 2 * i],
            chunk_send.at[0],
            column_recv.at[0],
            (plane_of(i) * INNER + x, y * CORES + core),
        )

    def stays(i, core):
        return jnp.logical_and(own_plane(i), c == core)

    def rise(i):
        for core in range(CORES):
            gathered = kept[block(spot(plane_of(i), x), seqs), core * quarter : (core + 1) * quarter]
            came = plane_in.at[i, core]
            remote(came, came, chunk_send.at[0], plane_recv.at[i, core], (e, t)).wait_recv()
            for step in range(len(around)):
                gathered = gathered + plane_in[i, core, step].astype(F32)
            column_out[i, core] = gathered.astype(BF16)

            @pl.when(jnp.logical_not(stays(i, core)))
            def _(i=i, core=core):
                climb(i, core).start()

    for i in order:
        if i == last:

            @pl.when(jnp.logical_not(far))
            def _(i=i):
                rise(i)
        else:
            rise(i)

    def took(start, stop):
        where = column_in.at[pl.ds(start, stop - start)]
        remote(where, where, chunk_send.at[0], column_recv.at[0], (e, t)).wait_recv()

    @pl.when(odd == 0)
    def _():
        column_in[0] = column_out[0, c]

    def finish(stop):
        for parity in range(2):

            @pl.when(odd == parity)
            def _(parity=parity):
                took(1 - parity, stop)

        out_ref[...] = (
            own_stream.astype(F32) + jnp.sum(column_in[:stop].astype(F32), axis=0)
        ).astype(BF16)

    @pl.when(edge)
    def _():
        finish(planes + len(around))

    @pl.when(jnp.logical_not(edge))
    def _():
        finish(planes)

    push(0).wait_send()
    push(1).wait_send()
    remote(heads_all, heads_all, heads_send.at[0], heads_recv.at[0], (e, t)).wait_send()

    def drained(count):
        where = ow.at[pl.ds(0, count * seqs), :]
        remote(where, where, chunk_send.at[0], column_recv.at[0], (e, t)).wait_send()

    hops = len(around)
    @pl.when(odd == 0)
    def _():
        for mask in range(1, n_ep):
            route_copy(mask).wait_send()

    for level in range(planes):
        for core in range(CORES):
            count = planes - 1 + hops + turns * CORES * (hops + 1)
            count += hops if level == planes - 1 else 0
            count += 1 if (level + core) % CORES else -1
            for plane in range(planes) if core == RELAY else ():
                if plane != level and plane - level != planes - 1:
                    count += CORES * (hops + (plane % CORES != RELAY))

            @pl.when(jnp.logical_and(z == level, c == core))
            def _(count=count):
                drained(count)


def settle(layer_ref, fresh_ref, layer_out, fresh_out, sem):
    first = pltpu.make_async_copy(layer_ref, layer_out, sem.at[0])
    second = pltpu.make_async_copy(fresh_ref, fresh_out, sem.at[1])
    first.start()
    second.start()
    first.wait()
    second.wait()


def near_call(n_ep, n_tp, arrays):
    (
        residual_in,
        lengths,
        kv_cache,
        norm_gain_attn,
        query_weight,
        key_weight,
        value_weight,
        diff_lambda,
        head_gain,
        out_weight,
        norm_gain_ffn,
        route_ids,
        route_weights,
        expert_gate,
        expert_up,
        expert_down,
        dense_gate,
        dense_up,
        dense_down,
        dense_mix,
    ) = arrays
    seqs, width = residual_in.shape
    held = lambda value: pltpu.with_memory_space_constraint(value, pltpu.HBM)
    groups, spots = kv_cache.shape[1:3]
    share = diff_lambda.shape[0] // groups
    inner = query_weight.shape[1]
    quarter = out_weight.shape[1]
    part = expert_gate.shape[2]
    hid = dense_gate.shape[1] // (n_tp // CORES)
    turns = n_ep // INNER // CORES
    blocks = turns * INNER
    rows = blocks * seqs
    lanes = -(-n_ep // LANES) * LANES
    topk = route_ids.shape[1]
    vmem = pl.BlockSpec(memory_space=pltpu.VMEM)
    hbm = pl.BlockSpec(memory_space=pltpu.HBM)
    dma = pltpu.SemaphoreType.DMA
    layer_out, fresh = pl.pallas_call(
        functools.partial(near_kernel, n_ep, n_tp),
        out_shape=(
            jax.ShapeDtypeStruct((seqs, quarter), BF16),
            jax.ShapeDtypeStruct((seqs, groups * kv_cache.shape[3]), BF16),
        ),
        in_specs=[hbm] * 20,
        out_specs=(vmem, vmem),
        scratch_shapes=[
            pltpu.SMEM(lengths.shape, jnp.int32),
            pltpu.SMEM(diff_lambda.shape, F32),
            pltpu.VMEM(residual_in.shape, BF16),
            pltpu.VMEM((1, width), F32),
            pltpu.VMEM((1, head_gain.shape[0]), F32),
            pltpu.VMEM((1, width), F32),
            pltpu.VMEM((1, width), F32),
            pltpu.VMEM((topk, seqs), jnp.int32),
            pltpu.VMEM((topk, seqs), F32),
            pltpu.VMEM((width, inner + key_weight.shape[1] + value_weight.shape[1]), BF16),
            pltpu.VMEM(kv_cache.shape, BF16),
            pltpu.VMEM((groups, seqs, 2 * share, LANES), F32),
            pltpu.VMEM((groups, seqs * 2 * share, 2 * LANES), BF16),
            pltpu.VMEM((groups, seqs, 2 * share, spots), F32),
            pltpu.VMEM((groups, seqs, 2 * share, LANES), F32),
            pltpu.VMEM((seqs, inner), BF16),
            pltpu.VMEM(out_weight.shape, BF16),
            pltpu.VMEM((CORES, width, 2 * part), BF16),
            pltpu.VMEM((CORES * part, width), BF16),
            pltpu.VMEM((width, hid), BF16),
            pltpu.VMEM((width, hid), BF16),
            pltpu.VMEM((hid, width), BF16),
            pltpu.VMEM((n_tp - 1, seqs, inner), BF16),
            pltpu.VMEM((seqs, quarter), BF16),
            pltpu.VMEM((n_ep * seqs, width), BF16),
            pltpu.VMEM((rows, width), BF16),
            pltpu.VMEM((blocks, seqs, lanes), F32),
            pltpu.VMEM((rows, CORES * part), BF16),
            pltpu.VMEM((rows, hid), BF16),
            pltpu.VMEM((2, rows, CORES * quarter), BF16),
            pltpu.VMEM((rows, CORES * quarter), F32),
            pltpu.VMEM((turns, CORES, 3, seqs, quarter), BF16),
            pltpu.VMEM((turns, CORES, seqs, quarter), BF16),
            pltpu.VMEM((n_ep // INNER + 3, seqs, quarter), BF16),
            dma((Q_CHUNKS + CACHE_CHUNKS + 4,)),
            dma((1,)),
            dma((2,)),
            dma((1,)),
            dma((1,)),
            dma((1,)),
            dma((n_tp // CORES,)),
            dma((1,)),
            dma((n_ep // INNER, CORES)),
            dma((turns, INNER)),
            dma((turns, CORES)),
            dma((1,)),
        ],
        compiler_params=pltpu.CompilerParams(
            collective_id=0, has_side_effects=True, vmem_limit_bytes=36 * 1024 * 1024
        ),
    )(
        held(lengths),
        held(diff_lambda),
        held(residual_in),
        held(norm_gain_attn[None, :]),
        held(head_gain[None, :]),
        held(norm_gain_ffn[None, :]),
        held(dense_mix[None, :]),
        held(route_ids.T),
        held(route_weights.T),
        held(query_weight),
        held(key_weight),
        held(value_weight),
        held(kv_cache),
        held(out_weight),
        held(expert_gate),
        held(expert_up),
        held(expert_down),
        held(dense_gate),
        held(dense_up),
        held(dense_down),
    )
    layer_out, fresh = pl.pallas_call(
        settle,
        out_shape=(
            jax.ShapeDtypeStruct(layer_out.shape, BF16),
            jax.ShapeDtypeStruct(fresh.shape, BF16),
        ),
        in_specs=[vmem, vmem],
        out_specs=(hbm, hbm),
        scratch_shapes=[dma((2,))],
        compiler_params=pltpu.CompilerParams(vmem_limit_bytes=1024 * 1024),
    )(layer_out, fresh)
    return layer_out, fresh.reshape(seqs, groups, kv_cache.shape[3])


def on_device(
    residual_in,
    lengths,
    kv_cache,
    norm_gain_attn,
    query_weight,
    key_weight,
    value_weight,
    diff_lambda,
    head_gain,
    out_weight,
    norm_gain_ffn,
    route_ids,
    route_weights,
    expert_gate,
    expert_up,
    expert_down,
    dense_gate,
    dense_up,
    dense_down,
    dense_mix,
):
    n_ep = lax.axis_size("ep")
    n_tp = lax.axis_size("tp")
    half = n_tp // 2
    if (
        n_tp == 2 * CORES
        and n_ep in (4, 8, 16)
        and expert_gate.shape[0] == 1
        and dense_gate.shape[1] // half % LANES == 0
        and expert_gate.shape[2] % LANES == 0
    ):
        return near_call(
            n_ep,
            n_tp,
            (
                residual_in,
                lengths,
                kv_cache,
                norm_gain_attn,
                query_weight,
                key_weight,
                value_weight,
                diff_lambda,
                head_gain,
                out_weight,
                norm_gain_ffn,
                route_ids,
                route_weights,
                expert_gate,
                expert_up,
                expert_down,
                dense_gate,
                dense_up,
                dense_down,
                dense_mix,
            ),
        )
    seqs, width = residual_in.shape
    groups, spots = kv_cache.shape[1:3]
    share = diff_lambda.shape[0] // groups
    inner = query_weight.shape[1]
    quarter = out_weight.shape[1]
    held, _, part = expert_gate.shape
    rows = n_ep * seqs
    own = dense_gate.shape[1] // n_tp
    split = own % LANES == 0
    hid = own if split else dense_gate.shape[1]
    lanes = -(-n_ep * held // LANES) * LANES
    vmem = pl.BlockSpec(memory_space=pltpu.VMEM)
    smem = pl.BlockSpec(memory_space=pltpu.SMEM)
    hbm = pl.BlockSpec(memory_space=pl.ANY)
    dma = pltpu.SemaphoreType.DMA
    layer_out, fresh = pl.pallas_call(
        functools.partial(layer_kernel, n_ep, n_tp, split),
        out_shape=(
            jax.ShapeDtypeStruct((seqs, quarter), F32),
            jax.ShapeDtypeStruct((seqs, groups * kv_cache.shape[3]), F32),
        ),
        in_specs=[smem] * 2 + [vmem] * 7 + [hbm] * 11,
        out_specs=(vmem, vmem),
        scratch_shapes=[
            pltpu.VMEM(query_weight.shape, BF16),
            pltpu.VMEM(key_weight.shape, BF16),
            pltpu.VMEM(value_weight.shape, BF16),
            pltpu.VMEM(kv_cache.shape, BF16),
            pltpu.VMEM((groups, seqs, 2 * share, LANES), F32),
            pltpu.VMEM((groups, seqs, 2 * share, spots), F32),
            pltpu.VMEM((groups, seqs, 2 * share, LANES), F32),
            pltpu.VMEM((seqs, inner), BF16),
            pltpu.VMEM(out_weight.shape, BF16),
            pltpu.VMEM(expert_gate.shape, BF16),
            pltpu.VMEM(expert_up.shape, BF16),
            pltpu.VMEM(expert_down.shape, BF16),
            pltpu.VMEM((width, hid), BF16),
            pltpu.VMEM((width, hid), BF16),
            pltpu.VMEM((hid, width), BF16),
            pltpu.VMEM((n_tp - 1, seqs, inner), BF16),
            pltpu.VMEM((rows, width), BF16),
            pltpu.VMEM((rows, width), BF16),
            pltpu.VMEM((rows, LANES), F32),
            pltpu.VMEM((rows, lanes), F32),
            pltpu.VMEM((held, rows, part), BF16),
            pltpu.VMEM((rows, hid), BF16),
            pltpu.VMEM((half, rows, quarter), BF16),
            pltpu.VMEM((half, rows, quarter), BF16),
            pltpu.VMEM((half, rows, quarter), BF16),
            pltpu.VMEM((n_ep * half, seqs, quarter), BF16),
            dma((7,)),
            dma((Q_CHUNKS + 2,)),
            dma((seqs,)),
            dma((n_ep - 1,)),
            dma((n_ep - 1,)),
            dma((n_tp - 1,)),
            dma((n_tp - 1,)),
            dma((n_ep,)),
            dma((half, n_ep)),
            dma((max(half - 1, 1), n_ep)),
            dma((n_tp, n_ep)),
            dma((half,)),
            dma((half,)),
            dma((half, n_ep)),
            dma((n_ep * half,)),
        ],
        compiler_params=pltpu.CompilerParams(
            collective_id=0, has_side_effects=True, vmem_limit_bytes=60 * 1024 * 1024
        ),
    )(
        lengths,
        diff_lambda,
        residual_in,
        norm_gain_attn[None, :],
        head_gain[None, :],
        norm_gain_ffn[None, :],
        dense_mix[None, :],
        route_ids.T,
        route_weights.T,
        query_weight,
        key_weight,
        value_weight,
        kv_cache,
        out_weight,
        expert_gate,
        expert_up,
        expert_down,
        dense_gate,
        dense_up,
        dense_down,
    )
    new_rows = fresh.astype(BF16).reshape(seqs, groups, kv_cache.shape[3])
    return (layer_out.astype(BF16), new_rows)


def solution(mesh):
    placed = (
        P("ep", None),
        P("ep"),
        P("ep", "tp", None, None),
        P(),
        P(None, "tp"),
        P(None, "tp"),
        P(None, "tp"),
        P("tp"),
        P(),
        P(None, "tp"),
        P(),
        P("ep", None),
        P("ep", None),
        P("ep", None, "tp"),
        P("ep", None, "tp"),
        P("ep", "tp", None),
        P(None, "ep"),
        P(None, "ep"),
        P("ep", None),
        P(),
    )
    return jax.shard_map(
        on_device,
        mesh=mesh,
        in_specs=placed,
        out_specs=(P("ep", "tp"), P("ep", "tp", None)),
        check_vma=False,
    )
```

```python
import functools
import math

import jax
import jax.numpy as jnp
from jax import lax
from jax.experimental import pallas as pl
from jax.experimental.pallas import tpu as pltpu
from jax.sharding import PartitionSpec as P

QK_DIM = 64
EPS = 1e-06
MESH = pl.DeviceIdType.MESH
F32 = jnp.float32
BF16 = jnp.bfloat16
LANES = 128
Q_CHUNKS = 4
INNER = 2
CORES = 2
RELAY = 1
CACHE_CHUNKS = 4


def flip(value, mask):
    bit = 1
    while bit <= mask:
        if mask & bit:
            value = value + bit * (1 - 2 * ((value // bit) % 2))
        bit *= 2
    return value


def each(count, body, order=None):
    if count <= 16:
        for index in order if order is not None else range(count):
            body(index)
    else:

        def step(index, carry):
            body(index)
            return carry

        lax.fori_loop(0, count, step, 0)


def block(start, size):
    return pl.ds(pl.multiple_of(start * size, size), size)


def remote(source, target, send, recv, where):
    return pltpu.make_async_remote_copy(
        src_ref=source,
        dst_ref=target,
        send_sem=send,
        recv_sem=recv,
        device_id=where,
        device_id_type=MESH,
    )


def dot(left, right):
    return jnp.dot(left, right, preferred_element_type=F32)


def column(row):
    count = row.shape[1]
    square = (count, count)
    same = lax.broadcasted_iota(jnp.int32, square, 0) == lax.broadcasted_iota(jnp.int32, square, 1)
    return jnp.sum(jnp.where(same, row, jnp.zeros_like(row)), axis=1, keepdims=True)


def layer_kernel(
    n_ep,
    n_tp,
    split,
    lengths_ref,
    lam_ref,
    resid_ref,
    first_gain_ref,
    head_gain_ref,
    gain_ref,
    mixw_ref,
    ids_ref,
    rw_ref,
    qw_hbm,
    kw_hbm,
    vw_hbm,
    cache_hbm,
    ow_hbm,
    eg_hbm,
    eu_hbm,
    ed_hbm,
    dg_hbm,
    du_hbm,
    dd_hbm,
    out_ref,
    new_ref,
    qw,
    kw,
    vw,
    cache,
    pairs,
    scores,
    mixed,
    heads_ref,
    ow,
    eg,
    eu,
    ed,
    dg,
    du,
    dd,
    heads_all,
    stream,
    ffn,
    mix,
    route,
    eh,
    dh,
    away,
    came,
    summed,
    landed,
    w_sem,
    q_sem,
    cache_sem,
    route_send,
    route_recv,
    heads_send,
    heads_recv,
    first_send,
    second_send,
    relay_send,
    stream_recv,
    pair_send,
    pair_recv,
    back_send,
    back_recv,
):
    e = lax.axis_index("ep")
    t = lax.axis_index("tp")
    half = n_tp // 2
    mate = flip(t, 1)
    core = t % 2
    seqs, width = resid_ref.shape
    quarter = out_ref.shape[1]
    held, _, part = eg.shape
    hid = dg.shape[1]
    rows_all = n_ep * seqs
    evens = [2 * i for i in range(1, half)]

    depth = qw.shape[0] // Q_CHUNKS
    q_loads = [
        pltpu.make_async_copy(
            qw_hbm.at[pl.ds(i * depth, depth), :], qw.at[pl.ds(i * depth, depth), :], q_sem.at[i]
        )
        for i in range(Q_CHUNKS)
    ] + [
        pltpu.make_async_copy(kw_hbm, kw, q_sem.at[Q_CHUNKS]),
        pltpu.make_async_copy(vw_hbm, vw, q_sem.at[Q_CHUNKS + 1]),
    ]
    for load in q_loads:
        load.start()
    cache_loads = [
        pltpu.make_async_copy(cache_hbm.at[s], cache.at[s], cache_sem.at[s]) for s in range(seqs)
    ]
    for load in cache_loads:
        load.start()

    barrier = pltpu.get_barrier_semaphore()

    def greet(index):
        where = (index // half, 2 * (index % half) + core)

        @pl.when(jnp.logical_or(where[0] != e, where[1] != t))
        def _():
            pl.semaphore_signal(barrier, inc=1, device_id=where, device_id_type=MESH)

    each(n_ep * half, greet)
    for i in range(half):
        pl.semaphore_signal(
            barrier, inc=1, device_id=(e, 2 * i + 1 - core), device_id_type=MESH
        )

    if split:
        cols = block(t, hid)
        dense_parts = (dg_hbm.at[:, cols], du_hbm.at[:, cols], dd_hbm.at[cols, :])
    else:
        dense_parts = (dg_hbm, du_hbm, dd_hbm)
    loads = [
        pltpu.make_async_copy(src, dst, w_sem.at[i])
        for i, (src, dst) in enumerate(
            zip((ow_hbm, eg_hbm, eu_hbm) + dense_parts[:2] + (ed_hbm, dense_parts[2]), (ow, eg, eu, dg, du, ed, dd))
        )
    ]

    lane = lax.broadcasted_iota(jnp.int32, (seqs, route.shape[1]), 1)
    table = jnp.zeros((seqs, route.shape[1]), F32)
    for k in range(ids_ref.shape[0]):
        wanted = column(ids_ref[k : k + 1, :])
        table = table + jnp.where(lane == wanted, column(rw_ref[k : k + 1, :]), 0.0)
    own_rows = block(e, seqs)
    route[own_rows, :] = table

    resid = resid_ref[...].astype(F32)
    mean_sq = jnp.mean(resid * resid, axis=-1, keepdims=True)
    normed = (resid * lax.rsqrt(mean_sq + EPS) * first_gain_ref[...]).astype(BF16)
    row = lax.broadcasted_iota(jnp.int32, (seqs, LANES), 0)
    entry = lax.broadcasted_iota(jnp.int32, (seqs, LANES), 1) % QK_DIM
    position = jnp.zeros((seqs, LANES), F32)
    for s in range(seqs):
        position = jnp.where(row == s, lengths_ref[s].astype(F32), position)
    turn = QK_DIM // 2
    power = (entry % turn).astype(F32) * (-1.0 / turn)
    angle = position * jnp.exp(power * math.log(10000.0))
    cosine = jnp.cos(angle)
    sine = jnp.where(entry < turn, -jnp.sin(angle), jnp.sin(angle))

    def rotate(values):
        other = jnp.where(
            entry < turn, pltpu.roll(values, LANES - turn, 1), pltpu.roll(values, turn, 1)
        )
        return (values * cosine + other * sine).astype(BF16).astype(F32)

    query = jnp.zeros((seqs, qw.shape[1]), F32)
    for i in range(Q_CHUNKS):
        q_loads[i].wait()
        query = query + dot(
            normed[:, i * depth : (i + 1) * depth], qw[i * depth : (i + 1) * depth, :]
        )
    for load in q_loads[Q_CHUNKS:]:
        load.wait()
    keys_raw = dot(normed, kw[...])
    values_raw = dot(normed, vw[...])
    for load in loads:
        load.start()

    groups, spots = cache.shape[1], cache.shape[2]
    share = query.shape[1] // LANES // groups
    lower = lax.broadcasted_iota(jnp.int32, (seqs, LANES), 1) < QK_DIM
    fresh = []
    for g in range(groups):
        key = rotate(keys_raw[:, g * LANES : (g + 1) * LANES])
        value = values_raw[:, g * LANES : (g + 1) * LANES].astype(BF16).astype(F32)
        new_ref[:, 2 * g * LANES : (2 * g + 1) * LANES] = key
        new_ref[:, (2 * g + 1) * LANES : (2 * g + 2) * LANES] = value
        fresh.append((key, value))
        for j in range(share):
            at = (g * share + j) * LANES
            head = rotate(query[:, at : at + LANES])
            pairs[g, :, j, :] = jnp.where(lower, head, 0.0)
            pairs[g, :, share + j, :] = jnp.where(lower, 0.0, head)

    pl.semaphore_wait(barrier, n_ep * half - 1 + half)

    def route_copy(d):
        there = (e + d) % n_ep
        return remote(
            route.at[own_rows, :],
            route.at[own_rows, :],
            route_send.at[d - 1],
            route_recv.at[d - 1],
            (there, t),
        )

    def route_wait(d):
        came_from = (e + n_ep - d) % n_ep
        spot = route.at[block(came_from, seqs), :]
        remote(spot, spot, route_send.at[d - 1], route_recv.at[d - 1], (e, t)).wait_recv()

    each(n_ep - 1, lambda i: route_copy(i + 1).start())

    scale = QK_DIM**-0.5
    lines = 2 * share
    for s in range(seqs):
        cache_loads[s].wait()
        for g in range(groups):
            both = pairs[g, s].astype(BF16)
            scores[g, s] = (
                lax.dot_general(
                    both,
                    cache[s, g, :, :LANES],
                    (((1,), (1,)), ((), ())),
                    preferred_element_type=F32,
                )
                * scale
            )
    length = jnp.zeros((seqs, lines, 1), jnp.int32)
    which = lax.broadcasted_iota(jnp.int32, (seqs, lines, 1), 0)
    for s in range(seqs):
        length = jnp.where(which == s, lengths_ref[s], length)
    place = lax.broadcasted_iota(jnp.int32, (seqs, lines, spots), 2)
    valid = place < length
    line = lax.broadcasted_iota(jnp.int32, (lines, 1), 0)
    for g in range(groups):
        key, value = fresh[g]
        latest = jnp.sum(pairs[g] * key[:, None, :], axis=-1, keepdims=True) * scale
        masked = jnp.where(valid, scores[g], -jnp.inf)
        top = jnp.maximum(jnp.max(masked, axis=-1, keepdims=True), latest)
        raised = jnp.exp(masked - top)
        raised_new = jnp.exp(latest - top)
        total = jnp.sum(raised, axis=-1, keepdims=True) + raised_new
        prob = raised / total
        prob_new = jnp.broadcast_to(raised_new / total, (seqs, lines, LANES))
        lam = jnp.zeros((lines, 1), F32)
        for j in range(share):
            lam = jnp.where(line == j, lam_ref[g * share + j], lam)
        scores[g] = prob - lam[None] * pltpu.roll(prob, share, 1)
        new_weight = (prob_new - lam[None] * pltpu.roll(prob_new, share, 1)).astype(BF16).astype(F32)
        fresh_part = new_weight * value[:, None, :]
        for s in range(seqs):
            mixed[g, s] = dot(scores[g, s].astype(BF16), cache[s, g, :, LANES:])
        whole = mixed[g] + fresh_part
        mean_sq = jnp.mean(whole * whole, axis=-1, keepdims=True)
        mixed[g] = whole * lax.rsqrt(mean_sq + EPS) * head_gain_ref[...][None]
        for j in range(share):
            at = (g * share + j) * LANES
            heads_ref[:, at : at + LANES] = mixed[g, :, j, :].astype(BF16)

    def heads_copy(mask):
        return remote(
            heads_ref,
            heads_all.at[mask - 1],
            heads_send.at[mask - 1],
            heads_recv.at[mask - 1],
            (e, flip(t, mask)),
        )

    for mask in range(n_tp - 1, 0, -1):
        heads_copy(mask).start()

    loads[0].wait()
    span = heads_ref.shape[1]
    total = dot(heads_ref[...], ow[block(t, span), :])
    for mask in range(1, n_tp):
        heads_copy(mask).wait_recv()
        total = total + dot(heads_all[mask - 1], ow[block(flip(t, mask), span), :])
    own_cols = block(t, quarter)
    own_stream = (resid_ref[:, own_cols].astype(F32) + total).astype(BF16)
    stream[own_rows, own_cols] = own_stream

    def spot(owner, column):
        return stream.at[block(owner, seqs), block(column, quarter)]

    def owner_of(d):
        return (e + n_ep - d) % n_ep

    def first(d):
        return remote(
            spot(e, t), spot(e, t), first_send.at[d], stream_recv.at[0, d], ((e + d) % n_ep, t)
        )

    def second(d, mask):
        index = mask // 2 if mask != 1 else 0
        where = spot(owner_of(d), t)
        return remote(
            where, where, second_send.at[index, d], stream_recv.at[mask, d], (e, flip(t, mask))
        )

    def relay(d, mask):
        where = spot(owner_of(d), flip(t, mask))
        return remote(
            where, where, relay_send.at[mask // 2 - 1, d], stream_recv.at[mask + 1, d], (e, mate)
        )

    def arrived(d, mask):
        where = spot(owner_of(d), flip(t, mask))
        remote(where, where, first_send.at[d], stream_recv.at[mask, d], (e, t)).wait_recv()

    def spread(d):
        for mask in evens:
            second(d, mask).start()
        second(d, 1).start()

    far_first = sorted(range(1, n_ep), key=lambda d: -min(d, n_ep - d)) if n_ep <= 16 else None
    near_first = [0] + far_first[::-1] if far_first is not None else None
    each(n_ep - 1 if far_first is None else 1, lambda i: first(i + 1).start(), order=None) if far_first is None else [
        first(d).start() for d in far_first
    ]

    def stage_two(d):
        if not (isinstance(d, int) and d == 0):
            arrived(d, 0)
        spread(d)

    def stage_three(d):
        for mask in evens:
            arrived(d, mask)
            relay(d, mask).start()

    def normalise(d):
        arrived(d, 1)
        for mask in evens:
            arrived(d, mask + 1)
        rows = block(owner_of(d), seqs)
        values = stream[rows, :].astype(F32)
        mean_sq = jnp.mean(values * values, axis=-1, keepdims=True)
        scaled = (values * lax.rsqrt(mean_sq + EPS) * gain_ref[...]).astype(BF16)
        ffn[rows, :] = scaled
        inner = jnp.sum(scaled.astype(F32) * mixw_ref[...], axis=-1, keepdims=True)
        mix[rows, :] = jnp.broadcast_to(jax.nn.sigmoid(inner), (seqs, LANES))

    if near_first is not None:
        for i, d in enumerate(near_first):
            stage_two(d)
            if i:
                stage_three(near_first[i - 1])
            if i > 1:
                normalise(near_first[i - 2])
        stage_three(near_first[-1])
        for d in near_first[-2:]:
            normalise(d)
    else:
        stage_two(0)
        each(n_ep - 1, lambda i: stage_two(i + 1))
        each(n_ep, stage_three)
        each(n_ep, normalise)
    each(n_ep - 1, lambda i: route_wait(i + 1))

    many = min(rows_all, 128)
    batches = rows_all // many
    for load in loads[1:5]:
        load.wait()

    def hidden(b):
        rows = block(b, many)
        a = ffn[rows, :]
        for j in range(held):
            eh[j, rows, :] = (jax.nn.silu(dot(a, eg[j])) * dot(a, eu[j])).astype(BF16)
        units = jax.nn.silu(dot(a, dg[...])) * dot(a, du[...])
        if not split:
            own = hid // n_tp
            unit = lax.broadcasted_iota(jnp.int32, units.shape, 1)
            units = jnp.where((unit >= t * own) & (unit < (t + 1) * own), units, 0.0)
        dh[rows, :] = units.astype(BF16)

    each(batches, hidden)
    for load in loads[5:]:
        load.wait()

    def result(b, q):
        rows = block(b, many)
        cols = block(q, quarter)
        total = mix[rows, :1] * dot(dh[rows, :], dd[:, cols])
        lanes = lax.broadcasted_iota(jnp.int32, (many, route.shape[1]), 1)
        for j in range(held):
            weight = jnp.sum(
                jnp.where(lanes == e * held + j, route[rows, :], 0.0), axis=1, keepdims=True
            )
            piece = dot(eh[j, rows, :], ed[j, :, cols]).astype(BF16)
            total = total + weight * piece.astype(F32)
        return total

    def pair(j):
        return remote(away.at[j], came.at[j], pair_send.at[j], pair_recv.at[j], (e, mate))

    for j in range(half):

        def leave(b, j=j):
            away[j, block(b, many), :] = result(b, 2 * j + 1 - core).astype(BF16)

        each(batches, leave)
        pair(j).start()

    me = e * half + t // 2

    def back(j, d):
        there = (e + d) % n_ep
        return remote(
            summed.at[j, block(there, seqs), :],
            landed.at[me],
            back_send.at[j, d],
            back_recv.at[me],
            (there, 2 * j + core),
        )

    def same(j, d):
        return jnp.logical_and(jnp.asarray(d == 0), 2 * j + core == t)

    for j in range(half):

        def keep(b, j=j):
            summed[j, block(b, many), :] = result(b, 2 * j + core).astype(BF16)

        each(batches, keep)
    for j in range(half):
        pair(j).wait_recv()

        def add(b, j=j):
            rows = block(b, many)
            summed[j, rows, :] = (summed[j, rows, :].astype(F32) + came[j, rows, :].astype(F32)).astype(BF16)

        each(batches, add)

        def send(d, j=j):
            @pl.when(jnp.logical_not(same(j, d)))
            def _():
                back(j, d).start()

        each(n_ep, send, order=None if far_first is None else far_first + [0])

    landed[me] = summed[t // 2, own_rows, :]

    def take(index):
        @pl.when(index != me)
        def _():
            where = landed.at[index]
            remote(where, where, back_send.at[0, 0], back_recv.at[index], (e, t)).wait_recv()

    each(n_ep * half, take)
    out_ref[...] = own_stream.astype(F32) + jnp.sum(landed[...].astype(F32), axis=0)

    for mask in range(1, n_tp):
        heads_copy(mask).wait_send()
    each(n_ep - 1, lambda i: route_copy(i + 1).wait_send())
    each(n_ep - 1, lambda i: first(i + 1).wait_send())

    def sent(d):
        second(d, 1).wait_send()
        for mask in evens:
            second(d, mask).wait_send()
            relay(d, mask).wait_send()

    each(n_ep, sent)
    for j in range(half):
        pair(j).wait_send()

        def gone(d, j=j):
            @pl.when(jnp.logical_not(same(j, d)))
            def _():
                back(j, d).wait_send()

        each(n_ep, gone)


def keeps(plane):
    return (plane + 1) % CORES


def near_kernel(
    n_ep,
    n_tp,
    lengths_hbm,
    lam_hbm,
    resid_hbm,
    first_gain_hbm,
    head_gain_hbm,
    gain_hbm,
    mixw_hbm,
    ids_hbm,
    rw_hbm,
    qw_hbm,
    kw_hbm,
    vw_hbm,
    cache_hbm,
    ow_hbm,
    eg_hbm,
    eu_hbm,
    ed_hbm,
    dg_hbm,
    du_hbm,
    dd_hbm,
    out_ref,
    new_ref,
    lengths_ref,
    lam_ref,
    resid_ref,
    first_gain_ref,
    head_gain_ref,
    gain_ref,
    mixw_ref,
    ids_ref,
    rw_ref,
    qkv,
    cache,
    pairs,
    asked,
    scores,
    mixed,
    heads_ref,
    ow,
    gu,
    ed,
    dg,
    du,
    dd,
    heads_all,
    mine,
    stream,
    ffn,
    route,
    eh,
    dh,
    leaving,
    kept,
    plane_in,
    column_out,
    column_in,
    local_sem,
    push_send,
    push_recv,
    route_send,
    route_recv,
    heads_send,
    heads_recv,
    chunk_send,
    climb_recv,
    group_recv,
    plane_recv,
    column_recv,
):
    e = lax.axis_index("ep")
    t = lax.axis_index("tp")
    planes = n_ep // INNER
    z = e // INNER
    x = e % INNER
    y = t // CORES
    c = t % CORES
    keeper = keeps(z)
    odd = (c + keeper) % CORES
    turns = planes // CORES
    seqs, width = resid_ref.shape
    quarter = out_ref.shape[1]
    part = eg_hbm.shape[2]
    hid = dg.shape[1]
    mate = flip(t, 1)

    def gather_loads(sem, *routes):
        return [pltpu.make_async_copy(src, dst, local_sem.at[sem]) for src, dst in routes]

    first_loads = gather_loads(
        0, (resid_hbm, resid_ref), (first_gain_hbm, first_gain_ref), (lengths_hbm, lengths_ref)
    )
    for load in first_loads:
        load.start()
    depth = qkv.shape[0] // Q_CHUNKS
    inner = qw_hbm.shape[1]
    side = kw_hbm.shape[1]
    for i in range(Q_CHUNKS):
        deep = pl.ds(i * depth, depth)
        for load in gather_loads(
            1 + i,
            (qw_hbm.at[deep, :], qkv.at[deep, :inner]),
            (kw_hbm.at[deep, :], qkv.at[deep, inner : inner + side]),
            (vw_hbm.at[deep, :], qkv.at[deep, inner + side :]),
        ):
            load.start()

    barrier = pltpu.get_barrier_semaphore()
    for index in range(n_ep * n_tp):
        where = (index // n_tp, index % n_tp)

        @pl.when(jnp.logical_or(where[0] != e, where[1] != t))
        def _():
            pl.semaphore_signal(barrier, inc=1, device_id=where, device_id_type=MESH)

    for load in first_loads:
        load.wait()
    bunch = seqs // CACHE_CHUNKS
    cache_loads = [
        gather_loads(
            1 + Q_CHUNKS + i,
            (cache_hbm.at[pl.ds(i * bunch, bunch)], cache.at[pl.ds(i * bunch, bunch)]),
        )[0]
        for i in range(CACHE_CHUNKS)
    ]
    for load in cache_loads:
        load.start()
    late = 1 + Q_CHUNKS + CACHE_CHUNKS
    late_loads = gather_loads(
        late,
        (ids_hbm, ids_ref),
        (rw_hbm, rw_ref),
        (lam_hbm, lam_ref),
        (head_gain_hbm, head_gain_ref),
        (gain_hbm, gain_ref),
        (mixw_hbm, mixw_ref),
    )
    for load in late_loads:
        load.start()
    cols = block(y, hid)
    e_loads = gather_loads(
        late + 1, (eg_hbm.at[0], gu.at[c, :, :part]), (eu_hbm.at[0], gu.at[c, :, part:])
    ) + gather_loads(late + 2, (ed_hbm.at[0], ed.at[block(c, part), :]))
    loads = [
        gather_loads(1 + i, route)[0]
        for i, route in enumerate(
            (
                (ow_hbm, ow),
                (dg_hbm.at[:, cols], dg),
                (du_hbm.at[:, cols], du),
                (dd_hbm.at[cols, :], dd),
            )
        )
    ]
    resid = resid_ref[...].astype(F32)
    mean_sq = jnp.mean(resid * resid, axis=-1, keepdims=True)
    normed = (resid * lax.rsqrt(mean_sq + EPS) * first_gain_ref[...]).astype(BF16)
    row = lax.broadcasted_iota(jnp.int32, (seqs, LANES), 0)
    entry = lax.broadcasted_iota(jnp.int32, (seqs, LANES), 1) % QK_DIM
    position = jnp.zeros((seqs, LANES), F32)
    for s in range(seqs):
        position = jnp.where(row == s, lengths_ref[s].astype(F32), position)
    turn = QK_DIM // 2
    power = (entry % turn).astype(F32) * (-1.0 / turn)
    angle = position * jnp.exp(power * math.log(10000.0))
    cosine = jnp.cos(angle)
    sine = jnp.where(entry < turn, -jnp.sin(angle), jnp.sin(angle))

    def rotate(values):
        other = jnp.where(
            entry < turn, pltpu.roll(values, LANES - turn, 1), pltpu.roll(values, turn, 1)
        )
        return (values * cosine + other * sine).astype(BF16).astype(F32)

    def spot(plane, inner):
        return plane // CORES * INNER + inner

    own_spot = spot(z, x)
    projected = jnp.zeros((seqs, qkv.shape[1]), F32)
    for i in range(Q_CHUNKS):
        deep = pl.ds(i * depth, depth)
        pltpu.make_async_copy(qkv.at[deep, :], qkv.at[deep, :], local_sem.at[1 + i]).wait()
        projected = projected + dot(normed[:, i * depth : (i + 1) * depth], qkv[deep, :])
    query = projected[:, :inner]
    keys_raw = projected[:, inner : inner + side]
    values_raw = projected[:, inner + side :]
    for load in e_loads + loads:
        load.start()

    groups, spots = cache.shape[1], cache.shape[2]
    share = query.shape[1] // LANES // groups
    scale = QK_DIM**-0.5
    lines = 2 * share
    lower = lax.broadcasted_iota(jnp.int32, (seqs, LANES), 1) < QK_DIM
    fresh = []
    for g in range(groups):
        key = rotate(keys_raw[:, g * LANES : (g + 1) * LANES])
        value = values_raw[:, g * LANES : (g + 1) * LANES].astype(BF16).astype(F32)
        new_ref[:, 2 * g * LANES : (2 * g + 1) * LANES] = key.astype(BF16)
        new_ref[:, (2 * g + 1) * LANES : (2 * g + 2) * LANES] = value.astype(BF16)
        fresh.append((key, value))
        for j in range(share):
            at = (g * share + j) * LANES
            head = rotate(query[:, at : at + LANES])
            pairs[g, :, j, :] = jnp.where(lower, head, 0.0)
            pairs[g, :, share + j, :] = jnp.where(lower, 0.0, head)
        spread = (pairs[g] * scale).reshape(seqs * lines, LANES).astype(BF16)
        turn_of = lax.broadcasted_iota(jnp.int32, spread.shape, 0) // lines % 2
        asked[g, :, :LANES] = jnp.where(turn_of == 0, spread, jnp.zeros_like(spread))
        asked[g, :, LANES:] = jnp.where(turn_of == 0, jnp.zeros_like(spread), spread)

    def push(index):
        where = (gu.at[c], ed.at[block(c, part), :])[index]
        return remote(where, where, push_send.at[0], push_recv.at[index], (e, mate))

    def pushed(index):
        where = (gu.at[1 - c], ed.at[block(1 - c, part), :])[index]
        remote(where, where, push_send.at[0], push_recv.at[index], (e, mate)).wait_recv()

    def beside(s, g, lanes):
        return jnp.concatenate([cache[s, g, :, lanes], cache[s + 1, g, :, lanes]], axis=1)

    place = lax.broadcasted_iota(jnp.int32, (bunch, lines, spots), 2)
    line = lax.broadcasted_iota(jnp.int32, (lines, 1), 0)

    def score(start):
        for s in range(start, start + bunch, 2):
            for g in range(groups):
                scores[g, s : s + 2] = lax.dot_general(
                    asked[g, s * lines : (s + 2) * lines, :],
                    beside(s, g, slice(0, LANES)),
                    (((1,), (1,)), ((), ())),
                    preferred_element_type=F32,
                ).reshape(2, lines, spots)

    def attend(start):
        stop = start + bunch
        length = jnp.zeros((bunch, lines, 1), jnp.int32)
        which = lax.broadcasted_iota(jnp.int32, (bunch, lines, 1), 0)
        for s in range(bunch):
            length = jnp.where(which == s, lengths_ref[start + s], length)
        valid = place < length
        for g in range(groups):
            key, value = (half[start:stop] for half in fresh[g])
            latest = jnp.sum(pairs[g, start:stop] * key[:, None, :], axis=-1, keepdims=True) * scale
            masked = jnp.where(valid, scores[g, start:stop], -jnp.inf)
            top = jnp.maximum(jnp.max(masked, axis=-1, keepdims=True), latest)
            raised = jnp.exp(masked - top)
            raised_new = jnp.exp(latest - top)
            total = jnp.sum(raised, axis=-1, keepdims=True) + raised_new
            lam = jnp.full((lines, 1), 1.0, F32)
            for j in range(share):
                lam = jnp.where(line == share + j, lam_ref[g * share + j], lam)
            part_of = lam[None] / total
            prob = raised * part_of
            prob_new = jnp.broadcast_to(raised_new * part_of, (bunch, lines, LANES))
            weights = (prob - pltpu.roll(prob, share, 1)).astype(BF16)
            new_weight = (
                (prob_new - pltpu.roll(prob_new, share, 1)).astype(BF16).astype(F32)
            )
            fresh_part = new_weight * value[:, None, :]
            for s in range(0, bunch, 2):
                both = dot(
                    weights[s : s + 2].reshape(2 * lines, spots),
                    beside(start + s, g, slice(LANES, None)),
                )
                mixed[g, start + s] = both[:lines, :LANES]
                mixed[g, start + s + 1] = both[lines:, LANES:]
            whole = mixed[g, start:stop] + fresh_part
            mean_sq = jnp.mean(whole * whole, axis=-1, keepdims=True)
            mixed[g, start:stop] = whole * lax.rsqrt(mean_sq + EPS) * head_gain_ref[...][None]

    for i in range(CACHE_CHUNKS):
        if i == CACHE_CHUNKS - 1:
            for load in late_loads:
                load.wait()
        cache_loads[i].wait()
        score(i * bunch)
        if i == CACHE_CHUNKS - 1:
            for k in range(CACHE_CHUNKS):
                attend(k * bunch)
    for g in range(groups):
        for j in range(share):
            at = (g * share + j) * LANES
            heads_ref[:, at : at + LANES] = mixed[g, :, j, :].astype(BF16)

    def heads_copy(mask):
        return remote(
            heads_ref,
            heads_all.at[mask - 1],
            heads_send.at[0],
            heads_recv.at[mask // CORES],
            (e, flip(t, mask)),
        )

    pl.semaphore_wait(barrier, n_ep * n_tp - 1)
    for mask in range(n_tp - 1, 0, -1):
        heads_copy(mask).start()

    for load in e_loads:
        load.wait()
    push(0).start()
    push(1).start()

    lane = lax.broadcasted_iota(jnp.int32, (seqs, route.shape[2]), 1)
    table = jnp.zeros((seqs, route.shape[2]), F32)
    for k in range(ids_ref.shape[0]):
        wanted = column(ids_ref[k : k + 1, :])
        table = table + jnp.where(lane == wanted, column(rw_ref[k : k + 1, :]), 0.0)

    @pl.when(odd == 0)
    def _():
        route[own_spot] = table

    def route_copy(mask):
        where = route.at[own_spot]
        return remote(
            where, where, route_send.at[0], route_recv.at[0], (flip(e, mask), t)
        )

    @pl.when(odd == 0)
    def _():
        for mask in range(1, n_ep):
            route_copy(mask).start()


    loads[0].wait()
    span = heads_ref.shape[1]
    total = dot(heads_ref[...], ow[block(t, span), :])
    for far in range(n_tp // CORES):
        batch = heads_all.at[pl.ds(0, 1) if far == 0 else pl.ds(far * CORES - 1, CORES)]
        remote(batch, batch, heads_send.at[0], heads_recv.at[far], (e, t)).wait_recv()
        for mask in range(max(far * CORES, 1), (far + 1) * CORES):
            total = total + dot(heads_all[mask - 1], ow[block(flip(t, mask), span), :])
    own_cols = block(t, quarter)
    own_stream = (resid_ref[:, own_cols].astype(F32) + total).astype(BF16)
    mine[...] = own_stream

    around = ((1, 1), (1, 0), (0, 1))
    last = turns - 1
    edge = jnp.logical_or(z == 0, z == planes - 1)
    far = jnp.logical_and(edge, odd == 1)

    def chunk(group, owner):
        return stream.at[block(group, seqs), block(owner, quarter)]

    def to_plane(step):
        dx, dy = around[step]
        there = (z * INNER + flip(x, dx), flip(y, dy) * CORES + keeper)
        return remote(
            mine, chunk(e, t), chunk_send.at[0], group_recv.at[z // CORES, dx], there
        )

    def to_column(d):
        core = jnp.where(z == planes - 1, keeper, RELAY) if d == planes - 1 else RELAY
        there = (flip(z, d) * INNER + x, y * CORES + core)
        return remote(mine, chunk(e, t), chunk_send.at[0], climb_recv.at[z, c], there)

    def to_mate():
        return remote(mine, chunk(e, t), chunk_send.at[0], climb_recv.at[z, c], (e, mate))

    def to_far(step):
        dx, dy = around[step]
        there = (flip(z, planes - 1) * INNER + flip(x, dx), flip(y, dy) * CORES + keeper)
        return remote(
            mine, chunk(e, t), chunk_send.at[0], group_recv.at[z // CORES, dx], there
        )

    for d in range(planes - 2, 0, -1):
        to_column(d).start()

    @pl.when(z == planes - 1)
    def _():
        for step in range(len(around)):
            to_far(step).start()

    to_column(planes - 1).start()
    for step in range(len(around)):
        to_plane(step).start()

    @pl.when(odd == 1)
    def _():
        to_mate().start()

    @pl.when(odd == 0)
    def _():
        stream[block(e, seqs), own_cols] = own_stream

    near = z + odd * (1 - 2 * (z % 2))

    def plane_of(i):
        return flip(near, 2 * i)

    def arrived(plane, core):
        where = chunk(plane * INNER + x, y * CORES + core)
        remote(where, where, chunk_send.at[0], climb_recv.at[plane, core], (e, t)).wait_recv()

    def forward(plane, core, step):
        dx, dy = around[step]
        where = chunk(plane * INNER + x, y * CORES + core)
        return remote(
            where,
            where,
            chunk_send.at[0],
            group_recv.at[plane // CORES, dx],
            (z * INNER + flip(x, dx), flip(y, dy) * CORES + keeps(plane)),
        )

    def hand_over(plane, core):
        where = chunk(plane * INNER + x, y * CORES + core)
        return remote(where, where, chunk_send.at[0], climb_recv.at[plane, core], (e, mate))

    @pl.when(c == RELAY)
    def _():
        for plane in range(planes):
            passes = plane != z
            if plane == planes - 1:
                passes = jnp.logical_and(passes, z != 0)

            @pl.when(passes)
            def _(plane=plane):
                for core in range(CORES):
                    arrived(plane, core)
                    for step in range(len(around)):
                        forward(plane, core, step).start()
                    if keeps(plane) != RELAY:
                        hand_over(plane, core).start()

    def normalise(i):
        plane = CORES * i + keeps(c)

        @pl.when(plane == z)
        def _():
            arrived(plane, 1 - c)

        leapt = jnp.logical_and(plane == planes - 1, z == 0)

        @pl.when(jnp.logical_and(plane != z, jnp.logical_or(c != RELAY, leapt)))
        def _():
            for core in range(CORES):
                arrived(plane, core)

        for inner in range(INNER):
            group = plane * INNER + flip(x, inner)
            came = stream.at[
                block(group, seqs),
                pl.ds(0, width) if inner else block(flip(y, 1), CORES * quarter),
            ]
            remote(
                came, came, chunk_send.at[0], group_recv.at[plane // CORES, inner], (e, t)
            ).wait_recv()
            values = stream[block(group, seqs), :].astype(F32)
            mean_sq = jnp.mean(values * values, axis=-1, keepdims=True)
            scaled = (values * lax.rsqrt(mean_sq + EPS) * gain_ref[...]).astype(BF16)
            ffn[block(spot(plane, flip(x, inner)), seqs), :] = scaled

    for i in range(turns):
        normalise(i)

    def route_wait(count):
        where = route.at[pl.ds(0, count)]
        remote(where, where, route_send.at[0], route_recv.at[0], (e, t)).wait_recv()

    @pl.when(odd == 0)
    def _():
        route_wait(route.shape[0] - 1)

    @pl.when(odd == 1)
    def _():
        route_wait(route.shape[0])

    rows_all = ffn.shape[0]
    pushed(0)
    pushed(1)
    for load in loads[1:]:
        load.wait()
    a = ffn[...]
    for core in range(CORES):
        both = dot(a, gu[core])
        eh[:, core * part : (core + 1) * part] = (
            jax.nn.silu(both[:, :part]) * both[:, part:]
        ).astype(BF16)
    for at in range(0, hid, 2 * LANES):
        piece = slice(at, at + 2 * LANES)
        dh[:, piece] = (jax.nn.silu(dot(a, dg[:, piece])) * dot(a, du[:, piece])).astype(BF16)
    blend = jax.nn.sigmoid(jnp.sum(a.astype(F32) * mixw_ref[...], axis=-1, keepdims=True))
    lanes = lax.broadcasted_iota(jnp.int32, (rows_all, route.shape[2]), 1)
    weight = jnp.sum(
        jnp.where(lanes == e, route[...].reshape(rows_all, route.shape[2]), 0.0),
        axis=1,
        keepdims=True,
    )
    half = CORES * quarter
    def project(dy):
        cols = block(flip(y, dy), half)
        sparse = weight * dot(eh[...], ed[:, cols])
        return sparse + blend * dot(dh[...], dd[:, cols])

    leaving[1] = project(1).astype(BF16)

    def own_plane(i):
        return jnp.logical_and(odd == 0, i == 0)

    def leave(i, core, step):
        dx, dy = around[step]
        where = spot(plane_of(i), flip(x, dx))
        summer = jnp.where(own_plane(i), c, RELAY)
        return remote(
            leaving.at[dy, block(where, seqs), pl.ds(core * quarter, quarter)],
            plane_in.at[c, i, core, step],
            chunk_send.at[0],
            plane_recv.at[c, i, core],
            (z * INNER + flip(x, dx), flip(y, dy) * CORES + summer),
        )

    def pass_over(i, core):
        where = spot(plane_of(i), x)
        return remote(
            leaving.at[0, block(where, seqs), pl.ds(core * quarter, quarter)],
            plane_in.at[c, i, core, len(around)],
            chunk_send.at[0],
            plane_recv.at[c, i, core],
            (e, mate),
        )

    def leap(core, step):
        dx, dy = around[step] if step < len(around) else (0, 0)
        where = spot(plane_of(last), flip(x, dx))
        return remote(
            leaving.at[dy, block(where, seqs), pl.ds(core * quarter, quarter)],
            column_in.at[planes - 1 + (step + 1) % (len(around) + 1)],
            chunk_send.at[0],
            column_recv.at[0],
            (plane_of(last) * INNER + flip(x, dx), flip(y, dy) * CORES + core),
        )

    order = range(turns - 1, -1, -1)
    for dy in (1, 0):
        if not dy:
            total = project(0)
            leaving[0] = total.astype(BF16)
            kept[...] = total
        steps = [step for step in range(len(around)) if around[step][1] == dy]

        @pl.when(far)
        def _():
            for step in steps + [len(around)] * (1 - dy):
                for core in range(CORES):
                    leap(core, step).start()

        for i in order:

            def depart(i=i):
                for core in range(CORES):
                    for step in steps:
                        leave(i, core, step).start()
                if not dy:

                    @pl.when(jnp.logical_and(c != RELAY, jnp.logical_not(own_plane(i))))
                    def _():
                        for core in range(CORES):
                            pass_over(i, core).start()

            if i == last:
                pl.when(jnp.logical_not(far))(depart)
            else:
                depart()

    def climb(lane, i, core):
        skew = (lane + keeper) % CORES
        level = flip(z + skew * (1 - 2 * (z % 2)), 2 * i)
        return remote(
            column_out.at[lane, i, core],
            column_in.at[skew + 2 * i],
            chunk_send.at[0],
            column_recv.at[0],
            (level * INNER + x, y * CORES + core),
        )

    def stays(i, core):
        return jnp.logical_and(own_plane(i), c == core)

    def rise(i):
        for core in range(CORES):
            gathered = kept[block(spot(plane_of(i), x), seqs), core * quarter : (core + 1) * quarter]
            came = plane_in.at[c, i, core, pl.ds(0, len(around))]
            remote(came, came, chunk_send.at[0], plane_recv.at[c, i, core], (e, t)).wait_recv()
            for step in range(len(around)):
                gathered = gathered + plane_in[c, i, core, step].astype(F32)
            column_out[c, i, core] = gathered.astype(BF16)

            @pl.when(jnp.logical_not(stays(i, core)))
            def _(i=i, core=core):
                climb(c, i, core).start()

    low = 1 - RELAY

    def lift(i):
        for core in range(CORES):
            came = plane_in.at[low, i, core]
            remote(came, came, chunk_send.at[0], plane_recv.at[low, i, core], (e, t)).wait_recv()
            gathered = plane_in[low, i, core, 0].astype(F32)
            for step in range(1, len(around) + 1):
                gathered = gathered + plane_in[low, i, core, step].astype(F32)
            column_out[low, i, core] = gathered.astype(BF16)
            climb(low, i, core).start()

    for i in order:
        sums = jnp.logical_or(c == RELAY, own_plane(i))
        if i == last:
            sums = jnp.logical_and(sums, jnp.logical_not(far))

        @pl.when(sums)
        def _(i=i):
            rise(i)

    slant = (low + keeper) % CORES == 1
    for i in order:
        theirs = c == RELAY
        if i == 0:
            theirs = jnp.logical_and(theirs, slant)
        if i == last:
            theirs = jnp.logical_and(theirs, jnp.logical_not(jnp.logical_and(edge, slant)))

        @pl.when(theirs)
        def _(i=i):
            lift(i)

    def took(start, stop):
        where = column_in.at[pl.ds(start, stop - start)]
        remote(where, where, chunk_send.at[0], column_recv.at[0], (e, t)).wait_recv()

    @pl.when(odd == 0)
    def _():
        column_in[0] = column_out[c, 0, c]

    def finish(stop):
        for parity in range(2):

            @pl.when(odd == parity)
            def _(parity=parity):
                took(1 - parity, stop)

        out_ref[...] = (
            own_stream.astype(F32) + jnp.sum(column_in[:stop].astype(F32), axis=0)
        ).astype(BF16)

    @pl.when(edge)
    def _():
        finish(planes + len(around))

    @pl.when(jnp.logical_not(edge))
    def _():
        finish(planes)

    push(0).wait_send()
    push(1).wait_send()
    remote(heads_all, heads_all, heads_send.at[0], heads_recv.at[0], (e, t)).wait_send()

    def drained(count):
        where = ow.at[pl.ds(0, count * seqs), :]
        remote(where, where, chunk_send.at[0], column_recv.at[0], (e, t)).wait_send()

    hops = len(around)
    @pl.when(odd == 0)
    def _():
        for mask in range(1, n_ep):
            route_copy(mask).wait_send()

    for level in range(planes):
        for core in range(CORES):
            count = planes - 1 + hops + turns * CORES * (hops + 1)
            count += hops if level == planes - 1 else 0
            count += 1 if core != keeps(level) else -1
            if core == RELAY:
                skew = (1 - RELAY + keeps(level)) % CORES
                lower = [level ^ skew ^ (CORES * i) for i in range(turns)]
                count += CORES * sum(
                    plane != level and abs(plane - level) != planes - 1 for plane in lower
                )
            for plane in range(planes) if core == RELAY else ():
                if plane != level and plane - level != planes - 1:
                    count += CORES * (hops + (keeps(plane) != RELAY))

            @pl.when(jnp.logical_and(z == level, c == core))
            def _(count=count):
                drained(count)


def settle(layer_ref, fresh_ref, layer_out, fresh_out, sem):
    first = pltpu.make_async_copy(layer_ref, layer_out, sem.at[0])
    second = pltpu.make_async_copy(fresh_ref, fresh_out, sem.at[1])
    first.start()
    second.start()
    first.wait()
    second.wait()


def near_call(n_ep, n_tp, arrays):
    (
        residual_in,
        lengths,
        kv_cache,
        norm_gain_attn,
        query_weight,
        key_weight,
        value_weight,
        diff_lambda,
        head_gain,
        out_weight,
        norm_gain_ffn,
        route_ids,
        route_weights,
        expert_gate,
        expert_up,
        expert_down,
        dense_gate,
        dense_up,
        dense_down,
        dense_mix,
    ) = arrays
    seqs, width = residual_in.shape
    held = lambda value: pltpu.with_memory_space_constraint(value, pltpu.HBM)
    groups, spots = kv_cache.shape[1:3]
    share = diff_lambda.shape[0] // groups
    inner = query_weight.shape[1]
    quarter = out_weight.shape[1]
    part = expert_gate.shape[2]
    hid = dense_gate.shape[1] // (n_tp // CORES)
    turns = n_ep // INNER // CORES
    blocks = turns * INNER
    rows = blocks * seqs
    lanes = -(-n_ep // LANES) * LANES
    topk = route_ids.shape[1]
    vmem = pl.BlockSpec(memory_space=pltpu.VMEM)
    hbm = pl.BlockSpec(memory_space=pltpu.HBM)
    dma = pltpu.SemaphoreType.DMA
    layer_out, fresh = pl.pallas_call(
        functools.partial(near_kernel, n_ep, n_tp),
        out_shape=(
            jax.ShapeDtypeStruct((seqs, quarter), BF16),
            jax.ShapeDtypeStruct((seqs, groups * kv_cache.shape[3]), BF16),
        ),
        in_specs=[hbm] * 20,
        out_specs=(vmem, vmem),
        scratch_shapes=[
            pltpu.SMEM(lengths.shape, jnp.int32),
            pltpu.SMEM(diff_lambda.shape, F32),
            pltpu.VMEM(residual_in.shape, BF16),
            pltpu.VMEM((1, width), F32),
            pltpu.VMEM((1, head_gain.shape[0]), F32),
            pltpu.VMEM((1, width), F32),
            pltpu.VMEM((1, width), F32),
            pltpu.VMEM((topk, seqs), jnp.int32),
            pltpu.VMEM((topk, seqs), F32),
            pltpu.VMEM((width, inner + key_weight.shape[1] + value_weight.shape[1]), BF16),
            pltpu.VMEM(kv_cache.shape, BF16),
            pltpu.VMEM((groups, seqs, 2 * share, LANES), F32),
            pltpu.VMEM((groups, seqs * 2 * share, 2 * LANES), BF16),
            pltpu.VMEM((groups, seqs, 2 * share, spots), F32),
            pltpu.VMEM((groups, seqs, 2 * share, LANES), F32),
            pltpu.VMEM((seqs, inner), BF16),
            pltpu.VMEM(out_weight.shape, BF16),
            pltpu.VMEM((CORES, width, 2 * part), BF16),
            pltpu.VMEM((CORES * part, width), BF16),
            pltpu.VMEM((width, hid), BF16),
            pltpu.VMEM((width, hid), BF16),
            pltpu.VMEM((hid, width), BF16),
            pltpu.VMEM((n_tp - 1, seqs, inner), BF16),
            pltpu.VMEM((seqs, quarter), BF16),
            pltpu.VMEM((n_ep * seqs, width), BF16),
            pltpu.VMEM((rows, width), BF16),
            pltpu.VMEM((blocks, seqs, lanes), F32),
            pltpu.VMEM((rows, CORES * part), BF16),
            pltpu.VMEM((rows, hid), BF16),
            pltpu.VMEM((2, rows, CORES * quarter), BF16),
            pltpu.VMEM((rows, CORES * quarter), F32),
            pltpu.VMEM((CORES, turns, CORES, 4, seqs, quarter), BF16),
            pltpu.VMEM((CORES, turns, CORES, seqs, quarter), BF16),
            pltpu.VMEM((n_ep // INNER + 3, seqs, quarter), BF16),
            dma((Q_CHUNKS + CACHE_CHUNKS + 4,)),
            dma((1,)),
            dma((2,)),
            dma((1,)),
            dma((1,)),
            dma((1,)),
            dma((n_tp // CORES,)),
            dma((1,)),
            dma((n_ep // INNER, CORES)),
            dma((turns, INNER)),
            dma((CORES, turns, CORES)),
            dma((1,)),
        ],
        compiler_params=pltpu.CompilerParams(
            collective_id=0, has_side_effects=True, vmem_limit_bytes=36 * 1024 * 1024
        ),
    )(
        held(lengths),
        held(diff_lambda),
        held(residual_in),
        held(norm_gain_attn[None, :]),
        held(head_gain[None, :]),
        held(norm_gain_ffn[None, :]),
        held(dense_mix[None, :]),
        held(route_ids.T),
        held(route_weights.T),
        held(query_weight),
        held(key_weight),
        held(value_weight),
        held(kv_cache),
        held(out_weight),
        held(expert_gate),
        held(expert_up),
        held(expert_down),
        held(dense_gate),
        held(dense_up),
        held(dense_down),
    )
    layer_out, fresh = pl.pallas_call(
        settle,
        out_shape=(
            jax.ShapeDtypeStruct(layer_out.shape, BF16),
            jax.ShapeDtypeStruct(fresh.shape, BF16),
        ),
        in_specs=[vmem, vmem],
        out_specs=(hbm, hbm),
        scratch_shapes=[dma((2,))],
        compiler_params=pltpu.CompilerParams(vmem_limit_bytes=1024 * 1024),
    )(layer_out, fresh)
    return layer_out, fresh.reshape(seqs, groups, kv_cache.shape[3])


def on_device(
    residual_in,
    lengths,
    kv_cache,
    norm_gain_attn,
    query_weight,
    key_weight,
    value_weight,
    diff_lambda,
    head_gain,
    out_weight,
    norm_gain_ffn,
    route_ids,
    route_weights,
    expert_gate,
    expert_up,
    expert_down,
    dense_gate,
    dense_up,
    dense_down,
    dense_mix,
):
    n_ep = lax.axis_size("ep")
    n_tp = lax.axis_size("tp")
    half = n_tp // 2
    if (
        n_tp == 2 * CORES
        and n_ep in (4, 8, 16)
        and expert_gate.shape[0] == 1
        and dense_gate.shape[1] // half % LANES == 0
        and expert_gate.shape[2] % LANES == 0
    ):
        return near_call(
            n_ep,
            n_tp,
            (
                residual_in,
                lengths,
                kv_cache,
                norm_gain_attn,
                query_weight,
                key_weight,
                value_weight,
                diff_lambda,
                head_gain,
                out_weight,
                norm_gain_ffn,
                route_ids,
                route_weights,
                expert_gate,
                expert_up,
                expert_down,
                dense_gate,
                dense_up,
                dense_down,
                dense_mix,
            ),
        )
    seqs, width = residual_in.shape
    groups, spots = kv_cache.shape[1:3]
    share = diff_lambda.shape[0] // groups
    inner = query_weight.shape[1]
    quarter = out_weight.shape[1]
    held, _, part = expert_gate.shape
    rows = n_ep * seqs
    own = dense_gate.shape[1] // n_tp
    split = own % LANES == 0
    hid = own if split else dense_gate.shape[1]
    lanes = -(-n_ep * held // LANES) * LANES
    vmem = pl.BlockSpec(memory_space=pltpu.VMEM)
    smem = pl.BlockSpec(memory_space=pltpu.SMEM)
    hbm = pl.BlockSpec(memory_space=pl.ANY)
    dma = pltpu.SemaphoreType.DMA
    layer_out, fresh = pl.pallas_call(
        functools.partial(layer_kernel, n_ep, n_tp, split),
        out_shape=(
            jax.ShapeDtypeStruct((seqs, quarter), F32),
            jax.ShapeDtypeStruct((seqs, groups * kv_cache.shape[3]), F32),
        ),
        in_specs=[smem] * 2 + [vmem] * 7 + [hbm] * 11,
        out_specs=(vmem, vmem),
        scratch_shapes=[
            pltpu.VMEM(query_weight.shape, BF16),
            pltpu.VMEM(key_weight.shape, BF16),
            pltpu.VMEM(value_weight.shape, BF16),
            pltpu.VMEM(kv_cache.shape, BF16),
            pltpu.VMEM((groups, seqs, 2 * share, LANES), F32),
            pltpu.VMEM((groups, seqs, 2 * share, spots), F32),
            pltpu.VMEM((groups, seqs, 2 * share, LANES), F32),
            pltpu.VMEM((seqs, inner), BF16),
            pltpu.VMEM(out_weight.shape, BF16),
            pltpu.VMEM(expert_gate.shape, BF16),
            pltpu.VMEM(expert_up.shape, BF16),
            pltpu.VMEM(expert_down.shape, BF16),
            pltpu.VMEM((width, hid), BF16),
            pltpu.VMEM((width, hid), BF16),
            pltpu.VMEM((hid, width), BF16),
            pltpu.VMEM((n_tp - 1, seqs, inner), BF16),
            pltpu.VMEM((rows, width), BF16),
            pltpu.VMEM((rows, width), BF16),
            pltpu.VMEM((rows, LANES), F32),
            pltpu.VMEM((rows, lanes), F32),
            pltpu.VMEM((held, rows, part), BF16),
            pltpu.VMEM((rows, hid), BF16),
            pltpu.VMEM((half, rows, quarter), BF16),
            pltpu.VMEM((half, rows, quarter), BF16),
            pltpu.VMEM((half, rows, quarter), BF16),
            pltpu.VMEM((n_ep * half, seqs, quarter), BF16),
            dma((7,)),
            dma((Q_CHUNKS + 2,)),
            dma((seqs,)),
            dma((n_ep - 1,)),
            dma((n_ep - 1,)),
            dma((n_tp - 1,)),
            dma((n_tp - 1,)),
            dma((n_ep,)),
            dma((half, n_ep)),
            dma((max(half - 1, 1), n_ep)),
            dma((n_tp, n_ep)),
            dma((half,)),
            dma((half,)),
            dma((half, n_ep)),
            dma((n_ep * half,)),
        ],
        compiler_params=pltpu.CompilerParams(
            collective_id=0, has_side_effects=True, vmem_limit_bytes=60 * 1024 * 1024
        ),
    )(
        lengths,
        diff_lambda,
        residual_in,
        norm_gain_attn[None, :],
        head_gain[None, :],
        norm_gain_ffn[None, :],
        dense_mix[None, :],
        route_ids.T,
        route_weights.T,
        query_weight,
        key_weight,
        value_weight,
        kv_cache,
        out_weight,
        expert_gate,
        expert_up,
        expert_down,
        dense_gate,
        dense_up,
        dense_down,
    )
    new_rows = fresh.astype(BF16).reshape(seqs, groups, kv_cache.shape[3])
    return (layer_out.astype(BF16), new_rows)


def solution(mesh):
    placed = (
        P("ep", None),
        P("ep"),
        P("ep", "tp", None, None),
        P(),
        P(None, "tp"),
        P(None, "tp"),
        P(None, "tp"),
        P("tp"),
        P(),
        P(None, "tp"),
        P(),
        P("ep", None),
        P("ep", None),
        P("ep", None, "tp"),
        P("ep", None, "tp"),
        P("ep", "tp", None),
        P(None, "ep"),
        P(None, "ep"),
        P("ep", None),
        P(),
    )
    return jax.shard_map(
        on_device,
        mesh=mesh,
        in_specs=placed,
        out_specs=(P("ep", "tp"), P("ep", "tp", None)),
        check_vma=False,
    )
```

```python
import functools
import math

import jax
import jax.numpy as jnp
from jax import lax
from jax.experimental import pallas as pl
from jax.experimental.pallas import tpu as pltpu
from jax.sharding import PartitionSpec as P

QK_DIM = 64
EPS = 1e-06
MESH = pl.DeviceIdType.MESH
F32 = jnp.float32
BF16 = jnp.bfloat16
LANES = 128
Q_CHUNKS = 4
INNER = 2
CORES = 2
RELAY = 1
CACHE_CHUNKS = 4


def flip(value, mask):
    bit = 1
    while bit <= mask:
        if mask & bit:
            value = value + bit * (1 - 2 * ((value // bit) % 2))
        bit *= 2
    return value


def each(count, body, order=None):
    if count <= 16:
        for index in order if order is not None else range(count):
            body(index)
    else:

        def step(index, carry):
            body(index)
            return carry

        lax.fori_loop(0, count, step, 0)


def block(start, size):
    return pl.ds(pl.multiple_of(start * size, size), size)


def remote(source, target, send, recv, where):
    return pltpu.make_async_remote_copy(
        src_ref=source,
        dst_ref=target,
        send_sem=send,
        recv_sem=recv,
        device_id=where,
        device_id_type=MESH,
    )


def dot(left, right):
    return jnp.dot(left, right, preferred_element_type=F32)


def column(row):
    count = row.shape[1]
    square = (count, count)
    same = lax.broadcasted_iota(jnp.int32, square, 0) == lax.broadcasted_iota(jnp.int32, square, 1)
    return jnp.sum(jnp.where(same, row, jnp.zeros_like(row)), axis=1, keepdims=True)


def layer_kernel(
    n_ep,
    n_tp,
    split,
    lengths_ref,
    lam_ref,
    resid_ref,
    first_gain_ref,
    head_gain_ref,
    gain_ref,
    mixw_ref,
    ids_ref,
    rw_ref,
    qw_hbm,
    kw_hbm,
    vw_hbm,
    cache_hbm,
    ow_hbm,
    eg_hbm,
    eu_hbm,
    ed_hbm,
    dg_hbm,
    du_hbm,
    dd_hbm,
    out_ref,
    new_ref,
    qw,
    kw,
    vw,
    cache,
    pairs,
    scores,
    mixed,
    heads_ref,
    ow,
    eg,
    eu,
    ed,
    dg,
    du,
    dd,
    heads_all,
    stream,
    ffn,
    mix,
    route,
    eh,
    dh,
    away,
    came,
    summed,
    landed,
    w_sem,
    q_sem,
    cache_sem,
    route_send,
    route_recv,
    heads_send,
    heads_recv,
    first_send,
    second_send,
    relay_send,
    stream_recv,
    pair_send,
    pair_recv,
    back_send,
    back_recv,
):
    e = lax.axis_index("ep")
    t = lax.axis_index("tp")
    half = n_tp // 2
    mate = flip(t, 1)
    core = t % 2
    seqs, width = resid_ref.shape
    quarter = out_ref.shape[1]
    held, _, part = eg.shape
    hid = dg.shape[1]
    rows_all = n_ep * seqs
    evens = [2 * i for i in range(1, half)]

    depth = qw.shape[0] // Q_CHUNKS
    q_loads = [
        pltpu.make_async_copy(
            qw_hbm.at[pl.ds(i * depth, depth), :], qw.at[pl.ds(i * depth, depth), :], q_sem.at[i]
        )
        for i in range(Q_CHUNKS)
    ] + [
        pltpu.make_async_copy(kw_hbm, kw, q_sem.at[Q_CHUNKS]),
        pltpu.make_async_copy(vw_hbm, vw, q_sem.at[Q_CHUNKS + 1]),
    ]
    for load in q_loads:
        load.start()
    cache_loads = [
        pltpu.make_async_copy(cache_hbm.at[s], cache.at[s], cache_sem.at[s]) for s in range(seqs)
    ]
    for load in cache_loads:
        load.start()

    barrier = pltpu.get_barrier_semaphore()

    def greet(index):
        where = (index // half, 2 * (index % half) + core)

        @pl.when(jnp.logical_or(where[0] != e, where[1] != t))
        def _():
            pl.semaphore_signal(barrier, inc=1, device_id=where, device_id_type=MESH)

    each(n_ep * half, greet)
    for i in range(half):
        pl.semaphore_signal(
            barrier, inc=1, device_id=(e, 2 * i + 1 - core), device_id_type=MESH
        )

    if split:
        cols = block(t, hid)
        dense_parts = (dg_hbm.at[:, cols], du_hbm.at[:, cols], dd_hbm.at[cols, :])
    else:
        dense_parts = (dg_hbm, du_hbm, dd_hbm)
    loads = [
        pltpu.make_async_copy(src, dst, w_sem.at[i])
        for i, (src, dst) in enumerate(
            zip((ow_hbm, eg_hbm, eu_hbm) + dense_parts[:2] + (ed_hbm, dense_parts[2]), (ow, eg, eu, dg, du, ed, dd))
        )
    ]

    lane = lax.broadcasted_iota(jnp.int32, (seqs, route.shape[1]), 1)
    table = jnp.zeros((seqs, route.shape[1]), F32)
    for k in range(ids_ref.shape[0]):
        wanted = column(ids_ref[k : k + 1, :])
        table = table + jnp.where(lane == wanted, column(rw_ref[k : k + 1, :]), 0.0)
    own_rows = block(e, seqs)
    route[own_rows, :] = table

    resid = resid_ref[...].astype(F32)
    mean_sq = jnp.mean(resid * resid, axis=-1, keepdims=True)
    normed = (resid * lax.rsqrt(mean_sq + EPS) * first_gain_ref[...]).astype(BF16)
    row = lax.broadcasted_iota(jnp.int32, (seqs, LANES), 0)
    entry = lax.broadcasted_iota(jnp.int32, (seqs, LANES), 1) % QK_DIM
    position = jnp.zeros((seqs, LANES), F32)
    for s in range(seqs):
        position = jnp.where(row == s, lengths_ref[s].astype(F32), position)
    turn = QK_DIM // 2
    power = (entry % turn).astype(F32) * (-1.0 / turn)
    angle = position * jnp.exp(power * math.log(10000.0))
    cosine = jnp.cos(angle)
    sine = jnp.where(entry < turn, -jnp.sin(angle), jnp.sin(angle))

    def rotate(values):
        other = jnp.where(
            entry < turn, pltpu.roll(values, LANES - turn, 1), pltpu.roll(values, turn, 1)
        )
        return (values * cosine + other * sine).astype(BF16).astype(F32)

    query = jnp.zeros((seqs, qw.shape[1]), F32)
    for i in range(Q_CHUNKS):
        q_loads[i].wait()
        query = query + dot(
            normed[:, i * depth : (i + 1) * depth], qw[i * depth : (i + 1) * depth, :]
        )
    for load in q_loads[Q_CHUNKS:]:
        load.wait()
    keys_raw = dot(normed, kw[...])
    values_raw = dot(normed, vw[...])
    for load in loads:
        load.start()

    groups, spots = cache.shape[1], cache.shape[2]
    share = query.shape[1] // LANES // groups
    lower = lax.broadcasted_iota(jnp.int32, (seqs, LANES), 1) < QK_DIM
    fresh = []
    for g in range(groups):
        key = rotate(keys_raw[:, g * LANES : (g + 1) * LANES])
        value = values_raw[:, g * LANES : (g + 1) * LANES].astype(BF16).astype(F32)
        new_ref[:, 2 * g * LANES : (2 * g + 1) * LANES] = key
        new_ref[:, (2 * g + 1) * LANES : (2 * g + 2) * LANES] = value
        fresh.append((key, value))
        for j in range(share):
            at = (g * share + j) * LANES
            head = rotate(query[:, at : at + LANES])
            pairs[g, :, j, :] = jnp.where(lower, head, 0.0)
            pairs[g, :, share + j, :] = jnp.where(lower, 0.0, head)

    pl.semaphore_wait(barrier, n_ep * half - 1 + half)

    def route_copy(d):
        there = (e + d) % n_ep
        return remote(
            route.at[own_rows, :],
            route.at[own_rows, :],
            route_send.at[d - 1],
            route_recv.at[d - 1],
            (there, t),
        )

    def route_wait(d):
        came_from = (e + n_ep - d) % n_ep
        spot = route.at[block(came_from, seqs), :]
        remote(spot, spot, route_send.at[d - 1], route_recv.at[d - 1], (e, t)).wait_recv()

    each(n_ep - 1, lambda i: route_copy(i + 1).start())

    scale = QK_DIM**-0.5
    lines = 2 * share
    for s in range(seqs):
        cache_loads[s].wait()
        for g in range(groups):
            both = pairs[g, s].astype(BF16)
            scores[g, s] = (
                lax.dot_general(
                    both,
                    cache[s, g, :, :LANES],
                    (((1,), (1,)), ((), ())),
                    preferred_element_type=F32,
                )
                * scale
            )
    length = jnp.zeros((seqs, lines, 1), jnp.int32)
    which = lax.broadcasted_iota(jnp.int32, (seqs, lines, 1), 0)
    for s in range(seqs):
        length = jnp.where(which == s, lengths_ref[s], length)
    place = lax.broadcasted_iota(jnp.int32, (seqs, lines, spots), 2)
    valid = place < length
    line = lax.broadcasted_iota(jnp.int32, (lines, 1), 0)
    for g in range(groups):
        key, value = fresh[g]
        latest = jnp.sum(pairs[g] * key[:, None, :], axis=-1, keepdims=True) * scale
        masked = jnp.where(valid, scores[g], -jnp.inf)
        top = jnp.maximum(jnp.max(masked, axis=-1, keepdims=True), latest)
        raised = jnp.exp(masked - top)
        raised_new = jnp.exp(latest - top)
        total = jnp.sum(raised, axis=-1, keepdims=True) + raised_new
        prob = raised / total
        prob_new = jnp.broadcast_to(raised_new / total, (seqs, lines, LANES))
        lam = jnp.zeros((lines, 1), F32)
        for j in range(share):
            lam = jnp.where(line == j, lam_ref[g * share + j], lam)
        scores[g] = prob - lam[None] * pltpu.roll(prob, share, 1)
        new_weight = (prob_new - lam[None] * pltpu.roll(prob_new, share, 1)).astype(BF16).astype(F32)
        fresh_part = new_weight * value[:, None, :]
        for s in range(seqs):
            mixed[g, s] = dot(scores[g, s].astype(BF16), cache[s, g, :, LANES:])
        whole = mixed[g] + fresh_part
        mean_sq = jnp.mean(whole * whole, axis=-1, keepdims=True)
        mixed[g] = whole * lax.rsqrt(mean_sq + EPS) * head_gain_ref[...][None]
        for j in range(share):
            at = (g * share + j) * LANES
            heads_ref[:, at : at + LANES] = mixed[g, :, j, :].astype(BF16)

    def heads_copy(mask):
        return remote(
            heads_ref,
            heads_all.at[mask - 1],
            heads_send.at[mask - 1],
            heads_recv.at[mask - 1],
            (e, flip(t, mask)),
        )

    for mask in range(n_tp - 1, 0, -1):
        heads_copy(mask).start()

    loads[0].wait()
    span = heads_ref.shape[1]
    total = dot(heads_ref[...], ow[block(t, span), :])
    for mask in range(1, n_tp):
        heads_copy(mask).wait_recv()
        total = total + dot(heads_all[mask - 1], ow[block(flip(t, mask), span), :])
    own_cols = block(t, quarter)
    own_stream = (resid_ref[:, own_cols].astype(F32) + total).astype(BF16)
    stream[own_rows, own_cols] = own_stream

    def spot(owner, column):
        return stream.at[block(owner, seqs), block(column, quarter)]

    def owner_of(d):
        return (e + n_ep - d) % n_ep

    def first(d):
        return remote(
            spot(e, t), spot(e, t), first_send.at[d], stream_recv.at[0, d], ((e + d) % n_ep, t)
        )

    def second(d, mask):
        index = mask // 2 if mask != 1 else 0
        where = spot(owner_of(d), t)
        return remote(
            where, where, second_send.at[index, d], stream_recv.at[mask, d], (e, flip(t, mask))
        )

    def relay(d, mask):
        where = spot(owner_of(d), flip(t, mask))
        return remote(
            where, where, relay_send.at[mask // 2 - 1, d], stream_recv.at[mask + 1, d], (e, mate)
        )

    def arrived(d, mask):
        where = spot(owner_of(d), flip(t, mask))
        remote(where, where, first_send.at[d], stream_recv.at[mask, d], (e, t)).wait_recv()

    def spread(d):
        for mask in evens:
            second(d, mask).start()
        second(d, 1).start()

    far_first = sorted(range(1, n_ep), key=lambda d: -min(d, n_ep - d)) if n_ep <= 16 else None
    near_first = [0] + far_first[::-1] if far_first is not None else None
    each(n_ep - 1 if far_first is None else 1, lambda i: first(i + 1).start(), order=None) if far_first is None else [
        first(d).start() for d in far_first
    ]

    def stage_two(d):
        if not (isinstance(d, int) and d == 0):
            arrived(d, 0)
        spread(d)

    def stage_three(d):
        for mask in evens:
            arrived(d, mask)
            relay(d, mask).start()

    def normalise(d):
        arrived(d, 1)
        for mask in evens:
            arrived(d, mask + 1)
        rows = block(owner_of(d), seqs)
        values = stream[rows, :].astype(F32)
        mean_sq = jnp.mean(values * values, axis=-1, keepdims=True)
        scaled = (values * lax.rsqrt(mean_sq + EPS) * gain_ref[...]).astype(BF16)
        ffn[rows, :] = scaled
        inner = jnp.sum(scaled.astype(F32) * mixw_ref[...], axis=-1, keepdims=True)
        mix[rows, :] = jnp.broadcast_to(jax.nn.sigmoid(inner), (seqs, LANES))

    if near_first is not None:
        for i, d in enumerate(near_first):
            stage_two(d)
            if i:
                stage_three(near_first[i - 1])
            if i > 1:
                normalise(near_first[i - 2])
        stage_three(near_first[-1])
        for d in near_first[-2:]:
            normalise(d)
    else:
        stage_two(0)
        each(n_ep - 1, lambda i: stage_two(i + 1))
        each(n_ep, stage_three)
        each(n_ep, normalise)
    each(n_ep - 1, lambda i: route_wait(i + 1))

    many = min(rows_all, 128)
    batches = rows_all // many
    for load in loads[1:5]:
        load.wait()

    def hidden(b):
        rows = block(b, many)
        a = ffn[rows, :]
        for j in range(held):
            eh[j, rows, :] = (jax.nn.silu(dot(a, eg[j])) * dot(a, eu[j])).astype(BF16)
        units = jax.nn.silu(dot(a, dg[...])) * dot(a, du[...])
        if not split:
            own = hid // n_tp
            unit = lax.broadcasted_iota(jnp.int32, units.shape, 1)
            units = jnp.where((unit >= t * own) & (unit < (t + 1) * own), units, 0.0)
        dh[rows, :] = units.astype(BF16)

    each(batches, hidden)
    for load in loads[5:]:
        load.wait()

    def result(b, q):
        rows = block(b, many)
        cols = block(q, quarter)
        total = mix[rows, :1] * dot(dh[rows, :], dd[:, cols])
        lanes = lax.broadcasted_iota(jnp.int32, (many, route.shape[1]), 1)
        for j in range(held):
            weight = jnp.sum(
                jnp.where(lanes == e * held + j, route[rows, :], 0.0), axis=1, keepdims=True
            )
            piece = dot(eh[j, rows, :], ed[j, :, cols]).astype(BF16)
            total = total + weight * piece.astype(F32)
        return total

    def pair(j):
        return remote(away.at[j], came.at[j], pair_send.at[j], pair_recv.at[j], (e, mate))

    for j in range(half):

        def leave(b, j=j):
            away[j, block(b, many), :] = result(b, 2 * j + 1 - core).astype(BF16)

        each(batches, leave)
        pair(j).start()

    me = e * half + t // 2

    def back(j, d):
        there = (e + d) % n_ep
        return remote(
            summed.at[j, block(there, seqs), :],
            landed.at[me],
            back_send.at[j, d],
            back_recv.at[me],
            (there, 2 * j + core),
        )

    def same(j, d):
        return jnp.logical_and(jnp.asarray(d == 0), 2 * j + core == t)

    for j in range(half):

        def keep(b, j=j):
            summed[j, block(b, many), :] = result(b, 2 * j + core).astype(BF16)

        each(batches, keep)
    for j in range(half):
        pair(j).wait_recv()

        def add(b, j=j):
            rows = block(b, many)
            summed[j, rows, :] = (summed[j, rows, :].astype(F32) + came[j, rows, :].astype(F32)).astype(BF16)

        each(batches, add)

        def send(d, j=j):
            @pl.when(jnp.logical_not(same(j, d)))
            def _():
                back(j, d).start()

        each(n_ep, send, order=None if far_first is None else far_first + [0])

    landed[me] = summed[t // 2, own_rows, :]

    def take(index):
        @pl.when(index != me)
        def _():
            where = landed.at[index]
            remote(where, where, back_send.at[0, 0], back_recv.at[index], (e, t)).wait_recv()

    each(n_ep * half, take)
    out_ref[...] = own_stream.astype(F32) + jnp.sum(landed[...].astype(F32), axis=0)

    for mask in range(1, n_tp):
        heads_copy(mask).wait_send()
    each(n_ep - 1, lambda i: route_copy(i + 1).wait_send())
    each(n_ep - 1, lambda i: first(i + 1).wait_send())

    def sent(d):
        second(d, 1).wait_send()
        for mask in evens:
            second(d, mask).wait_send()
            relay(d, mask).wait_send()

    each(n_ep, sent)
    for j in range(half):
        pair(j).wait_send()

        def gone(d, j=j):
            @pl.when(jnp.logical_not(same(j, d)))
            def _():
                back(j, d).wait_send()

        each(n_ep, gone)


def keeps(plane):
    return (plane + 1) % CORES


def tells(planes, me, you):
    z, x, y, c = me
    level, inner, side, core = you
    other = (z != level) | (x != inner) | (y != side) | (c != core)
    column = (c == RELAY) & (x == inner) & (y == side)
    lane = (y == side) & (c == core)
    far = (z == 0) & (level == planes - 1) & (c == keeps(planes - 1))
    return other & ((z == level) | column | lane | far)


def near_kernel(
    n_ep,
    n_tp,
    lengths_hbm,
    lam_hbm,
    resid_hbm,
    first_gain_hbm,
    head_gain_hbm,
    gain_hbm,
    mixw_hbm,
    ids_hbm,
    rw_hbm,
    qw_hbm,
    kw_hbm,
    vw_hbm,
    cache_hbm,
    ow_hbm,
    eg_hbm,
    eu_hbm,
    ed_hbm,
    dg_hbm,
    du_hbm,
    dd_hbm,
    out_ref,
    new_ref,
    lengths_ref,
    lam_ref,
    resid_ref,
    first_gain_ref,
    head_gain_ref,
    gain_ref,
    mixw_ref,
    ids_ref,
    rw_ref,
    qkv,
    cache,
    pairs,
    asked,
    scores,
    mixed,
    heads_ref,
    ow,
    gu,
    ed,
    dg,
    du,
    dd,
    heads_all,
    mine,
    stream,
    ffn,
    route,
    eh,
    dh,
    leaving,
    kept,
    plane_in,
    column_out,
    column_in,
    local_sem,
    push_send,
    push_recv,
    route_send,
    route_recv,
    heads_send,
    heads_recv,
    chunk_send,
    climb_recv,
    group_recv,
    plane_recv,
    column_recv,
):
    e = lax.axis_index("ep")
    t = lax.axis_index("tp")
    planes = n_ep // INNER
    z = e // INNER
    x = e % INNER
    y = t // CORES
    c = t % CORES
    keeper = keeps(z)
    odd = (c + keeper) % CORES
    turns = planes // CORES
    seqs, width = resid_ref.shape
    quarter = out_ref.shape[1]
    part = eg_hbm.shape[2]
    hid = dg.shape[1]
    mate = flip(t, 1)

    def gather_loads(sem, *routes):
        return [pltpu.make_async_copy(src, dst, local_sem.at[sem]) for src, dst in routes]

    first_loads = gather_loads(
        0, (resid_hbm, resid_ref), (first_gain_hbm, first_gain_ref), (lengths_hbm, lengths_ref)
    )
    for load in first_loads:
        load.start()
    depth = qkv.shape[0] // Q_CHUNKS
    inner = qw_hbm.shape[1]
    side = kw_hbm.shape[1]
    for i in range(Q_CHUNKS):
        deep = pl.ds(i * depth, depth)
        for load in gather_loads(
            1 + i,
            (qw_hbm.at[deep, :], qkv.at[deep, :inner]),
            (kw_hbm.at[deep, :], qkv.at[deep, inner : inner + side]),
            (vw_hbm.at[deep, :], qkv.at[deep, inner + side :]),
        ):
            load.start()

    barrier = pltpu.get_barrier_semaphore()
    for index in range(n_ep * n_tp):
        there = (index // n_tp // INNER, index // n_tp % INNER, index % n_tp // CORES, index % CORES)

        @pl.when(tells(planes, (z, x, y, c), there))
        def _():
            pl.semaphore_signal(
                barrier, inc=1, device_id=(index // n_tp, index % n_tp), device_id_type=MESH
            )

    told = 0
    for level in range(planes):
        for core in range(CORES):
            count = sum(
                tells(planes, (i, j, k, m), (level, 0, 0, core))
                for i in range(planes)
                for j in range(INNER)
                for k in range(n_tp // CORES)
                for m in range(CORES)
            )
            told = jnp.where((z == level) & (c == core), count, told)

    for load in first_loads:
        load.wait()
    bunch = seqs // CACHE_CHUNKS
    cache_loads = [
        gather_loads(
            1 + Q_CHUNKS + i,
            (cache_hbm.at[pl.ds(i * bunch, bunch)], cache.at[pl.ds(i * bunch, bunch)]),
        )[0]
        for i in range(CACHE_CHUNKS)
    ]
    for load in cache_loads:
        load.start()
    late = 1 + Q_CHUNKS + CACHE_CHUNKS
    late_loads = gather_loads(
        late,
        (ids_hbm, ids_ref),
        (rw_hbm, rw_ref),
        (lam_hbm, lam_ref),
        (head_gain_hbm, head_gain_ref),
        (gain_hbm, gain_ref),
        (mixw_hbm, mixw_ref),
    )
    for load in late_loads:
        load.start()
    cols = block(y, hid)
    e_loads = gather_loads(
        late + 1, (eg_hbm.at[0], gu.at[c, :, :part]), (eu_hbm.at[0], gu.at[c, :, part:])
    ) + gather_loads(late + 2, (ed_hbm.at[0], ed.at[block(c, part), :]))
    loads = [
        gather_loads(1 + i, route)[0]
        for i, route in enumerate(
            (
                (ow_hbm, ow),
                (dg_hbm.at[:, cols], dg),
                (du_hbm.at[:, cols], du),
                (dd_hbm.at[cols, :], dd),
            )
        )
    ]
    resid = resid_ref[...].astype(F32)
    mean_sq = jnp.mean(resid * resid, axis=-1, keepdims=True)
    normed = (resid * lax.rsqrt(mean_sq + EPS) * first_gain_ref[...]).astype(BF16)
    row = lax.broadcasted_iota(jnp.int32, (seqs, LANES), 0)
    entry = lax.broadcasted_iota(jnp.int32, (seqs, LANES), 1) % QK_DIM
    position = jnp.zeros((seqs, LANES), F32)
    for s in range(seqs):
        position = jnp.where(row == s, lengths_ref[s].astype(F32), position)
    turn = QK_DIM // 2
    power = (entry % turn).astype(F32) * (-1.0 / turn)
    angle = position * jnp.exp(power * math.log(10000.0))
    cosine = jnp.cos(angle)
    sine = jnp.where(entry < turn, -jnp.sin(angle), jnp.sin(angle))

    def rotate(values):
        other = jnp.where(
            entry < turn, pltpu.roll(values, LANES - turn, 1), pltpu.roll(values, turn, 1)
        )
        return (values * cosine + other * sine).astype(BF16).astype(F32)

    def spot(plane, inner):
        return plane // CORES * INNER + inner

    own_spot = spot(z, x)
    projected = jnp.zeros((seqs, qkv.shape[1]), F32)
    for i in range(Q_CHUNKS):
        deep = pl.ds(i * depth, depth)
        pltpu.make_async_copy(qkv.at[deep, :], qkv.at[deep, :], local_sem.at[1 + i]).wait()
        projected = projected + dot(normed[:, i * depth : (i + 1) * depth], qkv[deep, :])
    query = projected[:, :inner]
    keys_raw = projected[:, inner : inner + side]
    values_raw = projected[:, inner + side :]
    for load in e_loads + loads:
        load.start()

    groups, spots = cache.shape[1], cache.shape[2]
    share = query.shape[1] // LANES // groups
    scale = QK_DIM**-0.5
    lines = 2 * share
    lower = lax.broadcasted_iota(jnp.int32, (seqs, LANES), 1) < QK_DIM
    fresh = []
    for g in range(groups):
        key = rotate(keys_raw[:, g * LANES : (g + 1) * LANES])
        value = values_raw[:, g * LANES : (g + 1) * LANES].astype(BF16).astype(F32)
        new_ref[:, 2 * g * LANES : (2 * g + 1) * LANES] = key.astype(BF16)
        new_ref[:, (2 * g + 1) * LANES : (2 * g + 2) * LANES] = value.astype(BF16)
        fresh.append((key, value))
        for j in range(share):
            at = (g * share + j) * LANES
            head = rotate(query[:, at : at + LANES])
            pairs[g, :, j, :] = jnp.where(lower, head, 0.0)
            pairs[g, :, share + j, :] = jnp.where(lower, 0.0, head)
        spread = (pairs[g] * scale).reshape(seqs * lines, LANES).astype(BF16)
        turn_of = lax.broadcasted_iota(jnp.int32, spread.shape, 0) // lines % 2
        asked[g, :, :LANES] = jnp.where(turn_of == 0, spread, jnp.zeros_like(spread))
        asked[g, :, LANES:] = jnp.where(turn_of == 0, jnp.zeros_like(spread), spread)

    def push(index):
        where = (gu.at[c], ed.at[block(c, part), :])[index]
        return remote(where, where, push_send.at[0], push_recv.at[index], (e, mate))

    def pushed(index):
        where = (gu.at[1 - c], ed.at[block(1 - c, part), :])[index]
        remote(where, where, push_send.at[0], push_recv.at[index], (e, mate)).wait_recv()

    def beside(s, g, lanes):
        return jnp.concatenate([cache[s, g, :, lanes], cache[s + 1, g, :, lanes]], axis=1)

    place = lax.broadcasted_iota(jnp.int32, (bunch, lines, spots), 2)
    line = lax.broadcasted_iota(jnp.int32, (lines, 1), 0)

    def score(start):
        for s in range(start, start + bunch, 2):
            for g in range(groups):
                scores[g, s : s + 2] = lax.dot_general(
                    asked[g, s * lines : (s + 2) * lines, :],
                    beside(s, g, slice(0, LANES)),
                    (((1,), (1,)), ((), ())),
                    preferred_element_type=F32,
                ).reshape(2, lines, spots)

    def attend(start):
        stop = start + bunch
        length = jnp.zeros((bunch, lines, 1), jnp.int32)
        which = lax.broadcasted_iota(jnp.int32, (bunch, lines, 1), 0)
        for s in range(bunch):
            length = jnp.where(which == s, lengths_ref[start + s], length)
        valid = place < length
        for g in range(groups):
            key, value = (half[start:stop] for half in fresh[g])
            latest = jnp.sum(pairs[g, start:stop] * key[:, None, :], axis=-1, keepdims=True) * scale
            masked = jnp.where(valid, scores[g, start:stop], -jnp.inf)
            top = jnp.maximum(jnp.max(masked, axis=-1, keepdims=True), latest)
            raised = jnp.exp(masked - top)
            raised_new = jnp.exp(latest - top)
            total = jnp.sum(raised, axis=-1, keepdims=True) + raised_new
            lam = jnp.full((lines, 1), 1.0, F32)
            for j in range(share):
                lam = jnp.where(line == share + j, lam_ref[g * share + j], lam)
            part_of = lam[None] / total
            prob = raised * part_of
            prob_new = jnp.broadcast_to(raised_new * part_of, (bunch, lines, LANES))
            weights = (prob - pltpu.roll(prob, share, 1)).astype(BF16)
            new_weight = (
                (prob_new - pltpu.roll(prob_new, share, 1)).astype(BF16).astype(F32)
            )
            fresh_part = new_weight * value[:, None, :]
            for s in range(0, bunch, 2):
                both = dot(
                    weights[s : s + 2].reshape(2 * lines, spots),
                    beside(start + s, g, slice(LANES, None)),
                )
                mixed[g, start + s] = both[:lines, :LANES]
                mixed[g, start + s + 1] = both[lines:, LANES:]
            whole = mixed[g, start:stop] + fresh_part
            mean_sq = jnp.mean(whole * whole, axis=-1, keepdims=True)
            mixed[g, start:stop] = whole * lax.rsqrt(mean_sq + EPS) * head_gain_ref[...][None]

    for i in range(CACHE_CHUNKS):
        if i == CACHE_CHUNKS - 1:
            for load in late_loads:
                load.wait()
        cache_loads[i].wait()
        score(i * bunch)
        if i == CACHE_CHUNKS - 1:
            for k in range(CACHE_CHUNKS):
                attend(k * bunch)
    for g in range(groups):
        for j in range(share):
            at = (g * share + j) * LANES
            heads_ref[:, at : at + LANES] = mixed[g, :, j, :].astype(BF16)

    def heads_copy(mask):
        return remote(
            heads_ref,
            heads_all.at[mask - 1],
            heads_send.at[0],
            heads_recv.at[mask // CORES],
            (e, flip(t, mask)),
        )

    pl.semaphore_wait(barrier, told)
    for mask in range(n_tp - 1, 0, -1):
        heads_copy(mask).start()

    for load in e_loads:
        load.wait()
    push(0).start()
    push(1).start()

    lane = lax.broadcasted_iota(jnp.int32, (seqs, route.shape[2]), 1)
    table = jnp.zeros((seqs, route.shape[2]), F32)
    for k in range(ids_ref.shape[0]):
        wanted = column(ids_ref[k : k + 1, :])
        table = table + jnp.where(lane == wanted, column(rw_ref[k : k + 1, :]), 0.0)

    @pl.when(odd == 0)
    def _():
        route[own_spot] = table

    def route_copy(mask):
        where = route.at[own_spot]
        return remote(
            where, where, route_send.at[0], route_recv.at[0], (flip(e, mask), t)
        )

    @pl.when(odd == 0)
    def _():
        for mask in range(1, n_ep):
            route_copy(mask).start()


    loads[0].wait()
    span = heads_ref.shape[1]
    total = dot(heads_ref[...], ow[block(t, span), :])
    for far in range(n_tp // CORES):
        batch = heads_all.at[pl.ds(0, 1) if far == 0 else pl.ds(far * CORES - 1, CORES)]
        remote(batch, batch, heads_send.at[0], heads_recv.at[far], (e, t)).wait_recv()
        for mask in range(max(far * CORES, 1), (far + 1) * CORES):
            total = total + dot(heads_all[mask - 1], ow[block(flip(t, mask), span), :])
    own_cols = block(t, quarter)
    own_stream = (resid_ref[:, own_cols].astype(F32) + total).astype(BF16)
    mine[...] = own_stream

    around = ((1, 1), (1, 0), (0, 1))
    last = turns - 1
    edge = jnp.logical_or(z == 0, z == planes - 1)
    far = jnp.logical_and(edge, odd == 1)

    def chunk(group, owner):
        return stream.at[block(group, seqs), block(owner, quarter)]

    def to_plane(step):
        dx, dy = around[step]
        there = (z * INNER + flip(x, dx), flip(y, dy) * CORES + keeper)
        return remote(
            mine, chunk(e, t), chunk_send.at[0], group_recv.at[z // CORES, dx], there
        )

    def to_column(d):
        core = jnp.where(z == planes - 1, keeper, RELAY) if d == planes - 1 else RELAY
        there = (flip(z, d) * INNER + x, y * CORES + core)
        return remote(mine, chunk(e, t), chunk_send.at[0], climb_recv.at[z, c], there)

    def to_mate():
        return remote(mine, chunk(e, t), chunk_send.at[0], climb_recv.at[z, c], (e, mate))

    def to_far(step):
        dx, dy = around[step]
        there = (flip(z, planes - 1) * INNER + flip(x, dx), flip(y, dy) * CORES + keeper)
        return remote(
            mine, chunk(e, t), chunk_send.at[0], group_recv.at[z // CORES, dx], there
        )

    for d in range(planes - 2, 0, -1):
        to_column(d).start()

    @pl.when(z == planes - 1)
    def _():
        for step in range(len(around)):
            to_far(step).start()

    to_column(planes - 1).start()
    for step in range(len(around)):
        to_plane(step).start()

    @pl.when(odd == 1)
    def _():
        to_mate().start()

    @pl.when(odd == 0)
    def _():
        stream[block(e, seqs), own_cols] = own_stream

    near = z + odd * (1 - 2 * (z % 2))

    def plane_of(i):
        return flip(near, 2 * i)

    def arrived(plane, core):
        where = chunk(plane * INNER + x, y * CORES + core)
        remote(where, where, chunk_send.at[0], climb_recv.at[plane, core], (e, t)).wait_recv()

    def forward(plane, core, step):
        dx, dy = around[step]
        where = chunk(plane * INNER + x, y * CORES + core)
        return remote(
            where,
            where,
            chunk_send.at[0],
            group_recv.at[plane // CORES, dx],
            (z * INNER + flip(x, dx), flip(y, dy) * CORES + keeps(plane)),
        )

    def hand_over(plane, core):
        where = chunk(plane * INNER + x, y * CORES + core)
        return remote(where, where, chunk_send.at[0], climb_recv.at[plane, core], (e, mate))

    @pl.when(c == RELAY)
    def _():
        for plane in range(planes):
            passes = plane != z
            if plane == planes - 1:
                passes = jnp.logical_and(passes, z != 0)

            @pl.when(passes)
            def _(plane=plane):
                for core in range(CORES):
                    arrived(plane, core)
                    for step in range(len(around)):
                        forward(plane, core, step).start()
                    if keeps(plane) != RELAY:
                        hand_over(plane, core).start()

    def normalise(i):
        plane = CORES * i + keeps(c)

        @pl.when(plane == z)
        def _():
            arrived(plane, 1 - c)

        leapt = jnp.logical_and(plane == planes - 1, z == 0)

        @pl.when(jnp.logical_and(plane != z, jnp.logical_or(c != RELAY, leapt)))
        def _():
            for core in range(CORES):
                arrived(plane, core)

        for inner in range(INNER):
            group = plane * INNER + flip(x, inner)
            came = stream.at[
                block(group, seqs),
                pl.ds(0, width) if inner else block(flip(y, 1), CORES * quarter),
            ]
            remote(
                came, came, chunk_send.at[0], group_recv.at[plane // CORES, inner], (e, t)
            ).wait_recv()
            values = stream[block(group, seqs), :].astype(F32)
            mean_sq = jnp.mean(values * values, axis=-1, keepdims=True)
            scaled = (values * lax.rsqrt(mean_sq + EPS) * gain_ref[...]).astype(BF16)
            ffn[block(spot(plane, flip(x, inner)), seqs), :] = scaled

    for i in range(turns):
        normalise(i)

    def route_wait(count):
        where = route.at[pl.ds(0, count)]
        remote(where, where, route_send.at[0], route_recv.at[0], (e, t)).wait_recv()

    @pl.when(odd == 0)
    def _():
        route_wait(route.shape[0] - 1)

    @pl.when(odd == 1)
    def _():
        route_wait(route.shape[0])

    rows_all = ffn.shape[0]
    pushed(0)
    pushed(1)
    for load in loads[1:]:
        load.wait()
    a = ffn[...]
    for core in range(CORES):
        both = dot(a, gu[core])
        eh[:, core * part : (core + 1) * part] = (
            jax.nn.silu(both[:, :part]) * both[:, part:]
        ).astype(BF16)
    for at in range(0, hid, 2 * LANES):
        piece = slice(at, at + 2 * LANES)
        dh[:, piece] = (jax.nn.silu(dot(a, dg[:, piece])) * dot(a, du[:, piece])).astype(BF16)
    blend = jax.nn.sigmoid(jnp.sum(a.astype(F32) * mixw_ref[...], axis=-1, keepdims=True))
    lanes = lax.broadcasted_iota(jnp.int32, (rows_all, route.shape[2]), 1)
    weight = jnp.sum(
        jnp.where(lanes == e, route[...].reshape(rows_all, route.shape[2]), 0.0),
        axis=1,
        keepdims=True,
    )
    half = CORES * quarter
    def project(dy):
        cols = block(flip(y, dy), half)
        sparse = weight * dot(eh[...], ed[:, cols])
        return sparse + blend * dot(dh[...], dd[:, cols])

    leaving[1] = project(1).astype(BF16)

    def own_plane(i):
        return jnp.logical_and(odd == 0, i == 0)

    def leave(i, core, step):
        dx, dy = around[step]
        where = spot(plane_of(i), flip(x, dx))
        summer = jnp.where(own_plane(i), c, RELAY)
        return remote(
            leaving.at[dy, block(where, seqs), pl.ds(core * quarter, quarter)],
            plane_in.at[c, i, core, step],
            chunk_send.at[0],
            plane_recv.at[c, i, core],
            (z * INNER + flip(x, dx), flip(y, dy) * CORES + summer),
        )

    def pass_over(i, core):
        where = spot(plane_of(i), x)
        return remote(
            leaving.at[0, block(where, seqs), pl.ds(core * quarter, quarter)],
            plane_in.at[c, i, core, len(around)],
            chunk_send.at[0],
            plane_recv.at[c, i, core],
            (e, mate),
        )

    def leap(core, step):
        dx, dy = around[step] if step < len(around) else (0, 0)
        where = spot(plane_of(last), flip(x, dx))
        return remote(
            leaving.at[dy, block(where, seqs), pl.ds(core * quarter, quarter)],
            column_in.at[planes - 1 + (step + 1) % (len(around) + 1)],
            chunk_send.at[0],
            column_recv.at[0],
            (plane_of(last) * INNER + flip(x, dx), flip(y, dy) * CORES + core),
        )

    order = range(turns - 1, -1, -1)
    for dy in (1, 0):
        if not dy:
            total = project(0)
            leaving[0] = total.astype(BF16)
            kept[...] = total
        steps = [step for step in range(len(around)) if around[step][1] == dy]

        @pl.when(far)
        def _():
            for step in steps + [len(around)] * (1 - dy):
                for core in range(CORES):
                    leap(core, step).start()

        for i in order:

            def depart(i=i):
                for core in range(CORES):
                    for step in steps:
                        leave(i, core, step).start()
                if not dy:

                    @pl.when(jnp.logical_and(c != RELAY, jnp.logical_not(own_plane(i))))
                    def _():
                        for core in range(CORES):
                            pass_over(i, core).start()

            if i == last:
                pl.when(jnp.logical_not(far))(depart)
            else:
                depart()

    def climb(lane, i, core):
        skew = (lane + keeper) % CORES
        level = flip(z + skew * (1 - 2 * (z % 2)), 2 * i)
        return remote(
            column_out.at[lane, i, core],
            column_in.at[skew + 2 * i],
            chunk_send.at[0],
            column_recv.at[0],
            (level * INNER + x, y * CORES + core),
        )

    def stays(i, core):
        return jnp.logical_and(own_plane(i), c == core)

    def rise(i):
        for core in range(CORES):
            gathered = kept[block(spot(plane_of(i), x), seqs), core * quarter : (core + 1) * quarter]
            came = plane_in.at[c, i, core, pl.ds(0, len(around))]
            remote(came, came, chunk_send.at[0], plane_recv.at[c, i, core], (e, t)).wait_recv()
            for step in range(len(around)):
                gathered = gathered + plane_in[c, i, core, step].astype(F32)
            column_out[c, i, core] = gathered.astype(BF16)

            @pl.when(jnp.logical_not(stays(i, core)))
            def _(i=i, core=core):
                climb(c, i, core).start()

    low = 1 - RELAY

    def lift(i):
        for core in range(CORES):
            came = plane_in.at[low, i, core]
            remote(came, came, chunk_send.at[0], plane_recv.at[low, i, core], (e, t)).wait_recv()
            gathered = plane_in[low, i, core, 0].astype(F32)
            for step in range(1, len(around) + 1):
                gathered = gathered + plane_in[low, i, core, step].astype(F32)
            column_out[low, i, core] = gathered.astype(BF16)
            climb(low, i, core).start()

    for i in order:
        sums = jnp.logical_or(c == RELAY, own_plane(i))
        if i == last:
            sums = jnp.logical_and(sums, jnp.logical_not(far))

        @pl.when(sums)
        def _(i=i):
            rise(i)

    slant = (low + keeper) % CORES == 1
    for i in order:
        theirs = c == RELAY
        if i == 0:
            theirs = jnp.logical_and(theirs, slant)
        if i == last:
            theirs = jnp.logical_and(theirs, jnp.logical_not(jnp.logical_and(edge, slant)))

        @pl.when(theirs)
        def _(i=i):
            lift(i)

    def took(start, stop):
        where = column_in.at[pl.ds(start, stop - start)]
        remote(where, where, chunk_send.at[0], column_recv.at[0], (e, t)).wait_recv()

    @pl.when(odd == 0)
    def _():
        column_in[0] = column_out[c, 0, c]

    def finish(stop):
        for parity in range(2):

            @pl.when(odd == parity)
            def _(parity=parity):
                took(1 - parity, stop)

        out_ref[...] = (
            own_stream.astype(F32) + jnp.sum(column_in[:stop].astype(F32), axis=0)
        ).astype(BF16)

    @pl.when(edge)
    def _():
        finish(planes + len(around))

    @pl.when(jnp.logical_not(edge))
    def _():
        finish(planes)

    push(0).wait_send()
    push(1).wait_send()
    remote(heads_all, heads_all, heads_send.at[0], heads_recv.at[0], (e, t)).wait_send()

    def drained(count):
        where = ow.at[pl.ds(0, count * seqs), :]
        remote(where, where, chunk_send.at[0], column_recv.at[0], (e, t)).wait_send()

    hops = len(around)
    @pl.when(odd == 0)
    def _():
        for mask in range(1, n_ep):
            route_copy(mask).wait_send()

    for level in range(planes):
        for core in range(CORES):
            count = planes - 1 + hops + turns * CORES * (hops + 1)
            count += hops if level == planes - 1 else 0
            count += 1 if core != keeps(level) else -1
            if core == RELAY:
                skew = (1 - RELAY + keeps(level)) % CORES
                lower = [level ^ skew ^ (CORES * i) for i in range(turns)]
                count += CORES * sum(
                    plane != level and abs(plane - level) != planes - 1 for plane in lower
                )
            for plane in range(planes) if core == RELAY else ():
                if plane != level and plane - level != planes - 1:
                    count += CORES * (hops + (keeps(plane) != RELAY))

            @pl.when(jnp.logical_and(z == level, c == core))
            def _(count=count):
                drained(count)


def settle(layer_ref, fresh_ref, layer_out, fresh_out, sem):
    first = pltpu.make_async_copy(layer_ref, layer_out, sem.at[0])
    second = pltpu.make_async_copy(fresh_ref, fresh_out, sem.at[1])
    first.start()
    second.start()
    first.wait()
    second.wait()


def near_call(n_ep, n_tp, arrays):
    (
        residual_in,
        lengths,
        kv_cache,
        norm_gain_attn,
        query_weight,
        key_weight,
        value_weight,
        diff_lambda,
        head_gain,
        out_weight,
        norm_gain_ffn,
        route_ids,
        route_weights,
        expert_gate,
        expert_up,
        expert_down,
        dense_gate,
        dense_up,
        dense_down,
        dense_mix,
    ) = arrays
    seqs, width = residual_in.shape
    held = lambda value: pltpu.with_memory_space_constraint(value, pltpu.HBM)
    groups, spots = kv_cache.shape[1:3]
    share = diff_lambda.shape[0] // groups
    inner = query_weight.shape[1]
    quarter = out_weight.shape[1]
    part = expert_gate.shape[2]
    hid = dense_gate.shape[1] // (n_tp // CORES)
    turns = n_ep // INNER // CORES
    blocks = turns * INNER
    rows = blocks * seqs
    lanes = -(-n_ep // LANES) * LANES
    topk = route_ids.shape[1]
    vmem = pl.BlockSpec(memory_space=pltpu.VMEM)
    hbm = pl.BlockSpec(memory_space=pltpu.HBM)
    dma = pltpu.SemaphoreType.DMA
    layer_out, fresh = pl.pallas_call(
        functools.partial(near_kernel, n_ep, n_tp),
        out_shape=(
            jax.ShapeDtypeStruct((seqs, quarter), BF16),
            jax.ShapeDtypeStruct((seqs, groups * kv_cache.shape[3]), BF16),
        ),
        in_specs=[hbm] * 20,
        out_specs=(vmem, vmem),
        scratch_shapes=[
            pltpu.SMEM(lengths.shape, jnp.int32),
            pltpu.SMEM(diff_lambda.shape, F32),
            pltpu.VMEM(residual_in.shape, BF16),
            pltpu.VMEM((1, width), F32),
            pltpu.VMEM((1, head_gain.shape[0]), F32),
            pltpu.VMEM((1, width), F32),
            pltpu.VMEM((1, width), F32),
            pltpu.VMEM((topk, seqs), jnp.int32),
            pltpu.VMEM((topk, seqs), F32),
            pltpu.VMEM((width, inner + key_weight.shape[1] + value_weight.shape[1]), BF16),
            pltpu.VMEM(kv_cache.shape, BF16),
            pltpu.VMEM((groups, seqs, 2 * share, LANES), F32),
            pltpu.VMEM((groups, seqs * 2 * share, 2 * LANES), BF16),
            pltpu.VMEM((groups, seqs, 2 * share, spots), F32),
            pltpu.VMEM((groups, seqs, 2 * share, LANES), F32),
            pltpu.VMEM((seqs, inner), BF16),
            pltpu.VMEM(out_weight.shape, BF16),
            pltpu.VMEM((CORES, width, 2 * part), BF16),
            pltpu.VMEM((CORES * part, width), BF16),
            pltpu.VMEM((width, hid), BF16),
            pltpu.VMEM((width, hid), BF16),
            pltpu.VMEM((hid, width), BF16),
            pltpu.VMEM((n_tp - 1, seqs, inner), BF16),
            pltpu.VMEM((seqs, quarter), BF16),
            pltpu.VMEM((n_ep * seqs, width), BF16),
            pltpu.VMEM((rows, width), BF16),
            pltpu.VMEM((blocks, seqs, lanes), F32),
            pltpu.VMEM((rows, CORES * part), BF16),
            pltpu.VMEM((rows, hid), BF16),
            pltpu.VMEM((2, rows, CORES * quarter), BF16),
            pltpu.VMEM((rows, CORES * quarter), F32),
            pltpu.VMEM((CORES, turns, CORES, 4, seqs, quarter), BF16),
            pltpu.VMEM((CORES, turns, CORES, seqs, quarter), BF16),
            pltpu.VMEM((n_ep // INNER + 3, seqs, quarter), BF16),
            dma((Q_CHUNKS + CACHE_CHUNKS + 4,)),
            dma((1,)),
            dma((2,)),
            dma((1,)),
            dma((1,)),
            dma((1,)),
            dma((n_tp // CORES,)),
            dma((1,)),
            dma((n_ep // INNER, CORES)),
            dma((turns, INNER)),
            dma((CORES, turns, CORES)),
            dma((1,)),
        ],
        compiler_params=pltpu.CompilerParams(
            collective_id=0, has_side_effects=True, vmem_limit_bytes=36 * 1024 * 1024
        ),
    )(
        held(lengths),
        held(diff_lambda),
        held(residual_in),
        held(norm_gain_attn[None, :]),
        held(head_gain[None, :]),
        held(norm_gain_ffn[None, :]),
        held(dense_mix[None, :]),
        held(route_ids.T),
        held(route_weights.T),
        held(query_weight),
        held(key_weight),
        held(value_weight),
        held(kv_cache),
        held(out_weight),
        held(expert_gate),
        held(expert_up),
        held(expert_down),
        held(dense_gate),
        held(dense_up),
        held(dense_down),
    )
    layer_out, fresh = pl.pallas_call(
        settle,
        out_shape=(
            jax.ShapeDtypeStruct(layer_out.shape, BF16),
            jax.ShapeDtypeStruct(fresh.shape, BF16),
        ),
        in_specs=[vmem, vmem],
        out_specs=(hbm, hbm),
        scratch_shapes=[dma((2,))],
        compiler_params=pltpu.CompilerParams(vmem_limit_bytes=1024 * 1024),
    )(layer_out, fresh)
    return layer_out, fresh.reshape(seqs, groups, kv_cache.shape[3])


def on_device(
    residual_in,
    lengths,
    kv_cache,
    norm_gain_attn,
    query_weight,
    key_weight,
    value_weight,
    diff_lambda,
    head_gain,
    out_weight,
    norm_gain_ffn,
    route_ids,
    route_weights,
    expert_gate,
    expert_up,
    expert_down,
    dense_gate,
    dense_up,
    dense_down,
    dense_mix,
):
    n_ep = lax.axis_size("ep")
    n_tp = lax.axis_size("tp")
    half = n_tp // 2
    if (
        n_tp == 2 * CORES
        and n_ep in (4, 8, 16)
        and expert_gate.shape[0] == 1
        and dense_gate.shape[1] // half % LANES == 0
        and expert_gate.shape[2] % LANES == 0
    ):
        return near_call(
            n_ep,
            n_tp,
            (
                residual_in,
                lengths,
                kv_cache,
                norm_gain_attn,
                query_weight,
                key_weight,
                value_weight,
                diff_lambda,
                head_gain,
                out_weight,
                norm_gain_ffn,
                route_ids,
                route_weights,
                expert_gate,
                expert_up,
                expert_down,
                dense_gate,
                dense_up,
                dense_down,
                dense_mix,
            ),
        )
    seqs, width = residual_in.shape
    groups, spots = kv_cache.shape[1:3]
    share = diff_lambda.shape[0] // groups
    inner = query_weight.shape[1]
    quarter = out_weight.shape[1]
    held, _, part = expert_gate.shape
    rows = n_ep * seqs
    own = dense_gate.shape[1] // n_tp
    split = own % LANES == 0
    hid = own if split else dense_gate.shape[1]
    lanes = -(-n_ep * held // LANES) * LANES
    vmem = pl.BlockSpec(memory_space=pltpu.VMEM)
    smem = pl.BlockSpec(memory_space=pltpu.SMEM)
    hbm = pl.BlockSpec(memory_space=pl.ANY)
    dma = pltpu.SemaphoreType.DMA
    layer_out, fresh = pl.pallas_call(
        functools.partial(layer_kernel, n_ep, n_tp, split),
        out_shape=(
            jax.ShapeDtypeStruct((seqs, quarter), F32),
            jax.ShapeDtypeStruct((seqs, groups * kv_cache.shape[3]), F32),
        ),
        in_specs=[smem] * 2 + [vmem] * 7 + [hbm] * 11,
        out_specs=(vmem, vmem),
        scratch_shapes=[
            pltpu.VMEM(query_weight.shape, BF16),
            pltpu.VMEM(key_weight.shape, BF16),
            pltpu.VMEM(value_weight.shape, BF16),
            pltpu.VMEM(kv_cache.shape, BF16),
            pltpu.VMEM((groups, seqs, 2 * share, LANES), F32),
            pltpu.VMEM((groups, seqs, 2 * share, spots), F32),
            pltpu.VMEM((groups, seqs, 2 * share, LANES), F32),
            pltpu.VMEM((seqs, inner), BF16),
            pltpu.VMEM(out_weight.shape, BF16),
            pltpu.VMEM(expert_gate.shape, BF16),
            pltpu.VMEM(expert_up.shape, BF16),
            pltpu.VMEM(expert_down.shape, BF16),
            pltpu.VMEM((width, hid), BF16),
            pltpu.VMEM((width, hid), BF16),
            pltpu.VMEM((hid, width), BF16),
            pltpu.VMEM((n_tp - 1, seqs, inner), BF16),
            pltpu.VMEM((rows, width), BF16),
            pltpu.VMEM((rows, width), BF16),
            pltpu.VMEM((rows, LANES), F32),
            pltpu.VMEM((rows, lanes), F32),
            pltpu.VMEM((held, rows, part), BF16),
            pltpu.VMEM((rows, hid), BF16),
            pltpu.VMEM((half, rows, quarter), BF16),
            pltpu.VMEM((half, rows, quarter), BF16),
            pltpu.VMEM((half, rows, quarter), BF16),
            pltpu.VMEM((n_ep * half, seqs, quarter), BF16),
            dma((7,)),
            dma((Q_CHUNKS + 2,)),
            dma((seqs,)),
            dma((n_ep - 1,)),
            dma((n_ep - 1,)),
            dma((n_tp - 1,)),
            dma((n_tp - 1,)),
            dma((n_ep,)),
            dma((half, n_ep)),
            dma((max(half - 1, 1), n_ep)),
            dma((n_tp, n_ep)),
            dma((half,)),
            dma((half,)),
            dma((half, n_ep)),
            dma((n_ep * half,)),
        ],
        compiler_params=pltpu.CompilerParams(
            collective_id=0, has_side_effects=True, vmem_limit_bytes=60 * 1024 * 1024
        ),
    )(
        lengths,
        diff_lambda,
        residual_in,
        norm_gain_attn[None, :],
        head_gain[None, :],
        norm_gain_ffn[None, :],
        dense_mix[None, :],
        route_ids.T,
        route_weights.T,
        query_weight,
        key_weight,
        value_weight,
        kv_cache,
        out_weight,
        expert_gate,
        expert_up,
        expert_down,
        dense_gate,
        dense_up,
        dense_down,
    )
    new_rows = fresh.astype(BF16).reshape(seqs, groups, kv_cache.shape[3])
    return (layer_out.astype(BF16), new_rows)


def solution(mesh):
    placed = (
        P("ep", None),
        P("ep"),
        P("ep", "tp", None, None),
        P(),
        P(None, "tp"),
        P(None, "tp"),
        P(None, "tp"),
        P("tp"),
        P(),
        P(None, "tp"),
        P(),
        P("ep", None),
        P("ep", None),
        P("ep", None, "tp"),
        P("ep", None, "tp"),
        P("ep", "tp", None),
        P(None, "ep"),
        P(None, "ep"),
        P("ep", None),
        P(),
    )
    return jax.shard_map(
        on_device,
        mesh=mesh,
        in_specs=placed,
        out_specs=(P("ep", "tp"), P("ep", "tp", None)),
        check_vma=False,
    )
```

```python
import functools
import math

import jax
import jax.numpy as jnp
from jax import lax
from jax.experimental import pallas as pl
from jax.experimental.pallas import tpu as pltpu
from jax.sharding import PartitionSpec as P

QK_DIM = 64
EPS = 1e-06
MESH = pl.DeviceIdType.MESH
F32 = jnp.float32
BF16 = jnp.bfloat16
LANES = 128
Q_CHUNKS = 4
INNER = 2
CORES = 2
RELAY = 1
CACHE_CHUNKS = 4


def flip(value, mask):
    bit = 1
    while bit <= mask:
        if mask & bit:
            value = value + bit * (1 - 2 * ((value // bit) % 2))
        bit *= 2
    return value


def each(count, body, order=None):
    if count <= 16:
        for index in order if order is not None else range(count):
            body(index)
    else:

        def step(index, carry):
            body(index)
            return carry

        lax.fori_loop(0, count, step, 0)


def block(start, size):
    return pl.ds(pl.multiple_of(start * size, size), size)


def remote(source, target, send, recv, where):
    return pltpu.make_async_remote_copy(
        src_ref=source,
        dst_ref=target,
        send_sem=send,
        recv_sem=recv,
        device_id=where,
        device_id_type=MESH,
    )


def dot(left, right):
    return jnp.dot(left, right, preferred_element_type=F32)


def column(row):
    count = row.shape[1]
    square = (count, count)
    same = lax.broadcasted_iota(jnp.int32, square, 0) == lax.broadcasted_iota(jnp.int32, square, 1)
    return jnp.sum(jnp.where(same, row, jnp.zeros_like(row)), axis=1, keepdims=True)


def layer_kernel(
    n_ep,
    n_tp,
    split,
    lengths_ref,
    lam_ref,
    resid_ref,
    first_gain_ref,
    head_gain_ref,
    gain_ref,
    mixw_ref,
    ids_ref,
    rw_ref,
    qw_hbm,
    kw_hbm,
    vw_hbm,
    cache_hbm,
    ow_hbm,
    eg_hbm,
    eu_hbm,
    ed_hbm,
    dg_hbm,
    du_hbm,
    dd_hbm,
    out_ref,
    new_ref,
    qw,
    kw,
    vw,
    cache,
    pairs,
    scores,
    mixed,
    heads_ref,
    ow,
    eg,
    eu,
    ed,
    dg,
    du,
    dd,
    heads_all,
    stream,
    ffn,
    mix,
    route,
    eh,
    dh,
    away,
    came,
    summed,
    landed,
    w_sem,
    q_sem,
    cache_sem,
    route_send,
    route_recv,
    heads_send,
    heads_recv,
    first_send,
    second_send,
    relay_send,
    stream_recv,
    pair_send,
    pair_recv,
    back_send,
    back_recv,
):
    e = lax.axis_index("ep")
    t = lax.axis_index("tp")
    half = n_tp // 2
    mate = flip(t, 1)
    core = t % 2
    seqs, width = resid_ref.shape
    quarter = out_ref.shape[1]
    held, _, part = eg.shape
    hid = dg.shape[1]
    rows_all = n_ep * seqs
    evens = [2 * i for i in range(1, half)]

    depth = qw.shape[0] // Q_CHUNKS
    q_loads = [
        pltpu.make_async_copy(
            qw_hbm.at[pl.ds(i * depth, depth), :], qw.at[pl.ds(i * depth, depth), :], q_sem.at[i]
        )
        for i in range(Q_CHUNKS)
    ] + [
        pltpu.make_async_copy(kw_hbm, kw, q_sem.at[Q_CHUNKS]),
        pltpu.make_async_copy(vw_hbm, vw, q_sem.at[Q_CHUNKS + 1]),
    ]
    for load in q_loads:
        load.start()
    cache_loads = [
        pltpu.make_async_copy(cache_hbm.at[s], cache.at[s], cache_sem.at[s]) for s in range(seqs)
    ]
    for load in cache_loads:
        load.start()

    barrier = pltpu.get_barrier_semaphore()

    def greet(index):
        where = (index // half, 2 * (index % half) + core)

        @pl.when(jnp.logical_or(where[0] != e, where[1] != t))
        def _():
            pl.semaphore_signal(barrier, inc=1, device_id=where, device_id_type=MESH)

    each(n_ep * half, greet)
    for i in range(half):
        pl.semaphore_signal(
            barrier, inc=1, device_id=(e, 2 * i + 1 - core), device_id_type=MESH
        )

    if split:
        cols = block(t, hid)
        dense_parts = (dg_hbm.at[:, cols], du_hbm.at[:, cols], dd_hbm.at[cols, :])
    else:
        dense_parts = (dg_hbm, du_hbm, dd_hbm)
    loads = [
        pltpu.make_async_copy(src, dst, w_sem.at[i])
        for i, (src, dst) in enumerate(
            zip((ow_hbm, eg_hbm, eu_hbm) + dense_parts[:2] + (ed_hbm, dense_parts[2]), (ow, eg, eu, dg, du, ed, dd))
        )
    ]

    lane = lax.broadcasted_iota(jnp.int32, (seqs, route.shape[1]), 1)
    table = jnp.zeros((seqs, route.shape[1]), F32)
    for k in range(ids_ref.shape[0]):
        wanted = column(ids_ref[k : k + 1, :])
        table = table + jnp.where(lane == wanted, column(rw_ref[k : k + 1, :]), 0.0)
    own_rows = block(e, seqs)
    route[own_rows, :] = table

    resid = resid_ref[...].astype(F32)
    mean_sq = jnp.mean(resid * resid, axis=-1, keepdims=True)
    normed = (resid * lax.rsqrt(mean_sq + EPS) * first_gain_ref[...]).astype(BF16)
    row = lax.broadcasted_iota(jnp.int32, (seqs, LANES), 0)
    entry = lax.broadcasted_iota(jnp.int32, (seqs, LANES), 1) % QK_DIM
    position = jnp.zeros((seqs, LANES), F32)
    for s in range(seqs):
        position = jnp.where(row == s, lengths_ref[s].astype(F32), position)
    turn = QK_DIM // 2
    power = (entry % turn).astype(F32) * (-1.0 / turn)
    angle = position * jnp.exp(power * math.log(10000.0))
    cosine = jnp.cos(angle)
    sine = jnp.where(entry < turn, -jnp.sin(angle), jnp.sin(angle))

    def rotate(values):
        other = jnp.where(
            entry < turn, pltpu.roll(values, LANES - turn, 1), pltpu.roll(values, turn, 1)
        )
        return (values * cosine + other * sine).astype(BF16).astype(F32)

    query = jnp.zeros((seqs, qw.shape[1]), F32)
    for i in range(Q_CHUNKS):
        q_loads[i].wait()
        query = query + dot(
            normed[:, i * depth : (i + 1) * depth], qw[i * depth : (i + 1) * depth, :]
        )
    for load in q_loads[Q_CHUNKS:]:
        load.wait()
    keys_raw = dot(normed, kw[...])
    values_raw = dot(normed, vw[...])
    for load in loads:
        load.start()

    groups, spots = cache.shape[1], cache.shape[2]
    share = query.shape[1] // LANES // groups
    lower = lax.broadcasted_iota(jnp.int32, (seqs, LANES), 1) < QK_DIM
    fresh = []
    for g in range(groups):
        key = rotate(keys_raw[:, g * LANES : (g + 1) * LANES])
        value = values_raw[:, g * LANES : (g + 1) * LANES].astype(BF16).astype(F32)
        new_ref[:, 2 * g * LANES : (2 * g + 1) * LANES] = key
        new_ref[:, (2 * g + 1) * LANES : (2 * g + 2) * LANES] = value
        fresh.append((key, value))
        for j in range(share):
            at = (g * share + j) * LANES
            head = rotate(query[:, at : at + LANES])
            pairs[g, :, j, :] = jnp.where(lower, head, 0.0)
            pairs[g, :, share + j, :] = jnp.where(lower, 0.0, head)

    pl.semaphore_wait(barrier, n_ep * half - 1 + half)

    def route_copy(d):
        there = (e + d) % n_ep
        return remote(
            route.at[own_rows, :],
            route.at[own_rows, :],
            route_send.at[d - 1],
            route_recv.at[d - 1],
            (there, t),
        )

    def route_wait(d):
        came_from = (e + n_ep - d) % n_ep
        spot = route.at[block(came_from, seqs), :]
        remote(spot, spot, route_send.at[d - 1], route_recv.at[d - 1], (e, t)).wait_recv()

    each(n_ep - 1, lambda i: route_copy(i + 1).start())

    scale = QK_DIM**-0.5
    lines = 2 * share
    for s in range(seqs):
        cache_loads[s].wait()
        for g in range(groups):
            both = pairs[g, s].astype(BF16)
            scores[g, s] = (
                lax.dot_general(
                    both,
                    cache[s, g, :, :LANES],
                    (((1,), (1,)), ((), ())),
                    preferred_element_type=F32,
                )
                * scale
            )
    length = jnp.zeros((seqs, lines, 1), jnp.int32)
    which = lax.broadcasted_iota(jnp.int32, (seqs, lines, 1), 0)
    for s in range(seqs):
        length = jnp.where(which == s, lengths_ref[s], length)
    place = lax.broadcasted_iota(jnp.int32, (seqs, lines, spots), 2)
    valid = place < length
    line = lax.broadcasted_iota(jnp.int32, (lines, 1), 0)
    for g in range(groups):
        key, value = fresh[g]
        latest = jnp.sum(pairs[g] * key[:, None, :], axis=-1, keepdims=True) * scale
        masked = jnp.where(valid, scores[g], -jnp.inf)
        top = jnp.maximum(jnp.max(masked, axis=-1, keepdims=True), latest)
        raised = jnp.exp(masked - top)
        raised_new = jnp.exp(latest - top)
        total = jnp.sum(raised, axis=-1, keepdims=True) + raised_new
        prob = raised / total
        prob_new = jnp.broadcast_to(raised_new / total, (seqs, lines, LANES))
        lam = jnp.zeros((lines, 1), F32)
        for j in range(share):
            lam = jnp.where(line == j, lam_ref[g * share + j], lam)
        scores[g] = prob - lam[None] * pltpu.roll(prob, share, 1)
        new_weight = (prob_new - lam[None] * pltpu.roll(prob_new, share, 1)).astype(BF16).astype(F32)
        fresh_part = new_weight * value[:, None, :]
        for s in range(seqs):
            mixed[g, s] = dot(scores[g, s].astype(BF16), cache[s, g, :, LANES:])
        whole = mixed[g] + fresh_part
        mean_sq = jnp.mean(whole * whole, axis=-1, keepdims=True)
        mixed[g] = whole * lax.rsqrt(mean_sq + EPS) * head_gain_ref[...][None]
        for j in range(share):
            at = (g * share + j) * LANES
            heads_ref[:, at : at + LANES] = mixed[g, :, j, :].astype(BF16)

    def heads_copy(mask):
        return remote(
            heads_ref,
            heads_all.at[mask - 1],
            heads_send.at[mask - 1],
            heads_recv.at[mask - 1],
            (e, flip(t, mask)),
        )

    for mask in range(n_tp - 1, 0, -1):
        heads_copy(mask).start()

    loads[0].wait()
    span = heads_ref.shape[1]
    total = dot(heads_ref[...], ow[block(t, span), :])
    for mask in range(1, n_tp):
        heads_copy(mask).wait_recv()
        total = total + dot(heads_all[mask - 1], ow[block(flip(t, mask), span), :])
    own_cols = block(t, quarter)
    own_stream = (resid_ref[:, own_cols].astype(F32) + total).astype(BF16)
    stream[own_rows, own_cols] = own_stream

    def spot(owner, column):
        return stream.at[block(owner, seqs), block(column, quarter)]

    def owner_of(d):
        return (e + n_ep - d) % n_ep

    def first(d):
        return remote(
            spot(e, t), spot(e, t), first_send.at[d], stream_recv.at[0, d], ((e + d) % n_ep, t)
        )

    def second(d, mask):
        index = mask // 2 if mask != 1 else 0
        where = spot(owner_of(d), t)
        return remote(
            where, where, second_send.at[index, d], stream_recv.at[mask, d], (e, flip(t, mask))
        )

    def relay(d, mask):
        where = spot(owner_of(d), flip(t, mask))
        return remote(
            where, where, relay_send.at[mask // 2 - 1, d], stream_recv.at[mask + 1, d], (e, mate)
        )

    def arrived(d, mask):
        where = spot(owner_of(d), flip(t, mask))
        remote(where, where, first_send.at[d], stream_recv.at[mask, d], (e, t)).wait_recv()

    def spread(d):
        for mask in evens:
            second(d, mask).start()
        second(d, 1).start()

    far_first = sorted(range(1, n_ep), key=lambda d: -min(d, n_ep - d)) if n_ep <= 16 else None
    near_first = [0] + far_first[::-1] if far_first is not None else None
    each(n_ep - 1 if far_first is None else 1, lambda i: first(i + 1).start(), order=None) if far_first is None else [
        first(d).start() for d in far_first
    ]

    def stage_two(d):
        if not (isinstance(d, int) and d == 0):
            arrived(d, 0)
        spread(d)

    def stage_three(d):
        for mask in evens:
            arrived(d, mask)
            relay(d, mask).start()

    def normalise(d):
        arrived(d, 1)
        for mask in evens:
            arrived(d, mask + 1)
        rows = block(owner_of(d), seqs)
        values = stream[rows, :].astype(F32)
        mean_sq = jnp.mean(values * values, axis=-1, keepdims=True)
        scaled = (values * lax.rsqrt(mean_sq + EPS) * gain_ref[...]).astype(BF16)
        ffn[rows, :] = scaled
        inner = jnp.sum(scaled.astype(F32) * mixw_ref[...], axis=-1, keepdims=True)
        mix[rows, :] = jnp.broadcast_to(jax.nn.sigmoid(inner), (seqs, LANES))

    if near_first is not None:
        for i, d in enumerate(near_first):
            stage_two(d)
            if i:
                stage_three(near_first[i - 1])
            if i > 1:
                normalise(near_first[i - 2])
        stage_three(near_first[-1])
        for d in near_first[-2:]:
            normalise(d)
    else:
        stage_two(0)
        each(n_ep - 1, lambda i: stage_two(i + 1))
        each(n_ep, stage_three)
        each(n_ep, normalise)
    each(n_ep - 1, lambda i: route_wait(i + 1))

    many = min(rows_all, 128)
    batches = rows_all // many
    for load in loads[1:5]:
        load.wait()

    def hidden(b):
        rows = block(b, many)
        a = ffn[rows, :]
        for j in range(held):
            eh[j, rows, :] = (jax.nn.silu(dot(a, eg[j])) * dot(a, eu[j])).astype(BF16)
        units = jax.nn.silu(dot(a, dg[...])) * dot(a, du[...])
        if not split:
            own = hid // n_tp
            unit = lax.broadcasted_iota(jnp.int32, units.shape, 1)
            units = jnp.where((unit >= t * own) & (unit < (t + 1) * own), units, 0.0)
        dh[rows, :] = units.astype(BF16)

    each(batches, hidden)
    for load in loads[5:]:
        load.wait()

    def result(b, q):
        rows = block(b, many)
        cols = block(q, quarter)
        total = mix[rows, :1] * dot(dh[rows, :], dd[:, cols])
        lanes = lax.broadcasted_iota(jnp.int32, (many, route.shape[1]), 1)
        for j in range(held):
            weight = jnp.sum(
                jnp.where(lanes == e * held + j, route[rows, :], 0.0), axis=1, keepdims=True
            )
            piece = dot(eh[j, rows, :], ed[j, :, cols]).astype(BF16)
            total = total + weight * piece.astype(F32)
        return total

    def pair(j):
        return remote(away.at[j], came.at[j], pair_send.at[j], pair_recv.at[j], (e, mate))

    for j in range(half):

        def leave(b, j=j):
            away[j, block(b, many), :] = result(b, 2 * j + 1 - core).astype(BF16)

        each(batches, leave)
        pair(j).start()

    me = e * half + t // 2

    def back(j, d):
        there = (e + d) % n_ep
        return remote(
            summed.at[j, block(there, seqs), :],
            landed.at[me],
            back_send.at[j, d],
            back_recv.at[me],
            (there, 2 * j + core),
        )

    def same(j, d):
        return jnp.logical_and(jnp.asarray(d == 0), 2 * j + core == t)

    for j in range(half):

        def keep(b, j=j):
            summed[j, block(b, many), :] = result(b, 2 * j + core).astype(BF16)

        each(batches, keep)
    for j in range(half):
        pair(j).wait_recv()

        def add(b, j=j):
            rows = block(b, many)
            summed[j, rows, :] = (summed[j, rows, :].astype(F32) + came[j, rows, :].astype(F32)).astype(BF16)

        each(batches, add)

        def send(d, j=j):
            @pl.when(jnp.logical_not(same(j, d)))
            def _():
                back(j, d).start()

        each(n_ep, send, order=None if far_first is None else far_first + [0])

    landed[me] = summed[t // 2, own_rows, :]

    def take(index):
        @pl.when(index != me)
        def _():
            where = landed.at[index]
            remote(where, where, back_send.at[0, 0], back_recv.at[index], (e, t)).wait_recv()

    each(n_ep * half, take)
    out_ref[...] = own_stream.astype(F32) + jnp.sum(landed[...].astype(F32), axis=0)

    for mask in range(1, n_tp):
        heads_copy(mask).wait_send()
    each(n_ep - 1, lambda i: route_copy(i + 1).wait_send())
    each(n_ep - 1, lambda i: first(i + 1).wait_send())

    def sent(d):
        second(d, 1).wait_send()
        for mask in evens:
            second(d, mask).wait_send()
            relay(d, mask).wait_send()

    each(n_ep, sent)
    for j in range(half):
        pair(j).wait_send()

        def gone(d, j=j):
            @pl.when(jnp.logical_not(same(j, d)))
            def _():
                back(j, d).wait_send()

        each(n_ep, gone)


def keeps(plane):
    return (plane + 1) % CORES


def tells(planes, me, you):
    z, x, y, c = me
    level, inner, side, core = you
    other = (z != level) | (x != inner) | (y != side) | (c != core)
    column = (c == RELAY) & (x == inner) & (y == side)
    lane = (y == side) & (c == core)
    far = (z == 0) & (level == planes - 1) & (c == keeps(planes - 1))
    return other & ((z == level) | column | lane | far)


def near_kernel(
    n_ep,
    n_tp,
    lengths_hbm,
    lam_hbm,
    resid_hbm,
    first_gain_hbm,
    head_gain_hbm,
    gain_hbm,
    mixw_hbm,
    ids_hbm,
    rw_hbm,
    qw_hbm,
    kw_hbm,
    vw_hbm,
    cache_hbm,
    ow_hbm,
    eg_hbm,
    eu_hbm,
    ed_hbm,
    dg_hbm,
    du_hbm,
    dd_hbm,
    out_ref,
    new_ref,
    lengths_ref,
    lam_ref,
    resid_ref,
    first_gain_ref,
    head_gain_ref,
    gain_ref,
    mixw_ref,
    ids_ref,
    rw_ref,
    qkv,
    cache,
    pairs,
    asked,
    scores,
    mixed,
    heads_ref,
    ow,
    gu,
    ed,
    dg,
    du,
    dd,
    heads_all,
    mine,
    stream,
    ffn,
    route,
    eh,
    dh,
    leaving,
    kept,
    plane_in,
    column_out,
    column_in,
    local_sem,
    push_send,
    push_recv,
    route_send,
    route_recv,
    heads_send,
    heads_recv,
    chunk_send,
    climb_recv,
    group_recv,
    plane_recv,
    column_recv,
):
    e = lax.axis_index("ep")
    t = lax.axis_index("tp")
    planes = n_ep // INNER
    z = e // INNER
    x = e % INNER
    y = t // CORES
    c = t % CORES
    keeper = keeps(z)
    odd = (c + keeper) % CORES
    turns = planes // CORES
    seqs, width = resid_ref.shape
    quarter = out_ref.shape[1]
    part = eg_hbm.shape[2]
    hid = dg.shape[1]
    mate = flip(t, 1)

    def gather_loads(sem, *routes):
        return [pltpu.make_async_copy(src, dst, local_sem.at[sem]) for src, dst in routes]

    first_loads = gather_loads(
        0, (resid_hbm, resid_ref), (first_gain_hbm, first_gain_ref), (lengths_hbm, lengths_ref)
    )
    for load in first_loads:
        load.start()
    depth = qkv.shape[0] // Q_CHUNKS
    inner = qw_hbm.shape[1]
    side = kw_hbm.shape[1]
    for i in range(Q_CHUNKS):
        deep = pl.ds(i * depth, depth)
        for load in gather_loads(
            1 + i,
            (qw_hbm.at[deep, :], qkv.at[deep, :inner]),
            (kw_hbm.at[deep, :], qkv.at[deep, inner : inner + side]),
            (vw_hbm.at[deep, :], qkv.at[deep, inner + side :]),
        ):
            load.start()

    barrier = pltpu.get_barrier_semaphore()
    for index in range(n_ep * n_tp):
        there = (index // n_tp // INNER, index // n_tp % INNER, index % n_tp // CORES, index % CORES)

        @pl.when(tells(planes, (z, x, y, c), there))
        def _():
            pl.semaphore_signal(
                barrier, inc=1, device_id=(index // n_tp, index % n_tp), device_id_type=MESH
            )

    told = 0
    for level in range(planes):
        for core in range(CORES):
            count = sum(
                tells(planes, (i, j, k, m), (level, 0, 0, core))
                for i in range(planes)
                for j in range(INNER)
                for k in range(n_tp // CORES)
                for m in range(CORES)
            )
            told = jnp.where((z == level) & (c == core), count, told)

    for load in first_loads:
        load.wait()
    bunch = seqs // CACHE_CHUNKS
    cache_loads = [
        gather_loads(
            1 + Q_CHUNKS + i,
            (cache_hbm.at[pl.ds(i * bunch, bunch)], cache.at[pl.ds(i * bunch, bunch)]),
        )[0]
        for i in range(CACHE_CHUNKS)
    ]
    for load in cache_loads:
        load.start()
    late = 1 + Q_CHUNKS + CACHE_CHUNKS
    late_loads = gather_loads(
        late,
        (ids_hbm, ids_ref),
        (rw_hbm, rw_ref),
        (lam_hbm, lam_ref),
        (head_gain_hbm, head_gain_ref),
        (gain_hbm, gain_ref),
        (mixw_hbm, mixw_ref),
    )
    for load in late_loads:
        load.start()
    cols = block(y, hid)
    e_loads = gather_loads(
        late + 1, (eg_hbm.at[0], gu.at[c, :, :part]), (eu_hbm.at[0], gu.at[c, :, part:])
    ) + gather_loads(late + 2, (ed_hbm.at[0], ed.at[block(c, part), :]))
    loads = [
        gather_loads(1 + i, route)[0]
        for i, route in enumerate(
            (
                (ow_hbm, ow),
                (dg_hbm.at[:, cols], dg),
                (du_hbm.at[:, cols], du),
                (dd_hbm.at[cols, :], dd),
            )
        )
    ]
    resid = resid_ref[...].astype(F32)
    mean_sq = jnp.mean(resid * resid, axis=-1, keepdims=True)
    normed = (resid * lax.rsqrt(mean_sq + EPS) * first_gain_ref[...]).astype(BF16)
    row = lax.broadcasted_iota(jnp.int32, (seqs, LANES), 0)
    entry = lax.broadcasted_iota(jnp.int32, (seqs, LANES), 1) % QK_DIM
    position = jnp.zeros((seqs, LANES), F32)
    for s in range(seqs):
        position = jnp.where(row == s, lengths_ref[s].astype(F32), position)
    turn = QK_DIM // 2
    power = (entry % turn).astype(F32) * (-1.0 / turn)
    angle = position * jnp.exp(power * math.log(10000.0))
    cosine = jnp.cos(angle)
    sine = jnp.where(entry < turn, -jnp.sin(angle), jnp.sin(angle))

    def rotate(values):
        other = jnp.where(
            entry < turn, pltpu.roll(values, LANES - turn, 1), pltpu.roll(values, turn, 1)
        )
        return (values * cosine + other * sine).astype(BF16).astype(F32)

    def spot(plane, inner):
        return plane // CORES * INNER + inner

    own_spot = spot(z, x)
    projected = jnp.zeros((seqs, qkv.shape[1]), F32)
    for i in range(Q_CHUNKS):
        deep = pl.ds(i * depth, depth)
        pltpu.make_async_copy(qkv.at[deep, :], qkv.at[deep, :], local_sem.at[1 + i]).wait()
        projected = projected + dot(normed[:, i * depth : (i + 1) * depth], qkv[deep, :])
    query = projected[:, :inner]
    keys_raw = projected[:, inner : inner + side]
    values_raw = projected[:, inner + side :]
    for load in e_loads + loads:
        load.start()

    groups, spots = cache.shape[1], cache.shape[2]
    share = query.shape[1] // LANES // groups
    scale = QK_DIM**-0.5
    lines = 2 * share
    lower = lax.broadcasted_iota(jnp.int32, (seqs, LANES), 1) < QK_DIM
    fresh = []
    for g in range(groups):
        key = rotate(keys_raw[:, g * LANES : (g + 1) * LANES])
        value = values_raw[:, g * LANES : (g + 1) * LANES].astype(BF16).astype(F32)
        new_ref[:, 2 * g * LANES : (2 * g + 1) * LANES] = key.astype(BF16)
        new_ref[:, (2 * g + 1) * LANES : (2 * g + 2) * LANES] = value.astype(BF16)
        fresh.append((key, value))
        for j in range(share):
            at = (g * share + j) * LANES
            head = rotate(query[:, at : at + LANES])
            pairs[g, :, j, :] = jnp.where(lower, head, 0.0)
            pairs[g, :, share + j, :] = jnp.where(lower, 0.0, head)
        spread = (pairs[g] * scale).reshape(seqs * lines, LANES).astype(BF16)
        turn_of = lax.broadcasted_iota(jnp.int32, spread.shape, 0) // lines % 2
        asked[g, :, :LANES] = jnp.where(turn_of == 0, spread, jnp.zeros_like(spread))
        asked[g, :, LANES:] = jnp.where(turn_of == 0, jnp.zeros_like(spread), spread)

    def push(index):
        where = (gu.at[c], ed.at[block(c, part), :])[index]
        return remote(where, where, push_send.at[0], push_recv.at[index], (e, mate))

    def pushed(index):
        where = (gu.at[1 - c], ed.at[block(1 - c, part), :])[index]
        remote(where, where, push_send.at[0], push_recv.at[index], (e, mate)).wait_recv()

    def beside(s, g, lanes):
        return jnp.concatenate([cache[s, g, :, lanes], cache[s + 1, g, :, lanes]], axis=1)

    place = lax.broadcasted_iota(jnp.int32, (bunch, lines, spots), 2)
    line = lax.broadcasted_iota(jnp.int32, (lines, 1), 0)

    def score(start):
        for s in range(start, start + bunch, 2):
            for g in range(groups):
                scores[g, s : s + 2] = lax.dot_general(
                    asked[g, s * lines : (s + 2) * lines, :],
                    beside(s, g, slice(0, LANES)),
                    (((1,), (1,)), ((), ())),
                    preferred_element_type=F32,
                ).reshape(2, lines, spots)

    def attend(start):
        stop = start + bunch
        length = jnp.zeros((bunch, lines, 1), jnp.int32)
        which = lax.broadcasted_iota(jnp.int32, (bunch, lines, 1), 0)
        for s in range(bunch):
            length = jnp.where(which == s, lengths_ref[start + s], length)
        valid = place < length
        for g in range(groups):
            key, value = (half[start:stop] for half in fresh[g])
            latest = jnp.sum(pairs[g, start:stop] * key[:, None, :], axis=-1, keepdims=True) * scale
            masked = jnp.where(valid, scores[g, start:stop], -jnp.inf)
            top = jnp.maximum(jnp.max(masked, axis=-1, keepdims=True), latest)
            raised = jnp.exp(masked - top)
            raised_new = jnp.exp(latest - top)
            total = jnp.sum(raised, axis=-1, keepdims=True) + raised_new
            lam = jnp.full((lines, 1), 1.0, F32)
            for j in range(share):
                lam = jnp.where(line == share + j, lam_ref[g * share + j], lam)
            part_of = lam[None] / total
            prob = raised * part_of
            prob_new = jnp.broadcast_to(raised_new * part_of, (bunch, lines, LANES))
            weights = (prob - pltpu.roll(prob, share, 1)).astype(BF16)
            new_weight = (
                (prob_new - pltpu.roll(prob_new, share, 1)).astype(BF16).astype(F32)
            )
            fresh_part = new_weight * value[:, None, :]
            for s in range(0, bunch, 2):
                both = dot(
                    weights[s : s + 2].reshape(2 * lines, spots),
                    beside(start + s, g, slice(LANES, None)),
                )
                mixed[g, start + s] = both[:lines, :LANES]
                mixed[g, start + s + 1] = both[lines:, LANES:]
            whole = mixed[g, start:stop] + fresh_part
            mean_sq = jnp.mean(whole * whole, axis=-1, keepdims=True)
            mixed[g, start:stop] = whole * lax.rsqrt(mean_sq + EPS) * head_gain_ref[...][None]

    for i in range(CACHE_CHUNKS):
        if i == CACHE_CHUNKS - 1:
            for load in late_loads:
                load.wait()
        cache_loads[i].wait()
        score(i * bunch)
        if i == CACHE_CHUNKS - 1:
            for k in range(CACHE_CHUNKS):
                attend(k * bunch)
    for g in range(groups):
        for j in range(share):
            at = (g * share + j) * LANES
            heads_ref[:, at : at + LANES] = mixed[g, :, j, :].astype(BF16)

    def heads_copy(mask):
        return remote(
            heads_ref,
            heads_all.at[mask - 1],
            heads_send.at[0],
            heads_recv.at[mask // CORES],
            (e, flip(t, mask)),
        )

    pl.semaphore_wait(barrier, told)
    for core in range(CORES):
        skew = (c + core) % CORES
        remote(
            heads_ref,
            heads_all.at[CORES - 1 + skew],
            heads_send.at[0],
            heads_recv.at[1],
            (e, flip(y, 1) * CORES + core),
        ).start()
    heads_copy(1).start()

    for load in e_loads:
        load.wait()
    push(0).start()
    push(1).start()

    lane = lax.broadcasted_iota(jnp.int32, (seqs, route.shape[2]), 1)
    table = jnp.zeros((seqs, route.shape[2]), F32)
    for k in range(ids_ref.shape[0]):
        wanted = column(ids_ref[k : k + 1, :])
        table = table + jnp.where(lane == wanted, column(rw_ref[k : k + 1, :]), 0.0)

    @pl.when(odd == 0)
    def _():
        route[own_spot] = table

    def route_copy(mask):
        where = route.at[own_spot]
        return remote(
            where, where, route_send.at[0], route_recv.at[0], (flip(e, mask), t)
        )

    @pl.when(odd == 0)
    def _():
        for mask in range(1, n_ep):
            route_copy(mask).start()


    loads[0].wait()
    span = heads_ref.shape[1]
    total = dot(heads_ref[...], ow[block(t, span), :])
    for far in range(n_tp // CORES):
        batch = heads_all.at[pl.ds(0, 1) if far == 0 else pl.ds(far * CORES - 1, CORES)]
        remote(batch, batch, heads_send.at[0], heads_recv.at[far], (e, t)).wait_recv()
        for mask in range(max(far * CORES, 1), (far + 1) * CORES):
            total = total + dot(heads_all[mask - 1], ow[block(flip(t, mask), span), :])
    own_cols = block(t, quarter)
    own_stream = (resid_ref[:, own_cols].astype(F32) + total).astype(BF16)
    mine[...] = own_stream

    around = ((1, 1), (1, 0), (0, 1))
    last = turns - 1
    edge = jnp.logical_or(z == 0, z == planes - 1)
    far = jnp.logical_and(edge, odd == 1)

    def chunk(group, owner):
        return stream.at[block(group, seqs), block(owner, quarter)]

    def to_plane(step):
        dx, dy = around[step]
        there = (z * INNER + flip(x, dx), flip(y, dy) * CORES + keeper)
        return remote(
            mine, chunk(e, t), chunk_send.at[0], group_recv.at[z // CORES, dx], there
        )

    def to_column(d):
        core = jnp.where(z == planes - 1, keeper, RELAY) if d == planes - 1 else RELAY
        there = (flip(z, d) * INNER + x, y * CORES + core)
        return remote(mine, chunk(e, t), chunk_send.at[0], climb_recv.at[z, c], there)

    def to_mate():
        return remote(mine, chunk(e, t), chunk_send.at[0], climb_recv.at[z, c], (e, mate))

    def to_far(step):
        dx, dy = around[step]
        there = (flip(z, planes - 1) * INNER + flip(x, dx), flip(y, dy) * CORES + keeper)
        return remote(
            mine, chunk(e, t), chunk_send.at[0], group_recv.at[z // CORES, dx], there
        )

    for d in range(planes - 2, 0, -1):
        to_column(d).start()

    @pl.when(z == planes - 1)
    def _():
        for step in range(len(around)):
            to_far(step).start()

    to_column(planes - 1).start()
    for step in range(len(around)):
        to_plane(step).start()

    @pl.when(odd == 1)
    def _():
        to_mate().start()

    @pl.when(odd == 0)
    def _():
        stream[block(e, seqs), own_cols] = own_stream

    near = z + odd * (1 - 2 * (z % 2))

    def plane_of(i):
        return flip(near, 2 * i)

    def arrived(plane, core):
        where = chunk(plane * INNER + x, y * CORES + core)
        remote(where, where, chunk_send.at[0], climb_recv.at[plane, core], (e, t)).wait_recv()

    def forward(plane, core, step):
        dx, dy = around[step]
        where = chunk(plane * INNER + x, y * CORES + core)
        return remote(
            where,
            where,
            chunk_send.at[0],
            group_recv.at[plane // CORES, dx],
            (z * INNER + flip(x, dx), flip(y, dy) * CORES + keeps(plane)),
        )

    def hand_over(plane, core):
        where = chunk(plane * INNER + x, y * CORES + core)
        return remote(where, where, chunk_send.at[0], climb_recv.at[plane, core], (e, mate))

    @pl.when(c == RELAY)
    def _():
        for plane in sorted(range(planes), key=lambda plane: keeps(plane) != RELAY):
            passes = plane != z
            if plane == planes - 1:
                passes = jnp.logical_and(passes, z != 0)

            @pl.when(passes)
            def _(plane=plane):
                for core in (RELAY, 1 - RELAY):
                    arrived(plane, core)
                    for step in range(len(around)):
                        forward(plane, core, step).start()
                    if keeps(plane) != RELAY:
                        hand_over(plane, core).start()

    def normalise(i):
        plane = CORES * i + keeps(c)

        @pl.when(plane == z)
        def _():
            arrived(plane, 1 - c)

        leapt = jnp.logical_and(plane == planes - 1, z == 0)

        @pl.when(jnp.logical_and(plane != z, jnp.logical_or(c != RELAY, leapt)))
        def _():
            for core in range(CORES):
                arrived(plane, core)

        for inner in range(INNER):
            group = plane * INNER + flip(x, inner)
            came = stream.at[
                block(group, seqs),
                pl.ds(0, width) if inner else block(flip(y, 1), CORES * quarter),
            ]
            remote(
                came, came, chunk_send.at[0], group_recv.at[plane // CORES, inner], (e, t)
            ).wait_recv()
            values = stream[block(group, seqs), :].astype(F32)
            mean_sq = jnp.mean(values * values, axis=-1, keepdims=True)
            scaled = (values * lax.rsqrt(mean_sq + EPS) * gain_ref[...]).astype(BF16)
            ffn[block(spot(plane, flip(x, inner)), seqs), :] = scaled

    for i in range(turns):
        normalise(i)

    def route_wait(count):
        where = route.at[pl.ds(0, count)]
        remote(where, where, route_send.at[0], route_recv.at[0], (e, t)).wait_recv()

    @pl.when(odd == 0)
    def _():
        route_wait(route.shape[0] - 1)

    @pl.when(odd == 1)
    def _():
        route_wait(route.shape[0])

    rows_all = ffn.shape[0]
    pushed(0)
    pushed(1)
    for load in loads[1:]:
        load.wait()
    a = ffn[...]
    for core in range(CORES):
        both = dot(a, gu[core])
        eh[:, core * part : (core + 1) * part] = (
            jax.nn.silu(both[:, :part]) * both[:, part:]
        ).astype(BF16)
    for at in range(0, hid, 2 * LANES):
        piece = slice(at, at + 2 * LANES)
        dh[:, piece] = (jax.nn.silu(dot(a, dg[:, piece])) * dot(a, du[:, piece])).astype(BF16)
    blend = jax.nn.sigmoid(jnp.sum(a.astype(F32) * mixw_ref[...], axis=-1, keepdims=True))
    lanes = lax.broadcasted_iota(jnp.int32, (rows_all, route.shape[2]), 1)
    weight = jnp.sum(
        jnp.where(lanes == e, route[...].reshape(rows_all, route.shape[2]), 0.0),
        axis=1,
        keepdims=True,
    )
    half = CORES * quarter
    def project(dy):
        cols = block(flip(y, dy), half)
        sparse = weight * dot(eh[...], ed[:, cols])
        return sparse + blend * dot(dh[...], dd[:, cols])

    leaving[1] = project(1).astype(BF16)

    def own_plane(i):
        return jnp.logical_and(odd == 0, i == 0)

    def leave(i, core, step):
        dx, dy = around[step]
        where = spot(plane_of(i), flip(x, dx))
        summer = jnp.where(own_plane(i), c, RELAY)
        return remote(
            leaving.at[dy, block(where, seqs), pl.ds(core * quarter, quarter)],
            plane_in.at[c, i, core, step],
            chunk_send.at[0],
            plane_recv.at[c, i, core],
            (z * INNER + flip(x, dx), flip(y, dy) * CORES + summer),
        )

    def pass_over(i, core):
        where = spot(plane_of(i), x)
        return remote(
            leaving.at[0, block(where, seqs), pl.ds(core * quarter, quarter)],
            plane_in.at[c, i, core, len(around)],
            chunk_send.at[0],
            plane_recv.at[c, i, core],
            (e, mate),
        )

    def leap(core, step):
        dx, dy = around[step] if step < len(around) else (0, 0)
        where = spot(plane_of(last), flip(x, dx))
        return remote(
            leaving.at[dy, block(where, seqs), pl.ds(core * quarter, quarter)],
            column_in.at[planes - 1 + (step + 1) % (len(around) + 1)],
            chunk_send.at[0],
            column_recv.at[0],
            (plane_of(last) * INNER + flip(x, dx), flip(y, dy) * CORES + core),
        )

    order = range(turns - 1, -1, -1)
    for dy in (1, 0):
        if not dy:
            total = project(0)
            leaving[0] = total.astype(BF16)
            kept[...] = total
        steps = [step for step in range(len(around)) if around[step][1] == dy]

        @pl.when(far)
        def _():
            for step in steps + [len(around)] * (1 - dy):
                for core in range(CORES):
                    leap(core, step).start()

        for i in order:

            def depart(i=i):
                for core in range(CORES):
                    for step in steps:
                        leave(i, core, step).start()
                if not dy:

                    @pl.when(jnp.logical_and(c != RELAY, jnp.logical_not(own_plane(i))))
                    def _():
                        for core in range(CORES):
                            pass_over(i, core).start()

            if i == last:
                pl.when(jnp.logical_not(far))(depart)
            else:
                depart()

    def climb(lane, i, core):
        skew = (lane + keeper) % CORES
        level = flip(z + skew * (1 - 2 * (z % 2)), 2 * i)
        return remote(
            column_out.at[lane, i, core],
            column_in.at[skew + 2 * i],
            chunk_send.at[0],
            column_recv.at[0],
            (level * INNER + x, y * CORES + core),
        )

    def stays(i, core):
        return jnp.logical_and(own_plane(i), c == core)

    def rise(i):
        for core in range(CORES):
            gathered = kept[block(spot(plane_of(i), x), seqs), core * quarter : (core + 1) * quarter]
            came = plane_in.at[c, i, core, pl.ds(0, len(around))]
            remote(came, came, chunk_send.at[0], plane_recv.at[c, i, core], (e, t)).wait_recv()
            for step in range(len(around)):
                gathered = gathered + plane_in[c, i, core, step].astype(F32)
            column_out[c, i, core] = gathered.astype(BF16)

            @pl.when(jnp.logical_not(stays(i, core)))
            def _(i=i, core=core):
                climb(c, i, core).start()

    low = 1 - RELAY

    def lift(i):
        for core in range(CORES):
            came = plane_in.at[low, i, core]
            remote(came, came, chunk_send.at[0], plane_recv.at[low, i, core], (e, t)).wait_recv()
            gathered = plane_in[low, i, core, 0].astype(F32)
            for step in range(1, len(around) + 1):
                gathered = gathered + plane_in[low, i, core, step].astype(F32)
            column_out[low, i, core] = gathered.astype(BF16)
            climb(low, i, core).start()

    for i in order:
        sums = jnp.logical_or(c == RELAY, own_plane(i))
        if i == last:
            sums = jnp.logical_and(sums, jnp.logical_not(far))

        @pl.when(sums)
        def _(i=i):
            rise(i)

    slant = (low + keeper) % CORES == 1
    for i in order:
        theirs = c == RELAY
        if i == 0:
            theirs = jnp.logical_and(theirs, slant)
        if i == last:
            theirs = jnp.logical_and(theirs, jnp.logical_not(jnp.logical_and(edge, slant)))

        @pl.when(theirs)
        def _(i=i):
            lift(i)

    def took(start, stop):
        where = column_in.at[pl.ds(start, stop - start)]
        remote(where, where, chunk_send.at[0], column_recv.at[0], (e, t)).wait_recv()

    @pl.when(odd == 0)
    def _():
        column_in[0] = column_out[c, 0, c]

    def finish(stop):
        for parity in range(2):

            @pl.when(odd == parity)
            def _(parity=parity):
                took(1 - parity, stop)

        out_ref[...] = (
            own_stream.astype(F32) + jnp.sum(column_in[:stop].astype(F32), axis=0)
        ).astype(BF16)

    @pl.when(edge)
    def _():
        finish(planes + len(around))

    @pl.when(jnp.logical_not(edge))
    def _():
        finish(planes)

    push(0).wait_send()
    push(1).wait_send()
    remote(heads_all, heads_all, heads_send.at[0], heads_recv.at[0], (e, t)).wait_send()

    def drained(count):
        where = ow.at[pl.ds(0, count * seqs), :]
        remote(where, where, chunk_send.at[0], column_recv.at[0], (e, t)).wait_send()

    hops = len(around)
    @pl.when(odd == 0)
    def _():
        for mask in range(1, n_ep):
            route_copy(mask).wait_send()

    for level in range(planes):
        for core in range(CORES):
            count = planes - 1 + hops + turns * CORES * (hops + 1)
            count += hops if level == planes - 1 else 0
            count += 1 if core != keeps(level) else -1
            if core == RELAY:
                skew = (1 - RELAY + keeps(level)) % CORES
                lower = [level ^ skew ^ (CORES * i) for i in range(turns)]
                count += CORES * sum(
                    plane != level and abs(plane - level) != planes - 1 for plane in lower
                )
            for plane in range(planes) if core == RELAY else ():
                if plane != level and plane - level != planes - 1:
                    count += CORES * (hops + (keeps(plane) != RELAY))

            @pl.when(jnp.logical_and(z == level, c == core))
            def _(count=count):
                drained(count)


def settle(layer_ref, fresh_ref, layer_out, fresh_out, sem):
    first = pltpu.make_async_copy(layer_ref, layer_out, sem.at[0])
    second = pltpu.make_async_copy(fresh_ref, fresh_out, sem.at[1])
    first.start()
    second.start()
    first.wait()
    second.wait()


def near_call(n_ep, n_tp, arrays):
    (
        residual_in,
        lengths,
        kv_cache,
        norm_gain_attn,
        query_weight,
        key_weight,
        value_weight,
        diff_lambda,
        head_gain,
        out_weight,
        norm_gain_ffn,
        route_ids,
        route_weights,
        expert_gate,
        expert_up,
        expert_down,
        dense_gate,
        dense_up,
        dense_down,
        dense_mix,
    ) = arrays
    seqs, width = residual_in.shape
    held = lambda value: pltpu.with_memory_space_constraint(value, pltpu.HBM)
    groups, spots = kv_cache.shape[1:3]
    share = diff_lambda.shape[0] // groups
    inner = query_weight.shape[1]
    quarter = out_weight.shape[1]
    part = expert_gate.shape[2]
    hid = dense_gate.shape[1] // (n_tp // CORES)
    turns = n_ep // INNER // CORES
    blocks = turns * INNER
    rows = blocks * seqs
    lanes = -(-n_ep // LANES) * LANES
    topk = route_ids.shape[1]
    vmem = pl.BlockSpec(memory_space=pltpu.VMEM)
    hbm = pl.BlockSpec(memory_space=pltpu.HBM)
    dma = pltpu.SemaphoreType.DMA
    layer_out, fresh = pl.pallas_call(
        functools.partial(near_kernel, n_ep, n_tp),
        out_shape=(
            jax.ShapeDtypeStruct((seqs, quarter), BF16),
            jax.ShapeDtypeStruct((seqs, groups * kv_cache.shape[3]), BF16),
        ),
        in_specs=[hbm] * 20,
        out_specs=(vmem, vmem),
        scratch_shapes=[
            pltpu.SMEM(lengths.shape, jnp.int32),
            pltpu.SMEM(diff_lambda.shape, F32),
            pltpu.VMEM(residual_in.shape, BF16),
            pltpu.VMEM((1, width), F32),
            pltpu.VMEM((1, head_gain.shape[0]), F32),
            pltpu.VMEM((1, width), F32),
            pltpu.VMEM((1, width), F32),
            pltpu.VMEM((topk, seqs), jnp.int32),
            pltpu.VMEM((topk, seqs), F32),
            pltpu.VMEM((width, inner + key_weight.shape[1] + value_weight.shape[1]), BF16),
            pltpu.VMEM(kv_cache.shape, BF16),
            pltpu.VMEM((groups, seqs, 2 * share, LANES), F32),
            pltpu.VMEM((groups, seqs * 2 * share, 2 * LANES), BF16),
            pltpu.VMEM((groups, seqs, 2 * share, spots), F32),
            pltpu.VMEM((groups, seqs, 2 * share, LANES), F32),
            pltpu.VMEM((seqs, inner), BF16),
            pltpu.VMEM(out_weight.shape, BF16),
            pltpu.VMEM((CORES, width, 2 * part), BF16),
            pltpu.VMEM((CORES * part, width), BF16),
            pltpu.VMEM((width, hid), BF16),
            pltpu.VMEM((width, hid), BF16),
            pltpu.VMEM((hid, width), BF16),
            pltpu.VMEM((n_tp - 1, seqs, inner), BF16),
            pltpu.VMEM((seqs, quarter), BF16),
            pltpu.VMEM((n_ep * seqs, width), BF16),
            pltpu.VMEM((rows, width), BF16),
            pltpu.VMEM((blocks, seqs, lanes), F32),
            pltpu.VMEM((rows, CORES * part), BF16),
            pltpu.VMEM((rows, hid), BF16),
            pltpu.VMEM((2, rows, CORES * quarter), BF16),
            pltpu.VMEM((rows, CORES * quarter), F32),
            pltpu.VMEM((CORES, turns, CORES, 4, seqs, quarter), BF16),
            pltpu.VMEM((CORES, turns, CORES, seqs, quarter), BF16),
            pltpu.VMEM((n_ep // INNER + 3, seqs, quarter), BF16),
            dma((Q_CHUNKS + CACHE_CHUNKS + 4,)),
            dma((1,)),
            dma((2,)),
            dma((1,)),
            dma((1,)),
            dma((1,)),
            dma((n_tp // CORES,)),
            dma((1,)),
            dma((n_ep // INNER, CORES)),
            dma((turns, INNER)),
            dma((CORES, turns, CORES)),
            dma((1,)),
        ],
        compiler_params=pltpu.CompilerParams(
            collective_id=0, has_side_effects=True, vmem_limit_bytes=36 * 1024 * 1024
        ),
    )(
        held(lengths),
        held(diff_lambda),
        held(residual_in),
        held(norm_gain_attn[None, :]),
        held(head_gain[None, :]),
        held(norm_gain_ffn[None, :]),
        held(dense_mix[None, :]),
        held(route_ids.T),
        held(route_weights.T),
        held(query_weight),
        held(key_weight),
        held(value_weight),
        held(kv_cache),
        held(out_weight),
        held(expert_gate),
        held(expert_up),
        held(expert_down),
        held(dense_gate),
        held(dense_up),
        held(dense_down),
    )
    layer_out, fresh = pl.pallas_call(
        settle,
        out_shape=(
            jax.ShapeDtypeStruct(layer_out.shape, BF16),
            jax.ShapeDtypeStruct(fresh.shape, BF16),
        ),
        in_specs=[vmem, vmem],
        out_specs=(hbm, hbm),
        scratch_shapes=[dma((2,))],
        compiler_params=pltpu.CompilerParams(vmem_limit_bytes=1024 * 1024),
    )(layer_out, fresh)
    return layer_out, fresh.reshape(seqs, groups, kv_cache.shape[3])


def on_device(
    residual_in,
    lengths,
    kv_cache,
    norm_gain_attn,
    query_weight,
    key_weight,
    value_weight,
    diff_lambda,
    head_gain,
    out_weight,
    norm_gain_ffn,
    route_ids,
    route_weights,
    expert_gate,
    expert_up,
    expert_down,
    dense_gate,
    dense_up,
    dense_down,
    dense_mix,
):
    n_ep = lax.axis_size("ep")
    n_tp = lax.axis_size("tp")
    half = n_tp // 2
    if (
        n_tp == 2 * CORES
        and n_ep in (4, 8, 16)
        and expert_gate.shape[0] == 1
        and dense_gate.shape[1] // half % LANES == 0
        and expert_gate.shape[2] % LANES == 0
    ):
        return near_call(
            n_ep,
            n_tp,
            (
                residual_in,
                lengths,
                kv_cache,
                norm_gain_attn,
                query_weight,
                key_weight,
                value_weight,
                diff_lambda,
                head_gain,
                out_weight,
                norm_gain_ffn,
                route_ids,
                route_weights,
                expert_gate,
                expert_up,
                expert_down,
                dense_gate,
                dense_up,
                dense_down,
                dense_mix,
            ),
        )
    seqs, width = residual_in.shape
    groups, spots = kv_cache.shape[1:3]
    share = diff_lambda.shape[0] // groups
    inner = query_weight.shape[1]
    quarter = out_weight.shape[1]
    held, _, part = expert_gate.shape
    rows = n_ep * seqs
    own = dense_gate.shape[1] // n_tp
    split = own % LANES == 0
    hid = own if split else dense_gate.shape[1]
    lanes = -(-n_ep * held // LANES) * LANES
    vmem = pl.BlockSpec(memory_space=pltpu.VMEM)
    smem = pl.BlockSpec(memory_space=pltpu.SMEM)
    hbm = pl.BlockSpec(memory_space=pl.ANY)
    dma = pltpu.SemaphoreType.DMA
    layer_out, fresh = pl.pallas_call(
        functools.partial(layer_kernel, n_ep, n_tp, split),
        out_shape=(
            jax.ShapeDtypeStruct((seqs, quarter), F32),
            jax.ShapeDtypeStruct((seqs, groups * kv_cache.shape[3]), F32),
        ),
        in_specs=[smem] * 2 + [vmem] * 7 + [hbm] * 11,
        out_specs=(vmem, vmem),
        scratch_shapes=[
            pltpu.VMEM(query_weight.shape, BF16),
            pltpu.VMEM(key_weight.shape, BF16),
            pltpu.VMEM(value_weight.shape, BF16),
            pltpu.VMEM(kv_cache.shape, BF16),
            pltpu.VMEM((groups, seqs, 2 * share, LANES), F32),
            pltpu.VMEM((groups, seqs, 2 * share, spots), F32),
            pltpu.VMEM((groups, seqs, 2 * share, LANES), F32),
            pltpu.VMEM((seqs, inner), BF16),
            pltpu.VMEM(out_weight.shape, BF16),
            pltpu.VMEM(expert_gate.shape, BF16),
            pltpu.VMEM(expert_up.shape, BF16),
            pltpu.VMEM(expert_down.shape, BF16),
            pltpu.VMEM((width, hid), BF16),
            pltpu.VMEM((width, hid), BF16),
            pltpu.VMEM((hid, width), BF16),
            pltpu.VMEM((n_tp - 1, seqs, inner), BF16),
            pltpu.VMEM((rows, width), BF16),
            pltpu.VMEM((rows, width), BF16),
            pltpu.VMEM((rows, LANES), F32),
            pltpu.VMEM((rows, lanes), F32),
            pltpu.VMEM((held, rows, part), BF16),
            pltpu.VMEM((rows, hid), BF16),
            pltpu.VMEM((half, rows, quarter), BF16),
            pltpu.VMEM((half, rows, quarter), BF16),
            pltpu.VMEM((half, rows, quarter), BF16),
            pltpu.VMEM((n_ep * half, seqs, quarter), BF16),
            dma((7,)),
            dma((Q_CHUNKS + 2,)),
            dma((seqs,)),
            dma((n_ep - 1,)),
            dma((n_ep - 1,)),
            dma((n_tp - 1,)),
            dma((n_tp - 1,)),
            dma((n_ep,)),
            dma((half, n_ep)),
            dma((max(half - 1, 1), n_ep)),
            dma((n_tp, n_ep)),
            dma((half,)),
            dma((half,)),
            dma((half, n_ep)),
            dma((n_ep * half,)),
        ],
        compiler_params=pltpu.CompilerParams(
            collective_id=0, has_side_effects=True, vmem_limit_bytes=60 * 1024 * 1024
        ),
    )(
        lengths,
        diff_lambda,
        residual_in,
        norm_gain_attn[None, :],
        head_gain[None, :],
        norm_gain_ffn[None, :],
        dense_mix[None, :],
        route_ids.T,
        route_weights.T,
        query_weight,
        key_weight,
        value_weight,
        kv_cache,
        out_weight,
        expert_gate,
        expert_up,
        expert_down,
        dense_gate,
        dense_up,
        dense_down,
    )
    new_rows = fresh.astype(BF16).reshape(seqs, groups, kv_cache.shape[3])
    return (layer_out.astype(BF16), new_rows)


def solution(mesh):
    placed = (
        P("ep", None),
        P("ep"),
        P("ep", "tp", None, None),
        P(),
        P(None, "tp"),
        P(None, "tp"),
        P(None, "tp"),
        P("tp"),
        P(),
        P(None, "tp"),
        P(),
        P("ep", None),
        P("ep", None),
        P("ep", None, "tp"),
        P("ep", None, "tp"),
        P("ep", "tp", None),
        P(None, "ep"),
        P(None, "ep"),
        P("ep", None),
        P(),
    )
    return jax.shard_map(
        on_device,
        mesh=mesh,
        in_specs=placed,
        out_specs=(P("ep", "tp"), P("ep", "tp", None)),
        check_vma=False,
    )
```

```python
import functools
import math

import jax
import jax.numpy as jnp
from jax import lax
from jax.experimental import pallas as pl
from jax.experimental.pallas import tpu as pltpu
from jax.sharding import PartitionSpec as P

QK_DIM = 64
EPS = 1e-06
MESH = pl.DeviceIdType.MESH
F32 = jnp.float32
BF16 = jnp.bfloat16
LANES = 128
Q_CHUNKS = 4
INNER = 2
CORES = 2
RELAY = 1
CACHE_CHUNKS = 4


def flip(value, mask):
    bit = 1
    while bit <= mask:
        if mask & bit:
            value = value + bit * (1 - 2 * ((value // bit) % 2))
        bit *= 2
    return value


def each(count, body, order=None):
    if count <= 16:
        for index in order if order is not None else range(count):
            body(index)
    else:

        def step(index, carry):
            body(index)
            return carry

        lax.fori_loop(0, count, step, 0)


def block(start, size):
    return pl.ds(pl.multiple_of(start * size, size), size)


def remote(source, target, send, recv, where):
    return pltpu.make_async_remote_copy(
        src_ref=source,
        dst_ref=target,
        send_sem=send,
        recv_sem=recv,
        device_id=where,
        device_id_type=MESH,
    )


def dot(left, right):
    return jnp.dot(left, right, preferred_element_type=F32)


def column(row):
    count = row.shape[1]
    square = (count, count)
    same = lax.broadcasted_iota(jnp.int32, square, 0) == lax.broadcasted_iota(jnp.int32, square, 1)
    return jnp.sum(jnp.where(same, row, jnp.zeros_like(row)), axis=1, keepdims=True)


def layer_kernel(
    n_ep,
    n_tp,
    split,
    lengths_ref,
    lam_ref,
    resid_ref,
    first_gain_ref,
    head_gain_ref,
    gain_ref,
    mixw_ref,
    ids_ref,
    rw_ref,
    qw_hbm,
    kw_hbm,
    vw_hbm,
    cache_hbm,
    ow_hbm,
    eg_hbm,
    eu_hbm,
    ed_hbm,
    dg_hbm,
    du_hbm,
    dd_hbm,
    out_ref,
    new_ref,
    qw,
    kw,
    vw,
    cache,
    pairs,
    scores,
    mixed,
    heads_ref,
    ow,
    eg,
    eu,
    ed,
    dg,
    du,
    dd,
    heads_all,
    stream,
    ffn,
    mix,
    route,
    eh,
    dh,
    away,
    came,
    summed,
    landed,
    w_sem,
    q_sem,
    cache_sem,
    route_send,
    route_recv,
    heads_send,
    heads_recv,
    first_send,
    second_send,
    relay_send,
    stream_recv,
    pair_send,
    pair_recv,
    back_send,
    back_recv,
):
    e = lax.axis_index("ep")
    t = lax.axis_index("tp")
    half = n_tp // 2
    mate = flip(t, 1)
    core = t % 2
    seqs, width = resid_ref.shape
    quarter = out_ref.shape[1]
    held, _, part = eg.shape
    hid = dg.shape[1]
    rows_all = n_ep * seqs
    evens = [2 * i for i in range(1, half)]

    depth = qw.shape[0] // Q_CHUNKS
    q_loads = [
        pltpu.make_async_copy(
            qw_hbm.at[pl.ds(i * depth, depth), :], qw.at[pl.ds(i * depth, depth), :], q_sem.at[i]
        )
        for i in range(Q_CHUNKS)
    ] + [
        pltpu.make_async_copy(kw_hbm, kw, q_sem.at[Q_CHUNKS]),
        pltpu.make_async_copy(vw_hbm, vw, q_sem.at[Q_CHUNKS + 1]),
    ]
    for load in q_loads:
        load.start()
    cache_loads = [
        pltpu.make_async_copy(cache_hbm.at[s], cache.at[s], cache_sem.at[s]) for s in range(seqs)
    ]
    for load in cache_loads:
        load.start()

    barrier = pltpu.get_barrier_semaphore()

    def greet(index):
        where = (index // half, 2 * (index % half) + core)

        @pl.when(jnp.logical_or(where[0] != e, where[1] != t))
        def _():
            pl.semaphore_signal(barrier, inc=1, device_id=where, device_id_type=MESH)

    each(n_ep * half, greet)
    for i in range(half):
        pl.semaphore_signal(
            barrier, inc=1, device_id=(e, 2 * i + 1 - core), device_id_type=MESH
        )

    if split:
        cols = block(t, hid)
        dense_parts = (dg_hbm.at[:, cols], du_hbm.at[:, cols], dd_hbm.at[cols, :])
    else:
        dense_parts = (dg_hbm, du_hbm, dd_hbm)
    loads = [
        pltpu.make_async_copy(src, dst, w_sem.at[i])
        for i, (src, dst) in enumerate(
            zip((ow_hbm, eg_hbm, eu_hbm) + dense_parts[:2] + (ed_hbm, dense_parts[2]), (ow, eg, eu, dg, du, ed, dd))
        )
    ]

    lane = lax.broadcasted_iota(jnp.int32, (seqs, route.shape[1]), 1)
    table = jnp.zeros((seqs, route.shape[1]), F32)
    for k in range(ids_ref.shape[0]):
        wanted = column(ids_ref[k : k + 1, :])
        table = table + jnp.where(lane == wanted, column(rw_ref[k : k + 1, :]), 0.0)
    own_rows = block(e, seqs)
    route[own_rows, :] = table

    resid = resid_ref[...].astype(F32)
    mean_sq = jnp.mean(resid * resid, axis=-1, keepdims=True)
    normed = (resid * lax.rsqrt(mean_sq + EPS) * first_gain_ref[...]).astype(BF16)
    row = lax.broadcasted_iota(jnp.int32, (seqs, LANES), 0)
    entry = lax.broadcasted_iota(jnp.int32, (seqs, LANES), 1) % QK_DIM
    position = jnp.zeros((seqs, LANES), F32)
    for s in range(seqs):
        position = jnp.where(row == s, lengths_ref[s].astype(F32), position)
    turn = QK_DIM // 2
    power = (entry % turn).astype(F32) * (-1.0 / turn)
    angle = position * jnp.exp(power * math.log(10000.0))
    cosine = jnp.cos(angle)
    sine = jnp.where(entry < turn, -jnp.sin(angle), jnp.sin(angle))

    def rotate(values):
        other = jnp.where(
            entry < turn, pltpu.roll(values, LANES - turn, 1), pltpu.roll(values, turn, 1)
        )
        return (values * cosine + other * sine).astype(BF16).astype(F32)

    query = jnp.zeros((seqs, qw.shape[1]), F32)
    for i in range(Q_CHUNKS):
        q_loads[i].wait()
        query = query + dot(
            normed[:, i * depth : (i + 1) * depth], qw[i * depth : (i + 1) * depth, :]
        )
    for load in q_loads[Q_CHUNKS:]:
        load.wait()
    keys_raw = dot(normed, kw[...])
    values_raw = dot(normed, vw[...])
    for load in loads:
        load.start()

    groups, spots = cache.shape[1], cache.shape[2]
    share = query.shape[1] // LANES // groups
    lower = lax.broadcasted_iota(jnp.int32, (seqs, LANES), 1) < QK_DIM
    fresh = []
    for g in range(groups):
        key = rotate(keys_raw[:, g * LANES : (g + 1) * LANES])
        value = values_raw[:, g * LANES : (g + 1) * LANES].astype(BF16).astype(F32)
        new_ref[:, 2 * g * LANES : (2 * g + 1) * LANES] = key
        new_ref[:, (2 * g + 1) * LANES : (2 * g + 2) * LANES] = value
        fresh.append((key, value))
        for j in range(share):
            at = (g * share + j) * LANES
            head = rotate(query[:, at : at + LANES])
            pairs[g, :, j, :] = jnp.where(lower, head, 0.0)
            pairs[g, :, share + j, :] = jnp.where(lower, 0.0, head)

    pl.semaphore_wait(barrier, n_ep * half - 1 + half)

    def route_copy(d):
        there = (e + d) % n_ep
        return remote(
            route.at[own_rows, :],
            route.at[own_rows, :],
            route_send.at[d - 1],
            route_recv.at[d - 1],
            (there, t),
        )

    def route_wait(d):
        came_from = (e + n_ep - d) % n_ep
        spot = route.at[block(came_from, seqs), :]
        remote(spot, spot, route_send.at[d - 1], route_recv.at[d - 1], (e, t)).wait_recv()

    each(n_ep - 1, lambda i: route_copy(i + 1).start())

    scale = QK_DIM**-0.5
    lines = 2 * share
    for s in range(seqs):
        cache_loads[s].wait()
        for g in range(groups):
            both = pairs[g, s].astype(BF16)
            scores[g, s] = (
                lax.dot_general(
                    both,
                    cache[s, g, :, :LANES],
                    (((1,), (1,)), ((), ())),
                    preferred_element_type=F32,
                )
                * scale
            )
    length = jnp.zeros((seqs, lines, 1), jnp.int32)
    which = lax.broadcasted_iota(jnp.int32, (seqs, lines, 1), 0)
    for s in range(seqs):
        length = jnp.where(which == s, lengths_ref[s], length)
    place = lax.broadcasted_iota(jnp.int32, (seqs, lines, spots), 2)
    valid = place < length
    line = lax.broadcasted_iota(jnp.int32, (lines, 1), 0)
    for g in range(groups):
        key, value = fresh[g]
        latest = jnp.sum(pairs[g] * key[:, None, :], axis=-1, keepdims=True) * scale
        masked = jnp.where(valid, scores[g], -jnp.inf)
        top = jnp.maximum(jnp.max(masked, axis=-1, keepdims=True), latest)
        raised = jnp.exp(masked - top)
        raised_new = jnp.exp(latest - top)
        total = jnp.sum(raised, axis=-1, keepdims=True) + raised_new
        prob = raised / total
        prob_new = jnp.broadcast_to(raised_new / total, (seqs, lines, LANES))
        lam = jnp.zeros((lines, 1), F32)
        for j in range(share):
            lam = jnp.where(line == j, lam_ref[g * share + j], lam)
        scores[g] = prob - lam[None] * pltpu.roll(prob, share, 1)
        new_weight = (prob_new - lam[None] * pltpu.roll(prob_new, share, 1)).astype(BF16).astype(F32)
        fresh_part = new_weight * value[:, None, :]
        for s in range(seqs):
            mixed[g, s] = dot(scores[g, s].astype(BF16), cache[s, g, :, LANES:])
        whole = mixed[g] + fresh_part
        mean_sq = jnp.mean(whole * whole, axis=-1, keepdims=True)
        mixed[g] = whole * lax.rsqrt(mean_sq + EPS) * head_gain_ref[...][None]
        for j in range(share):
            at = (g * share + j) * LANES
            heads_ref[:, at : at + LANES] = mixed[g, :, j, :].astype(BF16)

    def heads_copy(mask):
        return remote(
            heads_ref,
            heads_all.at[mask - 1],
            heads_send.at[mask - 1],
            heads_recv.at[mask - 1],
            (e, flip(t, mask)),
        )

    for mask in range(n_tp - 1, 0, -1):
        heads_copy(mask).start()

    loads[0].wait()
    span = heads_ref.shape[1]
    total = dot(heads_ref[...], ow[block(t, span), :])
    for mask in range(1, n_tp):
        heads_copy(mask).wait_recv()
        total = total + dot(heads_all[mask - 1], ow[block(flip(t, mask), span), :])
    own_cols = block(t, quarter)
    own_stream = (resid_ref[:, own_cols].astype(F32) + total).astype(BF16)
    stream[own_rows, own_cols] = own_stream

    def spot(owner, column):
        return stream.at[block(owner, seqs), block(column, quarter)]

    def owner_of(d):
        return (e + n_ep - d) % n_ep

    def first(d):
        return remote(
            spot(e, t), spot(e, t), first_send.at[d], stream_recv.at[0, d], ((e + d) % n_ep, t)
        )

    def second(d, mask):
        index = mask // 2 if mask != 1 else 0
        where = spot(owner_of(d), t)
        return remote(
            where, where, second_send.at[index, d], stream_recv.at[mask, d], (e, flip(t, mask))
        )

    def relay(d, mask):
        where = spot(owner_of(d), flip(t, mask))
        return remote(
            where, where, relay_send.at[mask // 2 - 1, d], stream_recv.at[mask + 1, d], (e, mate)
        )

    def arrived(d, mask):
        where = spot(owner_of(d), flip(t, mask))
        remote(where, where, first_send.at[d], stream_recv.at[mask, d], (e, t)).wait_recv()

    def spread(d):
        for mask in evens:
            second(d, mask).start()
        second(d, 1).start()

    far_first = sorted(range(1, n_ep), key=lambda d: -min(d, n_ep - d)) if n_ep <= 16 else None
    near_first = [0] + far_first[::-1] if far_first is not None else None
    each(n_ep - 1 if far_first is None else 1, lambda i: first(i + 1).start(), order=None) if far_first is None else [
        first(d).start() for d in far_first
    ]

    def stage_two(d):
        if not (isinstance(d, int) and d == 0):
            arrived(d, 0)
        spread(d)

    def stage_three(d):
        for mask in evens:
            arrived(d, mask)
            relay(d, mask).start()

    def normalise(d):
        arrived(d, 1)
        for mask in evens:
            arrived(d, mask + 1)
        rows = block(owner_of(d), seqs)
        values = stream[rows, :].astype(F32)
        mean_sq = jnp.mean(values * values, axis=-1, keepdims=True)
        scaled = (values * lax.rsqrt(mean_sq + EPS) * gain_ref[...]).astype(BF16)
        ffn[rows, :] = scaled
        inner = jnp.sum(scaled.astype(F32) * mixw_ref[...], axis=-1, keepdims=True)
        mix[rows, :] = jnp.broadcast_to(jax.nn.sigmoid(inner), (seqs, LANES))

    if near_first is not None:
        for i, d in enumerate(near_first):
            stage_two(d)
            if i:
                stage_three(near_first[i - 1])
            if i > 1:
                normalise(near_first[i - 2])
        stage_three(near_first[-1])
        for d in near_first[-2:]:
            normalise(d)
    else:
        stage_two(0)
        each(n_ep - 1, lambda i: stage_two(i + 1))
        each(n_ep, stage_three)
        each(n_ep, normalise)
    each(n_ep - 1, lambda i: route_wait(i + 1))

    many = min(rows_all, 128)
    batches = rows_all // many
    for load in loads[1:5]:
        load.wait()

    def hidden(b):
        rows = block(b, many)
        a = ffn[rows, :]
        for j in range(held):
            eh[j, rows, :] = (jax.nn.silu(dot(a, eg[j])) * dot(a, eu[j])).astype(BF16)
        units = jax.nn.silu(dot(a, dg[...])) * dot(a, du[...])
        if not split:
            own = hid // n_tp
            unit = lax.broadcasted_iota(jnp.int32, units.shape, 1)
            units = jnp.where((unit >= t * own) & (unit < (t + 1) * own), units, 0.0)
        dh[rows, :] = units.astype(BF16)

    each(batches, hidden)
    for load in loads[5:]:
        load.wait()

    def result(b, q):
        rows = block(b, many)
        cols = block(q, quarter)
        total = mix[rows, :1] * dot(dh[rows, :], dd[:, cols])
        lanes = lax.broadcasted_iota(jnp.int32, (many, route.shape[1]), 1)
        for j in range(held):
            weight = jnp.sum(
                jnp.where(lanes == e * held + j, route[rows, :], 0.0), axis=1, keepdims=True
            )
            piece = dot(eh[j, rows, :], ed[j, :, cols]).astype(BF16)
            total = total + weight * piece.astype(F32)
        return total

    def pair(j):
        return remote(away.at[j], came.at[j], pair_send.at[j], pair_recv.at[j], (e, mate))

    for j in range(half):

        def leave(b, j=j):
            away[j, block(b, many), :] = result(b, 2 * j + 1 - core).astype(BF16)

        each(batches, leave)
        pair(j).start()

    me = e * half + t // 2

    def back(j, d):
        there = (e + d) % n_ep
        return remote(
            summed.at[j, block(there, seqs), :],
            landed.at[me],
            back_send.at[j, d],
            back_recv.at[me],
            (there, 2 * j + core),
        )

    def same(j, d):
        return jnp.logical_and(jnp.asarray(d == 0), 2 * j + core == t)

    for j in range(half):

        def keep(b, j=j):
            summed[j, block(b, many), :] = result(b, 2 * j + core).astype(BF16)

        each(batches, keep)
    for j in range(half):
        pair(j).wait_recv()

        def add(b, j=j):
            rows = block(b, many)
            summed[j, rows, :] = (summed[j, rows, :].astype(F32) + came[j, rows, :].astype(F32)).astype(BF16)

        each(batches, add)

        def send(d, j=j):
            @pl.when(jnp.logical_not(same(j, d)))
            def _():
                back(j, d).start()

        each(n_ep, send, order=None if far_first is None else far_first + [0])

    landed[me] = summed[t // 2, own_rows, :]

    def take(index):
        @pl.when(index != me)
        def _():
            where = landed.at[index]
            remote(where, where, back_send.at[0, 0], back_recv.at[index], (e, t)).wait_recv()

    each(n_ep * half, take)
    out_ref[...] = own_stream.astype(F32) + jnp.sum(landed[...].astype(F32), axis=0)

    for mask in range(1, n_tp):
        heads_copy(mask).wait_send()
    each(n_ep - 1, lambda i: route_copy(i + 1).wait_send())
    each(n_ep - 1, lambda i: first(i + 1).wait_send())

    def sent(d):
        second(d, 1).wait_send()
        for mask in evens:
            second(d, mask).wait_send()
            relay(d, mask).wait_send()

    each(n_ep, sent)
    for j in range(half):
        pair(j).wait_send()

        def gone(d, j=j):
            @pl.when(jnp.logical_not(same(j, d)))
            def _():
                back(j, d).wait_send()

        each(n_ep, gone)


def keeps(plane):
    return (plane + 1) % CORES


def tells(planes, me, you):
    z, x, y, c = me
    level, inner, side, core = you
    other = (z != level) | (x != inner) | (y != side) | (c != core)
    column = (c == RELAY) & (x == inner) & (y == side)
    lane = (y == side) & (c == core)
    far = (z == 0) & (level == planes - 1) & (c == keeps(planes - 1))
    return other & ((z == level) | column | lane | far)


def near_kernel(
    n_ep,
    n_tp,
    lengths_hbm,
    lam_hbm,
    resid_hbm,
    first_gain_hbm,
    head_gain_hbm,
    gain_hbm,
    mixw_hbm,
    ids_hbm,
    rw_hbm,
    qw_hbm,
    kw_hbm,
    vw_hbm,
    cache_hbm,
    ow_hbm,
    eg_hbm,
    eu_hbm,
    ed_hbm,
    dg_hbm,
    du_hbm,
    dd_hbm,
    out_ref,
    new_ref,
    lengths_ref,
    lam_ref,
    resid_ref,
    first_gain_ref,
    head_gain_ref,
    gain_ref,
    mixw_ref,
    ids_ref,
    rw_ref,
    qkv,
    cache,
    pairs,
    asked,
    scores,
    mixed,
    heads_ref,
    ow,
    gu,
    ed,
    dg,
    du,
    dd,
    heads_all,
    mine,
    stream,
    ffn,
    route,
    eh,
    dh,
    leaving,
    kept,
    plane_in,
    column_out,
    column_in,
    local_sem,
    push_send,
    push_recv,
    route_send,
    route_recv,
    heads_send,
    heads_recv,
    chunk_send,
    climb_recv,
    group_recv,
    plane_recv,
    column_recv,
):
    e = lax.axis_index("ep")
    t = lax.axis_index("tp")
    planes = n_ep // INNER
    z = e // INNER
    x = e % INNER
    y = t // CORES
    c = t % CORES
    keeper = keeps(z)
    odd = (c + keeper) % CORES
    turns = planes // CORES
    seqs, width = resid_ref.shape
    quarter = out_ref.shape[1]
    part = eg_hbm.shape[2]
    hid = dg.shape[1]
    mate = flip(t, 1)

    def gather_loads(sem, *routes):
        return [pltpu.make_async_copy(src, dst, local_sem.at[sem]) for src, dst in routes]

    first_loads = gather_loads(
        0, (resid_hbm, resid_ref), (first_gain_hbm, first_gain_ref), (lengths_hbm, lengths_ref)
    )
    for load in first_loads:
        load.start()
    depth = qkv.shape[0] // Q_CHUNKS
    inner = qw_hbm.shape[1]
    side = kw_hbm.shape[1]
    for i in range(Q_CHUNKS):
        deep = pl.ds(i * depth, depth)
        for load in gather_loads(
            1 + i,
            (qw_hbm.at[deep, :], qkv.at[deep, :inner]),
            (kw_hbm.at[deep, :], qkv.at[deep, inner : inner + side]),
            (vw_hbm.at[deep, :], qkv.at[deep, inner + side :]),
        ):
            load.start()

    barrier = pltpu.get_barrier_semaphore()
    for index in range(n_ep * n_tp):
        there = (index // n_tp // INNER, index // n_tp % INNER, index % n_tp // CORES, index % CORES)

        @pl.when(tells(planes, (z, x, y, c), there))
        def _():
            pl.semaphore_signal(
                barrier, inc=1, device_id=(index // n_tp, index % n_tp), device_id_type=MESH
            )

    told = 0
    for level in range(planes):
        for core in range(CORES):
            count = sum(
                tells(planes, (i, j, k, m), (level, 0, 0, core))
                for i in range(planes)
                for j in range(INNER)
                for k in range(n_tp // CORES)
                for m in range(CORES)
            )
            told = jnp.where((z == level) & (c == core), count, told)

    for load in first_loads:
        load.wait()
    bunch = seqs // CACHE_CHUNKS
    cache_loads = [
        gather_loads(
            1 + Q_CHUNKS + i,
            (cache_hbm.at[pl.ds(i * bunch, bunch)], cache.at[pl.ds(i * bunch, bunch)]),
        )[0]
        for i in range(CACHE_CHUNKS)
    ]
    for load in cache_loads:
        load.start()
    late = 1 + Q_CHUNKS + CACHE_CHUNKS
    late_loads = gather_loads(
        late,
        (ids_hbm, ids_ref),
        (rw_hbm, rw_ref),
        (lam_hbm, lam_ref),
        (head_gain_hbm, head_gain_ref),
        (gain_hbm, gain_ref),
        (mixw_hbm, mixw_ref),
    )
    for load in late_loads:
        load.start()
    cols = block(y, hid)
    e_loads = gather_loads(
        late + 1, (eg_hbm.at[0], gu.at[c, :, :part]), (eu_hbm.at[0], gu.at[c, :, part:])
    ) + gather_loads(late + 2, (ed_hbm.at[0], ed.at[block(c, part), :]))
    loads = [
        gather_loads(1 + i, route)[0]
        for i, route in enumerate(
            (
                (ow_hbm, ow),
                (dg_hbm.at[:, cols], dg),
                (du_hbm.at[:, cols], du),
                (dd_hbm.at[cols, :], dd),
            )
        )
    ]
    resid = resid_ref[...].astype(F32)
    mean_sq = jnp.mean(resid * resid, axis=-1, keepdims=True)
    normed = (resid * lax.rsqrt(mean_sq + EPS) * first_gain_ref[...]).astype(BF16)
    row = lax.broadcasted_iota(jnp.int32, (seqs, LANES), 0)
    entry = lax.broadcasted_iota(jnp.int32, (seqs, LANES), 1) % QK_DIM
    position = jnp.zeros((seqs, LANES), F32)
    for s in range(seqs):
        position = jnp.where(row == s, lengths_ref[s].astype(F32), position)
    turn = QK_DIM // 2
    power = (entry % turn).astype(F32) * (-1.0 / turn)
    angle = position * jnp.exp(power * math.log(10000.0))
    cosine = jnp.cos(angle)
    sine = jnp.where(entry < turn, -jnp.sin(angle), jnp.sin(angle))

    def rotate(values):
        other = jnp.where(
            entry < turn, pltpu.roll(values, LANES - turn, 1), pltpu.roll(values, turn, 1)
        )
        return (values * cosine + other * sine).astype(BF16).astype(F32)

    def spot(plane, inner):
        return plane // CORES * INNER + inner

    own_spot = spot(z, x)
    projected = jnp.zeros((seqs, qkv.shape[1]), F32)
    for i in range(Q_CHUNKS):
        deep = pl.ds(i * depth, depth)
        pltpu.make_async_copy(qkv.at[deep, :], qkv.at[deep, :], local_sem.at[1 + i]).wait()
        projected = projected + dot(normed[:, i * depth : (i + 1) * depth], qkv[deep, :])
    query = projected[:, :inner]
    keys_raw = projected[:, inner : inner + side]
    values_raw = projected[:, inner + side :]
    for load in e_loads + loads:
        load.start()

    groups, spots = cache.shape[1], cache.shape[2]
    share = query.shape[1] // LANES // groups
    scale = QK_DIM**-0.5
    lines = 2 * share
    lower = lax.broadcasted_iota(jnp.int32, (seqs, LANES), 1) < QK_DIM
    fresh = []
    for g in range(groups):
        key = rotate(keys_raw[:, g * LANES : (g + 1) * LANES])
        value = values_raw[:, g * LANES : (g + 1) * LANES].astype(BF16).astype(F32)
        new_ref[:, 2 * g * LANES : (2 * g + 1) * LANES] = key.astype(BF16)
        new_ref[:, (2 * g + 1) * LANES : (2 * g + 2) * LANES] = value.astype(BF16)
        fresh.append((key, value))
        for j in range(share):
            at = (g * share + j) * LANES
            head = rotate(query[:, at : at + LANES])
            pairs[g, :, j, :] = jnp.where(lower, head, 0.0)
            pairs[g, :, share + j, :] = jnp.where(lower, 0.0, head)
        spread = (pairs[g] * scale).reshape(seqs * lines, LANES).astype(BF16)
        turn_of = lax.broadcasted_iota(jnp.int32, spread.shape, 0) // lines % 2
        asked[g, :, :LANES] = jnp.where(turn_of == 0, spread, jnp.zeros_like(spread))
        asked[g, :, LANES:] = jnp.where(turn_of == 0, jnp.zeros_like(spread), spread)

    def push(index):
        where = (gu.at[c], ed.at[block(c, part), :])[index]
        return remote(where, where, push_send.at[0], push_recv.at[index], (e, mate))

    def pushed(index):
        where = (gu.at[1 - c], ed.at[block(1 - c, part), :])[index]
        remote(where, where, push_send.at[0], push_recv.at[index], (e, mate)).wait_recv()

    def beside(s, g, lanes):
        return jnp.concatenate([cache[s, g, :, lanes], cache[s + 1, g, :, lanes]], axis=1)

    place = lax.broadcasted_iota(jnp.int32, (bunch, lines, spots), 2)
    line = lax.broadcasted_iota(jnp.int32, (lines, 1), 0)

    def score(start):
        for s in range(start, start + bunch, 2):
            for g in range(groups):
                scores[g, s : s + 2] = lax.dot_general(
                    asked[g, s * lines : (s + 2) * lines, :],
                    beside(s, g, slice(0, LANES)),
                    (((1,), (1,)), ((), ())),
                    preferred_element_type=F32,
                ).reshape(2, lines, spots)

    def attend(start):
        stop = start + bunch
        length = jnp.zeros((bunch, lines, 1), jnp.int32)
        which = lax.broadcasted_iota(jnp.int32, (bunch, lines, 1), 0)
        for s in range(bunch):
            length = jnp.where(which == s, lengths_ref[start + s], length)
        valid = place < length
        for g in range(groups):
            key, value = (half[start:stop] for half in fresh[g])
            latest = jnp.sum(pairs[g, start:stop] * key[:, None, :], axis=-1, keepdims=True) * scale
            masked = jnp.where(valid, scores[g, start:stop], -jnp.inf)
            top = jnp.maximum(jnp.max(masked, axis=-1, keepdims=True), latest)
            raised = jnp.exp(masked - top)
            raised_new = jnp.exp(latest - top)
            total = jnp.sum(raised, axis=-1, keepdims=True) + raised_new
            lam = jnp.full((lines, 1), 1.0, F32)
            for j in range(share):
                lam = jnp.where(line == share + j, lam_ref[g * share + j], lam)
            part_of = lam[None] / total
            prob = raised * part_of
            prob_new = jnp.broadcast_to(raised_new * part_of, (bunch, lines, LANES))
            weights = (prob - pltpu.roll(prob, share, 1)).astype(BF16)
            new_weight = (
                (prob_new - pltpu.roll(prob_new, share, 1)).astype(BF16).astype(F32)
            )
            fresh_part = new_weight * value[:, None, :]
            for s in range(0, bunch, 2):
                both = dot(
                    weights[s : s + 2].reshape(2 * lines, spots),
                    beside(start + s, g, slice(LANES, None)),
                )
                mixed[g, start + s] = both[:lines, :LANES]
                mixed[g, start + s + 1] = both[lines:, LANES:]
            whole = mixed[g, start:stop] + fresh_part
            mean_sq = jnp.mean(whole * whole, axis=-1, keepdims=True)
            mixed[g, start:stop] = whole * lax.rsqrt(mean_sq + EPS) * head_gain_ref[...][None]

    for i in range(CACHE_CHUNKS):
        if i == CACHE_CHUNKS - 1:
            for load in late_loads:
                load.wait()
        cache_loads[i].wait()
        score(i * bunch)
        if i == CACHE_CHUNKS - 1:
            for k in range(CACHE_CHUNKS):
                attend(k * bunch)
    for g in range(groups):
        for j in range(share):
            at = (g * share + j) * LANES
            heads_ref[:, at : at + LANES] = mixed[g, :, j, :].astype(BF16)

    def heads_copy(mask):
        return remote(
            heads_ref,
            heads_all.at[mask - 1],
            heads_send.at[0],
            heads_recv.at[mask // CORES],
            (e, flip(t, mask)),
        )

    pl.semaphore_wait(barrier, told)
    for core in range(CORES):
        skew = (c + core) % CORES
        remote(
            heads_ref,
            heads_all.at[CORES - 1 + skew],
            heads_send.at[0],
            heads_recv.at[1],
            (e, flip(y, 1) * CORES + core),
        ).start()
    heads_copy(1).start()


    lane = lax.broadcasted_iota(jnp.int32, (seqs, route.shape[2]), 1)
    table = jnp.zeros((seqs, route.shape[2]), F32)
    for k in range(ids_ref.shape[0]):
        wanted = column(ids_ref[k : k + 1, :])
        table = table + jnp.where(lane == wanted, column(rw_ref[k : k + 1, :]), 0.0)

    @pl.when(odd == 0)
    def _():
        route[own_spot] = table

    def route_copy(mask):
        where = route.at[own_spot]
        return remote(
            where, where, route_send.at[0], route_recv.at[0], (flip(e, mask), t)
        )

    @pl.when(odd == 0)
    def _():
        for mask in range(1, n_ep):
            route_copy(mask).start()


    loads[0].wait()
    span = heads_ref.shape[1]
    total = dot(heads_ref[...], ow[block(t, span), :])
    for far in range(n_tp // CORES):
        batch = heads_all.at[pl.ds(0, 1) if far == 0 else pl.ds(far * CORES - 1, CORES)]
        remote(batch, batch, heads_send.at[0], heads_recv.at[far], (e, t)).wait_recv()
        for mask in range(max(far * CORES, 1), (far + 1) * CORES):
            total = total + dot(heads_all[mask - 1], ow[block(flip(t, mask), span), :])
    own_cols = block(t, quarter)
    own_stream = (resid_ref[:, own_cols].astype(F32) + total).astype(BF16)
    mine[...] = own_stream

    around = ((1, 1), (1, 0), (0, 1))
    last = turns - 1
    edge = jnp.logical_or(z == 0, z == planes - 1)
    far = jnp.logical_and(edge, odd == 1)

    def chunk(group, owner):
        return stream.at[block(group, seqs), block(owner, quarter)]

    def to_plane(step):
        dx, dy = around[step]
        there = (z * INNER + flip(x, dx), flip(y, dy) * CORES + keeper)
        return remote(
            mine, chunk(e, t), chunk_send.at[0], group_recv.at[z // CORES, dx], there
        )

    def to_column(d):
        core = jnp.where(z == planes - 1, keeper, RELAY) if d == planes - 1 else RELAY
        there = (flip(z, d) * INNER + x, y * CORES + core)
        return remote(mine, chunk(e, t), chunk_send.at[0], climb_recv.at[z, c], there)

    def to_mate():
        return remote(mine, chunk(e, t), chunk_send.at[0], climb_recv.at[z, c], (e, mate))

    def to_far(step):
        dx, dy = around[step]
        there = (flip(z, planes - 1) * INNER + flip(x, dx), flip(y, dy) * CORES + keeper)
        return remote(
            mine, chunk(e, t), chunk_send.at[0], group_recv.at[z // CORES, dx], there
        )

    for d in range(planes - 2, 0, -1):
        to_column(d).start()

    @pl.when(z == planes - 1)
    def _():
        for step in range(len(around)):
            to_far(step).start()

    to_column(planes - 1).start()
    for step in range(len(around)):
        to_plane(step).start()

    @pl.when(odd == 1)
    def _():
        to_mate().start()

    @pl.when(odd == 0)
    def _():
        stream[block(e, seqs), own_cols] = own_stream

    for load in e_loads:
        load.wait()
    push(0).start()
    push(1).start()

    near = z + odd * (1 - 2 * (z % 2))

    def plane_of(i):
        return flip(near, 2 * i)

    def arrived(plane, core):
        where = chunk(plane * INNER + x, y * CORES + core)
        remote(where, where, chunk_send.at[0], climb_recv.at[plane, core], (e, t)).wait_recv()

    def forward(plane, core, step):
        dx, dy = around[step]
        where = chunk(plane * INNER + x, y * CORES + core)
        return remote(
            where,
            where,
            chunk_send.at[0],
            group_recv.at[plane // CORES, dx],
            (z * INNER + flip(x, dx), flip(y, dy) * CORES + keeps(plane)),
        )

    def hand_over(plane, core):
        where = chunk(plane * INNER + x, y * CORES + core)
        return remote(where, where, chunk_send.at[0], climb_recv.at[plane, core], (e, mate))

    @pl.when(c == RELAY)
    def _():
        for plane in sorted(range(planes), key=lambda plane: keeps(plane) != RELAY):
            passes = plane != z
            if plane == planes - 1:
                passes = jnp.logical_and(passes, z != 0)

            @pl.when(passes)
            def _(plane=plane):
                for core in (RELAY, 1 - RELAY):
                    arrived(plane, core)
                    for step in range(len(around)):
                        forward(plane, core, step).start()
                    if keeps(plane) != RELAY:
                        hand_over(plane, core).start()

    def normalise(i):
        plane = CORES * i + keeps(c)

        @pl.when(plane == z)
        def _():
            arrived(plane, 1 - c)

        leapt = jnp.logical_and(plane == planes - 1, z == 0)

        @pl.when(jnp.logical_and(plane != z, jnp.logical_or(c != RELAY, leapt)))
        def _():
            for core in range(CORES):
                arrived(plane, core)

        for inner in range(INNER):
            group = plane * INNER + flip(x, inner)
            came = stream.at[
                block(group, seqs),
                pl.ds(0, width) if inner else block(flip(y, 1), CORES * quarter),
            ]
            remote(
                came, came, chunk_send.at[0], group_recv.at[plane // CORES, inner], (e, t)
            ).wait_recv()
            values = stream[block(group, seqs), :].astype(F32)
            mean_sq = jnp.mean(values * values, axis=-1, keepdims=True)
            scaled = (values * lax.rsqrt(mean_sq + EPS) * gain_ref[...]).astype(BF16)
            ffn[block(spot(plane, flip(x, inner)), seqs), :] = scaled

    for i in range(turns):
        normalise(i)

    def route_wait(count):
        where = route.at[pl.ds(0, count)]
        remote(where, where, route_send.at[0], route_recv.at[0], (e, t)).wait_recv()

    @pl.when(odd == 0)
    def _():
        route_wait(route.shape[0] - 1)

    @pl.when(odd == 1)
    def _():
        route_wait(route.shape[0])

    rows_all = ffn.shape[0]
    pushed(0)
    pushed(1)
    for load in loads[1:]:
        load.wait()
    a = ffn[...]
    for core in range(CORES):
        both = dot(a, gu[core])
        eh[:, core * part : (core + 1) * part] = (
            jax.nn.silu(both[:, :part]) * both[:, part:]
        ).astype(BF16)
    for at in range(0, hid, 2 * LANES):
        piece = slice(at, at + 2 * LANES)
        dh[:, piece] = (jax.nn.silu(dot(a, dg[:, piece])) * dot(a, du[:, piece])).astype(BF16)
    blend = jax.nn.sigmoid(jnp.sum(a.astype(F32) * mixw_ref[...], axis=-1, keepdims=True))
    lanes = lax.broadcasted_iota(jnp.int32, (rows_all, route.shape[2]), 1)
    weight = jnp.sum(
        jnp.where(lanes == e, route[...].reshape(rows_all, route.shape[2]), 0.0),
        axis=1,
        keepdims=True,
    )
    half = CORES * quarter
    def project(dy):
        cols = block(flip(y, dy), half)
        sparse = weight * dot(eh[...], ed[:, cols])
        return sparse + blend * dot(dh[...], dd[:, cols])

    leaving[1] = project(1).astype(BF16)

    def own_plane(i):
        return jnp.logical_and(odd == 0, i == 0)

    def leave(i, core, step):
        dx, dy = around[step]
        where = spot(plane_of(i), flip(x, dx))
        summer = jnp.where(own_plane(i), c, RELAY)
        return remote(
            leaving.at[dy, block(where, seqs), pl.ds(core * quarter, quarter)],
            plane_in.at[c, i, core, step],
            chunk_send.at[0],
            plane_recv.at[c, i, core],
            (z * INNER + flip(x, dx), flip(y, dy) * CORES + summer),
        )

    def pass_over(i, core):
        where = spot(plane_of(i), x)
        return remote(
            leaving.at[0, block(where, seqs), pl.ds(core * quarter, quarter)],
            plane_in.at[c, i, core, len(around)],
            chunk_send.at[0],
            plane_recv.at[c, i, core],
            (e, mate),
        )

    def leap(core, step):
        dx, dy = around[step] if step < len(around) else (0, 0)
        where = spot(plane_of(last), flip(x, dx))
        return remote(
            leaving.at[dy, block(where, seqs), pl.ds(core * quarter, quarter)],
            column_in.at[planes - 1 + (step + 1) % (len(around) + 1)],
            chunk_send.at[0],
            column_recv.at[0],
            (plane_of(last) * INNER + flip(x, dx), flip(y, dy) * CORES + core),
        )

    order = range(turns - 1, -1, -1)
    for dy in (1, 0):
        if not dy:
            total = project(0)
            leaving[0] = total.astype(BF16)
            kept[...] = total
        steps = [step for step in range(len(around)) if around[step][1] == dy]

        @pl.when(far)
        def _():
            for step in steps + [len(around)] * (1 - dy):
                for core in range(CORES):
                    leap(core, step).start()

        for i in order:

            def depart(i=i):
                for core in range(CORES):
                    for step in steps:
                        leave(i, core, step).start()
                if not dy:

                    @pl.when(jnp.logical_and(c != RELAY, jnp.logical_not(own_plane(i))))
                    def _():
                        for core in range(CORES):
                            pass_over(i, core).start()

            if i == last:
                pl.when(jnp.logical_not(far))(depart)
            else:
                depart()

    def climb(lane, i, core):
        skew = (lane + keeper) % CORES
        level = flip(z + skew * (1 - 2 * (z % 2)), 2 * i)
        return remote(
            column_out.at[lane, i, core],
            column_in.at[skew + 2 * i],
            chunk_send.at[0],
            column_recv.at[0],
            (level * INNER + x, y * CORES + core),
        )

    def stays(i, core):
        return jnp.logical_and(own_plane(i), c == core)

    def rise(i):
        for core in range(CORES):
            gathered = kept[block(spot(plane_of(i), x), seqs), core * quarter : (core + 1) * quarter]
            came = plane_in.at[c, i, core, pl.ds(0, len(around))]
            remote(came, came, chunk_send.at[0], plane_recv.at[c, i, core], (e, t)).wait_recv()
            for step in range(len(around)):
                gathered = gathered + plane_in[c, i, core, step].astype(F32)
            column_out[c, i, core] = gathered.astype(BF16)

            @pl.when(jnp.logical_not(stays(i, core)))
            def _(i=i, core=core):
                climb(c, i, core).start()

    low = 1 - RELAY

    def lift(i):
        for core in range(CORES):
            came = plane_in.at[low, i, core]
            remote(came, came, chunk_send.at[0], plane_recv.at[low, i, core], (e, t)).wait_recv()
            gathered = plane_in[low, i, core, 0].astype(F32)
            for step in range(1, len(around) + 1):
                gathered = gathered + plane_in[low, i, core, step].astype(F32)
            column_out[low, i, core] = gathered.astype(BF16)
            climb(low, i, core).start()

    for i in order:
        sums = jnp.logical_or(c == RELAY, own_plane(i))
        if i == last:
            sums = jnp.logical_and(sums, jnp.logical_not(far))

        @pl.when(sums)
        def _(i=i):
            rise(i)

    slant = (low + keeper) % CORES == 1
    for i in order:
        theirs = c == RELAY
        if i == 0:
            theirs = jnp.logical_and(theirs, slant)
        if i == last:
            theirs = jnp.logical_and(theirs, jnp.logical_not(jnp.logical_and(edge, slant)))

        @pl.when(theirs)
        def _(i=i):
            lift(i)

    def took(start, stop):
        where = column_in.at[pl.ds(start, stop - start)]
        remote(where, where, chunk_send.at[0], column_recv.at[0], (e, t)).wait_recv()

    @pl.when(odd == 0)
    def _():
        column_in[0] = column_out[c, 0, c]

    def finish(stop):
        for parity in range(2):

            @pl.when(odd == parity)
            def _(parity=parity):
                took(1 - parity, stop)

        out_ref[...] = (
            own_stream.astype(F32) + jnp.sum(column_in[:stop].astype(F32), axis=0)
        ).astype(BF16)

    @pl.when(edge)
    def _():
        finish(planes + len(around))

    @pl.when(jnp.logical_not(edge))
    def _():
        finish(planes)

    push(0).wait_send()
    push(1).wait_send()
    remote(heads_all, heads_all, heads_send.at[0], heads_recv.at[0], (e, t)).wait_send()

    def drained(count):
        where = ow.at[pl.ds(0, count * seqs), :]
        remote(where, where, chunk_send.at[0], column_recv.at[0], (e, t)).wait_send()

    hops = len(around)
    @pl.when(odd == 0)
    def _():
        for mask in range(1, n_ep):
            route_copy(mask).wait_send()

    for level in range(planes):
        for core in range(CORES):
            count = planes - 1 + hops + turns * CORES * (hops + 1)
            count += hops if level == planes - 1 else 0
            count += 1 if core != keeps(level) else -1
            if core == RELAY:
                skew = (1 - RELAY + keeps(level)) % CORES
                lower = [level ^ skew ^ (CORES * i) for i in range(turns)]
                count += CORES * sum(
                    plane != level and abs(plane - level) != planes - 1 for plane in lower
                )
            for plane in range(planes) if core == RELAY else ():
                if plane != level and plane - level != planes - 1:
                    count += CORES * (hops + (keeps(plane) != RELAY))

            @pl.when(jnp.logical_and(z == level, c == core))
            def _(count=count):
                drained(count)


def settle(layer_ref, fresh_ref, layer_out, fresh_out, sem):
    first = pltpu.make_async_copy(layer_ref, layer_out, sem.at[0])
    second = pltpu.make_async_copy(fresh_ref, fresh_out, sem.at[1])
    first.start()
    second.start()
    first.wait()
    second.wait()


def near_call(n_ep, n_tp, arrays):
    (
        residual_in,
        lengths,
        kv_cache,
        norm_gain_attn,
        query_weight,
        key_weight,
        value_weight,
        diff_lambda,
        head_gain,
        out_weight,
        norm_gain_ffn,
        route_ids,
        route_weights,
        expert_gate,
        expert_up,
        expert_down,
        dense_gate,
        dense_up,
        dense_down,
        dense_mix,
    ) = arrays
    seqs, width = residual_in.shape
    held = lambda value: pltpu.with_memory_space_constraint(value, pltpu.HBM)
    groups, spots = kv_cache.shape[1:3]
    share = diff_lambda.shape[0] // groups
    inner = query_weight.shape[1]
    quarter = out_weight.shape[1]
    part = expert_gate.shape[2]
    hid = dense_gate.shape[1] // (n_tp // CORES)
    turns = n_ep // INNER // CORES
    blocks = turns * INNER
    rows = blocks * seqs
    lanes = -(-n_ep // LANES) * LANES
    topk = route_ids.shape[1]
    vmem = pl.BlockSpec(memory_space=pltpu.VMEM)
    hbm = pl.BlockSpec(memory_space=pltpu.HBM)
    dma = pltpu.SemaphoreType.DMA
    layer_out, fresh = pl.pallas_call(
        functools.partial(near_kernel, n_ep, n_tp),
        out_shape=(
            jax.ShapeDtypeStruct((seqs, quarter), BF16),
            jax.ShapeDtypeStruct((seqs, groups * kv_cache.shape[3]), BF16),
        ),
        in_specs=[hbm] * 20,
        out_specs=(vmem, vmem),
        scratch_shapes=[
            pltpu.SMEM(lengths.shape, jnp.int32),
            pltpu.SMEM(diff_lambda.shape, F32),
            pltpu.VMEM(residual_in.shape, BF16),
            pltpu.VMEM((1, width), F32),
            pltpu.VMEM((1, head_gain.shape[0]), F32),
            pltpu.VMEM((1, width), F32),
            pltpu.VMEM((1, width), F32),
            pltpu.VMEM((topk, seqs), jnp.int32),
            pltpu.VMEM((topk, seqs), F32),
            pltpu.VMEM((width, inner + key_weight.shape[1] + value_weight.shape[1]), BF16),
            pltpu.VMEM(kv_cache.shape, BF16),
            pltpu.VMEM((groups, seqs, 2 * share, LANES), F32),
            pltpu.VMEM((groups, seqs * 2 * share, 2 * LANES), BF16),
            pltpu.VMEM((groups, seqs, 2 * share, spots), F32),
            pltpu.VMEM((groups, seqs, 2 * share, LANES), F32),
            pltpu.VMEM((seqs, inner), BF16),
            pltpu.VMEM(out_weight.shape, BF16),
            pltpu.VMEM((CORES, width, 2 * part), BF16),
            pltpu.VMEM((CORES * part, width), BF16),
            pltpu.VMEM((width, hid), BF16),
            pltpu.VMEM((width, hid), BF16),
            pltpu.VMEM((hid, width), BF16),
            pltpu.VMEM((n_tp - 1, seqs, inner), BF16),
            pltpu.VMEM((seqs, quarter), BF16),
            pltpu.VMEM((n_ep * seqs, width), BF16),
            pltpu.VMEM((rows, width), BF16),
            pltpu.VMEM((blocks, seqs, lanes), F32),
            pltpu.VMEM((rows, CORES * part), BF16),
            pltpu.VMEM((rows, hid), BF16),
            pltpu.VMEM((2, rows, CORES * quarter), BF16),
            pltpu.VMEM((rows, CORES * quarter), F32),
            pltpu.VMEM((CORES, turns, CORES, 4, seqs, quarter), BF16),
            pltpu.VMEM((CORES, turns, CORES, seqs, quarter), BF16),
            pltpu.VMEM((n_ep // INNER + 3, seqs, quarter), BF16),
            dma((Q_CHUNKS + CACHE_CHUNKS + 4,)),
            dma((1,)),
            dma((2,)),
            dma((1,)),
            dma((1,)),
            dma((1,)),
            dma((n_tp // CORES,)),
            dma((1,)),
            dma((n_ep // INNER, CORES)),
            dma((turns, INNER)),
            dma((CORES, turns, CORES)),
            dma((1,)),
        ],
        compiler_params=pltpu.CompilerParams(
            collective_id=0, has_side_effects=True, vmem_limit_bytes=36 * 1024 * 1024
        ),
    )(
        held(lengths),
        held(diff_lambda),
        held(residual_in),
        held(norm_gain_attn[None, :]),
        held(head_gain[None, :]),
        held(norm_gain_ffn[None, :]),
        held(dense_mix[None, :]),
        held(route_ids.T),
        held(route_weights.T),
        held(query_weight),
        held(key_weight),
        held(value_weight),
        held(kv_cache),
        held(out_weight),
        held(expert_gate),
        held(expert_up),
        held(expert_down),
        held(dense_gate),
        held(dense_up),
        held(dense_down),
    )
    layer_out, fresh = pl.pallas_call(
        settle,
        out_shape=(
            jax.ShapeDtypeStruct(layer_out.shape, BF16),
            jax.ShapeDtypeStruct(fresh.shape, BF16),
        ),
        in_specs=[vmem, vmem],
        out_specs=(hbm, hbm),
        scratch_shapes=[dma((2,))],
        compiler_params=pltpu.CompilerParams(vmem_limit_bytes=1024 * 1024),
    )(layer_out, fresh)
    return layer_out, fresh.reshape(seqs, groups, kv_cache.shape[3])


def on_device(
    residual_in,
    lengths,
    kv_cache,
    norm_gain_attn,
    query_weight,
    key_weight,
    value_weight,
    diff_lambda,
    head_gain,
    out_weight,
    norm_gain_ffn,
    route_ids,
    route_weights,
    expert_gate,
    expert_up,
    expert_down,
    dense_gate,
    dense_up,
    dense_down,
    dense_mix,
):
    n_ep = lax.axis_size("ep")
    n_tp = lax.axis_size("tp")
    half = n_tp // 2
    if (
        n_tp == 2 * CORES
        and n_ep in (4, 8, 16)
        and expert_gate.shape[0] == 1
        and dense_gate.shape[1] // half % LANES == 0
        and expert_gate.shape[2] % LANES == 0
    ):
        return near_call(
            n_ep,
            n_tp,
            (
                residual_in,
                lengths,
                kv_cache,
                norm_gain_attn,
                query_weight,
                key_weight,
                value_weight,
                diff_lambda,
                head_gain,
                out_weight,
                norm_gain_ffn,
                route_ids,
                route_weights,
                expert_gate,
                expert_up,
                expert_down,
                dense_gate,
                dense_up,
                dense_down,
                dense_mix,
            ),
        )
    seqs, width = residual_in.shape
    groups, spots = kv_cache.shape[1:3]
    share = diff_lambda.shape[0] // groups
    inner = query_weight.shape[1]
    quarter = out_weight.shape[1]
    held, _, part = expert_gate.shape
    rows = n_ep * seqs
    own = dense_gate.shape[1] // n_tp
    split = own % LANES == 0
    hid = own if split else dense_gate.shape[1]
    lanes = -(-n_ep * held // LANES) * LANES
    vmem = pl.BlockSpec(memory_space=pltpu.VMEM)
    smem = pl.BlockSpec(memory_space=pltpu.SMEM)
    hbm = pl.BlockSpec(memory_space=pl.ANY)
    dma = pltpu.SemaphoreType.DMA
    layer_out, fresh = pl.pallas_call(
        functools.partial(layer_kernel, n_ep, n_tp, split),
        out_shape=(
            jax.ShapeDtypeStruct((seqs, quarter), F32),
            jax.ShapeDtypeStruct((seqs, groups * kv_cache.shape[3]), F32),
        ),
        in_specs=[smem] * 2 + [vmem] * 7 + [hbm] * 11,
        out_specs=(vmem, vmem),
        scratch_shapes=[
            pltpu.VMEM(query_weight.shape, BF16),
            pltpu.VMEM(key_weight.shape, BF16),
            pltpu.VMEM(value_weight.shape, BF16),
            pltpu.VMEM(kv_cache.shape, BF16),
            pltpu.VMEM((groups, seqs, 2 * share, LANES), F32),
            pltpu.VMEM((groups, seqs, 2 * share, spots), F32),
            pltpu.VMEM((groups, seqs, 2 * share, LANES), F32),
            pltpu.VMEM((seqs, inner), BF16),
            pltpu.VMEM(out_weight.shape, BF16),
            pltpu.VMEM(expert_gate.shape, BF16),
            pltpu.VMEM(expert_up.shape, BF16),
            pltpu.VMEM(expert_down.shape, BF16),
            pltpu.VMEM((width, hid), BF16),
            pltpu.VMEM((width, hid), BF16),
            pltpu.VMEM((hid, width), BF16),
            pltpu.VMEM((n_tp - 1, seqs, inner), BF16),
            pltpu.VMEM((rows, width), BF16),
            pltpu.VMEM((rows, width), BF16),
            pltpu.VMEM((rows, LANES), F32),
            pltpu.VMEM((rows, lanes), F32),
            pltpu.VMEM((held, rows, part), BF16),
            pltpu.VMEM((rows, hid), BF16),
            pltpu.VMEM((half, rows, quarter), BF16),
            pltpu.VMEM((half, rows, quarter), BF16),
            pltpu.VMEM((half, rows, quarter), BF16),
            pltpu.VMEM((n_ep * half, seqs, quarter), BF16),
            dma((7,)),
            dma((Q_CHUNKS + 2,)),
            dma((seqs,)),
            dma((n_ep - 1,)),
            dma((n_ep - 1,)),
            dma((n_tp - 1,)),
            dma((n_tp - 1,)),
            dma((n_ep,)),
            dma((half, n_ep)),
            dma((max(half - 1, 1), n_ep)),
            dma((n_tp, n_ep)),
            dma((half,)),
            dma((half,)),
            dma((half, n_ep)),
            dma((n_ep * half,)),
        ],
        compiler_params=pltpu.CompilerParams(
            collective_id=0, has_side_effects=True, vmem_limit_bytes=60 * 1024 * 1024
        ),
    )(
        lengths,
        diff_lambda,
        residual_in,
        norm_gain_attn[None, :],
        head_gain[None, :],
        norm_gain_ffn[None, :],
        dense_mix[None, :],
        route_ids.T,
        route_weights.T,
        query_weight,
        key_weight,
        value_weight,
        kv_cache,
        out_weight,
        expert_gate,
        expert_up,
        expert_down,
        dense_gate,
        dense_up,
        dense_down,
    )
    new_rows = fresh.astype(BF16).reshape(seqs, groups, kv_cache.shape[3])
    return (layer_out.astype(BF16), new_rows)


def solution(mesh):
    placed = (
        P("ep", None),
        P("ep"),
        P("ep", "tp", None, None),
        P(),
        P(None, "tp"),
        P(None, "tp"),
        P(None, "tp"),
        P("tp"),
        P(),
        P(None, "tp"),
        P(),
        P("ep", None),
        P("ep", None),
        P("ep", None, "tp"),
        P("ep", None, "tp"),
        P("ep", "tp", None),
        P(None, "ep"),
        P(None, "ep"),
        P("ep", None),
        P(),
    )
    return jax.shard_map(
        on_device,
        mesh=mesh,
        in_specs=placed,
        out_specs=(P("ep", "tp"), P("ep", "tp", None)),
        check_vma=False,
    )
```
